128 devices in a mesh: sp: 32 (over z, y, core), tp: 4 (over x).
Axes of the slice: x: 4, y: 4, z: 4, core: 2. Of those that a mesh axis runs over, the one named last changes fastest.
Arguments:
- input_activations: bfloat16 [32768, 2048], P(('sp', 'tp')), may hold values from -6 to 6
- norm_gain: float32 [2048], replicated, may hold values from 0.5 to 1.5
- w_gate: bfloat16 [2048, 2048], P('sp', 'tp'), may hold values from -0.125 to 0.125
- w_value: bfloat16 [2048, 2048], P('sp', 'tp'), may hold values from -0.125 to 0.125
- w_state_in: bfloat16 [2048, 1024], P('sp', 'tp'), may hold values from -0.125 to 0.125
- w_state_out: bfloat16 [2048, 1024], P('sp', 'tp'), may hold values from -0.125 to 0.125
- w_step_forward: bfloat16 [2048, 32], P('sp', 'tp'), may hold values from -0.03125 to 0.03125
- w_step_backward: bfloat16 [2048, 32], P('sp', 'tp'), may hold values from -0.03125 to 0.03125
- step_offset: float32 [2, 32], P(None, 'tp'), may hold values from -0.5 to 0.5
- fading_speed: float32 [2, 32], P(None, 'tp'), may hold values from 0.3 to 1
- conv_value: float32 [3, 2048], P(None, 'tp'), may hold values from -3.5 to 3.5
- conv_state_in: float32 [3, 1024], P(None, 'tp'), may hold values from -3.5 to 3.5
- conv_state_out: float32 [3, 1024], P(None, 'tp'), may hold values from -3.5 to 3.5
- out_gain: float32 [2048], P('tp'), may hold values from 0.5 to 1.5
- w_out: bfloat16 [2048, 2048], P('tp', 'sp'), may hold values from -0.125 to 0.125
Outputs:
- mixer_out: bfloat16 [32768, 2048], P(('sp', 'tp'))
The draws below stay inside these ranges and needn't reach their ends.
All inputs are finite; a program needn't handle non-finite values.
Results may differ from the reference program's by a relative error of at most 0.015.
Values may be sent and summed in bfloat16 or wider, within the bound.
A program may use at most 128 MiB of HBM per device.

```python
import math
import jax
import jax.numpy as jnp
from jax import lax

D = 2048
HEADS = 32
HEAD_DIM = 64
GROUPS = 8
STATE = 128
BLOCK = 128
WIDTH = 2048
SEQ = 32768


def block_levels(rng, dims, split, low, high):
    gain, own = 1.0, jax.random.fold_in(rng, 6)
    for axis_at, shards_of in split:
        heights = jnp.exp(jax.random.uniform(jax.random.fold_in(own, axis_at), (shards_of,), jnp.float32, low / len(split), high / len(split)))
        gain = gain * jnp.repeat(heights, dims[axis_at] // shards_of).reshape([-1 if axis == axis_at else 1 for axis in range(len(dims))])
    return gain


def gaussian(rng, extent, spread, bound, shards=(), dtype=jnp.bfloat16):
    drawn = jax.random.normal(rng, extent, jnp.float32) * spread
    if len(shards) > 0:
        drawn = block_levels(rng, extent, shards, -0.22, 0.18) * drawn
    return jnp.clip(drawn, min=-bound, max=bound).astype(dtype)


def setup_inputs(seed: int = 0) -> dict:
    key_list = jax.random.split(jax.random.key(seed), 16)
    return {
        "input_activations": gaussian(key_list[0], (SEQ, D), 1.0, 6.0, ((0, 128),)),
        "norm_gain": jnp.clip(1.0 + 0.1 * jax.random.normal(key_list[1], (D,), jnp.float32), 0.5, 1.5),
        "w_gate": gaussian(key_list[2], (D, WIDTH), D ** -0.5, 0.125, ((0, 32), (1, 4))),
        "w_value": gaussian(key_list[3], (D, WIDTH), D ** -0.5, 0.125, ((0, 32), (1, 4))),
        "w_state_in": gaussian(key_list[4], (D, GROUPS * STATE), D ** -0.5, 0.125, ((0, 32), (1, 4))),
        "w_state_out": gaussian(key_list[5], (D, GROUPS * STATE), D ** -0.5, 0.125, ((0, 32), (1, 4))),
        "w_step_forward": gaussian(key_list[6], (D, HEADS), (16 * D) ** -0.5, 0.03125, ((0, 32), (1, 4))),
        "w_step_backward": gaussian(key_list[7], (D, HEADS), (16 * D) ** -0.5, 0.03125, ((0, 32), (1, 4))),
        "step_offset": jnp.clip(jax.random.uniform(key_list[8], (2, HEADS), jnp.float32, -0.5, 0.5) * block_levels(key_list[8], (2, HEADS), ((1, 4),), -0.4, 0.0), -0.5, 0.5),
        "fading_speed": jnp.clip(jnp.exp(math.log(1.0) - 1.2039728 * jax.random.uniform(key_list[9], (2, HEADS), jnp.float32) ** block_levels(key_list[9], (2, HEADS), ((1, 4),), -0.2, 0.2)), 0.3, 1.0),
        "conv_value": gaussian(key_list[10], (3, WIDTH), 3 ** -0.5, 3.5, ((1, 4),), jnp.float32),
        "conv_state_in": gaussian(key_list[11], (3, GROUPS * STATE), 3 ** -0.5, 3.5, ((1, 4),), jnp.float32),
        "conv_state_out": gaussian(key_list[12], (3, GROUPS * STATE), 3 ** -0.5, 3.5, ((1, 4),), jnp.float32),
        "out_gain": jnp.clip(1.0 + 0.1 * jax.random.normal(key_list[13], (WIDTH,), jnp.float32), 0.5, 1.5),
        "w_out": gaussian(key_list[14], (WIDTH, D), WIDTH ** -0.5, 0.125, ((0, 4), (1, 32))),
    }


epsilon = 1e-06
HIGHEST_PRECISION = lax.Precision.HIGHEST

def rms_rows(values):
    wide = values.astype(jnp.float32)
    return wide * lax.rsqrt(lax.optimization_barrier(jnp.mean(wide * wide, axis=-1, keepdims=True)) + epsilon)

def short_filter(values, taps):
    wide = values.astype(jnp.float32)
    padded = jnp.pad(wide, ((1, 1), (0, 0)))
    mixed = taps[0] * padded[:-2] + taps[1] * padded[1:-1] + taps[2] * padded[2:]
    return jax.nn.silu(mixed).astype(jnp.bfloat16)

def sweep(signal, step_size, rate, inward, outward):
    sequence_extent = signal.shape[0]
    count = sequence_extent // BLOCK
    ratio = HEADS // GROUPS
    blocks = signal.reshape(count, BLOCK, GROUPS, ratio, HEAD_DIM).astype(jnp.float32)
    step_blocks = step_size.reshape(count, BLOCK, GROUPS, ratio)
    inward_blocks = inward.reshape(count, BLOCK, GROUPS, STATE).astype(jnp.float32)
    outward_blocks = outward.reshape(count, BLOCK, GROUPS, STATE).astype(jnp.float32)
    log_decay = -step_blocks * rate.reshape(GROUPS, ratio)
    lower = (jnp.arange(BLOCK)[:, None] >= jnp.arange(BLOCK)[None, :])[:, :, None, None]

    def advance(state, inputs):
        values, steps, inner, outer, logs = inputs
        within = jnp.cumsum(logs, axis=0)
        gaps = within[:, None] - within[None]
        decay = jnp.where(lower, jnp.exp(jnp.where(lower, gaps, 0.0)), 0.0)
        intersect = jnp.einsum('qgn,kgn->qkg', outer, inner, precision=HIGHEST_PRECISION)
        weights_mix = intersect[..., None] * decay * steps[None]
        result = jnp.einsum('qkgr,kgrp->qgrp', weights_mix, values, precision=HIGHEST_PRECISION)
        result = result + jnp.einsum('qgn,grpn->qgrp', outer, state, precision=HIGHEST_PRECISION) * jnp.exp(within)[..., None]
        final = within[-1]
        scaling_factor = jnp.exp(final[None] - within) * steps
        added = jnp.einsum('qgn,qgrp->grpn', inner, values * scaling_factor[..., None], precision=HIGHEST_PRECISION)
        return (state * jnp.exp(final)[..., None, None] + added, result)
    start_state = jnp.zeros((GROUPS, ratio, HEAD_DIM, STATE), jnp.float32)
    _, outputs = lax.scan(advance, start_state, (blocks, step_blocks, inward_blocks, outward_blocks, log_decay))
    return outputs.reshape(sequence_extent, WIDTH)

def reference(input_activations, norm_gain, w_gate, w_value, w_state_in, w_state_out, w_step_forward, w_step_backward, step_offset, fading_speed, conv_value, conv_state_in, conv_state_out, out_gain, w_out):
    normed = (rms_rows(input_activations) * norm_gain).astype(jnp.bfloat16)

    def project(scaling_factor):
        return jnp.dot(normed, scaling_factor, preferred_element_type=jnp.float32).astype(jnp.bfloat16)
    gate = project(w_gate)
    value = project(w_value)
    inward_raw = project(w_state_in)
    outward_raw = project(w_state_out)
    raw_forward = project(w_step_forward)
    raw_backward = project(w_step_backward)
    shift = math.log(SEQ)
    step_forward = jax.nn.softplus(raw_forward.astype(jnp.float32) + step_offset[0] - shift)
    step_backward = jax.nn.softplus(raw_backward.astype(jnp.float32) + step_offset[1] - shift)
    signal = short_filter(value, conv_value).reshape(SEQ, HEADS, HEAD_DIM)
    inward = short_filter(inward_raw, conv_state_in).reshape(SEQ, GROUPS, STATE)
    outward = short_filter(outward_raw, conv_state_out).reshape(SEQ, GROUPS, STATE)
    forward = sweep(signal, step_forward, fading_speed[0], inward, outward)
    backward = sweep(signal[::-1], step_backward[::-1], fading_speed[1], inward[::-1], outward[::-1])[::-1]
    gated = (forward + backward) * jax.nn.silu(gate.astype(jnp.float32))
    grouped = rms_rows(gated.reshape(SEQ, GROUPS, WIDTH // GROUPS)).reshape(SEQ, WIDTH)
    mixed = (grouped * out_gain).astype(jnp.bfloat16)
    return jnp.dot(mixed, w_out, preferred_element_type=jnp.float32).astype(jnp.bfloat16)
```

```python
import functools
import math

import jax
import jax.numpy as jnp
from jax import lax
from jax.experimental import pallas as pl
from jax.experimental.pallas import tpu as pltpu
from jax.sharding import PartitionSpec as P

HEAD_DIM = 64
STATE = 128
BLOCK = 128
LANES = 128
EPSILON = 1e-06
HIGHEST = lax.Precision.HIGHEST
VMEM_LIMIT = 60 * 1024 * 1024
SIDE = 4


def rms_rows(values):
    wide = values.astype(jnp.float32)
    return wide * lax.rsqrt(jnp.mean(wide * wide, axis=-1, keepdims=True) + EPSILON)


def sigmoid(values):
    return 1.0 / (1.0 + jnp.exp(-values))


def softplus(values):
    return jnp.maximum(values, 0.0) + jnp.log1p(jnp.exp(-jnp.abs(values)))


def spread(columns, first, count):
    rows = columns.shape[0]
    lane = lax.broadcasted_iota(jnp.int32, (rows, LANES), 1)
    tiles = []
    for at in range(first, first + count, 2):
        low = jnp.broadcast_to(columns[:, at : at + 1], (rows, LANES))
        high = jnp.broadcast_to(columns[:, at + 1 : at + 2], (rows, LANES))
        tiles.append(jnp.where(lane < HEAD_DIM, low, high))
    return jnp.concatenate(tiles, axis=1)


def greet(peers):
    barrier = pltpu.get_barrier_semaphore()
    for peer in peers:
        pl.semaphore_signal(
            barrier, inc=1, device_id=peer, device_id_type=pl.DeviceIdType.MESH
        )
    return lambda: pl.semaphore_wait(barrier, len(peers))


def remote(source, target, send, receive, peer):
    return pltpu.make_async_remote_copy(
        src_ref=source,
        dst_ref=target,
        send_sem=send,
        recv_sem=receive,
        device_id=peer,
        device_id_type=pl.DeviceIdType.MESH,
    )


def place():
    me = lax.axis_index("sp")
    return me // (2 * SIDE), me // 2 % SIDE, me % 2


def plane_gather(whole, half, send, receive):
    z, y, c = place()
    part = lax.axis_index("tp")

    def origin(first, second):
        over_z = (z + c * first + (1 - c) * second + 2 * SIDE) % SIDE
        over_y = (y + (1 - c) * first + c * second + 2 * SIDE) % SIDE
        return (over_z * SIDE + over_y) * 2 + c

    along = [(origin(1, 0), part), (origin(-1, 0), part)]
    cross = [(origin(0, 1), part), (origin(0, -1), part)]
    partner = ((z * SIDE + y) * 2 + 1 - c, part)
    copies = []

    def go(block, peer):
        at = len(copies)
        copy = remote(block, block, send.at[at], receive.at[at], peer)
        copy.start()
        copies.append(copy)
        return copy

    over, shared = {}, []

    def spread_line(first):
        over[first] = [go(whole(origin(first, 0)), peer) for peer in cross]
        shared.append(go(whole(origin(first, 0)), partner))

    def forward(first):
        halves = []
        for way in range(2):
            over[first][way].wait_recv()
            source = origin(first, (-1, 1)[way])
            halves.append(go(half(source, way), cross[way]))
        for way in range(2):
            shared.append(go(whole(origin(first, (-1, 1)[way])), partner))
        over[first] = halves

    line = [go(whole(origin(0, 0)), peer) for peer in along]
    spread_line(0)
    yield
    far = []
    for way in range(2):
        line[way].wait_recv()
        first = (-1, 1)[way]
        far.append(go(half(origin(first, 0), way), along[way]))
        spread_line(first)
    yield
    forward(0)
    yield
    for copy in far:
        copy.wait_recv()
    spread_line(2)
    yield
    forward(-1)
    yield
    forward(1)
    yield
    forward(2)
    yield
    for first in (0, -1, 1, 2):
        for copy in over[first]:
            copy.wait_recv()
        shared.append(go(whole(origin(first, 2)), partner))
    yield
    for copy in shared:
        copy.wait_recv()
    yield
    for copy in copies:
        copy.wait_send()
    yield


GATHER_COPIES = 36


def mixer_kernel(
    shift,
    x_ref,
    norm_gain_ref,
    gate_weights_ref,
    value_weights_ref,
    in_weights_ref,
    out_weights_ref,
    ahead_weights_ref,
    behind_weights_ref,
    offset_ref,
    speed_ref,
    taps_value_ref,
    taps_in_ref,
    taps_out_ref,
    gain_ref,
    w_out_ref,
    result_ref,
    tokens,
    weights,
    full_out,
    placed,
    paired,
    padded,
    gates,
    raw_steps,
    halo,
    signal_ref,
    inward_ref,
    outward_ref,
    within_ref,
    rows_ref,
    block_states_ref,
    block_logs_ref,
    sent,
    slices,
    returned,
    incoming,
    total,
    staged,
    mixed,
    weights_send,
    weights_receive,
    out_send,
    out_receive,
    pair_send,
    pair_receive,
    cross_send,
    cross_receive,
    token_send,
    token_receive,
    onward_send,
    onward_receive,
    halo_send,
    halo_receive,
    scan_send,
    scan_receive,
    back_send,
    back_receive,
    mixed_send,
    mixed_receive,
):
    me, part = lax.axis_index("sp"), lax.axis_index("tp")
    core = me % 2
    stretches = slices.shape[0]
    parts, chunk, features = tokens.shape
    extent = parts * chunk
    depth = value_weights_ref.shape[0]
    content = value_weights_ref.shape[1]
    state_width = in_weights_ref.shape[1]
    heads = ahead_weights_ref.shape[1]
    groups = state_width // STATE
    ratio = heads // groups
    span = ratio * HEAD_DIM
    channels = content + 2 * state_width
    count = extent // BLOCK
    f32, bf16 = jnp.float32, jnp.bfloat16

    peers = [((me + hop) % stretches, part) for hop in range(1, stretches)]
    across = [(me, (part + hop) % parts) for hop in range(1, parts)]
    settle = greet(peers + across)

    rows = 16

    def normalize(at, _):
        here = pl.ds(pl.multiple_of(at * rows, rows), rows)
        tokens[part, here, :] = (rms_rows(x_ref[here, :]) * norm_gain_ref[...]).astype(bf16)
        return 0

    lax.fori_loop(0, chunk // rows, normalize, 0)
    own_rows = pl.ds(pl.multiple_of(me * depth, depth), depth)
    weights[own_rows, 0:content] = value_weights_ref[...]
    weights[own_rows, content : content + state_width] = in_weights_ref[...]
    weights[own_rows, content + state_width : channels] = out_weights_ref[...]
    weights[own_rows, channels : channels + content] = gate_weights_ref[...]
    head_row = lax.broadcasted_iota(jnp.int32, (heads, LANES), 0)
    head_lane = lax.broadcasted_iota(jnp.int32, (heads, LANES), 1)
    to_ahead = (head_row == head_lane).astype(bf16)
    to_behind = (head_row + heads == head_lane).astype(bf16)
    weights[own_rows, channels + content :] = (
        jnp.dot(ahead_weights_ref[...], to_ahead, preferred_element_type=f32)
        + jnp.dot(behind_weights_ref[...], to_behind, preferred_element_type=f32)
    ).astype(bf16)
    width = w_out_ref.shape[1]
    move_row = lax.broadcasted_iota(jnp.int32, (width, LANES), 0)
    move_lane = lax.broadcasted_iota(jnp.int32, (width, LANES), 1)
    to_half = (move_row + core * width == move_lane).astype(bf16)
    half_rows = w_out_ref.shape[0] // 2
    for side in range(2):
        placed[side] = jnp.dot(
            w_out_ref[side * half_rows : (side + 1) * half_rows, :],
            to_half,
            preferred_element_type=f32,
        ).astype(bf16)
    settle()

    quarter = chunk // 4
    right, left = (me, (part + 1) % parts), (me, (part + parts - 1) % parts)
    before, after = (part + parts - 1) % parts, (part + 1) % parts
    opposite = (part + 2) % parts

    def piece(source, at):
        return tokens.at[source, pl.ds(at * quarter, quarter)]

    orders = ((0, 1, 2, 3), (3, 2, 1, 0))
    ring = [[], []]

    def send_own(step):
        for way, peer in enumerate((right, left)):
            block = piece(part, orders[way][step])
            copy = remote(
                block, block, token_send.at[way, step], token_receive.at[way, step], peer
            )
            copy.start()
            ring[way].append(copy)

    onward_copies = []

    def pass_on(step):
        for way, peer in enumerate((right, left)):
            ring[way][step].wait_recv()
            block = piece((before, after)[way], orders[way][step])
            copy = remote(
                block, block, onward_send.at[way, step], onward_receive.at[way, step], peer
            )
            copy.start()
            onward_copies.append(copy)

    weights_steps = plane_gather(
        lambda at: weights.at[pl.ds(pl.multiple_of(at * depth, depth), depth)],
        lambda at, side: weights.at[
            pl.ds(pl.multiple_of(at * depth + side * (depth // 2), depth // 2), depth // 2)
        ],
        weights_send,
        weights_receive,
    )
    out_steps = plane_gather(
        lambda at: full_out.at[at],
        lambda at, side: full_out.at[at, pl.ds(side * (parts // 2), parts // 2)],
        out_send,
        out_receive,
    )

    z, y, _ = place()
    partner = ((z * SIDE + y) * 2 + 1 - core, part)
    pair = remote(placed.at[1 - core], paired, pair_send.at[0], pair_receive.at[0], partner)
    pair.start()
    send_own(0)
    next(weights_steps)
    pair.wait_recv()
    full_out[me, part] = placed[core] + paired[...]
    send_own(1)
    next(weights_steps)
    crossing = []
    for hop, peer in enumerate(across):
        block = full_out.at[me, part]
        copy = remote(block, block, cross_send.at[hop], cross_receive.at[hop], peer)
        copy.start()
        crossing.append(copy)
    send_own(2)
    send_own(3)
    next(weights_steps)
    pass_on(0)
    next(weights_steps)
    next(weights_steps)
    pass_on(1)
    next(weights_steps)
    next(weights_steps)
    for copy in crossing:
        copy.wait_recv()
    next(out_steps)
    next(weights_steps)
    next(out_steps)
    next(weights_steps)

    def project(source):
        start = pl.multiple_of(source * chunk, chunk)

        def product(columns):
            return jnp.dot(tokens[source], weights[:, columns], preferred_element_type=f32)

        wide = 2 * LANES

        def filtered(at, _):
            columns = pl.ds(pl.multiple_of(at * wide, wide), wide)
            padded[pl.ds(start + 8, chunk), columns] = product(columns).astype(bf16).astype(f32)
            return 0

        lax.fori_loop(0, channels // wide, filtered, 0)

        def gated(at, _):
            columns = pl.ds(pl.multiple_of(channels + at * wide, wide), wide)
            gates[pl.ds(start, chunk), pl.ds(pl.multiple_of(at * wide, wide), wide)] = product(
                columns
            ).astype(bf16)
            return 0

        lax.fori_loop(0, content // wide, gated, 0)
        raw_steps[pl.ds(start, chunk), :] = (
            product(slice(channels + content, channels + content + LANES)).astype(bf16).astype(f32)
        )

    project(part)
    next(out_steps)
    for copy in ring[0][2:]:
        copy.wait_recv()
    project(before)
    next(out_steps)
    for copy in ring[1][2:]:
        copy.wait_recv()
    project(after)
    next(out_steps)
    for copy in onward_copies:
        copy.wait_recv()
    project(opposite)

    edges = []
    for way, hop in enumerate((1, stretches - 1)):
        peer = ((me + hop) % stretches, part)
        block = padded.at[pl.ds((extent, 8)[way], 8)]
        copy = remote(block, halo.at[way], halo_send.at[way], halo_receive.at[way], peer)
        copy.start()
        edges.append(copy)
    next(out_steps)

    row = lax.broadcasted_iota(jnp.int32, (BLOCK, BLOCK), 0)
    column = lax.broadcasted_iota(jnp.int32, (BLOCK, BLOCK), 1)
    lower = (row >= column).astype(f32)
    upper = (row <= column).astype(f32)
    lane = lax.broadcasted_iota(jnp.int32, (1, LANES), 1)
    spare = jnp.zeros((1, LANES - 2 * heads), f32)
    offset = jnp.concatenate([offset_ref[0:1, :], offset_ref[1:2, :], spare], axis=1)
    rate = jnp.concatenate([speed_ref[0:1, :], speed_ref[1:2, :], spare], axis=1)

    def block(at, _):
        start = pl.multiple_of(at * BLOCK, BLOCK)
        here = pl.ds(start, BLOCK)
        filtered = []
        for first in range(0, channels, 2 * LANES):
            part_rows = padded[pl.ds(start, BLOCK + 16), first : first + 2 * LANES]
            if first < content:
                taps = taps_value_ref[:, first : first + 2 * LANES]
            elif first < content + state_width:
                taps = taps_in_ref[:, first - content : first - content + 2 * LANES]
            else:
                base = first - content - state_width
                taps = taps_out_ref[:, base : base + 2 * LANES]
            mixed_rows = (
                taps[0:1] * part_rows[7 : 7 + BLOCK]
                + taps[1:2] * part_rows[8 : 8 + BLOCK]
                + taps[2:3] * part_rows[9 : 9 + BLOCK]
            )
            filtered.append((mixed_rows * sigmoid(mixed_rows)).astype(bf16))
        filtered = jnp.concatenate(filtered, axis=1)
        signal = filtered[:, :content]
        inward = filtered[:, content : content + state_width]
        signal_ref[here, :] = signal
        inward_ref[here, :] = inward
        outward_ref[here, :] = filtered[:, content + state_width :]
        steps = softplus(raw_steps[here, :] + offset - shift)
        logs = -steps * rate
        ahead = jnp.dot(lower, logs, precision=HIGHEST, preferred_element_type=f32)
        behind = jnp.dot(upper, logs, precision=HIGHEST, preferred_element_type=f32)
        within = jnp.where(lane < heads, ahead, behind)
        final = jnp.where(lane < heads, within[BLOCK - 1 : BLOCK], within[0:1])
        within_ref[here, :] = within
        rows_ref[0 : 2 * heads, here] = within.T[0 : 2 * heads]
        rows_ref[2 * heads : 4 * heads, here] = steps.T[0 : 2 * heads]
        scale = jnp.exp(final - within) * steps
        for group in range(groups):
            wide = signal[:, group * span : (group + 1) * span].astype(f32)
            scaled = jnp.concatenate(
                [wide * spread(scale, way * heads + group * ratio, ratio) for way in range(2)],
                axis=1,
            ).astype(bf16)
            block_states_ref[group, at] = lax.dot_general(
                inward[:, group * STATE : (group + 1) * STATE],
                scaled,
                (((0,), (0,)), ((), ())),
                preferred_element_type=f32,
            )
            block_logs_ref[group, at] = jnp.concatenate(
                [spread(final, way * heads + group * ratio, ratio) for way in range(2)], axis=1
            )
        return 0

    lax.fori_loop(1, count - 1, block, 0)
    for copy in edges:
        copy.wait()
    padded[0:8, :] = halo[0] * (me > 0).astype(f32)
    padded[pl.ds(extent + 8, 8), :] = halo[1] * (me < stretches - 1).astype(f32)
    lax.fori_loop(0, 2, lambda at, _: block(at * (count - 1), 0), 0)
    next(out_steps)

    slice_rows = sent.shape[1]
    per_state = STATE // slice_rows
    for group in range(groups):

        def onward(at, state):
            return state * jnp.exp(block_logs_ref[group, at][:, :span]) + block_states_ref[
                group, at
            ][:, :span]

        def back(at, state):
            at = count - 1 - at
            return state * jnp.exp(block_logs_ref[group, at][:, span:]) + block_states_ref[
                group, at
            ][:, span:]

        def sum_logs(at, carried):
            return carried + block_logs_ref[group, at]

        empty = jnp.zeros((STATE, span), f32)
        decayed = lax.fori_loop(0, count, sum_logs, jnp.zeros((1, 2 * span), f32))
        coarse = decayed.astype(bf16).astype(f32)
        fine = decayed - coarse
        for way, body in enumerate((onward, back)):
            state = lax.fori_loop(0, count, body, empty).astype(bf16)
            first = (way * groups + group) * per_state
            sent[first : first + per_state, :, 0:span] = state.reshape(
                per_state, slice_rows, span
            )
            base = way * span
            logs = jnp.concatenate(
                [
                    coarse[:, base : base + LANES],
                    coarse[:, base + LANES : base + 2 * LANES],
                    fine[:, base : base + LANES],
                    fine[:, base + LANES : base + 2 * LANES],
                    jnp.zeros((slice_rows - 4, LANES), f32),
                ],
                axis=0,
            ).astype(bf16)
            sent[first : first + per_state, :, span:] = jnp.broadcast_to(
                logs[None], (per_state, slice_rows, LANES)
            )

    def exchange(source, target, send, receive):
        copies = []
        for hop, peer in enumerate(peers):
            copy = remote(
                source.at[peer[0]], target.at[me], send.at[hop], receive.at[hop], peer
            )
            copy.start()
            copies.append(copy)
        target[me] = source[me]
        return copies

    scanning = exchange(sent, slices, scan_send, scan_receive)

    lanes = lax.broadcasted_iota(jnp.int32, (BLOCK, LANES), 1)

    def diagonal(at, _):
        here = pl.ds(pl.multiple_of(at * BLOCK, BLOCK), BLOCK)
        within = within_ref[here, :]
        for group in range(groups):
            intersect = lax.dot_general(
                outward_ref[here, group * STATE : (group + 1) * STATE],
                inward_ref[here, group * STATE : (group + 1) * STATE],
                (((1,), (1,)), ((), ())),
                preferred_element_type=f32,
            )
            products = []
            for head in range(group * ratio, (group + 1) * ratio):
                other = heads + head
                gap_ahead = within[:, head : head + 1] - rows_ref[head : head + 1, here]
                gap_behind = within[:, other : other + 1] - rows_ref[other : other + 1, here]
                step_ahead = rows_ref[2 * heads + head : 2 * heads + head + 1, here]
                step_behind = rows_ref[2 * heads + other : 2 * heads + other + 1, here]
                gap = jnp.where(row >= column, gap_ahead, gap_behind)
                step = jnp.where(
                    row > column,
                    step_ahead,
                    jnp.where(row < column, step_behind, step_ahead + step_behind),
                )
                mixing = (intersect * jnp.exp(gap) * step).astype(bf16)
                tile = head // 2 * 2 * HEAD_DIM
                products.append(
                    jnp.dot(
                        mixing,
                        signal_ref[here, tile : tile + LANES],
                        preferred_element_type=f32,
                    )
                )
            for two in range(ratio // 2):
                at_tile = (group * ratio + 2 * two) * HEAD_DIM
                total[here, at_tile : at_tile + LANES] = jnp.where(
                    lanes < HEAD_DIM, products[2 * two], products[2 * two + 1]
                )
        return 0

    lax.fori_loop(0, count // 2, diagonal, 0)
    next(out_steps)
    for copy in scanning:
        copy.wait_recv()

    reverse = me // (stretches // 2)

    def scan(at, state):
        source = at + reverse * (stretches - 1 - 2 * at)
        returned[source] = state.astype(bf16)
        logs = slices[source, :, span:].astype(f32)
        logs = jnp.concatenate([logs[0:1] + logs[2:3], logs[1:2] + logs[3:4]], axis=1)
        return state * jnp.exp(logs) + slices[source, :, 0:span].astype(f32)

    lax.fori_loop(0, stretches, scan, jnp.zeros((slice_rows, span), f32))
    returning = exchange(returned, incoming, back_send, back_receive)
    lax.fori_loop(count // 2, count, diagonal, 0)
    next(out_steps)
    for copy in returning:
        copy.wait_recv()

    def carried_in(way, group):
        first = (way * groups + group) * per_state
        return incoming[first : first + per_state].reshape(STATE, span).astype(f32)

    for group in range(groups):
        states = slice(group * STATE, (group + 1) * STATE)
        wide = slice(group * span, (group + 1) * span)

        def leave(hop, state):
            at = count - 1 - hop
            here = pl.ds(pl.multiple_of(at * BLOCK, BLOCK), BLOCK)
            carried = jnp.dot(
                outward_ref[here, states], state.astype(bf16), preferred_element_type=f32
            )
            decay = spread(jnp.exp(within_ref[here, :]), heads + group * ratio, ratio)
            total[here, wide] += carried * decay
            return (
                state * jnp.exp(block_logs_ref[group, at][:, span:])
                + block_states_ref[group, at][:, span:]
            )

        lax.fori_loop(0, count, leave, carried_in(1, group))

    carries = [carried_in(0, group) for group in range(groups)]
    blocks_in_chunk = chunk // BLOCK
    for target in range(parts):
        for group in range(groups):
            states = slice(group * STATE, (group + 1) * STATE)
            wide = slice(group * span, (group + 1) * span)

            def arrive(inner, state):
                at = target * blocks_in_chunk + inner
                here = pl.ds(pl.multiple_of(at * BLOCK, BLOCK), BLOCK)
                carried = jnp.dot(
                    outward_ref[here, states], state.astype(bf16), preferred_element_type=f32
                )
                decay = spread(jnp.exp(within_ref[here, :]), group * ratio, ratio)
                gate = gates[here, wide].astype(f32)
                gated = (total[here, wide] + carried * decay) * (gate * sigmoid(gate))
                scale = lax.rsqrt(jnp.mean(gated * gated, axis=-1, keepdims=True) + EPSILON)
                rows_in = pl.ds(pl.multiple_of(inner * BLOCK, BLOCK), BLOCK)
                staged[target, rows_in, wide] = (gated * scale * gain_ref[:, wide]).astype(bf16)
                return (
                    state * jnp.exp(block_logs_ref[group, at][:, :span])
                    + block_states_ref[group, at][:, :span]
                )

            carries[group] = lax.fori_loop(0, blocks_in_chunk, arrive, carries[group])

        @pl.when(part != target)
        def _():
            remote(
                staged.at[target],
                mixed.at[part],
                mixed_send.at[target],
                mixed_receive.at[part],
                (me, target),
            ).start()

        @pl.when(part == target)
        def _():
            mixed[target] = staged[target]

    for source in range(parts):

        @pl.when(part != source)
        def _():
            remote(
                staged.at[source],
                mixed.at[source],
                mixed_send.at[source],
                mixed_receive.at[source],
                (me, source),
            ).wait()

    half = content // 2

    def output(at, _):
        columns = pl.ds(pl.multiple_of(at * 2 * LANES, 2 * LANES), 2 * LANES)
        summed = jnp.zeros((chunk, 2 * LANES), f32)
        for source in range(parts):
            for side in range(2):
                tile = jnp.concatenate(
                    [full_out[4 * at + side, source], full_out[4 * at + 2 + side, source]], axis=1
                )
                summed += jnp.dot(
                    mixed[source, :, side * half : (side + 1) * half],
                    tile,
                    preferred_element_type=f32,
                )
        result_ref[:, columns] = summed.astype(bf16)
        return 0

    lax.fori_loop(0, features // (2 * LANES), output, 0)

    next(weights_steps)
    next(out_steps)
    pair.wait_send()
    for copy in crossing + ring[0] + ring[1] + onward_copies + scanning + returning:
        copy.wait_send()


def on_device(
    input_activations,
    norm_gain,
    w_gate,
    w_value,
    w_state_in,
    w_state_out,
    w_step_forward,
    w_step_backward,
    step_offset,
    fading_speed,
    conv_value,
    conv_state_in,
    conv_state_out,
    out_gain,
    w_out,
):
    stretches = lax.axis_size("sp")
    parts = lax.axis_size("tp")
    chunk, features = input_activations.shape
    extent = parts * chunk
    depth = w_gate.shape[0]
    content = w_value.shape[1]
    state_width = w_state_in.shape[1]
    heads = w_step_forward.shape[1]
    groups = state_width // STATE
    span = heads // groups * HEAD_DIM
    channels = content + 2 * state_width
    count = extent // BLOCK
    slice_rows = 2 * groups * STATE // stretches
    shift = math.log(extent * stretches)
    bf16, f32 = jnp.bfloat16, jnp.float32
    vmem, dma = pltpu.VMEM, pltpu.SemaphoreType.DMA
    space = pl.BlockSpec(memory_space=pltpu.VMEM)
    half_rows = w_out.shape[0] // 2
    return pl.pallas_call(
        functools.partial(mixer_kernel, shift),
        out_shape=jax.ShapeDtypeStruct((chunk, features), bf16),
        in_specs=[space] * 15,
        out_specs=space,
        scratch_shapes=[
            vmem((parts, chunk, features), bf16),
            vmem((stretches * depth, channels + content + LANES), bf16),
            vmem((stretches, parts, half_rows, LANES), bf16),
            vmem((2, half_rows, LANES), bf16),
            vmem((half_rows, LANES), bf16),
            vmem((extent + 16, channels), f32),
            vmem((extent, content), bf16),
            vmem((extent, LANES), f32),
            vmem((2, 8, channels), f32),
            vmem((extent, content), bf16),
            vmem((extent, state_width), bf16),
            vmem((extent, state_width), bf16),
            vmem((extent, LANES), f32),
            vmem((4 * heads, extent), f32),
            vmem((groups, count, STATE, 2 * span), f32),
            vmem((groups, count, 1, 2 * span), f32),
            vmem((stretches, slice_rows, span + LANES), bf16),
            vmem((stretches, slice_rows, span + LANES), bf16),
            vmem((stretches, slice_rows, span), bf16),
            vmem((stretches, slice_rows, span), bf16),
            vmem((extent, content), f32),
            vmem((parts, chunk, content), bf16),
            vmem((parts, chunk, content), bf16),
            dma((GATHER_COPIES,)),
            dma((GATHER_COPIES,)),
            dma((GATHER_COPIES,)),
            dma((GATHER_COPIES,)),
            dma((1,)),
            dma((1,)),
            dma((parts - 1,)),
            dma((parts - 1,)),
            dma((2, 4)),
            dma((2, 4)),
            dma((2, 2)),
            dma((2, 2)),
            dma((2,)),
            dma((2,)),
            dma((stretches - 1,)),
            dma((stretches - 1,)),
            dma((stretches - 1,)),
            dma((stretches - 1,)),
            dma((parts,)),
            dma((parts,)),
        ],
        cost_estimate=pl.CostEstimate(
            flops=int(3e10), bytes_accessed=1 << 20, transcendentals=0
        ),
        compiler_params=pltpu.CompilerParams(
            collective_id=1, has_side_effects=True, vmem_limit_bytes=VMEM_LIMIT
        ),
    )(
        input_activations,
        norm_gain.reshape(1, features),
        w_gate,
        w_value,
        w_state_in,
        w_state_out,
        w_step_forward,
        w_step_backward,
        step_offset,
        fading_speed,
        conv_value,
        conv_state_in,
        conv_state_out,
        out_gain.reshape(1, content),
        w_out,
    )


def solution(mesh):
    return jax.shard_map(
        on_device,
        mesh=mesh,
        in_specs=(
            P(("sp", "tp"), None),
            P(),
            P("sp", "tp"),
            P("sp", "tp"),
            P("sp", "tp"),
            P("sp", "tp"),
            P("sp", "tp"),
            P("sp", "tp"),
            P(None, "tp"),
            P(None, "tp"),
            P(None, "tp"),
            P(None, "tp"),
            P(None, "tp"),
            P("tp"),
            P("tp", "sp"),
        ),
        out_specs=P(("sp", "tp"), None),
        check_vma=False,
    )
```

```python
import functools
import math

import jax
import jax.numpy as jnp
from jax import lax
from jax.experimental import pallas as pl
from jax.experimental.pallas import tpu as pltpu
from jax.sharding import PartitionSpec as P

HEAD_DIM = 64
STATE = 128
BLOCK = 128
LANES = 128
EPSILON = 1e-06
HIGHEST = lax.Precision.HIGHEST
VMEM_LIMIT = 60 * 1024 * 1024
SIDE = 4


def rms_rows(values):
    wide = values.astype(jnp.float32)
    return wide * lax.rsqrt(jnp.mean(wide * wide, axis=-1, keepdims=True) + EPSILON)


def softplus(values):
    return jnp.maximum(values, 0.0) + jnp.log1p(jnp.exp(-jnp.abs(values)))


def spread(columns, first, count):
    rows = columns.shape[0]
    lane = lax.broadcasted_iota(jnp.int32, (rows, LANES), 1)
    tiles = []
    for at in range(first, first + count, 2):
        low = jnp.broadcast_to(columns[:, at : at + 1], (rows, LANES))
        high = jnp.broadcast_to(columns[:, at + 1 : at + 2], (rows, LANES))
        tiles.append(jnp.where(lane < HEAD_DIM, low, high))
    return jnp.concatenate(tiles, axis=1)


def silu(values):
    half = 0.5 * values
    return half + half * jnp.tanh(half)


def greet(peers):
    barrier = pltpu.get_barrier_semaphore()
    for peer in peers:
        pl.semaphore_signal(
            barrier, inc=1, device_id=peer, device_id_type=pl.DeviceIdType.MESH
        )
    return lambda: pl.semaphore_wait(barrier, len(peers))


def remote(source, target, send, receive, peer):
    return pltpu.make_async_remote_copy(
        src_ref=source,
        dst_ref=target,
        send_sem=send,
        recv_sem=receive,
        device_id=peer,
        device_id_type=pl.DeviceIdType.MESH,
    )


def place():
    me = lax.axis_index("sp")
    return me // (2 * SIDE), me // 2 % SIDE, me % 2


def plane_gather(whole, half, send, receive):
    z, y, c = place()
    part = lax.axis_index("tp")

    def origin(first, second):
        over_z = (z + c * first + (1 - c) * second + 2 * SIDE) % SIDE
        over_y = (y + (1 - c) * first + c * second + 2 * SIDE) % SIDE
        return (over_z * SIDE + over_y) * 2 + c

    along = [(origin(1, 0), part), (origin(-1, 0), part)]
    cross = [(origin(0, 1), part), (origin(0, -1), part)]
    partner = ((z * SIDE + y) * 2 + 1 - c, part)
    copies = []

    def go(block, peer):
        at = len(copies)
        copy = remote(block, block, send.at[at], receive.at[at], peer)
        copy.start()
        copies.append(copy)
        return copy

    over, shared = {}, []

    def spread_line(first):
        over[first] = [go(whole(origin(first, 0)), peer) for peer in cross]
        shared.append(go(whole(origin(first, 0)), partner))

    def forward(first):
        halves = []
        for way in range(2):
            over[first][way].wait_recv()
            source = origin(first, (-1, 1)[way])
            halves.append(go(half(source, way), cross[way]))
        for way in range(2):
            shared.append(go(whole(origin(first, (-1, 1)[way])), partner))
        over[first] = halves

    line = [go(whole(origin(0, 0)), peer) for peer in along]
    spread_line(0)
    yield
    far = []
    for way in range(2):
        line[way].wait_recv()
        first = (-1, 1)[way]
        far.append(go(half(origin(first, 0), way), along[way]))
        spread_line(first)
    yield
    forward(0)
    yield
    for copy in far:
        copy.wait_recv()
    spread_line(2)
    yield
    forward(-1)
    yield
    forward(1)
    yield
    forward(2)
    yield
    for first in (0, -1, 1, 2):
        for copy in over[first]:
            copy.wait_recv()
        shared.append(go(whole(origin(first, 2)), partner))
    yield
    for copy in shared:
        copy.wait_recv()
    yield
    for copy in copies:
        copy.wait_send()
    yield


GATHER_COPIES = 36


def mixer_kernel(
    shift,
    x_ref,
    norm_gain_ref,
    gate_weights_ref,
    value_weights_ref,
    in_weights_ref,
    out_weights_ref,
    ahead_weights_ref,
    behind_weights_ref,
    offset_ref,
    speed_ref,
    taps_value_ref,
    taps_in_ref,
    taps_out_ref,
    gain_ref,
    w_out_ref,
    result_ref,
    tokens,
    weights,
    full_out,
    placed,
    paired,
    padded,
    gates,
    raw_steps,
    halo,
    signal_ref,
    inward_ref,
    outward_ref,
    within_ref,
    rows_ref,
    block_states_ref,
    block_logs_ref,
    sent,
    slices,
    returned,
    incoming,
    total,
    staged,
    mixed,
    wide_gates,
    summed_ref,
    relay,
    weights_send,
    weights_receive,
    out_send,
    out_receive,
    pair_send,
    pair_receive,
    cross_send,
    cross_receive,
    token_send,
    token_receive,
    onward_send,
    onward_receive,
    halo_send,
    halo_receive,
    scan_send,
    scan_receive,
    back_send,
    back_receive,
    mixed_send,
    mixed_receive,
    relay_send,
    relay_receive,
    handed_send,
    handed_receive,
):
    me, part = lax.axis_index("sp"), lax.axis_index("tp")
    core = me % 2
    stretches = slices.shape[0]
    parts, chunk, features = tokens.shape
    extent = parts * chunk
    depth = value_weights_ref.shape[0]
    content = value_weights_ref.shape[1]
    state_width = in_weights_ref.shape[1]
    heads = ahead_weights_ref.shape[0]
    groups = state_width // STATE
    ratio = heads // groups
    span = ratio * HEAD_DIM
    channels = content + 2 * state_width
    count = extent // BLOCK
    f32, bf16 = jnp.float32, jnp.bfloat16

    peers = [((me + hop) % stretches, part) for hop in range(1, stretches)]
    across = [(me, (part + hop) % parts) for hop in range(1, parts)]
    settle = greet(peers + across)

    rows = 16

    def normalize(at, _):
        here = pl.ds(pl.multiple_of(at * rows, rows), rows)
        tokens[part, here, :] = (rms_rows(x_ref[here, :]) * norm_gain_ref[...]).astype(bf16)
        return 0

    lax.fori_loop(0, chunk // rows, normalize, 0)
    own_rows = pl.ds(pl.multiple_of(me * depth, depth), depth)
    weights[own_rows, 0:content] = value_weights_ref[...]
    weights[own_rows, content : content + state_width] = in_weights_ref[...]
    weights[own_rows, content + state_width : channels] = out_weights_ref[...]
    weights[own_rows, channels : channels + content] = gate_weights_ref[...]

    def across_rows(left, right):
        return lax.dot_general(left, right, (((0,), (0,)), ((), ())), preferred_element_type=f32)

    head_row = lax.broadcasted_iota(jnp.int32, (heads, LANES), 0)
    head_lane = lax.broadcasted_iota(jnp.int32, (heads, LANES), 1)
    to_ahead = (head_row == head_lane).astype(bf16)
    to_behind = (head_row + heads == head_lane).astype(bf16)
    weights[own_rows, channels + content :] = (
        across_rows(ahead_weights_ref[...], to_ahead)
        + across_rows(behind_weights_ref[...], to_behind)
    ).astype(bf16)
    width = w_out_ref.shape[0]
    move_row = lax.broadcasted_iota(jnp.int32, (width, LANES), 0)
    move_lane = lax.broadcasted_iota(jnp.int32, (width, LANES), 1)
    to_half = (move_row + core * width == move_lane).astype(bf16)
    half_rows = w_out_ref.shape[1] // 2
    for side in range(2):
        placed[side] = across_rows(
            w_out_ref[:, side * half_rows : (side + 1) * half_rows], to_half
        ).astype(bf16)
    settle()

    quarter = chunk // 4
    right, left = (me, (part + 1) % parts), (me, (part + parts - 1) % parts)
    before, after = (part + parts - 1) % parts, (part + 1) % parts
    opposite = (part + 2) % parts

    def piece(source, at):
        return tokens.at[source, pl.ds(at * quarter, quarter)]

    orders = ((0, 1, 2, 3), (3, 2, 1, 0))
    ring = [[], []]

    def send_own(step):
        for way, peer in enumerate((right, left)):
            block = piece(part, orders[way][step])
            copy = remote(
                block, block, token_send.at[way, step], token_receive.at[way, step], peer
            )
            copy.start()
            ring[way].append(copy)

    onward_copies = []

    def pass_on(step):
        for way, peer in enumerate((right, left)):
            ring[way][step].wait_recv()
            block = piece((before, after)[way], orders[way][step])
            copy = remote(
                block, block, onward_send.at[way, step], onward_receive.at[way, step], peer
            )
            copy.start()
            onward_copies.append(copy)

    weights_steps = plane_gather(
        lambda at: weights.at[pl.ds(pl.multiple_of(at * depth, depth), depth)],
        lambda at, side: weights.at[
            pl.ds(pl.multiple_of(at * depth + side * (depth // 2), depth // 2), depth // 2)
        ],
        weights_send,
        weights_receive,
    )
    out_steps = plane_gather(
        lambda at: full_out.at[at],
        lambda at, side: full_out.at[at, pl.ds(side * (parts // 2), parts // 2)],
        out_send,
        out_receive,
    )

    z, y, _ = place()
    partner = ((z * SIDE + y) * 2 + 1 - core, part)
    pair = remote(placed.at[1 - core], paired, pair_send.at[0], pair_receive.at[0], partner)
    pair.start()
    send_own(0)
    next(weights_steps)
    pair.wait_recv()
    full_out[me, part] = placed[core] + paired[...]
    send_own(1)
    next(weights_steps)
    crossing = []
    for hop, peer in enumerate(across):
        block = full_out.at[me, part]
        copy = remote(block, block, cross_send.at[hop], cross_receive.at[hop], peer)
        copy.start()
        crossing.append(copy)
    send_own(2)
    send_own(3)
    next(weights_steps)
    next(weights_steps)
    pass_on(0)
    next(weights_steps)
    next(weights_steps)
    pass_on(1)
    next(weights_steps)
    next(weights_steps)
    for copy in crossing:
        copy.wait_recv()
    next(out_steps)
    next(weights_steps)

    wide_tile = 2 * LANES

    def product(source, columns):
        return jnp.dot(tokens[source], weights[:, columns], preferred_element_type=f32)

    def project(source):
        start = pl.multiple_of(source * chunk, chunk)

        def filtered(at, _):
            columns = pl.ds(pl.multiple_of(at * wide_tile, wide_tile), wide_tile)
            padded[pl.ds(start + 8, chunk), columns] = (
                product(source, columns).astype(bf16).astype(f32)
            )
            return 0

        lax.fori_loop(0, channels // wide_tile, filtered, 0)
        raw_steps[pl.ds(start, chunk), :] = (
            product(source, slice(channels + content, channels + content + LANES))
            .astype(bf16)
            .astype(f32)
        )

    def project_gate(source):
        start = pl.multiple_of(source * chunk, chunk)

        def gated(at, _):
            columns = pl.ds(pl.multiple_of(channels + at * wide_tile, wide_tile), wide_tile)
            gates[
                pl.ds(start, chunk), pl.ds(pl.multiple_of(at * wide_tile, wide_tile), wide_tile)
            ] = product(source, columns).astype(bf16)
            return 0

        lax.fori_loop(0, content // wide_tile, gated, 0)

    edges = []
    for way, hop in enumerate((1, stretches - 1)):
        peer = ((me + hop) % stretches, part)
        block = padded.at[pl.ds((extent, 8)[way], 8)]
        edges.append(
            remote(block, halo.at[way], halo_send.at[way], halo_receive.at[way], peer)
        )

    def send_edges():
        for copy in edges:
            copy.start()

    def take_edges():
        for copy in edges:
            copy.wait()
        padded[0:8, :] = halo[0] * (me > 0).astype(f32)
        padded[pl.ds(extent + 8, 8), :] = halo[1] * (me < stretches - 1).astype(f32)

    row = lax.broadcasted_iota(jnp.int32, (BLOCK, BLOCK), 0)
    column = lax.broadcasted_iota(jnp.int32, (BLOCK, BLOCK), 1)
    lower = (row >= column).astype(f32)
    upper = (row <= column).astype(f32)
    lane = lax.broadcasted_iota(jnp.int32, (1, LANES), 1)
    spare = jnp.zeros((1, LANES - 2 * heads), f32)
    offset = jnp.concatenate([offset_ref[0:1, :], offset_ref[1:2, :], spare], axis=1)
    rate = jnp.concatenate([speed_ref[0:1, :], speed_ref[1:2, :], spare], axis=1)

    def filter_columns(start, first):
        part_rows = padded[pl.ds(start, BLOCK + 16), first : first + wide_tile]
        if first < content:
            taps = taps_value_ref[:, first : first + wide_tile]
        elif first < content + state_width:
            taps = taps_in_ref[:, first - content : first - content + wide_tile]
        else:
            base = first - content - state_width
            taps = taps_out_ref[:, base : base + wide_tile]
        mixed_rows = (
            taps[0:1] * part_rows[7 : 7 + BLOCK]
            + taps[1:2] * part_rows[8 : 8 + BLOCK]
            + taps[2:3] * part_rows[9 : 9 + BLOCK]
        )
        return silu(mixed_rows).astype(bf16)

    def filter_outward(at):
        start = pl.multiple_of(at * BLOCK, BLOCK)
        for first in range(0, state_width, wide_tile):
            outward_ref[pl.ds(start, BLOCK), first : first + wide_tile] = filter_columns(
                start, content + state_width + first
            )

    def block(at):
        start = pl.multiple_of(at * BLOCK, BLOCK)
        here = pl.ds(start, BLOCK)
        filtered = jnp.concatenate(
            [
                filter_columns(start, first)
                for first in range(0, content + state_width, wide_tile)
            ],
            axis=1,
        )
        signal = filtered[:, :content]
        inward = filtered[:, content : content + state_width]
        signal_ref[here, :] = signal
        inward_ref[here, :] = inward
        steps = softplus(raw_steps[here, :] + offset - shift)
        logs = -steps * rate
        ahead = jnp.dot(lower, logs, precision=HIGHEST, preferred_element_type=f32)
        behind = jnp.dot(upper, logs, precision=HIGHEST, preferred_element_type=f32)
        within = jnp.where(lane < heads, ahead, behind)
        final = jnp.where(lane < heads, within[BLOCK - 1 : BLOCK], within[0:1])
        within_ref[here, :] = within
        rows_ref[0 : 2 * heads, here] = within.T[0 : 2 * heads]
        rows_ref[2 * heads : 4 * heads, here] = steps.T[0 : 2 * heads]
        scale = jnp.exp(final - within) * steps
        for group in range(groups):
            wide = signal[:, group * span : (group + 1) * span].astype(f32)
            scaled = jnp.concatenate(
                [wide * spread(scale, way * heads + group * ratio, ratio) for way in range(2)],
                axis=1,
            ).astype(bf16)
            block_states_ref[group, at] = lax.dot_general(
                inward[:, group * STATE : (group + 1) * STATE],
                scaled,
                (((0,), (0,)), ((), ())),
                preferred_element_type=f32,
            )
            block_logs_ref[group, at] = jnp.concatenate(
                [spread(final, way * heads + group * ratio, ratio) for way in range(2)], axis=1
            )

    project(part)
    project_gate(part)
    next(out_steps)
    for copy in ring[0][2:]:
        copy.wait_recv()
    project(before)
    project_gate(before)
    next(out_steps)
    for copy in ring[1][2:]:
        copy.wait_recv()
    project(after)

    early = part % 3 == 0

    @pl.when(early)
    def _():
        send_edges()

    project_gate(after)
    next(out_steps)
    ahead_of_last = 2 * opposite + 3
    turn = 2 - 2 * (part // 3)

    def early_block(step, _):
        at = (ahead_of_last + (step + turn) % 4) % count
        block(at)
        filter_outward(at)
        return 0

    lax.fori_loop(0, 2, early_block, 0)
    next(out_steps)

    @pl.when(early)
    def _():
        take_edges()

    lax.fori_loop(2, 4, early_block, 0)
    next(out_steps)
    for copy in onward_copies:
        copy.wait_recv()
    project(opposite)

    @pl.when(part % 3 != 0)
    def _():
        send_edges()

    late_turn = 2 * (part // 2) * (1 - part % 2)

    def late_at(step):
        return (ahead_of_last + 4 + (step + late_turn) % 4) % count

    def late_block(step, _):
        block(late_at(step))
        return 0

    lax.fori_loop(0, 2, late_block, 0)

    @pl.when(part % 3 != 0)
    def _():
        take_edges()

    lax.fori_loop(2, 4, late_block, 0)

    slice_rows = sent.shape[1]
    per_state = STATE // slice_rows
    for group in range(groups):

        def onward(at, carried):
            return enter(at, 0, *carried)

        def back(at, carried):
            return enter(count - 1 - at, span, *carried)

        def enter(at, base, state, logs):
            added = block_states_ref[group, at, :, base : base + span]
            decay = block_logs_ref[group, at, :, base : base + span]
            block_states_ref[group, at, :, base : base + span] = state
            block_logs_ref[group, at, :, base : base + span] = logs
            return state * jnp.exp(decay) + added, logs + decay

        empty = jnp.zeros((STATE, span), f32)
        still = jnp.zeros((1, span), f32)
        for way, body in enumerate((onward, back)):
            state, decayed = lax.fori_loop(0, count, body, (empty, still))
            state = state.astype(bf16)
            coarse = decayed.astype(bf16).astype(f32)
            fine = decayed - coarse
            first = (way * groups + group) * per_state
            sent[first : first + per_state, :, 0:span] = state.reshape(
                per_state, slice_rows, span
            )
            base = 0
            logs = jnp.concatenate(
                [
                    coarse[:, base : base + LANES],
                    coarse[:, base + LANES : base + 2 * LANES],
                    fine[:, base : base + LANES],
                    fine[:, base + LANES : base + 2 * LANES],
                    jnp.zeros((slice_rows - 4, LANES), f32),
                ],
                axis=0,
            ).astype(bf16)
            sent[first : first + per_state, :, span:] = jnp.broadcast_to(
                logs[None], (per_state, slice_rows, LANES)
            )

    def exchange(source, target, send, receive):
        copies = []
        for hop, peer in enumerate(peers):
            copy = remote(
                source.at[peer[0]], target.at[me], send.at[hop], receive.at[hop], peer
            )
            copy.start()
            copies.append(copy)
        target[me] = source[me]
        return copies

    scanning = exchange(sent, slices, scan_send, scan_receive)

    lanes = lax.broadcasted_iota(jnp.int32, (BLOCK, LANES), 1)

    def diagonal(at, _):
        here = pl.ds(pl.multiple_of(at * BLOCK, BLOCK), BLOCK)
        within = within_ref[here, :]
        wide_gates[here, :] = silu(gates[here, :].astype(f32))
        for group in range(groups):
            intersect = lax.dot_general(
                outward_ref[here, group * STATE : (group + 1) * STATE],
                inward_ref[here, group * STATE : (group + 1) * STATE],
                (((1,), (1,)), ((), ())),
                preferred_element_type=f32,
            )
            products = []
            for head in range(group * ratio, (group + 1) * ratio):
                other = heads + head
                gap_ahead = within[:, head : head + 1] - rows_ref[head : head + 1, here]
                gap_behind = within[:, other : other + 1] - rows_ref[other : other + 1, here]
                step_ahead = rows_ref[2 * heads + head : 2 * heads + head + 1, here]
                step_behind = rows_ref[2 * heads + other : 2 * heads + other + 1, here]
                gap = jnp.where(row >= column, gap_ahead, gap_behind)
                step = jnp.where(
                    row > column,
                    step_ahead,
                    jnp.where(row < column, step_behind, step_ahead + step_behind),
                )
                mixing = (intersect * jnp.exp(gap) * step).astype(bf16)
                tile = head // 2 * 2 * HEAD_DIM
                products.append(
                    jnp.dot(
                        mixing,
                        signal_ref[here, tile : tile + LANES],
                        preferred_element_type=f32,
                    )
                )
            for two in range(ratio // 2):
                at_tile = (group * ratio + 2 * two) * HEAD_DIM
                total[here, at_tile : at_tile + LANES] = jnp.where(
                    lanes < HEAD_DIM, products[2 * two], products[2 * two + 1]
                )
        return 0

    project_gate(opposite)
    next(out_steps)

    def late_outward(step, _):
        filter_outward(late_at(step))
        return 0

    lax.fori_loop(0, 4, late_outward, 0)
    lax.fori_loop(0, count // 2, diagonal, 0)
    next(out_steps)
    for copy in scanning:
        copy.wait_recv()

    reverse = me // (stretches // 2)

    def scan(at, state):
        source = at + reverse * (stretches - 1 - 2 * at)
        returned[source] = state.astype(bf16)
        logs = slices[source, :, span:].astype(f32)
        logs = jnp.concatenate([logs[0:1] + logs[2:3], logs[1:2] + logs[3:4]], axis=1)
        return state * jnp.exp(logs) + slices[source, :, 0:span].astype(f32)

    lax.fori_loop(0, stretches, scan, jnp.zeros((slice_rows, span), f32))
    returning = exchange(returned, incoming, back_send, back_receive)
    lax.fori_loop(count // 2, count, diagonal, 0)
    next(out_steps)
    for copy in returning:
        copy.wait_recv()

    def carried_in(way, group):
        first = (way * groups + group) * per_state
        return incoming[first : first + per_state].reshape(STATE, span).astype(f32)

    def finish(source, inner):
        at = source * (chunk // BLOCK) + inner
        here = pl.ds(pl.multiple_of(at * BLOCK, BLOCK), BLOCK)
        decays = jnp.exp(within_ref[here, :])
        for group in range(groups):
            wide = slice(group * span, (group + 1) * span)
            summed = total[here, wide]
            for way in range(2):
                base = way * span
                state = block_states_ref[group, at, :, base : base + span] + jnp.exp(
                    block_logs_ref[group, at, :, base : base + span]
                ) * carried_in(way, group)
                carried = jnp.dot(
                    outward_ref[here, group * STATE : (group + 1) * STATE],
                    state.astype(bf16),
                    preferred_element_type=f32,
                )
                summed += carried * spread(decays, way * heads + group * ratio, ratio)
            gated = summed * wide_gates[here, wide]
            scale = lax.rsqrt(jnp.mean(gated * gated, axis=-1, keepdims=True) + EPSILON)
            staged[source, pl.ds(pl.multiple_of(inner * BLOCK, BLOCK), BLOCK), wide] = (
                gated * scale * gain_ref[:, wide]
            ).astype(bf16)

    sides = (right, left)
    leaving, relays, handed = [], [], []
    half_chunk = chunk // 2

    def half_of(at):
        return pl.ds(at * half_chunk, half_chunk)

    def finish_half(source, at):
        def one(step, _):
            finish(source, step)
            return 0

        lax.fori_loop(at * half_chunk // BLOCK, (at + 1) * half_chunk // BLOCK, one, 0)

    for way in range(2):
        finish_half(opposite, way)
        copy = remote(
            staged.at[opposite, half_of(way)],
            relay.at[way],
            relay_send.at[way],
            relay_receive.at[way],
            sides[way],
        )
        copy.start()
        relays.append(copy)
    for at in range(2):
        for way, target in enumerate((after, before)):
            finish_half(target, at)
            copy = remote(
                staged.at[target, half_of(at)],
                mixed.at[part, half_of(at)],
                mixed_send.at[way, at],
                mixed_receive.at[way, at],
                sides[way],
            )
            copy.start()
            leaving.append(copy)
    for way in range(2):
        relays[way].wait_recv()
        copy = remote(
            relay.at[way],
            mixed.at[(before, after)[way], half_of(way)],
            handed_send.at[way],
            handed_receive.at[way],
            sides[way],
        )
        copy.start()
        handed.append(copy)
    for at in range(2):
        finish_half(part, at)

    half = content // 2

    def output(block_of, source, first, last):
        def tile(at, _):
            columns = pl.ds(pl.multiple_of(at * wide_tile, wide_tile), wide_tile)
            summed = 0.0 if first else summed_ref[:, columns]
            for side in range(2):
                weight = jnp.concatenate(
                    [full_out[4 * at + side, source], full_out[4 * at + 2 + side, source]], axis=1
                )
                summed += jnp.dot(
                    block_of[source, :, side * half : (side + 1) * half],
                    weight,
                    preferred_element_type=f32,
                )
            if last:
                result_ref[:, columns] = summed.astype(bf16)
            else:
                summed_ref[:, columns] = summed
            return 0

        lax.fori_loop(0, features // wide_tile, tile, 0)

    output(staged, part, True, False)
    for at in range(2):
        leaving[2 * at].wait_recv()
    output(mixed, before, False, False)
    for at in range(2):
        leaving[2 * at + 1].wait_recv()
    output(mixed, after, False, False)
    for copy in handed:
        copy.wait_recv()
    output(mixed, opposite, False, True)
    next(weights_steps)
    next(out_steps)
    pair.wait_send()
    for copy in crossing + ring[0] + ring[1] + onward_copies + scanning + returning + leaving + relays + handed:
        copy.wait_send()


def on_device(
    input_activations,
    norm_gain,
    w_gate,
    w_value,
    w_state_in,
    w_state_out,
    w_step_forward,
    w_step_backward,
    step_offset,
    fading_speed,
    conv_value,
    conv_state_in,
    conv_state_out,
    out_gain,
    w_out,
):
    stretches = lax.axis_size("sp")
    parts = lax.axis_size("tp")
    chunk, features = input_activations.shape
    extent = parts * chunk
    depth = w_gate.shape[0]
    content = w_value.shape[1]
    state_width = w_state_in.shape[1]
    heads = w_step_forward.shape[1]
    groups = state_width // STATE
    span = heads // groups * HEAD_DIM
    channels = content + 2 * state_width
    count = extent // BLOCK
    slice_rows = 2 * groups * STATE // stretches
    shift = math.log(extent * stretches)
    bf16, f32 = jnp.bfloat16, jnp.float32
    vmem, dma = pltpu.VMEM, pltpu.SemaphoreType.DMA
    space = pl.BlockSpec(memory_space=pltpu.VMEM)
    half_rows = w_out.shape[0] // 2
    return pl.pallas_call(
        functools.partial(mixer_kernel, shift),
        out_shape=jax.ShapeDtypeStruct((chunk, features), bf16),
        in_specs=[space] * 15,
        out_specs=space,
        scratch_shapes=[
            vmem((parts, chunk, features), bf16),
            vmem((stretches * depth, channels + content + LANES), bf16),
            vmem((stretches, parts, half_rows, LANES), bf16),
            vmem((2, half_rows, LANES), bf16),
            vmem((half_rows, LANES), bf16),
            vmem((extent + 16, channels), f32),
            vmem((extent, content), bf16),
            vmem((extent, LANES), f32),
            vmem((2, 8, channels), f32),
            vmem((extent, content), bf16),
            vmem((extent, state_width), bf16),
            vmem((extent, state_width), bf16),
            vmem((extent, LANES), f32),
            vmem((4 * heads, extent), f32),
            vmem((groups, count, STATE, 2 * span), f32),
            vmem((groups, count, 1, 2 * span), f32),
            vmem((stretches, slice_rows, span + LANES), bf16),
            vmem((stretches, slice_rows, span + LANES), bf16),
            vmem((stretches, slice_rows, span), bf16),
            vmem((stretches, slice_rows, span), bf16),
            vmem((extent, content), f32),
            vmem((parts, chunk, content), bf16),
            vmem((parts, chunk, content), bf16),
            vmem((extent, content), f32),
            vmem((chunk, features), f32),
            vmem((2, chunk // 2, content), bf16),
            dma((GATHER_COPIES,)),
            dma((GATHER_COPIES,)),
            dma((GATHER_COPIES,)),
            dma((GATHER_COPIES,)),
            dma((1,)),
            dma((1,)),
            dma((parts - 1,)),
            dma((parts - 1,)),
            dma((2, 4)),
            dma((2, 4)),
            dma((2, 2)),
            dma((2, 2)),
            dma((2,)),
            dma((2,)),
            dma((stretches - 1,)),
            dma((stretches - 1,)),
            dma((stretches - 1,)),
            dma((stretches - 1,)),
            dma((2, 2)),
            dma((2, 2)),
            dma((2,)),
            dma((2,)),
            dma((2,)),
            dma((2,)),
        ],
        cost_estimate=pl.CostEstimate(
            flops=int(3e10), bytes_accessed=1 << 20, transcendentals=0
        ),
        compiler_params=pltpu.CompilerParams(
            collective_id=1, has_side_effects=True, vmem_limit_bytes=VMEM_LIMIT
        ),
    )(
        input_activations,
        norm_gain.reshape(1, features),
        w_gate,
        w_value,
        w_state_in,
        w_state_out,
        w_step_forward.T,
        w_step_backward.T,
        step_offset,
        fading_speed,
        conv_value,
        conv_state_in,
        conv_state_out,
        out_gain.reshape(1, content),
        w_out.T,
    )


def solution(mesh):
    return jax.shard_map(
        on_device,
        mesh=mesh,
        in_specs=(
            P(("sp", "tp"), None),
            P(),
            P("sp", "tp"),
            P("sp", "tp"),
            P("sp", "tp"),
            P("sp", "tp"),
            P("sp", "tp"),
            P("sp", "tp"),
            P(None, "tp"),
            P(None, "tp"),
            P(None, "tp"),
            P(None, "tp"),
            P(None, "tp"),
            P("tp"),
            P("tp", "sp"),
        ),
        out_specs=P(("sp", "tp"), None),
        check_vma=False,
    )
```

```python
import functools
import math

import jax
import jax.numpy as jnp
from jax import lax
from jax.experimental import pallas as pl
from jax.experimental.pallas import tpu as pltpu
from jax.sharding import PartitionSpec as P

HEAD_DIM = 64
STATE = 128
BLOCK = 128
LANES = 128
EPSILON = 1e-06
HIGHEST = lax.Precision.HIGHEST
VMEM_LIMIT = 60 * 1024 * 1024
SIDE = 4


def rms_rows(values):
    wide = values.astype(jnp.float32)
    return wide * lax.rsqrt(jnp.mean(wide * wide, axis=-1, keepdims=True) + EPSILON)


def softplus(values):
    return jnp.maximum(values, 0.0) + jnp.log1p(jnp.exp(-jnp.abs(values)))


def spread(columns, first, count):
    rows = columns.shape[0]
    lane = lax.broadcasted_iota(jnp.int32, (rows, LANES), 1)
    tiles = []
    for at in range(first, first + count, 2):
        low = jnp.broadcast_to(columns[:, at : at + 1], (rows, LANES))
        high = jnp.broadcast_to(columns[:, at + 1 : at + 2], (rows, LANES))
        tiles.append(jnp.where(lane < HEAD_DIM, low, high))
    return jnp.concatenate(tiles, axis=1)


def silu(values):
    half = 0.5 * values
    return half + half * jnp.tanh(half)


def greet(peers):
    barrier = pltpu.get_barrier_semaphore()
    for peer in peers:
        pl.semaphore_signal(
            barrier, inc=1, device_id=peer, device_id_type=pl.DeviceIdType.MESH
        )
    return lambda: pl.semaphore_wait(barrier, len(peers))


def remote(source, target, send, receive, peer):
    return pltpu.make_async_remote_copy(
        src_ref=source,
        dst_ref=target,
        send_sem=send,
        recv_sem=receive,
        device_id=peer,
        device_id_type=pl.DeviceIdType.MESH,
    )


def place():
    me = lax.axis_index("sp")
    return me // (2 * SIDE), me // 2 % SIDE, me % 2


def plane_gather(whole, half, send, receive):
    z, y, c = place()
    part = lax.axis_index("tp")

    def origin(first, second):
        over_z = (z + c * first + (1 - c) * second + 2 * SIDE) % SIDE
        over_y = (y + (1 - c) * first + c * second + 2 * SIDE) % SIDE
        return (over_z * SIDE + over_y) * 2 + c

    along = [(origin(1, 0), part), (origin(-1, 0), part)]
    cross = [(origin(0, 1), part), (origin(0, -1), part)]
    partner = ((z * SIDE + y) * 2 + 1 - c, part)
    copies = []

    def go(block, peer):
        at = len(copies)
        copy = remote(block, block, send.at[at], receive.at[at], peer)
        copy.start()
        copies.append(copy)
        return copy

    over, shared = {}, []

    def spread_line(first):
        over[first] = [go(whole(origin(first, 0)), peer) for peer in cross]
        shared.append(go(whole(origin(first, 0)), partner))

    def forward(first):
        halves = []
        for way in range(2):
            over[first][way].wait_recv()
            source = origin(first, (-1, 1)[way])
            halves.append(go(half(source, way), cross[way]))
        for way in range(2):
            shared.append(go(whole(origin(first, (-1, 1)[way])), partner))
        over[first] = halves

    line = [go(whole(origin(0, 0)), peer) for peer in along]
    spread_line(0)
    yield
    far = []
    for way in range(2):
        line[way].wait_recv()
        first = (-1, 1)[way]
        far.append(go(half(origin(first, 0), way), along[way]))
        spread_line(first)
    yield
    forward(0)
    yield
    for copy in far:
        copy.wait_recv()
    spread_line(2)
    yield
    forward(-1)
    yield
    forward(1)
    yield
    forward(2)
    yield
    for first in (0, -1, 1, 2):
        for copy in over[first]:
            copy.wait_recv()
        shared.append(go(whole(origin(first, 2)), partner))
    yield
    for copy in shared:
        copy.wait_recv()
    yield
    for copy in copies:
        copy.wait_send()
    yield


GATHER_COPIES = 36


def mixer_kernel(
    shift,
    x_ref,
    norm_gain_ref,
    gate_weights_ref,
    value_weights_ref,
    in_weights_ref,
    out_weights_ref,
    ahead_weights_ref,
    behind_weights_ref,
    offset_ref,
    speed_ref,
    taps_value_ref,
    taps_in_ref,
    taps_out_ref,
    gain_ref,
    w_out_ref,
    result_ref,
    tokens,
    weights,
    full_out,
    placed,
    paired,
    padded,
    gates,
    raw_steps,
    halo,
    signal_ref,
    inward_ref,
    outward_ref,
    within_ref,
    rows_ref,
    block_states_ref,
    block_logs_ref,
    sent,
    slices,
    returned,
    incoming,
    total,
    staged,
    mixed,
    wide_gates,
    summed_ref,
    relay,
    raw_tokens,
    weights_send,
    weights_receive,
    out_send,
    out_receive,
    pair_send,
    pair_receive,
    cross_send,
    cross_receive,
    token_send,
    token_receive,
    onward_send,
    onward_receive,
    halo_send,
    halo_receive,
    scan_send,
    scan_receive,
    back_send,
    back_receive,
    mixed_send,
    mixed_receive,
    relay_send,
    relay_receive,
    handed_send,
    handed_receive,
    load,
):
    me, part = lax.axis_index("sp"), lax.axis_index("tp")
    core = me % 2
    stretches = slices.shape[0]
    parts, chunk, features = tokens.shape
    extent = parts * chunk
    depth = value_weights_ref.shape[0]
    content = value_weights_ref.shape[1]
    state_width = in_weights_ref.shape[1]
    heads = ahead_weights_ref.shape[0]
    groups = state_width // STATE
    ratio = heads // groups
    span = ratio * HEAD_DIM
    channels = content + 2 * state_width
    count = extent // BLOCK
    f32, bf16 = jnp.float32, jnp.bfloat16

    peers = [((me + hop) % stretches, part) for hop in range(1, stretches)]
    across = [(me, (part + hop) % parts) for hop in range(1, parts)]
    settle = greet(peers + across)

    quarter = chunk // 4
    loads = []
    for at in (0, 3, 1, 2):
        here = pl.ds(at * quarter, quarter)
        copy = pltpu.make_async_copy(x_ref.at[here], raw_tokens.at[here], load.at[at])
        copy.start()
        loads.append(copy)
    rows = 16

    def normalize(at):
        def some(step, _):
            here = pl.ds(pl.multiple_of(at * quarter + step * rows, rows), rows)
            normed = rms_rows(raw_tokens[here, :]) * norm_gain_ref[...]
            tokens[part, here, :] = normed.astype(bf16)
            return 0

        lax.fori_loop(0, quarter // rows, some, 0)

    own_rows = pl.ds(pl.multiple_of(me * depth, depth), depth)
    weights[own_rows, 0:content] = value_weights_ref[...]
    weights[own_rows, content : content + state_width] = in_weights_ref[...]
    weights[own_rows, content + state_width : channels] = out_weights_ref[...]
    weights[own_rows, channels : channels + content] = gate_weights_ref[...]

    def across_rows(left, right):
        return lax.dot_general(left, right, (((0,), (0,)), ((), ())), preferred_element_type=f32)

    head_row = lax.broadcasted_iota(jnp.int32, (heads, LANES), 0)
    head_lane = lax.broadcasted_iota(jnp.int32, (heads, LANES), 1)
    to_ahead = (head_row == head_lane).astype(bf16)
    to_behind = (head_row + heads == head_lane).astype(bf16)
    weights[own_rows, channels + content :] = (
        across_rows(ahead_weights_ref[...], to_ahead)
        + across_rows(behind_weights_ref[...], to_behind)
    ).astype(bf16)
    for at, copy in zip((0, 3), loads[:2]):
        copy.wait()
        normalize(at)
    settle()

    right, left = (me, (part + 1) % parts), (me, (part + parts - 1) % parts)
    before, after = (part + parts - 1) % parts, (part + 1) % parts
    opposite = (part + 2) % parts

    def piece(source, at):
        return tokens.at[source, pl.ds(at * quarter, quarter)]

    orders = ((0, 1, 2, 3), (3, 2, 1, 0))
    ring = [[], []]

    def send_own(step):
        for way, peer in enumerate((right, left)):
            block = piece(part, orders[way][step])
            copy = remote(
                block, block, token_send.at[way, step], token_receive.at[way, step], peer
            )
            copy.start()
            ring[way].append(copy)

    onward_copies = []

    def pass_on(step):
        for way, peer in enumerate((right, left)):
            ring[way][step].wait_recv()
            block = piece((before, after)[way], orders[way][step])
            copy = remote(
                block, block, onward_send.at[way, step], onward_receive.at[way, step], peer
            )
            copy.start()
            onward_copies.append(copy)

    weights_steps = plane_gather(
        lambda at: weights.at[pl.ds(pl.multiple_of(at * depth, depth), depth)],
        lambda at, side: weights.at[
            pl.ds(pl.multiple_of(at * depth + side * (depth // 2), depth // 2), depth // 2)
        ],
        weights_send,
        weights_receive,
    )
    out_steps = plane_gather(
        lambda at: full_out.at[at],
        lambda at, side: full_out.at[at, pl.ds(side * (parts // 2), parts // 2)],
        out_send,
        out_receive,
    )

    z, y, _ = place()
    partner = ((z * SIDE + y) * 2 + 1 - core, part)
    pair = remote(placed.at[1 - core], paired, pair_send.at[0], pair_receive.at[0], partner)
    send_own(0)
    next(weights_steps)
    width = w_out_ref.shape[0]
    move_row = lax.broadcasted_iota(jnp.int32, (width, LANES), 0)
    move_lane = lax.broadcasted_iota(jnp.int32, (width, LANES), 1)
    to_half = (move_row + core * width == move_lane).astype(bf16)
    half_rows = w_out_ref.shape[1] // 2
    for side in range(2):
        placed[side] = across_rows(
            w_out_ref[:, side * half_rows : (side + 1) * half_rows], to_half
        ).astype(bf16)
    pair.start()
    for at, copy in zip((1, 2), loads[2:]):
        copy.wait()
        normalize(at)
    send_own(1)
    send_own(2)
    pair.wait_recv()
    full_out[me, part] = placed[core] + paired[...]
    next(weights_steps)
    crossing = []
    for hop, peer in enumerate(across):
        block = full_out.at[me, part]
        copy = remote(block, block, cross_send.at[hop], cross_receive.at[hop], peer)
        copy.start()
        crossing.append(copy)
    send_own(3)
    next(weights_steps)
    next(weights_steps)
    pass_on(0)
    next(weights_steps)
    next(weights_steps)
    pass_on(1)
    next(weights_steps)
    for copy in crossing:
        copy.wait_recv()
    next(out_steps)
    next(weights_steps)
    next(weights_steps)

    wide_tile = 2 * LANES

    def product(source, columns):
        return jnp.dot(tokens[source], weights[:, columns], preferred_element_type=f32)

    def project(source):
        start = pl.multiple_of(source * chunk, chunk)

        for first in range(0, channels, wide_tile):
            columns = slice(first, first + wide_tile)
            padded[pl.ds(start + 8, chunk), columns] = (
                product(source, columns).astype(bf16).astype(f32)
            )
        raw_steps[pl.ds(start, chunk), :] = (
            product(source, slice(channels + content, channels + content + LANES))
            .astype(bf16)
            .astype(f32)
        )

    def project_gate(source):
        start = pl.multiple_of(source * chunk, chunk)

        for first in range(0, content, wide_tile):
            gates[pl.ds(start, chunk), first : first + wide_tile] = product(
                source, slice(channels + first, channels + first + wide_tile)
            ).astype(bf16)

    edges = []
    for way, hop in enumerate((1, stretches - 1)):
        peer = ((me + hop) % stretches, part)
        block = padded.at[pl.ds((extent, 8)[way], 8)]
        edges.append(
            remote(block, halo.at[way], halo_send.at[way], halo_receive.at[way], peer)
        )

    def send_edges():
        for copy in edges:
            copy.start()

    def take_edges():
        for copy in edges:
            copy.wait()
        padded[0:8, :] = halo[0] * (me > 0).astype(f32)
        padded[pl.ds(extent + 8, 8), :] = halo[1] * (me < stretches - 1).astype(f32)

    row = lax.broadcasted_iota(jnp.int32, (BLOCK, BLOCK), 0)
    column = lax.broadcasted_iota(jnp.int32, (BLOCK, BLOCK), 1)
    lower = (row >= column).astype(f32)
    upper = (row <= column).astype(f32)
    lane = lax.broadcasted_iota(jnp.int32, (1, LANES), 1)
    spare = jnp.zeros((1, LANES - 2 * heads), f32)
    offset = jnp.concatenate([offset_ref[0:1, :], offset_ref[1:2, :], spare], axis=1)
    rate = jnp.concatenate([speed_ref[0:1, :], speed_ref[1:2, :], spare], axis=1)

    def filter_columns(start, first):
        part_rows = padded[pl.ds(start, BLOCK + 16), first : first + wide_tile]
        if first < content:
            taps = taps_value_ref[:, first : first + wide_tile]
        elif first < content + state_width:
            taps = taps_in_ref[:, first - content : first - content + wide_tile]
        else:
            base = first - content - state_width
            taps = taps_out_ref[:, base : base + wide_tile]
        mixed_rows = (
            taps[0:1] * part_rows[7 : 7 + BLOCK]
            + taps[1:2] * part_rows[8 : 8 + BLOCK]
            + taps[2:3] * part_rows[9 : 9 + BLOCK]
        )
        return silu(mixed_rows).astype(bf16)

    def filter_outward(at):
        start = pl.multiple_of(at * BLOCK, BLOCK)
        for first in range(0, state_width, wide_tile):
            outward_ref[pl.ds(start, BLOCK), first : first + wide_tile] = filter_columns(
                start, content + state_width + first
            )

    def block(at):
        start = pl.multiple_of(at * BLOCK, BLOCK)
        here = pl.ds(start, BLOCK)
        filtered = jnp.concatenate(
            [
                filter_columns(start, first)
                for first in range(0, content + state_width, wide_tile)
            ],
            axis=1,
        )
        signal = filtered[:, :content]
        inward = filtered[:, content : content + state_width]
        signal_ref[here, :] = signal
        inward_ref[here, :] = inward
        steps = softplus(raw_steps[here, :] + offset - shift)
        logs = -steps * rate
        ahead = jnp.dot(lower, logs, precision=HIGHEST, preferred_element_type=f32)
        behind = jnp.dot(upper, logs, precision=HIGHEST, preferred_element_type=f32)
        within = jnp.where(lane < heads, ahead, behind)
        final = jnp.where(lane < heads, within[BLOCK - 1 : BLOCK], within[0:1])
        within_ref[here, :] = within
        rows_ref[0 : 2 * heads, here] = within.T[0 : 2 * heads]
        rows_ref[2 * heads : 4 * heads, here] = steps.T[0 : 2 * heads]
        scale = jnp.exp(final - within) * steps
        for group in range(groups):
            wide = signal[:, group * span : (group + 1) * span].astype(f32)
            scaled = jnp.concatenate(
                [wide * spread(scale, way * heads + group * ratio, ratio) for way in range(2)],
                axis=1,
            ).astype(bf16)
            block_states_ref[group, at] = lax.dot_general(
                inward[:, group * STATE : (group + 1) * STATE],
                scaled,
                (((0,), (0,)), ((), ())),
                preferred_element_type=f32,
            )
            block_logs_ref[group, at] = jnp.concatenate(
                [spread(final, way * heads + group * ratio, ratio) for way in range(2)], axis=1
            )

    project(part)
    project_gate(part)
    next(out_steps)
    next(out_steps)
    for copy in ring[0][2:]:
        copy.wait_recv()
    project(before)
    project_gate(before)
    for copy in ring[1][2:]:
        copy.wait_recv()
    project(after)

    early = part % 3 == 0

    @pl.when(early)
    def _():
        send_edges()

    project_gate(after)
    next(out_steps)
    ahead_of_last = 2 * opposite + 3
    turn = 2 - 2 * (part // 3)

    def early_block(step, _):
        at = (ahead_of_last + (step + turn) % 4) % count
        block(at)
        filter_outward(at)
        return 0

    lax.fori_loop(0, 2, early_block, 0)
    next(out_steps)

    @pl.when(early)
    def _():
        take_edges()

    lax.fori_loop(2, 4, early_block, 0)
    next(out_steps)
    for copy in onward_copies:
        copy.wait_recv()
    project(opposite)

    @pl.when(part % 3 != 0)
    def _():
        send_edges()

    next(out_steps)
    late_turn = 2 * (part // 2) * (1 - part % 2)

    def late_at(step):
        return (ahead_of_last + 4 + (step + late_turn) % 4) % count

    def late_block(step, _):
        block(late_at(step))
        return 0

    lax.fori_loop(0, 2, late_block, 0)

    @pl.when(part % 3 != 0)
    def _():
        take_edges()

    lax.fori_loop(2, 4, late_block, 0)

    slice_rows = sent.shape[1]
    per_state = STATE // slice_rows
    for group in range(groups):

        def onward(at, carried):
            return enter(at, 0, *carried)

        def back(at, carried):
            return enter(count - 1 - at, span, *carried)

        def enter(at, base, state, logs):
            added = block_states_ref[group, at, :, base : base + span]
            decay = block_logs_ref[group, at, :, base : base + span]
            block_states_ref[group, at, :, base : base + span] = state
            block_logs_ref[group, at, :, base : base + span] = logs
            return state * jnp.exp(decay) + added, logs + decay

        empty = jnp.zeros((STATE, span), f32)
        still = jnp.zeros((1, span), f32)
        for way, body in enumerate((onward, back)):
            state, decayed = lax.fori_loop(0, count, body, (empty, still))
            state = state.astype(bf16)
            coarse = decayed.astype(bf16).astype(f32)
            fine = decayed - coarse
            first = (way * groups + group) * per_state
            sent[first : first + per_state, :, 0:span] = state.reshape(
                per_state, slice_rows, span
            )
            base = 0
            logs = jnp.concatenate(
                [
                    coarse[:, base : base + LANES],
                    coarse[:, base + LANES : base + 2 * LANES],
                    fine[:, base : base + LANES],
                    fine[:, base + LANES : base + 2 * LANES],
                    jnp.zeros((slice_rows - 4, LANES), f32),
                ],
                axis=0,
            ).astype(bf16)
            sent[first : first + per_state, :, span:] = jnp.broadcast_to(
                logs[None], (per_state, slice_rows, LANES)
            )

    def exchange(source, target, send, receive):
        copies = []
        for hop, peer in enumerate(peers):
            copy = remote(
                source.at[peer[0]], target.at[me], send.at[hop], receive.at[hop], peer
            )
            copy.start()
            copies.append(copy)
        target[me] = source[me]
        return copies

    scanning = exchange(sent, slices, scan_send, scan_receive)

    lanes = lax.broadcasted_iota(jnp.int32, (BLOCK, LANES), 1)

    def diagonal(at, _):
        here = pl.ds(pl.multiple_of(at * BLOCK, BLOCK), BLOCK)
        within = within_ref[here, :]
        wide_gates[here, :] = silu(gates[here, :].astype(f32))
        for group in range(groups):
            intersect = lax.dot_general(
                outward_ref[here, group * STATE : (group + 1) * STATE],
                inward_ref[here, group * STATE : (group + 1) * STATE],
                (((1,), (1,)), ((), ())),
                preferred_element_type=f32,
            )
            products = []
            for head in range(group * ratio, (group + 1) * ratio):
                other = heads + head
                gap_ahead = within[:, head : head + 1] - rows_ref[head : head + 1, here]
                gap_behind = within[:, other : other + 1] - rows_ref[other : other + 1, here]
                step_ahead = rows_ref[2 * heads + head : 2 * heads + head + 1, here]
                step_behind = rows_ref[2 * heads + other : 2 * heads + other + 1, here]
                gap = jnp.where(row >= column, gap_ahead, gap_behind)
                step = jnp.where(
                    row > column,
                    step_ahead,
                    jnp.where(row < column, step_behind, step_ahead + step_behind),
                )
                mixing = (intersect * jnp.exp(gap) * step).astype(bf16)
                tile = head // 2 * 2 * HEAD_DIM
                products.append(
                    jnp.dot(
                        mixing,
                        signal_ref[here, tile : tile + LANES],
                        preferred_element_type=f32,
                    )
                )
            for two in range(ratio // 2):
                at_tile = (group * ratio + 2 * two) * HEAD_DIM
                total[here, at_tile : at_tile + LANES] = jnp.where(
                    lanes < HEAD_DIM, products[2 * two], products[2 * two + 1]
                )
        return 0

    project_gate(opposite)

    def late_outward(step, _):
        filter_outward(late_at(step))
        return 0

    lax.fori_loop(0, 4, late_outward, 0)
    lax.fori_loop(0, count // 2, diagonal, 0)
    next(out_steps)
    for copy in scanning:
        copy.wait_recv()

    reverse = me // (stretches // 2)

    def scan(at, state):
        source = at + reverse * (stretches - 1 - 2 * at)
        returned[source] = state.astype(bf16)
        logs = slices[source, :, span:].astype(f32)
        logs = jnp.concatenate([logs[0:1] + logs[2:3], logs[1:2] + logs[3:4]], axis=1)
        return state * jnp.exp(logs) + slices[source, :, 0:span].astype(f32)

    lax.fori_loop(0, stretches, scan, jnp.zeros((slice_rows, span), f32))
    returning = exchange(returned, incoming, back_send, back_receive)
    lax.fori_loop(count // 2, count, diagonal, 0)
    next(out_steps)
    for copy in returning:
        copy.wait_recv()

    def carried_in(way, group):
        first = (way * groups + group) * per_state
        return incoming[first : first + per_state].reshape(STATE, span).astype(f32)

    def finish(source, inner):
        at = source * (chunk // BLOCK) + inner
        here = pl.ds(pl.multiple_of(at * BLOCK, BLOCK), BLOCK)
        decays = jnp.exp(within_ref[here, :])
        for group in range(groups):
            wide = slice(group * span, (group + 1) * span)
            summed = total[here, wide]
            for way in range(2):
                base = way * span
                state = block_states_ref[group, at, :, base : base + span] + jnp.exp(
                    block_logs_ref[group, at, :, base : base + span]
                ) * carried_in(way, group)
                carried = jnp.dot(
                    outward_ref[here, group * STATE : (group + 1) * STATE],
                    state.astype(bf16),
                    preferred_element_type=f32,
                )
                summed += carried * spread(decays, way * heads + group * ratio, ratio)
            gated = summed * wide_gates[here, wide]
            scale = lax.rsqrt(jnp.mean(gated * gated, axis=-1, keepdims=True) + EPSILON)
            staged[source, pl.ds(pl.multiple_of(inner * BLOCK, BLOCK), BLOCK), wide] = (
                gated * scale * gain_ref[:, wide]
            ).astype(bf16)

    sides = (right, left)
    leaving, relays, handed = [], [], []
    half_chunk = chunk // 2

    def half_of(at):
        return pl.ds(at * half_chunk, half_chunk)

    def finish_half(source, at):
        def one(step, _):
            finish(source, step)
            return 0

        lax.fori_loop(at * half_chunk // BLOCK, (at + 1) * half_chunk // BLOCK, one, 0)

    for way in range(2):
        finish_half(opposite, way)
        copy = remote(
            staged.at[opposite, half_of(way)],
            relay.at[way],
            relay_send.at[way],
            relay_receive.at[way],
            sides[way],
        )
        copy.start()
        relays.append(copy)
    for at in range(2):
        for way, target in enumerate((after, before)):
            finish_half(target, at)
            copy = remote(
                staged.at[target, half_of(at)],
                mixed.at[part, half_of(at)],
                mixed_send.at[way, at],
                mixed_receive.at[way, at],
                sides[way],
            )
            copy.start()
            leaving.append(copy)
    for way in range(2):
        relays[way].wait_recv()
        copy = remote(
            relay.at[way],
            mixed.at[(before, after)[way], half_of(way)],
            handed_send.at[way],
            handed_receive.at[way],
            sides[way],
        )
        copy.start()
        handed.append(copy)
    for at in range(2):
        finish_half(part, at)

    half = content // 2

    def output(block_of, source, first, last):
        broad = 8 * LANES

        def tile(at, _):
            columns = pl.ds(pl.multiple_of(at * broad, broad), broad)
            summed = 0.0 if first else summed_ref[:, columns]
            for side in range(2):
                weight = jnp.concatenate(
                    [full_out[16 * at + 2 * place + side, source] for place in range(8)], axis=1
                )
                summed += jnp.dot(
                    block_of[source, :, side * half : (side + 1) * half],
                    weight,
                    preferred_element_type=f32,
                )
            if last:
                result_ref[:, columns] = summed.astype(bf16)
            else:
                summed_ref[:, columns] = summed
            return 0

        lax.fori_loop(0, features // broad, tile, 0)

    output(staged, part, True, False)
    for at in range(2):
        leaving[2 * at].wait_recv()
    output(mixed, before, False, False)
    for at in range(2):
        leaving[2 * at + 1].wait_recv()
    output(mixed, after, False, False)
    for copy in handed:
        copy.wait_recv()
    output(mixed, opposite, False, True)
    next(weights_steps)
    next(out_steps)
    pair.wait_send()
    for copy in crossing + ring[0] + ring[1] + onward_copies + scanning + returning + leaving + relays + handed:
        copy.wait_send()


def on_device(
    input_activations,
    norm_gain,
    w_gate,
    w_value,
    w_state_in,
    w_state_out,
    w_step_forward,
    w_step_backward,
    step_offset,
    fading_speed,
    conv_value,
    conv_state_in,
    conv_state_out,
    out_gain,
    w_out,
):
    stretches = lax.axis_size("sp")
    parts = lax.axis_size("tp")
    chunk, features = input_activations.shape
    extent = parts * chunk
    depth = w_gate.shape[0]
    content = w_value.shape[1]
    state_width = w_state_in.shape[1]
    heads = w_step_forward.shape[1]
    groups = state_width // STATE
    span = heads // groups * HEAD_DIM
    channels = content + 2 * state_width
    count = extent // BLOCK
    slice_rows = 2 * groups * STATE // stretches
    shift = math.log(extent * stretches)
    bf16, f32 = jnp.bfloat16, jnp.float32
    vmem, dma = pltpu.VMEM, pltpu.SemaphoreType.DMA
    space = pl.BlockSpec(memory_space=pltpu.VMEM)
    half_rows = w_out.shape[0] // 2
    return pl.pallas_call(
        functools.partial(mixer_kernel, shift),
        out_shape=pltpu.VMEM((chunk, features), bf16),
        in_specs=[pl.BlockSpec(memory_space=pl.ANY)] + [space] * 14,
        out_specs=space,
        scratch_shapes=[
            vmem((parts, chunk, features), bf16),
            vmem((stretches * depth, channels + content + LANES), bf16),
            vmem((stretches, parts, half_rows, LANES), bf16),
            vmem((2, half_rows, LANES), bf16),
            vmem((half_rows, LANES), bf16),
            vmem((extent + 16, channels), f32),
            vmem((extent, content), bf16),
            vmem((extent, LANES), f32),
            vmem((2, 8, channels), f32),
            vmem((extent, content), bf16),
            vmem((extent, state_width), bf16),
            vmem((extent, state_width), bf16),
            vmem((extent, LANES), f32),
            vmem((4 * heads, extent), f32),
            vmem((groups, count, STATE, 2 * span), f32),
            vmem((groups, count, 1, 2 * span), f32),
            vmem((stretches, slice_rows, span + LANES), bf16),
            vmem((stretches, slice_rows, span + LANES), bf16),
            vmem((stretches, slice_rows, span), bf16),
            vmem((stretches, slice_rows, span), bf16),
            vmem((extent, content), f32),
            vmem((parts, chunk, content), bf16),
            vmem((parts, chunk, content), bf16),
            vmem((extent, content), f32),
            vmem((chunk, features), f32),
            vmem((2, chunk // 2, content), bf16),
            vmem((chunk, features), bf16),
            dma((GATHER_COPIES,)),
            dma((GATHER_COPIES,)),
            dma((GATHER_COPIES,)),
            dma((GATHER_COPIES,)),
            dma((1,)),
            dma((1,)),
            dma((parts - 1,)),
            dma((parts - 1,)),
            dma((2, 4)),
            dma((2, 4)),
            dma((2, 2)),
            dma((2, 2)),
            dma((2,)),
            dma((2,)),
            dma((stretches - 1,)),
            dma((stretches - 1,)),
            dma((stretches - 1,)),
            dma((stretches - 1,)),
            dma((2, 2)),
            dma((2, 2)),
            dma((2,)),
            dma((2,)),
            dma((2,)),
            dma((2,)),
            dma((4,)),
        ],
        cost_estimate=pl.CostEstimate(
            flops=int(3e10), bytes_accessed=1 << 20, transcendentals=0
        ),
        compiler_params=pltpu.CompilerParams(
            collective_id=1, has_side_effects=True, vmem_limit_bytes=VMEM_LIMIT
        ),
    )(
        input_activations,
        norm_gain.reshape(1, features),
        w_gate,
        w_value,
        w_state_in,
        w_state_out,
        w_step_forward.T,
        w_step_backward.T,
        step_offset,
        fading_speed,
        conv_value,
        conv_state_in,
        conv_state_out,
        out_gain.reshape(1, content),
        w_out.T,
    )


def solution(mesh):
    return jax.shard_map(
        on_device,
        mesh=mesh,
        in_specs=(
            P(("sp", "tp"), None),
            P(),
            P("sp", "tp"),
            P("sp", "tp"),
            P("sp", "tp"),
            P("sp", "tp"),
            P("sp", "tp"),
            P("sp", "tp"),
            P(None, "tp"),
            P(None, "tp"),
            P(None, "tp"),
            P(None, "tp"),
            P(None, "tp"),
            P("tp"),
            P("tp", "sp"),
        ),
        out_specs=P(("sp", "tp"), None),
        check_vma=False,
    )
```

```python
import functools
import math

import jax
import jax.numpy as jnp
from jax import lax
from jax.experimental import pallas as pl
from jax.experimental.pallas import tpu as pltpu
from jax.sharding import PartitionSpec as P

HEAD_DIM = 64
STATE = 128
BLOCK = 128
LANES = 128
EPSILON = 1e-06
HIGHEST = lax.Precision.HIGHEST
VMEM_LIMIT = 60 * 1024 * 1024
SIDE = 4


def rms_rows(values):
    wide = values.astype(jnp.float32)
    return wide * lax.rsqrt(jnp.mean(wide * wide, axis=-1, keepdims=True) + EPSILON)


def softplus(values):
    return jnp.maximum(values, 0.0) + jnp.log1p(jnp.exp(-jnp.abs(values)))


def spread(columns, first, count):
    rows = columns.shape[0]
    lane = lax.broadcasted_iota(jnp.int32, (rows, LANES), 1)
    tiles = []
    for at in range(first, first + count, 2):
        low = jnp.broadcast_to(columns[:, at : at + 1], (rows, LANES))
        high = jnp.broadcast_to(columns[:, at + 1 : at + 2], (rows, LANES))
        tiles.append(jnp.where(lane < HEAD_DIM, low, high))
    return jnp.concatenate(tiles, axis=1)


def silu(values):
    half = 0.5 * values
    return half + half * jnp.tanh(half)


def greet(peers):
    barrier = pltpu.get_barrier_semaphore()
    for peer in peers:
        pl.semaphore_signal(
            barrier, inc=1, device_id=peer, device_id_type=pl.DeviceIdType.MESH
        )
    return lambda: pl.semaphore_wait(barrier, len(peers))


def remote(source, target, send, receive, peer):
    return pltpu.make_async_remote_copy(
        src_ref=source,
        dst_ref=target,
        send_sem=send,
        recv_sem=receive,
        device_id=peer,
        device_id_type=pl.DeviceIdType.MESH,
    )


def place():
    me = lax.axis_index("sp")
    return me // (2 * SIDE), me // 2 % SIDE, me % 2


def plane_gather(whole, half, many, send, receive):
    z, y, c = place()
    part = lax.axis_index("tp")

    def origin(first, second):
        over_z = (z + c * first + (1 - c) * second + 2 * SIDE) % SIDE
        over_y = (y + (1 - c) * first + c * second + 2 * SIDE) % SIDE
        return (over_z * SIDE + over_y) * 2 + c

    along = [(origin(1, 0), part), (origin(-1, 0), part)]
    cross = [(origin(0, 1), part), (origin(0, -1), part)]
    partner = ((z * SIDE + y) * 2 + 1 - c, part)
    lines = (0, -1, 1, 2)
    at_line, at_far, at_over, at_last, at_shared = 0, 1, 2, 6, 7

    def go(block, peer, kind):
        remote(block, block, send.at[0], receive.at[kind], peer).start()

    def arrived(shards, kind):
        remote(many(shards), many(shards), send.at[0], receive.at[kind], partner).wait_recv()

    def share(at):
        go(whole(at), partner, at_shared)

    def spread_line(first):
        for peer in cross:
            go(whole(origin(first, 0)), peer, at_over + lines.index(first))
        share(origin(first, 0))

    def forward(first):
        arrived(2, at_over + lines.index(first))
        for way in range(2):
            go(half(origin(first, (-1, 1)[way]), way), cross[way], at_last)
        for way in range(2):
            share(origin(first, (-1, 1)[way]))

    for peer in along:
        go(whole(origin(0, 0)), peer, at_line)
    spread_line(0)
    yield
    arrived(2, at_line)
    for way in range(2):
        go(half(origin((-1, 1)[way], 0), way), along[way], at_far)
    for way in range(2):
        spread_line((-1, 1)[way])
    yield
    forward(0)
    yield
    arrived(1, at_far)
    spread_line(2)
    yield
    forward(-1)
    yield
    forward(1)
    yield
    forward(2)
    yield
    arrived(4, at_last)
    for first in lines:
        share(origin(first, 2))
    yield
    arrived(16, at_shared)
    yield
    remote(many(31), many(31), send.at[0], receive.at[at_line], partner).wait_send()
    yield


GATHER_WAITS = 8


def mixer_kernel(
    shift,
    x_ref,
    norm_gain_ref,
    gate_weights_ref,
    value_weights_ref,
    in_weights_ref,
    out_weights_ref,
    ahead_weights_ref,
    behind_weights_ref,
    offset_ref,
    speed_ref,
    taps_value_ref,
    taps_in_ref,
    taps_out_ref,
    gain_ref,
    w_out_ref,
    result_ref,
    tokens,
    weights,
    full_out,
    placed,
    paired,
    padded,
    gates,
    scale_ref,
    halo,
    signal_ref,
    inward_ref,
    outward_ref,
    within_ref,
    rows_ref,
    block_states_ref,
    block_logs_ref,
    sent,
    slices,
    log_tiles,
    all_logs,
    returned,
    incoming,
    total,
    staged,
    mixed,
    wide_gates,
    summed_ref,
    relay,
    raw_tokens,
    weights_send,
    weights_receive,
    out_send,
    out_receive,
    pair_send,
    pair_receive,
    cross_send,
    cross_receive,
    token_send,
    token_receive,
    onward_receive,
    halo_send,
    halo_receive,
    logs_send,
    logs_receive,
    scan_send,
    scan_receive,
    back_send,
    back_receive,
    mixed_send,
    mixed_receive,
    relay_receive,
    handed_receive,
    load,
):
    me, part = lax.axis_index("sp"), lax.axis_index("tp")
    core = me % 2
    stretches = slices.shape[0]
    parts, chunk, features = tokens.shape
    extent = parts * chunk
    depth = value_weights_ref.shape[0]
    content = value_weights_ref.shape[1]
    state_width = in_weights_ref.shape[1]
    heads = ahead_weights_ref.shape[0]
    groups = state_width // STATE
    ratio = heads // groups
    span = ratio * HEAD_DIM
    channels = content + 2 * state_width
    count = extent // BLOCK
    f32, bf16 = jnp.float32, jnp.bfloat16

    peers = [((me + hop) % stretches, part) for hop in range(1, stretches)]
    across = [(me, (part + hop) % parts) for hop in range(1, parts)]
    settle = greet(peers + across)

    quarter = chunk // 4
    loads = []
    for at in (0, 3, 1, 2):
        here = pl.ds(at * quarter, quarter)
        copy = pltpu.make_async_copy(x_ref.at[here], raw_tokens.at[here], load.at[at])
        copy.start()
        loads.append(copy)
    rows = 16

    def normalize(at):
        for step in range(quarter // rows):
            here = pl.ds(at * quarter + step * rows, rows)
            normed = rms_rows(raw_tokens[here, :]) * norm_gain_ref[...]
            tokens[part, here, :] = normed.astype(bf16)

    own_rows = pl.ds(pl.multiple_of(me * depth, depth), depth)
    weights[own_rows, 0:content] = value_weights_ref[...]
    weights[own_rows, content : content + state_width] = in_weights_ref[...]
    weights[own_rows, content + state_width : channels] = out_weights_ref[...]
    weights[own_rows, channels : channels + content] = gate_weights_ref[...]

    def across_rows(left, right):
        return lax.dot_general(left, right, (((0,), (0,)), ((), ())), preferred_element_type=f32)

    head_row = lax.broadcasted_iota(jnp.int32, (heads, LANES), 0)
    head_lane = lax.broadcasted_iota(jnp.int32, (heads, LANES), 1)
    to_ahead = (head_row == head_lane).astype(bf16)
    to_behind = (head_row + heads == head_lane).astype(bf16)
    weights[own_rows, channels + content :] = (
        across_rows(ahead_weights_ref[...], to_ahead)
        + across_rows(behind_weights_ref[...], to_behind)
    ).astype(bf16)
    for at, copy in zip((0, 3), loads[:2]):
        copy.wait()
        normalize(at)
    settle()

    right, left = (me, (part + 1) % parts), (me, (part + parts - 1) % parts)
    before, after = (part + parts - 1) % parts, (part + 1) % parts
    opposite = (part + 2) % parts

    def piece(source, at):
        return tokens.at[source, pl.ds(at * quarter, quarter)]

    orders = ((0, 1, 2, 3), (3, 2, 1, 0))

    def arrived(block, semaphore):
        remote(block, block, semaphore, semaphore, right).wait_recv()

    def left_here(block, semaphore):
        remote(block, block, semaphore, semaphore, right).wait_send()

    def send_own(step):
        for way, peer in enumerate((right, left)):
            block = piece(part, orders[way][step])
            received = token_receive.at[way, min(step, 2)]
            remote(block, block, token_send.at[0], received, peer).start()

    def pass_on(step):
        for way, peer in enumerate((right, left)):
            block = piece((before, after)[way], orders[way][step])
            arrived(block, token_receive.at[way, step])
            remote(block, block, token_send.at[0], onward_receive.at[0], peer).start()

    weights_steps = plane_gather(
        lambda at: weights.at[pl.ds(pl.multiple_of(at * depth, depth), depth)],
        lambda at, side: weights.at[
            pl.ds(pl.multiple_of(at * depth + side * (depth // 2), depth // 2), depth // 2)
        ],
        lambda shards: weights.at[pl.ds(0, shards * depth)],
        weights_send,
        weights_receive,
    )
    out_steps = plane_gather(
        lambda at: full_out.at[at],
        lambda at, side: full_out.at[at, pl.ds(side * (parts // 2), parts // 2)],
        lambda shards: full_out.at[pl.ds(0, shards)],
        out_send,
        out_receive,
    )

    z, y, _ = place()
    partner = ((z * SIDE + y) * 2 + 1 - core, part)
    pair = remote(placed.at[1 - core], paired, pair_send.at[0], pair_receive.at[0], partner)
    send_own(0)
    next(weights_steps)
    width = w_out_ref.shape[0]
    move_row = lax.broadcasted_iota(jnp.int32, (width, LANES), 0)
    move_lane = lax.broadcasted_iota(jnp.int32, (width, LANES), 1)
    to_half = (move_row + core * width == move_lane).astype(bf16)
    half_rows = w_out_ref.shape[1] // 2
    for side in range(2):
        placed[side] = across_rows(
            w_out_ref[:, side * half_rows : (side + 1) * half_rows], to_half
        ).astype(bf16)
    pair.start()
    loads[2].wait()
    normalize(1)
    pair.wait_recv()
    full_out[me, part] = placed[core] + paired[...]
    loads[3].wait()
    normalize(2)
    for peer in (right, left):
        block = full_out.at[me, part]
        remote(block, block, cross_send.at[0], cross_receive.at[0], peer).start()
    send_own(1)
    next(weights_steps)
    both = full_out.at[me, pl.ds(0, 2)]
    arrived(both, cross_receive.at[0])
    block = full_out.at[me, (part + 3 + 2 * core) % parts]
    onward_peer = (me, (part + 1 + 2 * core) % parts)
    remote(block, block, cross_send.at[0], cross_receive.at[1], onward_peer).start()
    send_own(2)
    next(weights_steps)
    next(weights_steps)
    pass_on(0)
    send_own(3)
    next(weights_steps)
    next(weights_steps)
    pass_on(1)
    next(weights_steps)
    arrived(full_out.at[me, 0], cross_receive.at[1])
    next(out_steps)
    next(weights_steps)
    next(weights_steps)

    wide_tile = 2 * LANES

    def product(source, columns):
        return jnp.dot(tokens[source], weights[:, columns], preferred_element_type=f32)

    row = lax.broadcasted_iota(jnp.int32, (BLOCK, BLOCK), 0)
    column = lax.broadcasted_iota(jnp.int32, (BLOCK, BLOCK), 1)
    triangles = jnp.concatenate([row >= column, row <= column], axis=0).astype(bf16)
    lane = lax.broadcasted_iota(jnp.int32, (1, LANES), 1)
    spare = jnp.zeros((1, LANES - 2 * heads), f32)
    offset = jnp.concatenate([offset_ref[0:1, :], offset_ref[1:2, :], spare], axis=1)
    rate = jnp.concatenate([speed_ref[0:1, :], speed_ref[1:2, :], spare], axis=1)

    def decays_of(source, raw):
        steps = softplus(raw + offset - shift)
        logs = -steps * rate
        logs = jnp.concatenate([logs[:BLOCK], logs[BLOCK:]], axis=1)
        high = logs.astype(bf16)
        rest = logs - high.astype(f32)
        middle = rest.astype(bf16)
        low = (rest - middle.astype(f32)).astype(bf16)
        sums = jnp.dot(
            triangles,
            jnp.concatenate([high, middle, low], axis=1),
            preferred_element_type=f32,
        )
        sums = sums[:, : 2 * LANES] + (
            sums[:, 2 * LANES : 4 * LANES] + sums[:, 4 * LANES : 6 * LANES]
        )
        for inner in range(2):
            at = 2 * source + inner
            here = pl.ds(pl.multiple_of(at * BLOCK, BLOCK), BLOCK)
            lanes_of = slice(inner * LANES, (inner + 1) * LANES)
            within = jnp.where(lane < heads, sums[:BLOCK, lanes_of], sums[BLOCK:, lanes_of])
            final = jnp.where(lane < heads, within[BLOCK - 1 : BLOCK], within[0:1])
            step = steps[inner * BLOCK : (inner + 1) * BLOCK]
            within_ref[here, :] = within
            rows_ref[0 : 2 * heads, here] = within.T[0 : 2 * heads]
            rows_ref[2 * heads : 4 * heads, here] = step.T[0 : 2 * heads]
            scale_ref[here, :] = jnp.exp(final - within) * step
            for group in range(groups):
                block_logs_ref[group, at] = jnp.concatenate(
                    [spread(final, way * heads + group * ratio, ratio) for way in range(2)],
                    axis=1,
                )

    def project(source):
        start = pl.multiple_of(source * chunk, chunk)
        raw = product(source, slice(channels + content, channels + content + LANES))
        decays_of(source, raw.astype(bf16).astype(f32))

        for first in range(0, channels, wide_tile):
            columns = slice(first, first + wide_tile)
            padded[pl.ds(start + 8, chunk), columns] = (
                product(source, columns).astype(bf16).astype(f32)
            )
    def project_gate(source):
        start = pl.multiple_of(source * chunk, chunk)

        for first in range(0, content, wide_tile):
            gates[pl.ds(start, chunk), first : first + wide_tile] = product(
                source, slice(channels + first, channels + first + wide_tile)
            ).astype(bf16)

    edges = []
    for way, hop in enumerate((1, stretches - 1)):
        peer = ((me + hop) % stretches, part)
        block = padded.at[pl.ds((extent, 8)[way], 8)]
        edges.append(
            remote(block, halo.at[way], halo_send.at[0], halo_receive.at[0], peer)
        )

    def send_edges():
        for copy in edges:
            copy.start()

    def take_edges():
        arrived(halo, halo_receive.at[0])
        left_here(halo, halo_send.at[0])
        padded[0:8, :] = halo[0] * (me > 0).astype(f32)
        padded[pl.ds(extent + 8, 8), :] = halo[1] * (me < stretches - 1).astype(f32)

    def filter_columns(start, first):
        part_rows = padded[pl.ds(start, BLOCK + 16), first : first + wide_tile]
        if first < content:
            taps = taps_value_ref[:, first : first + wide_tile]
        elif first < content + state_width:
            taps = taps_in_ref[:, first - content : first - content + wide_tile]
        else:
            base = first - content - state_width
            taps = taps_out_ref[:, base : base + wide_tile]
        mixed_rows = (
            taps[0:1] * part_rows[7 : 7 + BLOCK]
            + taps[1:2] * part_rows[8 : 8 + BLOCK]
            + taps[2:3] * part_rows[9 : 9 + BLOCK]
        )
        return silu(mixed_rows).astype(bf16)

    def filter_outward(at):
        start = pl.multiple_of(at * BLOCK, BLOCK)
        for first in range(0, state_width, wide_tile):
            outward_ref[pl.ds(start, BLOCK), first : first + wide_tile] = filter_columns(
                start, content + state_width + first
            )

    def block(at):
        start = pl.multiple_of(at * BLOCK, BLOCK)
        here = pl.ds(start, BLOCK)
        filtered = jnp.concatenate(
            [
                filter_columns(start, first)
                for first in range(0, content + state_width, wide_tile)
            ],
            axis=1,
        )
        signal = filtered[:, :content]
        inward = filtered[:, content : content + state_width]
        signal_ref[here, :] = signal
        inward_ref[here, :] = inward
        scale = scale_ref[here, :]
        for group in range(groups):
            wide = signal[:, group * span : (group + 1) * span].astype(f32)
            scaled = jnp.concatenate(
                [wide * spread(scale, way * heads + group * ratio, ratio) for way in range(2)],
                axis=1,
            ).astype(bf16)
            block_states_ref[group, at] = lax.dot_general(
                inward[:, group * STATE : (group + 1) * STATE],
                scaled,
                (((0,), (0,)), ((), ())),
                preferred_element_type=f32,
            )

    project(part)
    project_gate(part)
    arrived(tokens.at[0, pl.ds(0, 2 * quarter)], token_receive.at[0, 2])
    project(before)
    project_gate(before)
    next(out_steps)
    next(out_steps)
    arrived(tokens.at[0, pl.ds(0, 2 * quarter)], token_receive.at[1, 2])
    project(after)

    early = part % 3 == 0

    @pl.when(early)
    def _():
        send_edges()

    project_gate(after)
    next(out_steps)
    ahead_of_last = 2 * opposite + 3
    turn = 2 - 2 * (part // 3)

    def early_block(step, _):
        at = (ahead_of_last + (step + turn) % 4) % count
        block(at)
        filter_outward(at)
        return 0

    early_block(0, 0)
    early_block(1, 0)
    next(out_steps)

    @pl.when(early)
    def _():
        take_edges()

    early_block(2, 0)
    early_block(3, 0)
    next(out_steps)
    arrived(tokens.at[0], onward_receive.at[0])
    project(opposite)

    @pl.when(part % 3 != 0)
    def _():
        send_edges()

    summed_logs = [
        functools.reduce(jnp.add, [block_logs_ref[group, at] for at in range(count)])
        for group in range(groups)
    ]
    for way in range(2):
        for group in range(groups):
            for lane_tile in range(span // LANES):
                first = way * span + lane_tile * LANES
                log_tiles[way * groups + group, lane_tile : lane_tile + 1, :] = summed_logs[group][
                    :, first : first + LANES
                ]
    next(out_steps)
    handled = stretches // (2 * groups)
    for peer in peers:
        remote(
            log_tiles.at[peer[0] // handled],
            all_logs.at[me],
            logs_send.at[0],
            logs_receive.at[0],
            peer,
        ).start()
    all_logs[me] = log_tiles[me // handled]
    late_turn = 2 * (part // 2) * (1 - part % 2)

    def late_at(step):
        return (ahead_of_last + 4 + (step + late_turn) % 4) % count

    def late_block(step, _):
        block(late_at(step))
        return 0

    late_block(0, 0)
    late_block(1, 0)

    @pl.when(part % 3 != 0)
    def _():
        take_edges()

    late_block(2, 0)
    late_block(3, 0)

    slice_rows = sent.shape[1]
    per_state = STATE // slice_rows
    for group in range(groups):

        def onward(at, carried):
            return enter(at, 0, *carried)

        def back(at, carried):
            return enter(count - 1 - at, span, *carried)

        def enter(at, base, state, logs):
            added = block_states_ref[group, at, :, base : base + span]
            decay = block_logs_ref[group, at, :, base : base + span]
            block_states_ref[group, at, :, base : base + span] = state
            block_logs_ref[group, at, :, base : base + span] = logs
            return state * jnp.exp(decay) + added, logs + decay

        empty = jnp.zeros((STATE, span), f32)
        still = jnp.zeros((1, span), f32)
        for way, body in enumerate((onward, back)):
            state, _ = lax.fori_loop(0, count, body, (empty, still))
            state = state.astype(bf16)
            first = (way * groups + group) * per_state
            sent[first : first + per_state] = state.reshape(per_state, slice_rows, span)

    def exchange(source, target, send, receive):
        for peer in peers:
            remote(source.at[peer[0]], target.at[me], send.at[0], receive.at[0], peer).start()
        target[me] = source[me]

    exchange(sent, slices, scan_send, scan_receive)

    lanes = lax.broadcasted_iota(jnp.int32, (BLOCK, LANES), 1)

    def diagonal(at, _):
        here = pl.ds(pl.multiple_of(at * BLOCK, BLOCK), BLOCK)
        within = within_ref[here, :]
        wide_gates[here, :] = silu(gates[here, :].astype(f32))
        for group in range(groups):
            intersect = lax.dot_general(
                outward_ref[here, group * STATE : (group + 1) * STATE],
                inward_ref[here, group * STATE : (group + 1) * STATE],
                (((1,), (1,)), ((), ())),
                preferred_element_type=f32,
            )
            products = []
            for head in range(group * ratio, (group + 1) * ratio):
                other = heads + head
                gap_ahead = within[:, head : head + 1] - rows_ref[head : head + 1, here]
                gap_behind = within[:, other : other + 1] - rows_ref[other : other + 1, here]
                step_ahead = rows_ref[2 * heads + head : 2 * heads + head + 1, here]
                step_behind = rows_ref[2 * heads + other : 2 * heads + other + 1, here]
                gap = jnp.where(row >= column, gap_ahead, gap_behind)
                step = jnp.where(
                    row > column,
                    step_ahead,
                    jnp.where(row < column, step_behind, step_ahead + step_behind),
                )
                mixing = (intersect * jnp.exp(gap) * step).astype(bf16)
                tile = head // 2 * 2 * HEAD_DIM
                products.append(
                    jnp.dot(
                        mixing,
                        signal_ref[here, tile : tile + LANES],
                        preferred_element_type=f32,
                    )
                )
            for two in range(ratio // 2):
                at_tile = (group * ratio + 2 * two) * HEAD_DIM
                total[here, at_tile : at_tile + LANES] = jnp.where(
                    lanes < HEAD_DIM, products[2 * two], products[2 * two + 1]
                )
        return 0

    project_gate(opposite)

    def late_outward(step, _):
        filter_outward(late_at(step))
        return 0

    lax.fori_loop(0, 4, late_outward, 0)
    lax.fori_loop(0, count // 2, diagonal, 0)
    next(out_steps)
    arrived(all_logs.at[pl.ds(0, stretches - 1)], logs_receive.at[0])
    arrived(slices.at[pl.ds(0, stretches - 1)], scan_receive.at[0])

    reverse = me // (stretches // 2)

    def scan(step, state):
        for inner in range(4):
            at = 4 * step + inner
            source = at + reverse * (stretches - 1 - 2 * at)
            returned[source] = state.astype(bf16)
            logs = jnp.concatenate(
                [all_logs[source, at_lane : at_lane + 1, :] for at_lane in range(span // LANES)],
                axis=1,
            )
            state = state * jnp.exp(logs) + slices[source].astype(f32)
        return state

    lax.fori_loop(0, stretches // 4, scan, jnp.zeros((slice_rows, span), f32))
    exchange(returned, incoming, back_send, back_receive)
    lax.fori_loop(count // 2, count, diagonal, 0)
    next(out_steps)
    arrived(incoming.at[pl.ds(0, stretches - 1)], back_receive.at[0])

    def carried_in(way, group):
        first = (way * groups + group) * per_state
        return incoming[first : first + per_state].reshape(STATE, span).astype(f32)

    def finish(source, inner):
        at = source * (chunk // BLOCK) + inner
        here = pl.ds(pl.multiple_of(at * BLOCK, BLOCK), BLOCK)
        decays = jnp.exp(within_ref[here, :])
        for group in range(groups):
            wide = slice(group * span, (group + 1) * span)
            summed = total[here, wide]
            for way in range(2):
                base = way * span
                state = block_states_ref[group, at, :, base : base + span] + jnp.exp(
                    block_logs_ref[group, at, :, base : base + span]
                ) * carried_in(way, group)
                carried = jnp.dot(
                    outward_ref[here, group * STATE : (group + 1) * STATE],
                    state.astype(bf16),
                    preferred_element_type=f32,
                )
                summed += carried * spread(decays, way * heads + group * ratio, ratio)
            gated = summed * wide_gates[here, wide]
            scale = lax.rsqrt(jnp.mean(gated * gated, axis=-1, keepdims=True) + EPSILON)
            staged[source, pl.ds(pl.multiple_of(inner * BLOCK, BLOCK), BLOCK), wide] = (
                gated * scale * gain_ref[:, wide]
            ).astype(bf16)

    sides = (right, left)
    half_chunk = chunk // 2

    def half_of(at):
        return pl.ds(at * half_chunk, half_chunk)

    def finish_half(source, at):
        def one(step, _):
            finish(source, step)
            return 0

        lax.fori_loop(at * half_chunk // BLOCK, (at + 1) * half_chunk // BLOCK, one, 0)

    for way in range(2):
        finish_half(opposite, way)
        remote(
            staged.at[opposite, half_of(way)],
            relay.at[way],
            mixed_send.at[0],
            relay_receive.at[way],
            sides[way],
        ).start()
    for at in range(2):
        for way, target in enumerate((after, before)):
            finish_half(target, at)
            remote(
                staged.at[target, half_of(at)],
                mixed.at[part, half_of(at)],
                mixed_send.at[0],
                mixed_receive.at[way],
                sides[way],
            ).start()
    for way in range(2):
        arrived(relay.at[way], relay_receive.at[way])
        remote(
            relay.at[way],
            mixed.at[(before, after)[way], half_of(way)],
            mixed_send.at[0],
            handed_receive.at[0],
            sides[way],
        ).start()
    for at in range(2):
        finish_half(part, at)

    half = content // 2

    def output(block_of, source, first, last):
        broad = 8 * LANES

        def tile(at, _):
            columns = pl.ds(pl.multiple_of(at * broad, broad), broad)
            summed = 0.0 if first else summed_ref[:, columns]
            for side in range(2):
                weight = jnp.concatenate(
                    [full_out[16 * at + 2 * place + side, source] for place in range(8)], axis=1
                )
                summed += jnp.dot(
                    block_of[source, :, side * half : (side + 1) * half],
                    weight,
                    preferred_element_type=f32,
                )
            if last:
                result_ref[:, columns] = summed.astype(bf16)
            else:
                summed_ref[:, columns] = summed
            return 0

        lax.fori_loop(0, features // broad, tile, 0)

    output(staged, part, True, False)
    arrived(mixed.at[before], mixed_receive.at[0])
    output(mixed, before, False, False)
    arrived(mixed.at[after], mixed_receive.at[1])
    output(mixed, after, False, False)
    arrived(mixed.at[opposite], handed_receive.at[0])
    output(mixed, opposite, False, True)
    next(weights_steps)
    next(out_steps)
    pair.wait_send()
    left_here(full_out.at[0, pl.ds(0, 3)], cross_send.at[0])
    left_here(tokens.at[pl.ds(0, 3)], token_send.at[0])
    left_here(all_logs.at[pl.ds(0, stretches - 1)], logs_send.at[0])
    left_here(slices.at[pl.ds(0, stretches - 1)], scan_send.at[0])
    left_here(incoming.at[pl.ds(0, stretches - 1)], back_send.at[0])
    left_here(mixed, mixed_send.at[0])


def on_device(
    input_activations,
    norm_gain,
    w_gate,
    w_value,
    w_state_in,
    w_state_out,
    w_step_forward,
    w_step_backward,
    step_offset,
    fading_speed,
    conv_value,
    conv_state_in,
    conv_state_out,
    out_gain,
    w_out,
):
    stretches = lax.axis_size("sp")
    parts = lax.axis_size("tp")
    chunk, features = input_activations.shape
    extent = parts * chunk
    depth = w_gate.shape[0]
    content = w_value.shape[1]
    state_width = w_state_in.shape[1]
    heads = w_step_forward.shape[1]
    groups = state_width // STATE
    span = heads // groups * HEAD_DIM
    channels = content + 2 * state_width
    count = extent // BLOCK
    slice_rows = 2 * groups * STATE // stretches
    shift = math.log(extent * stretches)
    bf16, f32 = jnp.bfloat16, jnp.float32
    vmem, dma = pltpu.VMEM, pltpu.SemaphoreType.DMA
    space = pl.BlockSpec(memory_space=pltpu.VMEM)
    half_rows = w_out.shape[0] // 2
    return pl.pallas_call(
        functools.partial(mixer_kernel, shift),
        out_shape=pltpu.VMEM((chunk, features), bf16),
        in_specs=[pl.BlockSpec(memory_space=pl.ANY)] + [space] * 14,
        out_specs=space,
        scratch_shapes=[
            vmem((parts, chunk, features), bf16),
            vmem((stretches * depth, channels + content + LANES), bf16),
            vmem((stretches, parts, half_rows, LANES), bf16),
            vmem((2, half_rows, LANES), bf16),
            vmem((half_rows, LANES), bf16),
            vmem((extent + 16, channels), f32),
            vmem((extent, content), bf16),
            vmem((extent, LANES), f32),
            vmem((2, 8, channels), f32),
            vmem((extent, content), bf16),
            vmem((extent, state_width), bf16),
            vmem((extent, state_width), bf16),
            vmem((extent, LANES), f32),
            vmem((4 * heads, extent), f32),
            vmem((groups, count, STATE, 2 * span), f32),
            vmem((groups, count, 1, 2 * span), f32),
            vmem((stretches, slice_rows, span), bf16),
            vmem((stretches, slice_rows, span), bf16),
            vmem((2 * groups, 8, LANES), f32),
            vmem((stretches, 8, LANES), f32),
            vmem((stretches, slice_rows, span), bf16),
            vmem((stretches, slice_rows, span), bf16),
            vmem((extent, content), f32),
            vmem((parts, chunk, content), bf16),
            vmem((parts, chunk, content), bf16),
            vmem((extent, content), f32),
            vmem((chunk, features), f32),
            vmem((2, chunk // 2, content), bf16),
            vmem((chunk, features), bf16),
            dma((1,)),
            dma((GATHER_WAITS,)),
            dma((1,)),
            dma((GATHER_WAITS,)),
            dma((1,)),
            dma((1,)),
            dma((1,)),
            dma((2,)),
            dma((1,)),
            dma((2, 3)),
            dma((1,)),
            dma((1,)),
            dma((1,)),
            dma((1,)),
            dma((1,)),
            dma((1,)),
            dma((1,)),
            dma((1,)),
            dma((1,)),
            dma((1,)),
            dma((2,)),
            dma((2,)),
            dma((1,)),
            dma((4,)),
        ],
        cost_estimate=pl.CostEstimate(
            flops=int(3e10), bytes_accessed=1 << 20, transcendentals=0
        ),
        compiler_params=pltpu.CompilerParams(
            collective_id=1, has_side_effects=True, vmem_limit_bytes=VMEM_LIMIT
        ),
    )(
        input_activations,
        norm_gain.reshape(1, features),
        w_gate,
        w_value,
        w_state_in,
        w_state_out,
        w_step_forward.T,
        w_step_backward.T,
        step_offset,
        fading_speed,
        conv_value,
        conv_state_in,
        conv_state_out,
        out_gain.reshape(1, content),
        w_out.T,
    )


def solution(mesh):
    return jax.shard_map(
        on_device,
        mesh=mesh,
        in_specs=(
            P(("sp", "tp"), None),
            P(),
            P("sp", "tp"),
            P("sp", "tp"),
            P("sp", "tp"),
            P("sp", "tp"),
            P("sp", "tp"),
            P("sp", "tp"),
            P(None, "tp"),
            P(None, "tp"),
            P(None, "tp"),
            P(None, "tp"),
            P(None, "tp"),
            P("tp"),
            P("tp", "sp"),
        ),
        out_specs=P(("sp", "tp"), None),
        check_vma=False,
    )
```

```python
import functools
import math

import jax
import jax.numpy as jnp
from jax import lax
from jax.experimental import pallas as pl
from jax.experimental.pallas import tpu as pltpu
from jax.sharding import PartitionSpec as P

HEAD_DIM = 64
STATE = 128
BLOCK = 128
LANES = 128
EPSILON = 1e-06
HIGHEST = lax.Precision.HIGHEST
VMEM_LIMIT = 60 * 1024 * 1024
SIDE = 4


def rms_rows(values):
    wide = values.astype(jnp.float32)
    return wide * lax.rsqrt(jnp.mean(wide * wide, axis=-1, keepdims=True) + EPSILON)


def softplus(values):
    return jnp.maximum(values, 0.0) + jnp.log1p(jnp.exp(-jnp.abs(values)))


def spread(columns, first, count):
    rows = columns.shape[0]
    lane = lax.broadcasted_iota(jnp.int32, (rows, LANES), 1)
    tiles = []
    for at in range(first, first + count, 2):
        low = jnp.broadcast_to(columns[:, at : at + 1], (rows, LANES))
        high = jnp.broadcast_to(columns[:, at + 1 : at + 2], (rows, LANES))
        tiles.append(jnp.where(lane < HEAD_DIM, low, high))
    return jnp.concatenate(tiles, axis=1)


def silu(values):
    half = 0.5 * values
    return half + half * jnp.tanh(half)


def greet(peers):
    barrier = pltpu.get_barrier_semaphore()
    for peer in peers:
        pl.semaphore_signal(
            barrier, inc=1, device_id=peer, device_id_type=pl.DeviceIdType.MESH
        )
    return lambda: pl.semaphore_wait(barrier, len(peers))


def remote(source, target, send, receive, peer):
    return pltpu.make_async_remote_copy(
        src_ref=source,
        dst_ref=target,
        send_sem=send,
        recv_sem=receive,
        device_id=peer,
        device_id_type=pl.DeviceIdType.MESH,
    )


def place():
    me = lax.axis_index("sp")
    return me // (2 * SIDE), me // 2 % SIDE, me % 2


def plane_gather(whole, half, many, send, receive):
    z, y, c = place()
    part = lax.axis_index("tp")

    def origin(first, second):
        over_z = (z + c * first + (1 - c) * second + 2 * SIDE) % SIDE
        over_y = (y + (1 - c) * first + c * second + 2 * SIDE) % SIDE
        return (over_z * SIDE + over_y) * 2 + c

    along = [(origin(1, 0), part), (origin(-1, 0), part)]
    cross = [(origin(0, 1), part), (origin(0, -1), part)]
    partner = ((z * SIDE + y) * 2 + 1 - c, part)
    lines = (0, -1, 1, 2)
    at_line, at_far, at_over, at_last, at_shared = 0, 1, 2, 6, 7

    def go(block, peer, kind):
        remote(block, block, send.at[0], receive.at[kind], peer).start()

    def arrived(shards, kind):
        remote(many(shards), many(shards), send.at[0], receive.at[kind], partner).wait_recv()

    def share(at):
        go(whole(at), partner, at_shared)

    def spread_line(first):
        for peer in cross:
            go(whole(origin(first, 0)), peer, at_over + lines.index(first))
        share(origin(first, 0))

    def forward(first):
        arrived(2, at_over + lines.index(first))
        for way in range(2):
            go(half(origin(first, (-1, 1)[way]), way), cross[way], at_last)
        for way in range(2):
            share(origin(first, (-1, 1)[way]))

    for peer in along:
        go(whole(origin(0, 0)), peer, at_line)
    spread_line(0)
    yield
    arrived(2, at_line)
    for way in range(2):
        go(half(origin((-1, 1)[way], 0), way), along[way], at_far)
    for way in range(2):
        spread_line((-1, 1)[way])
    yield
    forward(0)
    yield
    arrived(1, at_far)
    spread_line(2)
    yield
    forward(-1)
    yield
    forward(1)
    yield
    forward(2)
    yield
    arrived(4, at_last)
    for first in lines:
        share(origin(first, 2))
    yield
    arrived(16, at_shared)
    yield
    remote(many(31), many(31), send.at[0], receive.at[at_line], partner).wait_send()
    yield


GATHER_WAITS = 8


def mixer_kernel(
    shift,
    x_ref,
    norm_gain_ref,
    gate_weights_ref,
    value_weights_ref,
    in_weights_ref,
    out_weights_ref,
    ahead_weights_ref,
    behind_weights_ref,
    offset_ref,
    speed_ref,
    taps_value_ref,
    taps_in_ref,
    taps_out_ref,
    gain_ref,
    w_out_ref,
    result_ref,
    tokens,
    weights,
    full_out,
    placed,
    paired,
    padded,
    gates,
    scale_ref,
    halo,
    signal_ref,
    inward_ref,
    outward_ref,
    within_ref,
    rows_ref,
    block_states_ref,
    block_logs_ref,
    sent,
    slices,
    log_tiles,
    all_logs,
    returned,
    incoming,
    total,
    staged,
    mixed,
    wide_gates,
    summed_ref,
    relay,
    raw_tokens,
    weights_send,
    weights_receive,
    out_send,
    out_receive,
    pair_send,
    pair_receive,
    cross_send,
    cross_receive,
    token_send,
    token_receive,
    onward_receive,
    halo_send,
    halo_receive,
    logs_send,
    logs_receive,
    scan_send,
    scan_receive,
    back_send,
    back_receive,
    mixed_send,
    mixed_receive,
    relay_receive,
    handed_receive,
    load,
):
    me, part = lax.axis_index("sp"), lax.axis_index("tp")
    core = me % 2
    stretches = slices.shape[0]
    parts, chunk, features = tokens.shape
    extent = parts * chunk
    depth = value_weights_ref.shape[0]
    content = value_weights_ref.shape[1]
    state_width = in_weights_ref.shape[1]
    heads = ahead_weights_ref.shape[0]
    groups = state_width // STATE
    ratio = heads // groups
    span = ratio * HEAD_DIM
    channels = content + 2 * state_width
    count = extent // BLOCK
    f32, bf16 = jnp.float32, jnp.bfloat16

    peers = [((me + hop) % stretches, part) for hop in range(1, stretches)]
    across = [(me, (part + hop) % parts) for hop in range(1, parts)]
    settle = greet(peers + across)

    quarter = chunk // 4
    loads = []
    for at in (0, 3, 1, 2):
        here = pl.ds(at * quarter, quarter)
        copy = pltpu.make_async_copy(x_ref.at[here], raw_tokens.at[here], load.at[at])
        copy.start()
        loads.append(copy)
    rows = 16

    def normalize(at):
        for step in range(quarter // rows):
            here = pl.ds(at * quarter + step * rows, rows)
            normed = rms_rows(raw_tokens[here, :]) * norm_gain_ref[...]
            tokens[part, here, :] = normed.astype(bf16)

    own_rows = pl.ds(pl.multiple_of(me * depth, depth), depth)
    weights[own_rows, 0:content] = value_weights_ref[...]
    weights[own_rows, content : content + state_width] = in_weights_ref[...]
    weights[own_rows, content + state_width : channels] = out_weights_ref[...]
    weights[own_rows, channels : channels + content] = gate_weights_ref[...]

    def across_rows(left, right):
        return lax.dot_general(left, right, (((0,), (0,)), ((), ())), preferred_element_type=f32)

    head_row = lax.broadcasted_iota(jnp.int32, (heads, LANES), 0)
    head_lane = lax.broadcasted_iota(jnp.int32, (heads, LANES), 1)
    to_ahead = (head_row == head_lane).astype(bf16)
    to_behind = (head_row + heads == head_lane).astype(bf16)
    weights[own_rows, channels + content :] = (
        across_rows(ahead_weights_ref[...], to_ahead)
        + across_rows(behind_weights_ref[...], to_behind)
    ).astype(bf16)
    for at, copy in zip((0, 3), loads[:2]):
        copy.wait()
        normalize(at)
    settle()

    right, left = (me, (part + 1) % parts), (me, (part + parts - 1) % parts)
    before, after = (part + parts - 1) % parts, (part + 1) % parts
    opposite = (part + 2) % parts

    def piece(source, at):
        return tokens.at[source, pl.ds(at * quarter, quarter)]

    orders = ((0, 1, 2, 3), (3, 2, 1, 0))

    def arrived(block, semaphore):
        remote(block, block, semaphore, semaphore, right).wait_recv()

    def left_here(block, semaphore):
        remote(block, block, semaphore, semaphore, right).wait_send()

    def send_own(step):
        for way, peer in enumerate((right, left)):
            block = piece(part, orders[way][step])
            received = token_receive.at[way, min(step, 2)]
            remote(block, block, token_send.at[0], received, peer).start()

    def pass_on(step):
        for way, peer in enumerate((right, left)):
            block = piece((before, after)[way], orders[way][step])
            arrived(block, token_receive.at[way, step])
            remote(block, block, token_send.at[0], onward_receive.at[0], peer).start()

    weights_steps = plane_gather(
        lambda at: weights.at[pl.ds(pl.multiple_of(at * depth, depth), depth)],
        lambda at, side: weights.at[
            pl.ds(pl.multiple_of(at * depth + side * (depth // 2), depth // 2), depth // 2)
        ],
        lambda shards: weights.at[pl.ds(0, shards * depth)],
        weights_send,
        weights_receive,
    )
    out_steps = plane_gather(
        lambda at: full_out.at[at],
        lambda at, side: full_out.at[at, pl.ds(side * (parts // 2), parts // 2)],
        lambda shards: full_out.at[pl.ds(0, shards)],
        out_send,
        out_receive,
    )

    z, y, _ = place()
    partner = ((z * SIDE + y) * 2 + 1 - core, part)
    pair = remote(placed.at[1 - core], paired, pair_send.at[0], pair_receive.at[0], partner)
    send_own(0)
    next(weights_steps)
    width = w_out_ref.shape[0]
    move_row = lax.broadcasted_iota(jnp.int32, (width, LANES), 0)
    move_lane = lax.broadcasted_iota(jnp.int32, (width, LANES), 1)
    to_half = (move_row + core * width == move_lane).astype(bf16)
    half_rows = w_out_ref.shape[1] // 2
    for side in range(2):
        placed[side] = across_rows(
            w_out_ref[:, side * half_rows : (side + 1) * half_rows], to_half
        ).astype(bf16)
    pair.start()
    loads[2].wait()
    normalize(1)
    pair.wait_recv()
    full_out[me, part] = placed[core] + paired[...]
    loads[3].wait()
    normalize(2)
    for peer in (right, left):
        block = full_out.at[me, part]
        remote(block, block, cross_send.at[0], cross_receive.at[0], peer).start()
    send_own(1)
    next(weights_steps)
    next(weights_steps)
    both = full_out.at[me, pl.ds(0, 2)]
    arrived(both, cross_receive.at[0])
    block = full_out.at[me, (part + 3 + 2 * core) % parts]
    onward_peer = (me, (part + 1 + 2 * core) % parts)
    remote(block, block, cross_send.at[0], cross_receive.at[1], onward_peer).start()
    send_own(2)
    send_own(3)
    next(weights_steps)
    pass_on(0)
    next(weights_steps)
    next(weights_steps)
    pass_on(1)
    next(weights_steps)
    arrived(full_out.at[me, 0], cross_receive.at[1])
    next(out_steps)
    next(weights_steps)
    next(weights_steps)

    wide_tile = 2 * LANES

    def product(source, columns):
        return jnp.dot(tokens[source], weights[:, columns], preferred_element_type=f32)

    row = lax.broadcasted_iota(jnp.int32, (BLOCK, BLOCK), 0)
    column = lax.broadcasted_iota(jnp.int32, (BLOCK, BLOCK), 1)
    triangles = jnp.concatenate([row >= column, row <= column], axis=0).astype(bf16)
    lane = lax.broadcasted_iota(jnp.int32, (1, LANES), 1)
    spare = jnp.zeros((1, LANES - 2 * heads), f32)
    offset = jnp.concatenate([offset_ref[0:1, :], offset_ref[1:2, :], spare], axis=1)
    rate = jnp.concatenate([speed_ref[0:1, :], speed_ref[1:2, :], spare], axis=1)

    def decays_of(source, raw):
        steps = softplus(raw + offset - shift)
        logs = -steps * rate
        logs = jnp.concatenate([logs[:BLOCK], logs[BLOCK:]], axis=1)
        high = logs.astype(bf16)
        rest = logs - high.astype(f32)
        middle = rest.astype(bf16)
        low = (rest - middle.astype(f32)).astype(bf16)
        sums = jnp.dot(
            triangles,
            jnp.concatenate([high, middle, low], axis=1),
            preferred_element_type=f32,
        )
        sums = sums[:, : 2 * LANES] + (
            sums[:, 2 * LANES : 4 * LANES] + sums[:, 4 * LANES : 6 * LANES]
        )
        for inner in range(2):
            at = 2 * source + inner
            here = pl.ds(pl.multiple_of(at * BLOCK, BLOCK), BLOCK)
            lanes_of = slice(inner * LANES, (inner + 1) * LANES)
            within = jnp.where(lane < heads, sums[:BLOCK, lanes_of], sums[BLOCK:, lanes_of])
            final = jnp.where(lane < heads, within[BLOCK - 1 : BLOCK], within[0:1])
            step = steps[inner * BLOCK : (inner + 1) * BLOCK]
            within_ref[here, :] = within
            rows_ref[0 : 2 * heads, here] = within.T[0 : 2 * heads]
            rows_ref[2 * heads : 4 * heads, here] = step.T[0 : 2 * heads]
            scale_ref[here, :] = jnp.exp(final - within) * step
            for group in range(groups):
                block_logs_ref[group, at] = jnp.concatenate(
                    [spread(final, way * heads + group * ratio, ratio) for way in range(2)],
                    axis=1,
                )

    def project(source):
        start = pl.multiple_of(source * chunk, chunk)
        raw = product(source, slice(channels + content, channels + content + LANES))
        decays_of(source, raw.astype(bf16).astype(f32))

        for first in range(0, channels, wide_tile):
            columns = slice(first, first + wide_tile)
            padded[pl.ds(start + 8, chunk), columns] = (
                product(source, columns).astype(bf16).astype(f32)
            )
    def project_gate(source):
        start = pl.multiple_of(source * chunk, chunk)

        for first in range(0, content, wide_tile):
            gates[pl.ds(start, chunk), first : first + wide_tile] = product(
                source, slice(channels + first, channels + first + wide_tile)
            ).astype(bf16)

    edges = []
    for way, hop in enumerate((1, stretches - 1)):
        peer = ((me + hop) % stretches, part)
        block = padded.at[pl.ds((extent, 8)[way], 8)]
        edges.append(
            remote(block, halo.at[way], halo_send.at[0], halo_receive.at[0], peer)
        )

    def send_edges():
        for copy in edges:
            copy.start()

    def take_edges():
        arrived(halo, halo_receive.at[0])
        left_here(halo, halo_send.at[0])
        padded[0:8, :] = halo[0] * (me > 0).astype(f32)
        padded[pl.ds(extent + 8, 8), :] = halo[1] * (me < stretches - 1).astype(f32)

    def filter_columns(start, first):
        part_rows = padded[pl.ds(start, BLOCK + 16), first : first + wide_tile]
        if first < content:
            taps = taps_value_ref[:, first : first + wide_tile]
        elif first < content + state_width:
            taps = taps_in_ref[:, first - content : first - content + wide_tile]
        else:
            base = first - content - state_width
            taps = taps_out_ref[:, base : base + wide_tile]
        mixed_rows = (
            taps[0:1] * part_rows[7 : 7 + BLOCK]
            + taps[1:2] * part_rows[8 : 8 + BLOCK]
            + taps[2:3] * part_rows[9 : 9 + BLOCK]
        )
        return silu(mixed_rows).astype(bf16)

    def filter_outward(at):
        start = pl.multiple_of(at * BLOCK, BLOCK)
        for first in range(0, state_width, wide_tile):
            outward_ref[pl.ds(start, BLOCK), first : first + wide_tile] = filter_columns(
                start, content + state_width + first
            )

    def block(at):
        start = pl.multiple_of(at * BLOCK, BLOCK)
        here = pl.ds(start, BLOCK)
        filtered = jnp.concatenate(
            [
                filter_columns(start, first)
                for first in range(0, content + state_width, wide_tile)
            ],
            axis=1,
        )
        signal = filtered[:, :content]
        inward = filtered[:, content : content + state_width]
        signal_ref[here, :] = signal
        inward_ref[here, :] = inward
        scale = scale_ref[here, :]
        for group in range(groups):
            wide = signal[:, group * span : (group + 1) * span].astype(f32)
            scaled = jnp.concatenate(
                [wide * spread(scale, way * heads + group * ratio, ratio) for way in range(2)],
                axis=1,
            ).astype(bf16)
            block_states_ref[group, at] = lax.dot_general(
                inward[:, group * STATE : (group + 1) * STATE],
                scaled,
                (((0,), (0,)), ((), ())),
                preferred_element_type=f32,
            )

    project(part)
    project_gate(part)
    next(out_steps)
    next(out_steps)
    arrived(tokens.at[0, pl.ds(0, 2 * quarter)], token_receive.at[0, 2])
    project(before)
    project_gate(before)
    arrived(tokens.at[0, pl.ds(0, 2 * quarter)], token_receive.at[1, 2])
    project(after)

    early = part % 3 == 0

    @pl.when(early)
    def _():
        send_edges()

    project_gate(after)
    ahead_of_last = 2 * opposite + 3
    turn = 2 - 2 * (part // 3)

    def early_block(step, _):
        at = (ahead_of_last + (step + turn) % 4) % count
        block(at)
        filter_outward(at)
        return 0

    early_block(0, 0)
    early_block(1, 0)

    @pl.when(early)
    def _():
        take_edges()

    early_block(2, 0)
    early_block(3, 0)
    next(out_steps)
    arrived(tokens.at[0], onward_receive.at[0])
    project(opposite)

    @pl.when(part % 3 != 0)
    def _():
        send_edges()

    summed_logs = [
        functools.reduce(jnp.add, [block_logs_ref[group, at] for at in range(count)])
        for group in range(groups)
    ]
    for way in range(2):
        for group in range(groups):
            for lane_tile in range(span // LANES):
                first = way * span + lane_tile * LANES
                log_tiles[way * groups + group, lane_tile : lane_tile + 1, :] = summed_logs[group][
                    :, first : first + LANES
                ]
    handled = stretches // (2 * groups)
    for peer in peers:
        remote(
            log_tiles.at[peer[0] // handled],
            all_logs.at[me],
            logs_send.at[0],
            logs_receive.at[0],
            peer,
        ).start()
    all_logs[me] = log_tiles[me // handled]
    late_turn = 2 * (part // 2) * (1 - part % 2)

    def late_at(step):
        return (ahead_of_last + 4 + (step + late_turn) % 4) % count

    def late_block(step, _):
        block(late_at(step))
        return 0

    late_block(0, 0)
    late_block(1, 0)

    @pl.when(part % 3 != 0)
    def _():
        take_edges()

    late_block(2, 0)
    late_block(3, 0)

    slice_rows = sent.shape[1]
    per_state = STATE // slice_rows

    def decayed(state, group, at, lanes_of):
        return (
            state * jnp.exp(block_logs_ref[group, at, :, lanes_of])
            + block_states_ref[group, at, :, lanes_of]
        )

    for group in range(groups):
        for way in range(2):
            for lane_tile in range(span // LANES):
                first = way * span + lane_tile * LANES
                order = range(count) if way == 0 else range(count - 1, -1, -1)
                state = jnp.zeros((STATE, LANES), f32)
                for at in order:
                    state = decayed(state, group, at, slice(first, first + LANES))
                at_slice = (way * groups + group) * per_state
                here = slice(lane_tile * LANES, (lane_tile + 1) * LANES)
                sent[at_slice : at_slice + per_state, :, here] = state.astype(bf16).reshape(
                    per_state, slice_rows, LANES
                )

    def keep_entries(group):
        def onward(at, carried):
            return enter(at, 0, *carried)

        def back(at, carried):
            return enter(count - 1 - at, span, *carried)

        def enter(at, base, state, logs):
            added = block_states_ref[group, at, :, base : base + span]
            decay = block_logs_ref[group, at, :, base : base + span]
            block_states_ref[group, at, :, base : base + span] = state
            block_logs_ref[group, at, :, base : base + span] = logs
            return state * jnp.exp(decay) + added, logs + decay

        empty = jnp.zeros((STATE, span), f32)
        still = jnp.zeros((1, span), f32)
        for body in (onward, back):
            lax.fori_loop(0, count, body, (empty, still))

    def exchange(source, target, send, receive):
        for peer in peers:
            remote(source.at[peer[0]], target.at[me], send.at[0], receive.at[0], peer).start()
        target[me] = source[me]

    exchange(sent, slices, scan_send, scan_receive)

    lanes = lax.broadcasted_iota(jnp.int32, (BLOCK, LANES), 1)

    def diagonal(at, _):
        here = pl.ds(pl.multiple_of(at * BLOCK, BLOCK), BLOCK)
        within = within_ref[here, :]
        wide_gates[here, :] = silu(gates[here, :].astype(f32))
        for group in range(groups):
            intersect = lax.dot_general(
                outward_ref[here, group * STATE : (group + 1) * STATE],
                inward_ref[here, group * STATE : (group + 1) * STATE],
                (((1,), (1,)), ((), ())),
                preferred_element_type=f32,
            )
            products = []
            for head in range(group * ratio, (group + 1) * ratio):
                other = heads + head
                gap_ahead = within[:, head : head + 1] - rows_ref[head : head + 1, here]
                gap_behind = within[:, other : other + 1] - rows_ref[other : other + 1, here]
                step_ahead = rows_ref[2 * heads + head : 2 * heads + head + 1, here]
                step_behind = rows_ref[2 * heads + other : 2 * heads + other + 1, here]
                gap = jnp.where(row >= column, gap_ahead, gap_behind)
                step = jnp.where(
                    row > column,
                    step_ahead,
                    jnp.where(row < column, step_behind, step_ahead + step_behind),
                )
                mixing = (intersect * jnp.exp(gap) * step).astype(bf16)
                tile = head // 2 * 2 * HEAD_DIM
                products.append(
                    jnp.dot(
                        mixing,
                        signal_ref[here, tile : tile + LANES],
                        preferred_element_type=f32,
                    )
                )
            for two in range(ratio // 2):
                at_tile = (group * ratio + 2 * two) * HEAD_DIM
                total[here, at_tile : at_tile + LANES] = jnp.where(
                    lanes < HEAD_DIM, products[2 * two], products[2 * two + 1]
                )
        return 0

    project_gate(opposite)

    def late_outward(step, _):
        filter_outward(late_at(step))
        return 0

    lax.fori_loop(0, 4, late_outward, 0)
    for group in range(groups):
        keep_entries(group)
    lax.fori_loop(0, count // 2, diagonal, 0)
    arrived(all_logs.at[pl.ds(0, stretches - 1)], logs_receive.at[0])
    arrived(slices.at[pl.ds(0, stretches - 1)], scan_receive.at[0])

    reverse = me // (stretches // 2)

    def scan(step, state):
        for inner in range(4):
            at = 4 * step + inner
            source = at + reverse * (stretches - 1 - 2 * at)
            returned[source] = state.astype(bf16)
            logs = jnp.concatenate(
                [all_logs[source, at_lane : at_lane + 1, :] for at_lane in range(span // LANES)],
                axis=1,
            )
            state = state * jnp.exp(logs) + slices[source].astype(f32)
        return state

    lax.fori_loop(0, stretches // 4, scan, jnp.zeros((slice_rows, span), f32))
    exchange(returned, incoming, back_send, back_receive)
    lax.fori_loop(count // 2, count, diagonal, 0)
    arrived(incoming.at[pl.ds(0, stretches - 1)], back_receive.at[0])

    for _ in range(3):
        next(out_steps)
    def carried_in(way, group):
        first = (way * groups + group) * per_state
        return incoming[first : first + per_state].reshape(STATE, span).astype(f32)

    def finish(source, inner):
        at = source * (chunk // BLOCK) + inner
        here = pl.ds(pl.multiple_of(at * BLOCK, BLOCK), BLOCK)
        decays = jnp.exp(within_ref[here, :])
        for group in range(groups):
            wide = slice(group * span, (group + 1) * span)
            summed = total[here, wide]
            for way in range(2):
                base = way * span
                state = block_states_ref[group, at, :, base : base + span] + jnp.exp(
                    block_logs_ref[group, at, :, base : base + span]
                ) * carried_in(way, group)
                carried = jnp.dot(
                    outward_ref[here, group * STATE : (group + 1) * STATE],
                    state.astype(bf16),
                    preferred_element_type=f32,
                )
                summed += carried * spread(decays, way * heads + group * ratio, ratio)
            gated = summed * wide_gates[here, wide]
            scale = lax.rsqrt(jnp.mean(gated * gated, axis=-1, keepdims=True) + EPSILON)
            staged[source, pl.ds(pl.multiple_of(inner * BLOCK, BLOCK), BLOCK), wide] = (
                gated * scale * gain_ref[:, wide]
            ).astype(bf16)

    sides = (right, left)
    half_chunk = chunk // 2

    def half_of(at):
        return pl.ds(at * half_chunk, half_chunk)

    def finish_half(source, at):
        def one(step, _):
            finish(source, step)
            return 0

        lax.fori_loop(at * half_chunk // BLOCK, (at + 1) * half_chunk // BLOCK, one, 0)

    for way in range(2):
        finish_half(opposite, way)
        remote(
            staged.at[opposite, half_of(way)],
            relay.at[way],
            mixed_send.at[0],
            relay_receive.at[way],
            sides[way],
        ).start()
    for at in range(2):
        for way, target in enumerate((after, before)):
            finish_half(target, at)
            remote(
                staged.at[target, half_of(at)],
                mixed.at[part, half_of(at)],
                mixed_send.at[0],
                mixed_receive.at[way],
                sides[way],
            ).start()
    for way in range(2):
        arrived(relay.at[way], relay_receive.at[way])
        remote(
            relay.at[way],
            mixed.at[(before, after)[way], half_of(way)],
            mixed_send.at[0],
            handed_receive.at[0],
            sides[way],
        ).start()
    for at in range(2):
        finish_half(part, at)

    next(out_steps)
    next(out_steps)
    half = content // 2

    def output(block_of, source, first, last):
        broad = 8 * LANES

        def tile(at, _):
            columns = pl.ds(pl.multiple_of(at * broad, broad), broad)
            summed = 0.0 if first else summed_ref[:, columns]
            for side in range(2):
                weight = jnp.concatenate(
                    [full_out[16 * at + 2 * place + side, source] for place in range(8)], axis=1
                )
                summed += jnp.dot(
                    block_of[source, :, side * half : (side + 1) * half],
                    weight,
                    preferred_element_type=f32,
                )
            if last:
                result_ref[:, columns] = summed.astype(bf16)
            else:
                summed_ref[:, columns] = summed
            return 0

        lax.fori_loop(0, features // broad, tile, 0)

    output(staged, part, True, False)
    arrived(mixed.at[before], mixed_receive.at[0])
    output(mixed, before, False, False)
    arrived(mixed.at[after], mixed_receive.at[1])
    output(mixed, after, False, False)
    arrived(mixed.at[opposite], handed_receive.at[0])
    output(mixed, opposite, False, True)
    next(weights_steps)
    next(out_steps)
    pair.wait_send()
    left_here(full_out.at[0, pl.ds(0, 3)], cross_send.at[0])
    left_here(tokens.at[pl.ds(0, 3)], token_send.at[0])
    left_here(all_logs.at[pl.ds(0, stretches - 1)], logs_send.at[0])
    left_here(slices.at[pl.ds(0, stretches - 1)], scan_send.at[0])
    left_here(incoming.at[pl.ds(0, stretches - 1)], back_send.at[0])
    left_here(mixed, mixed_send.at[0])


def on_device(
    input_activations,
    norm_gain,
    w_gate,
    w_value,
    w_state_in,
    w_state_out,
    w_step_forward,
    w_step_backward,
    step_offset,
    fading_speed,
    conv_value,
    conv_state_in,
    conv_state_out,
    out_gain,
    w_out,
):
    stretches = lax.axis_size("sp")
    parts = lax.axis_size("tp")
    chunk, features = input_activations.shape
    extent = parts * chunk
    depth = w_gate.shape[0]
    content = w_value.shape[1]
    state_width = w_state_in.shape[1]
    heads = w_step_forward.shape[1]
    groups = state_width // STATE
    span = heads // groups * HEAD_DIM
    channels = content + 2 * state_width
    count = extent // BLOCK
    slice_rows = 2 * groups * STATE // stretches
    shift = math.log(extent * stretches)
    bf16, f32 = jnp.bfloat16, jnp.float32
    vmem, dma = pltpu.VMEM, pltpu.SemaphoreType.DMA
    space = pl.BlockSpec(memory_space=pltpu.VMEM)
    half_rows = w_out.shape[0] // 2
    return pl.pallas_call(
        functools.partial(mixer_kernel, shift),
        out_shape=pltpu.VMEM((chunk, features), bf16),
        in_specs=[pl.BlockSpec(memory_space=pl.ANY)] + [space] * 14,
        out_specs=space,
        scratch_shapes=[
            vmem((parts, chunk, features), bf16),
            vmem((stretches * depth, channels + content + LANES), bf16),
            vmem((stretches, parts, half_rows, LANES), bf16),
            vmem((2, half_rows, LANES), bf16),
            vmem((half_rows, LANES), bf16),
            vmem((extent + 16, channels), f32),
            vmem((extent, content), bf16),
            vmem((extent, LANES), f32),
            vmem((2, 8, channels), f32),
            vmem((extent, content), bf16),
            vmem((extent, state_width), bf16),
            vmem((extent, state_width), bf16),
            vmem((extent, LANES), f32),
            vmem((4 * heads, extent), f32),
            vmem((groups, count, STATE, 2 * span), f32),
            vmem((groups, count, 1, 2 * span), f32),
            vmem((stretches, slice_rows, span), bf16),
            vmem((stretches, slice_rows, span), bf16),
            vmem((2 * groups, 8, LANES), f32),
            vmem((stretches, 8, LANES), f32),
            vmem((stretches, slice_rows, span), bf16),
            vmem((stretches, slice_rows, span), bf16),
            vmem((extent, content), f32),
            vmem((parts, chunk, content), bf16),
            vmem((parts, chunk, content), bf16),
            vmem((extent, content), f32),
            vmem((chunk, features), f32),
            vmem((2, chunk // 2, content), bf16),
            vmem((chunk, features), bf16),
            dma((1,)),
            dma((GATHER_WAITS,)),
            dma((1,)),
            dma((GATHER_WAITS,)),
            dma((1,)),
            dma((1,)),
            dma((1,)),
            dma((2,)),
            dma((1,)),
            dma((2, 3)),
            dma((1,)),
            dma((1,)),
            dma((1,)),
            dma((1,)),
            dma((1,)),
            dma((1,)),
            dma((1,)),
            dma((1,)),
            dma((1,)),
            dma((1,)),
            dma((2,)),
            dma((2,)),
            dma((1,)),
            dma((4,)),
        ],
        cost_estimate=pl.CostEstimate(
            flops=int(3e10), bytes_accessed=1 << 20, transcendentals=0
        ),
        compiler_params=pltpu.CompilerParams(
            collective_id=1, has_side_effects=True, vmem_limit_bytes=VMEM_LIMIT
        ),
    )(
        input_activations,
        norm_gain.reshape(1, features),
        w_gate,
        w_value,
        w_state_in,
        w_state_out,
        w_step_forward.T,
        w_step_backward.T,
        step_offset,
        fading_speed,
        conv_value,
        conv_state_in,
        conv_state_out,
        out_gain.reshape(1, content),
        w_out.T,
    )


def solution(mesh):
    return jax.shard_map(
        on_device,
        mesh=mesh,
        in_specs=(
            P(("sp", "tp"), None),
            P(),
            P("sp", "tp"),
            P("sp", "tp"),
            P("sp", "tp"),
            P("sp", "tp"),
            P("sp", "tp"),
            P("sp", "tp"),
            P(None, "tp"),
            P(None, "tp"),
            P(None, "tp"),
            P(None, "tp"),
            P(None, "tp"),
            P("tp"),
            P("tp", "sp"),
        ),
        out_specs=P(("sp", "tp"), None),
        check_vma=False,
    )
```

```python
import functools
import math

import jax
import jax.numpy as jnp
from jax import lax
from jax.experimental import pallas as pl
from jax.experimental.pallas import tpu as pltpu
from jax.sharding import PartitionSpec as P

HEAD_DIM = 64
STATE = 128
BLOCK = 128
LANES = 128
EPSILON = 1e-06
HIGHEST = lax.Precision.HIGHEST
VMEM_LIMIT = 60 * 1024 * 1024
SIDE = 4


def rms_rows(values):
    wide = values.astype(jnp.float32)
    return wide * lax.rsqrt(jnp.mean(wide * wide, axis=-1, keepdims=True) + EPSILON)


def softplus(values):
    return jnp.maximum(values, 0.0) + jnp.log1p(jnp.exp(-jnp.abs(values)))


def spread(columns, first, count):
    rows = columns.shape[0]
    lane = lax.broadcasted_iota(jnp.int32, (rows, LANES), 1)
    tiles = []
    for at in range(first, first + count, 2):
        low = jnp.broadcast_to(columns[:, at : at + 1], (rows, LANES))
        high = jnp.broadcast_to(columns[:, at + 1 : at + 2], (rows, LANES))
        tiles.append(jnp.where(lane < HEAD_DIM, low, high))
    return jnp.concatenate(tiles, axis=1)


def silu(values):
    half = 0.5 * values
    return half + half * jnp.tanh(half)


def greet(peers):
    barrier = pltpu.get_barrier_semaphore()
    for peer in peers:
        pl.semaphore_signal(
            barrier, inc=1, device_id=peer, device_id_type=pl.DeviceIdType.MESH
        )
    return lambda: pl.semaphore_wait(barrier, len(peers))


def remote(source, target, send, receive, peer):
    return pltpu.make_async_remote_copy(
        src_ref=source,
        dst_ref=target,
        send_sem=send,
        recv_sem=receive,
        device_id=peer,
        device_id_type=pl.DeviceIdType.MESH,
    )


def place():
    me = lax.axis_index("sp")
    return me // (2 * SIDE), me // 2 % SIDE, me % 2


def plane_gather(whole, half, many, send, receive):
    z, y, c = place()
    part = lax.axis_index("tp")

    def origin(first, second):
        over_z = (z + c * first + (1 - c) * second + 2 * SIDE) % SIDE
        over_y = (y + (1 - c) * first + c * second + 2 * SIDE) % SIDE
        return (over_z * SIDE + over_y) * 2 + c

    along = [(origin(1, 0), part), (origin(-1, 0), part)]
    cross = [(origin(0, 1), part), (origin(0, -1), part)]
    partner = ((z * SIDE + y) * 2 + 1 - c, part)
    lines = (0, -1, 1, 2)
    at_line, at_far, at_over, at_last, at_shared = 0, 1, 2, 6, 7

    def go(block, peer, kind):
        remote(block, block, send.at[0], receive.at[kind], peer).start()

    def arrived(shards, kind):
        remote(many(shards), many(shards), send.at[0], receive.at[kind], partner).wait_recv()

    def share(at):
        go(whole(at), partner, at_shared)

    def spread_line(first):
        for peer in cross:
            go(whole(origin(first, 0)), peer, at_over + lines.index(first))
        share(origin(first, 0))

    def forward(first):
        arrived(2, at_over + lines.index(first))
        for way in range(2):
            go(half(origin(first, (-1, 1)[way]), way), cross[way], at_last)
        for way in range(2):
            share(origin(first, (-1, 1)[way]))

    for peer in along:
        go(whole(origin(0, 0)), peer, at_line)
    spread_line(0)
    yield
    arrived(2, at_line)
    for way in range(2):
        go(half(origin((-1, 1)[way], 0), way), along[way], at_far)
    for way in range(2):
        spread_line((-1, 1)[way])
    yield
    forward(0)
    yield
    arrived(1, at_far)
    spread_line(2)
    yield
    forward(-1)
    yield
    forward(1)
    yield
    forward(2)
    yield
    arrived(4, at_last)
    for first in lines:
        share(origin(first, 2))
    yield
    arrived(16, at_shared)
    yield
    remote(many(31), many(31), send.at[0], receive.at[at_line], partner).wait_send()
    yield


GATHER_WAITS = 8


def mixer_kernel(
    shift,
    x_ref,
    norm_gain_ref,
    gate_weights_ref,
    value_weights_ref,
    in_weights_ref,
    out_weights_ref,
    ahead_weights_ref,
    behind_weights_ref,
    offset_ref,
    speed_ref,
    taps_value_ref,
    taps_in_ref,
    taps_out_ref,
    gain_ref,
    w_out_ref,
    result_ref,
    tokens,
    weights,
    full_out,
    placed,
    paired,
    padded,
    gates,
    scale_ref,
    halo,
    signal_ref,
    inward_ref,
    outward_ref,
    within_ref,
    rows_ref,
    block_states_ref,
    block_logs_ref,
    sent,
    slices,
    log_tiles,
    all_logs,
    returned,
    incoming,
    total,
    staged,
    mixed,
    wide_gates,
    summed_ref,
    relay,
    raw_tokens,
    weights_send,
    weights_receive,
    out_send,
    out_receive,
    pair_send,
    pair_receive,
    cross_send,
    cross_receive,
    token_send,
    token_receive,
    onward_receive,
    halo_send,
    halo_receive,
    logs_send,
    logs_receive,
    scan_send,
    scan_receive,
    back_send,
    back_receive,
    mixed_send,
    mixed_receive,
    relay_receive,
    handed_receive,
    load,
):
    me, part = lax.axis_index("sp"), lax.axis_index("tp")
    core = me % 2
    stretches = slices.shape[0]
    parts, chunk, features = tokens.shape
    extent = parts * chunk
    depth = value_weights_ref.shape[0]
    content = value_weights_ref.shape[1]
    state_width = in_weights_ref.shape[1]
    heads = ahead_weights_ref.shape[0]
    groups = state_width // STATE
    ratio = heads // groups
    span = ratio * HEAD_DIM
    channels = content + 2 * state_width
    count = extent // BLOCK
    f32, bf16 = jnp.float32, jnp.bfloat16

    peers = [((me + hop) % stretches, part) for hop in range(1, stretches)]
    across = [(me, (part + hop) % parts) for hop in range(1, parts)]
    settle = greet(peers + across)

    quarter = chunk // 4
    loads = []
    for at in (0, 3, 1, 2):
        here = pl.ds(at * quarter, quarter)
        copy = pltpu.make_async_copy(x_ref.at[here], raw_tokens.at[here], load.at[at])
        copy.start()
        loads.append(copy)
    rows = 16

    def normalize(at):
        for step in range(quarter // rows):
            here = pl.ds(at * quarter + step * rows, rows)
            normed = rms_rows(raw_tokens[here, :]) * norm_gain_ref[...]
            tokens[part, here, :] = normed.astype(bf16)

    own_rows = pl.ds(pl.multiple_of(me * depth, depth), depth)
    weights[own_rows, 0:content] = value_weights_ref[...]
    weights[own_rows, content : content + state_width] = in_weights_ref[...]
    weights[own_rows, content + state_width : channels] = out_weights_ref[...]
    weights[own_rows, channels : channels + content] = gate_weights_ref[...]

    def across_rows(left, right):
        return lax.dot_general(left, right, (((0,), (0,)), ((), ())), preferred_element_type=f32)

    head_row = lax.broadcasted_iota(jnp.int32, (heads, LANES), 0)
    head_lane = lax.broadcasted_iota(jnp.int32, (heads, LANES), 1)
    to_ahead = (head_row == head_lane).astype(bf16)
    to_behind = (head_row + heads == head_lane).astype(bf16)
    weights[own_rows, channels + content :] = (
        across_rows(ahead_weights_ref[...], to_ahead)
        + across_rows(behind_weights_ref[...], to_behind)
    ).astype(bf16)
    for at, copy in zip((0, 3), loads[:2]):
        copy.wait()
        normalize(at)
    settle()

    right, left = (me, (part + 1) % parts), (me, (part + parts - 1) % parts)
    before, after = (part + parts - 1) % parts, (part + 1) % parts
    opposite = (part + 2) % parts

    def piece(source, at):
        return tokens.at[source, pl.ds(at * quarter, quarter)]

    orders = ((0, 1, 2, 3), (3, 2, 1, 0))

    def arrived(block, semaphore):
        remote(block, block, semaphore, semaphore, right).wait_recv()

    def left_here(block, semaphore):
        remote(block, block, semaphore, semaphore, right).wait_send()

    def send_own(step):
        for way, peer in enumerate((right, left)):
            block = piece(part, orders[way][step])
            received = token_receive.at[way, min(step, 2)]
            remote(block, block, token_send.at[0], received, peer).start()

    def pass_on(step):
        for way, peer in enumerate((right, left)):
            block = piece((before, after)[way], orders[way][step])
            arrived(block, token_receive.at[way, step])
            remote(block, block, token_send.at[0], onward_receive.at[0], peer).start()

    weights_steps = plane_gather(
        lambda at: weights.at[pl.ds(pl.multiple_of(at * depth, depth), depth)],
        lambda at, side: weights.at[
            pl.ds(pl.multiple_of(at * depth + side * (depth // 2), depth // 2), depth // 2)
        ],
        lambda shards: weights.at[pl.ds(0, shards * depth)],
        weights_send,
        weights_receive,
    )
    out_steps = plane_gather(
        lambda at: full_out.at[at],
        lambda at, side: full_out.at[at, pl.ds(side * (parts // 2), parts // 2)],
        lambda shards: full_out.at[pl.ds(0, shards)],
        out_send,
        out_receive,
    )

    z, y, _ = place()
    partner = ((z * SIDE + y) * 2 + 1 - core, part)
    pair = remote(placed.at[1 - core], paired, pair_send.at[0], pair_receive.at[0], partner)
    send_own(0)
    next(weights_steps)
    width = w_out_ref.shape[0]
    move_row = lax.broadcasted_iota(jnp.int32, (width, LANES), 0)
    move_lane = lax.broadcasted_iota(jnp.int32, (width, LANES), 1)
    to_half = (move_row + core * width == move_lane).astype(bf16)
    half_rows = w_out_ref.shape[1] // 2
    for side in range(2):
        placed[side] = across_rows(
            w_out_ref[:, side * half_rows : (side + 1) * half_rows], to_half
        ).astype(bf16)
    pair.start()
    loads[2].wait()
    normalize(1)
    pair.wait_recv()
    full_out[me, part] = placed[core] + paired[...]
    loads[3].wait()
    normalize(2)
    for peer in (right, left):
        block = full_out.at[me, part]
        remote(block, block, cross_send.at[0], cross_receive.at[0], peer).start()
    send_own(1)
    next(weights_steps)
    next(weights_steps)
    both = full_out.at[me, pl.ds(0, 2)]
    arrived(both, cross_receive.at[0])
    block = full_out.at[me, (part + 3 + 2 * core) % parts]
    onward_peer = (me, (part + 1 + 2 * core) % parts)
    remote(block, block, cross_send.at[0], cross_receive.at[1], onward_peer).start()
    send_own(2)
    send_own(3)
    next(weights_steps)
    pass_on(0)
    next(weights_steps)
    next(weights_steps)
    pass_on(1)
    next(weights_steps)
    arrived(full_out.at[me, 0], cross_receive.at[1])
    next(out_steps)
    next(weights_steps)
    next(weights_steps)

    wide_tile = 2 * LANES

    def product(source, columns):
        return jnp.dot(tokens[source], weights[:, columns], preferred_element_type=f32)

    row = lax.broadcasted_iota(jnp.int32, (BLOCK, BLOCK), 0)
    column = lax.broadcasted_iota(jnp.int32, (BLOCK, BLOCK), 1)
    triangles = jnp.concatenate([row >= column, row <= column], axis=0).astype(bf16)
    lane = lax.broadcasted_iota(jnp.int32, (1, LANES), 1)
    spare = jnp.zeros((1, LANES - 2 * heads), f32)
    offset = jnp.concatenate([offset_ref[0:1, :], offset_ref[1:2, :], spare], axis=1)
    rate = jnp.concatenate([speed_ref[0:1, :], speed_ref[1:2, :], spare], axis=1)

    def decays_of(source, raw):
        steps = softplus(raw + offset - shift)
        logs = -steps * rate
        logs = jnp.concatenate([logs[:BLOCK], logs[BLOCK:]], axis=1)
        high = logs.astype(bf16)
        rest = logs - high.astype(f32)
        middle = rest.astype(bf16)
        low = (rest - middle.astype(f32)).astype(bf16)
        sums = jnp.dot(
            triangles,
            jnp.concatenate([high, middle, low], axis=1),
            preferred_element_type=f32,
        )
        sums = sums[:, : 2 * LANES] + (
            sums[:, 2 * LANES : 4 * LANES] + sums[:, 4 * LANES : 6 * LANES]
        )
        for inner in range(2):
            at = 2 * source + inner
            here = pl.ds(pl.multiple_of(at * BLOCK, BLOCK), BLOCK)
            lanes_of = slice(inner * LANES, (inner + 1) * LANES)
            within = jnp.where(lane < heads, sums[:BLOCK, lanes_of], sums[BLOCK:, lanes_of])
            final = jnp.where(lane < heads, within[BLOCK - 1 : BLOCK], within[0:1])
            step = steps[inner * BLOCK : (inner + 1) * BLOCK]
            within_ref[here, :] = within
            rows_ref[0 : 2 * heads, here] = within.T[0 : 2 * heads]
            rows_ref[2 * heads : 4 * heads, here] = step.T[0 : 2 * heads]
            scale_ref[here, :] = jnp.exp(final - within) * step
            for group in range(groups):
                block_logs_ref[group, at] = jnp.concatenate(
                    [spread(final, way * heads + group * ratio, ratio) for way in range(2)],
                    axis=1,
                )

    def project(source):
        start = pl.multiple_of(source * chunk, chunk)
        raw = product(source, slice(channels + content, channels + content + LANES))
        decays_of(source, raw.astype(bf16).astype(f32))

        for first in range(0, channels, wide_tile):
            columns = slice(first, first + wide_tile)
            padded[pl.ds(start + 8, chunk), columns] = (
                product(source, columns).astype(bf16).astype(f32)
            )
    def project_gate(source):
        start = pl.multiple_of(source * chunk, chunk)

        for first in range(0, content, wide_tile):
            gates[pl.ds(start, chunk), first : first + wide_tile] = product(
                source, slice(channels + first, channels + first + wide_tile)
            ).astype(bf16)

    edges = []
    for way, hop in enumerate((1, stretches - 1)):
        peer = ((me + hop) % stretches, part)
        block = padded.at[pl.ds((extent, 8)[way], 8)]
        edges.append(
            remote(block, halo.at[way], halo_send.at[0], halo_receive.at[0], peer)
        )

    def send_edges():
        for copy in edges:
            copy.start()

    def take_edges():
        arrived(halo, halo_receive.at[0])
        left_here(halo, halo_send.at[0])
        padded[0:8, :] = halo[0] * (me > 0).astype(f32)
        padded[pl.ds(extent + 8, 8), :] = halo[1] * (me < stretches - 1).astype(f32)

    def filter_columns(start, first, width):
        part_rows = padded[pl.ds(start, BLOCK + 16), first : first + width]
        if first < content:
            taps = taps_value_ref[:, first : first + width]
        elif first < content + state_width:
            taps = taps_in_ref[:, first - content : first - content + width]
        else:
            base = first - content - state_width
            taps = taps_out_ref[:, base : base + width]
        mixed_rows = (
            taps[0:1] * part_rows[7 : 7 + BLOCK]
            + taps[1:2] * part_rows[8 : 8 + BLOCK]
            + taps[2:3] * part_rows[9 : 9 + BLOCK]
        )
        return silu(mixed_rows).astype(bf16)

    def filter_outward(at):
        start = pl.multiple_of(at * BLOCK, BLOCK)
        for first in range(0, state_width, wide_tile):
            outward_ref[pl.ds(start, BLOCK), first : first + wide_tile] = filter_columns(
                start, content + state_width + first, wide_tile
            )

    def block(at, group):
        start = pl.multiple_of(at * BLOCK, BLOCK)
        here = pl.ds(start, BLOCK)
        signal = filter_columns(start, group * span, span)
        inward = filter_columns(start, content + group * STATE, STATE)
        signal_ref[here, group * span : (group + 1) * span] = signal
        inward_ref[here, group * STATE : (group + 1) * STATE] = inward
        scale = scale_ref[here, :]
        wide = signal.astype(f32)
        scaled = jnp.concatenate(
            [wide * spread(scale, way * heads + group * ratio, ratio) for way in range(2)],
            axis=1,
        ).astype(bf16)
        block_states_ref[group, at] = lax.dot_general(
            inward, scaled, (((0,), (0,)), ((), ())), preferred_element_type=f32
        )

    project(part)
    project_gate(part)
    next(out_steps)
    next(out_steps)
    arrived(tokens.at[0, pl.ds(0, 2 * quarter)], token_receive.at[0, 2])
    project(before)
    project_gate(before)
    arrived(tokens.at[0, pl.ds(0, 2 * quarter)], token_receive.at[1, 2])
    project(after)

    early = part % 3 == 0

    @pl.when(early)
    def _():
        send_edges()

    project_gate(after)
    ahead_of_last = 2 * opposite + 3
    turn = 2 - 2 * (part // 3)

    def early_block(step, _):
        at = (ahead_of_last + (step + turn) % 4) % count
        for group in range(groups):
            block(at, group)
        filter_outward(at)
        return 0

    early_block(0, 0)
    early_block(1, 0)

    @pl.when(early)
    def _():
        take_edges()

    early_block(2, 0)
    early_block(3, 0)
    next(out_steps)
    arrived(tokens.at[0], onward_receive.at[0])
    project(opposite)

    @pl.when(part % 3 != 0)
    def _():
        send_edges()

    summed_logs = [
        functools.reduce(jnp.add, [block_logs_ref[group, at] for at in range(count)])
        for group in range(groups)
    ]
    for way in range(2):
        for group in range(groups):
            for lane_tile in range(span // LANES):
                first = way * span + lane_tile * LANES
                log_tiles[way * groups + group, lane_tile : lane_tile + 1, :] = summed_logs[group][
                    :, first : first + LANES
                ]
    handled = stretches // (2 * groups)
    for peer in peers:
        remote(
            log_tiles.at[peer[0] // handled],
            all_logs.at[me],
            logs_send.at[0],
            logs_receive.at[0],
            peer,
        ).start()
    all_logs[me] = log_tiles[me // handled]
    late_turn = 2 * (part // 2) * (1 - part % 2)

    def late_at(step):
        return (ahead_of_last + 4 + (step + late_turn) % 4) % count

    def late_block(step, group):
        block(late_at(step), group)

    slice_rows = sent.shape[1]
    per_state = STATE // slice_rows
    my_group = me // handled % groups
    my_index = me % handled + handled * (me // (groups * handled))

    def final_states(group):
        for way in range(2):
            order = range(count) if way == 0 else range(count - 1, -1, -1)
            for lane_tile in range(span // LANES):
                first = way * span + lane_tile * LANES
                state = jnp.zeros((STATE, LANES), f32)
                for at in order:
                    state = (
                        state * jnp.exp(block_logs_ref[group, at, :, first : first + LANES])
                        + block_states_ref[group, at, :, first : first + LANES]
                    )
                at_slice = (way * groups + group) * per_state
                here = slice(lane_tile * LANES, (lane_tile + 1) * LANES)
                sent[at_slice : at_slice + per_state, :, here] = state.astype(bf16).reshape(
                    per_state, slice_rows, LANES
                )

    def send_slices(group):
        scanners = 2 * handled
        for hop in range(scanners):
            index = (my_index + hop) % scanners
            target = index // handled * (groups * handled) + group * handled + index % handled

            def send():
                remote(
                    sent.at[target],
                    slices.at[me],
                    scan_send.at[0],
                    scan_receive.at[0],
                    (target, part),
                ).start()

            if hop:
                send()
            else:
                pl.when(my_group != group)(send)

        @pl.when(my_group == group)
        def _():
            slices[me] = sent[me]

    late_block(0, 0)
    late_block(1, 0)

    @pl.when(part % 3 != 0)
    def _():
        take_edges()

    late_block(2, 0)
    late_block(3, 0)
    final_states(0)
    send_slices(0)
    for step in range(4):
        late_block(step, 1)
    final_states(1)
    send_slices(1)

    def keep_entries(group):
        def onward(at, carried):
            return enter(at, 0, *carried)

        def back(at, carried):
            return enter(count - 1 - at, span, *carried)

        def enter(at, base, state, logs):
            added = block_states_ref[group, at, :, base : base + span]
            decay = block_logs_ref[group, at, :, base : base + span]
            block_states_ref[group, at, :, base : base + span] = state
            block_logs_ref[group, at, :, base : base + span] = logs
            return state * jnp.exp(decay) + added, logs + decay

        empty = jnp.zeros((STATE, span), f32)
        still = jnp.zeros((1, span), f32)
        for body in (onward, back):
            lax.fori_loop(0, count, body, (empty, still))

    lanes = lax.broadcasted_iota(jnp.int32, (BLOCK, LANES), 1)

    def diagonal(at, _):
        here = pl.ds(pl.multiple_of(at * BLOCK, BLOCK), BLOCK)
        within = within_ref[here, :]
        wide_gates[here, :] = silu(gates[here, :].astype(f32))
        for group in range(groups):
            intersect = lax.dot_general(
                outward_ref[here, group * STATE : (group + 1) * STATE],
                inward_ref[here, group * STATE : (group + 1) * STATE],
                (((1,), (1,)), ((), ())),
                preferred_element_type=f32,
            )
            products = []
            for head in range(group * ratio, (group + 1) * ratio):
                other = heads + head
                gap_ahead = within[:, head : head + 1] - rows_ref[head : head + 1, here]
                gap_behind = within[:, other : other + 1] - rows_ref[other : other + 1, here]
                step_ahead = rows_ref[2 * heads + head : 2 * heads + head + 1, here]
                step_behind = rows_ref[2 * heads + other : 2 * heads + other + 1, here]
                gap = jnp.where(row >= column, gap_ahead, gap_behind)
                step = jnp.where(
                    row > column,
                    step_ahead,
                    jnp.where(row < column, step_behind, step_ahead + step_behind),
                )
                mixing = (intersect * jnp.exp(gap) * step).astype(bf16)
                tile = head // 2 * 2 * HEAD_DIM
                products.append(
                    jnp.dot(
                        mixing,
                        signal_ref[here, tile : tile + LANES],
                        preferred_element_type=f32,
                    )
                )
            for two in range(ratio // 2):
                at_tile = (group * ratio + 2 * two) * HEAD_DIM
                total[here, at_tile : at_tile + LANES] = jnp.where(
                    lanes < HEAD_DIM, products[2 * two], products[2 * two + 1]
                )
        return 0

    next(out_steps)
    next(out_steps)
    project_gate(opposite)

    def late_outward(step, _):
        filter_outward(late_at(step))
        return 0

    lax.fori_loop(0, 4, late_outward, 0)
    for group in range(groups):
        keep_entries(group)
    lax.fori_loop(0, count // 4, diagonal, 0)

    reverse = me // (stretches // 2)

    def scan_slices(group):
        arrived(all_logs.at[pl.ds(0, stretches - 1)], logs_receive.at[0])
        arrived(slices.at[pl.ds(0, stretches - 1)], scan_receive.at[0])

        def scan(step, state):
            for inner in range(4):
                at = 4 * step + inner
                source = at + reverse * (stretches - 1 - 2 * at)
                returned[source] = state.astype(bf16)
                logs = jnp.concatenate(
                    [all_logs[source, tile : tile + 1, :] for tile in range(span // LANES)],
                    axis=1,
                )
                state = state * jnp.exp(logs) + slices[source].astype(f32)
            return state

        lax.fori_loop(0, stretches // 4, scan, jnp.zeros((slice_rows, span), f32))
        for peer in peers:
            remote(
                returned.at[peer[0]],
                incoming.at[me],
                back_send.at[0],
                back_receive.at[group],
                peer,
            ).start()
        incoming[me] = returned[me]

    def take_incoming(group):
        scanners = 2 * handled

        @pl.when(my_group == group)
        def _():
            arrived(incoming.at[pl.ds(0, scanners - 1)], back_receive.at[group])

        @pl.when(my_group != group)
        def _():
            arrived(incoming.at[pl.ds(0, scanners)], back_receive.at[group])

    @pl.when(my_group == 0)
    def _():
        scan_slices(0)

    lax.fori_loop(count // 4, count // 2, diagonal, 0)

    @pl.when(my_group == 1)
    def _():
        scan_slices(1)

    lax.fori_loop(count // 2, count, diagonal, 0)
    take_incoming(0)
    next(out_steps)
    def carried_in(way, group):
        first = (way * groups + group) * per_state
        return incoming[first : first + per_state].reshape(STATE, span).astype(f32)

    def finish(source, inner, group):
        at = source * (chunk // BLOCK) + inner
        here = pl.ds(pl.multiple_of(at * BLOCK, BLOCK), BLOCK)
        decays = jnp.exp(within_ref[here, :])
        wide = slice(group * span, (group + 1) * span)
        summed = total[here, wide]
        for way in range(2):
            base = way * span
            state = block_states_ref[group, at, :, base : base + span] + jnp.exp(
                block_logs_ref[group, at, :, base : base + span]
            ) * carried_in(way, group)
            carried = jnp.dot(
                outward_ref[here, group * STATE : (group + 1) * STATE],
                state.astype(bf16),
                preferred_element_type=f32,
            )
            summed += carried * spread(decays, way * heads + group * ratio, ratio)
        gated = summed * wide_gates[here, wide]
        scale = lax.rsqrt(jnp.mean(gated * gated, axis=-1, keepdims=True) + EPSILON)
        staged[group, source, pl.ds(inner * BLOCK, BLOCK), :] = (
            gated * scale * gain_ref[:, wide]
        ).astype(bf16)

    sides = (right, left)
    half_chunk = chunk // 2

    def half_of(at):
        return pl.ds(at * half_chunk, half_chunk)

    def send_mixed(group):
        for way in range(2):
            finish(opposite, way, group)
            remote(
                staged.at[group, opposite, half_of(way)],
                relay.at[group, way],
                mixed_send.at[0],
                relay_receive.at[2 * group + way],
                sides[way],
            ).start()
        for at in range(2):
            for way, target in enumerate((after, before)):
                finish(target, at, group)
                remote(
                    staged.at[group, target, half_of(at)],
                    mixed.at[group, part, half_of(at)],
                    mixed_send.at[0],
                    mixed_receive.at[2 * group + way],
                    sides[way],
                ).start()

    def pass_mixed(group):
        for way in range(2):
            arrived(relay.at[group, way], relay_receive.at[2 * group + way])
            remote(
                relay.at[group, way],
                mixed.at[group, (before, after)[way], half_of(way)],
                mixed_send.at[0],
                handed_receive.at[group],
                sides[way],
            ).start()

    send_mixed(0)
    take_incoming(1)
    send_mixed(1)
    pass_mixed(0)
    for group in range(groups):
        for at in range(2):
            finish(part, at, group)
    next(out_steps)
    pass_mixed(1)
    next(out_steps)

    def output(terms, first, last):
        broad = 8 * LANES

        def tile(at, _):
            columns = pl.ds(pl.multiple_of(at * broad, broad), broad)
            summed = 0.0 if first else summed_ref[:, columns]
            for block_of, group, source in terms:
                weight = jnp.concatenate(
                    [full_out[16 * at + 2 * place + group, source] for place in range(8)], axis=1
                )
                summed += jnp.dot(
                    block_of[group, source], weight, preferred_element_type=f32
                )
            if last:
                result_ref[:, columns] = summed.astype(bf16)
            else:
                summed_ref[:, columns] = summed
            return 0

        lax.fori_loop(0, features // broad, tile, 0)

    def take_sides(group):
        arrived(mixed.at[group, before], mixed_receive.at[2 * group])
        arrived(mixed.at[group, after], mixed_receive.at[2 * group + 1])

    take_sides(0)
    output(
        [(staged, 0, part), (staged, 1, part), (mixed, 0, before), (mixed, 0, after)],
        True,
        False,
    )
    take_sides(1)
    arrived(mixed.at[0, opposite], handed_receive.at[0])
    output([(mixed, 1, before), (mixed, 1, after), (mixed, 0, opposite)], False, False)
    arrived(mixed.at[1, opposite], handed_receive.at[1])
    output([(mixed, 1, opposite)], False, True)
    next(weights_steps)
    next(out_steps)
    pair.wait_send()
    left_here(full_out.at[0, pl.ds(0, 3)], cross_send.at[0])
    left_here(tokens.at[pl.ds(0, 3)], token_send.at[0])
    left_here(all_logs.at[pl.ds(0, stretches - 1)], logs_send.at[0])
    left_here(slices.at[pl.ds(0, stretches - 1)], scan_send.at[0])
    left_here(incoming.at[pl.ds(0, stretches - 1)], back_send.at[0])
    left_here(mixed, mixed_send.at[0])


def on_device(
    input_activations,
    norm_gain,
    w_gate,
    w_value,
    w_state_in,
    w_state_out,
    w_step_forward,
    w_step_backward,
    step_offset,
    fading_speed,
    conv_value,
    conv_state_in,
    conv_state_out,
    out_gain,
    w_out,
):
    stretches = lax.axis_size("sp")
    parts = lax.axis_size("tp")
    chunk, features = input_activations.shape
    extent = parts * chunk
    depth = w_gate.shape[0]
    content = w_value.shape[1]
    state_width = w_state_in.shape[1]
    heads = w_step_forward.shape[1]
    groups = state_width // STATE
    span = heads // groups * HEAD_DIM
    channels = content + 2 * state_width
    count = extent // BLOCK
    slice_rows = 2 * groups * STATE // stretches
    shift = math.log(extent * stretches)
    bf16, f32 = jnp.bfloat16, jnp.float32
    vmem, dma = pltpu.VMEM, pltpu.SemaphoreType.DMA
    space = pl.BlockSpec(memory_space=pltpu.VMEM)
    half_rows = w_out.shape[0] // 2
    return pl.pallas_call(
        functools.partial(mixer_kernel, shift),
        out_shape=pltpu.VMEM((chunk, features), bf16),
        in_specs=[pl.BlockSpec(memory_space=pl.ANY)] + [space] * 14,
        out_specs=space,
        scratch_shapes=[
            vmem((parts, chunk, features), bf16),
            vmem((stretches * depth, channels + content + LANES), bf16),
            vmem((stretches, parts, half_rows, LANES), bf16),
            vmem((2, half_rows, LANES), bf16),
            vmem((half_rows, LANES), bf16),
            vmem((extent + 16, channels), f32),
            vmem((extent, content), bf16),
            vmem((extent, LANES), f32),
            vmem((2, 8, channels), f32),
            vmem((extent, content), bf16),
            vmem((extent, state_width), bf16),
            vmem((extent, state_width), bf16),
            vmem((extent, LANES), f32),
            vmem((4 * heads, extent), f32),
            vmem((groups, count, STATE, 2 * span), f32),
            vmem((groups, count, 1, 2 * span), f32),
            vmem((stretches, slice_rows, span), bf16),
            vmem((stretches, slice_rows, span), bf16),
            vmem((2 * groups, 8, LANES), f32),
            vmem((stretches, 8, LANES), f32),
            vmem((stretches, slice_rows, span), bf16),
            vmem((stretches, slice_rows, span), bf16),
            vmem((extent, content), f32),
            vmem((groups, parts, chunk, span), bf16),
            vmem((groups, parts, chunk, span), bf16),
            vmem((extent, content), f32),
            vmem((chunk, features), f32),
            vmem((groups, 2, chunk // 2, span), bf16),
            vmem((chunk, features), bf16),
            dma((1,)),
            dma((GATHER_WAITS,)),
            dma((1,)),
            dma((GATHER_WAITS,)),
            dma((1,)),
            dma((1,)),
            dma((1,)),
            dma((2,)),
            dma((1,)),
            dma((2, 3)),
            dma((1,)),
            dma((1,)),
            dma((1,)),
            dma((1,)),
            dma((1,)),
            dma((1,)),
            dma((1,)),
            dma((1,)),
            dma((2,)),
            dma((1,)),
            dma((4,)),
            dma((4,)),
            dma((2,)),
            dma((4,)),
        ],
        cost_estimate=pl.CostEstimate(
            flops=int(3e10), bytes_accessed=1 << 20, transcendentals=0
        ),
        compiler_params=pltpu.CompilerParams(
            collective_id=1, has_side_effects=True, vmem_limit_bytes=VMEM_LIMIT
        ),
    )(
        input_activations,
        norm_gain.reshape(1, features),
        w_gate,
        w_value,
        w_state_in,
        w_state_out,
        w_step_forward.T,
        w_step_backward.T,
        step_offset,
        fading_speed,
        conv_value,
        conv_state_in,
        conv_state_out,
        out_gain.reshape(1, content),
        w_out.T,
    )


def solution(mesh):
    return jax.shard_map(
        on_device,
        mesh=mesh,
        in_specs=(
            P(("sp", "tp"), None),
            P(),
            P("sp", "tp"),
            P("sp", "tp"),
            P("sp", "tp"),
            P("sp", "tp"),
            P("sp", "tp"),
            P("sp", "tp"),
            P(None, "tp"),
            P(None, "tp"),
            P(None, "tp"),
            P(None, "tp"),
            P(None, "tp"),
            P("tp"),
            P("tp", "sp"),
        ),
        out_specs=P(("sp", "tp"), None),
        check_vma=False,
    )
```

```python
import functools
import math

import jax
import jax.numpy as jnp
from jax import lax
from jax.experimental import pallas as pl
from jax.experimental.pallas import tpu as pltpu
from jax.sharding import PartitionSpec as P

HEAD_DIM = 64
STATE = 128
BLOCK = 128
LANES = 128
EPSILON = 1e-06
HIGHEST = lax.Precision.HIGHEST
VMEM_LIMIT = 60 * 1024 * 1024
SIDE = 4


def rms_rows(values):
    wide = values.astype(jnp.float32)
    return wide * lax.rsqrt(jnp.mean(wide * wide, axis=-1, keepdims=True) + EPSILON)


def softplus(values):
    return jnp.maximum(values, 0.0) + jnp.log1p(jnp.exp(-jnp.abs(values)))


def spread(columns, first, count):
    rows = columns.shape[0]
    lane = lax.broadcasted_iota(jnp.int32, (rows, LANES), 1)
    tiles = []
    for at in range(first, first + count, 2):
        low = jnp.broadcast_to(columns[:, at : at + 1], (rows, LANES))
        high = jnp.broadcast_to(columns[:, at + 1 : at + 2], (rows, LANES))
        tiles.append(jnp.where(lane < HEAD_DIM, low, high))
    return jnp.concatenate(tiles, axis=1)


def silu(values):
    half = 0.5 * values
    return half + half * jnp.tanh(half)


def greet(peers):
    barrier = pltpu.get_barrier_semaphore()
    for peer in peers:
        pl.semaphore_signal(
            barrier, inc=1, device_id=peer, device_id_type=pl.DeviceIdType.MESH
        )
    return lambda: pl.semaphore_wait(barrier, len(peers))


def remote(source, target, send, receive, peer):
    return pltpu.make_async_remote_copy(
        src_ref=source,
        dst_ref=target,
        send_sem=send,
        recv_sem=receive,
        device_id=peer,
        device_id_type=pl.DeviceIdType.MESH,
    )


def place():
    me = lax.axis_index("sp")
    return me // (2 * SIDE), me // 2 % SIDE, me % 2


def plane_gather(whole, half, many, send, receive):
    z, y, c = place()
    part = lax.axis_index("tp")

    def origin(first, second):
        over_z = (z + c * first + (1 - c) * second + 2 * SIDE) % SIDE
        over_y = (y + (1 - c) * first + c * second + 2 * SIDE) % SIDE
        return (over_z * SIDE + over_y) * 2 + c

    along = [(origin(1, 0), part), (origin(-1, 0), part)]
    cross = [(origin(0, 1), part), (origin(0, -1), part)]
    partner = ((z * SIDE + y) * 2 + 1 - c, part)
    lines = (0, -1, 1, 2)
    at_line, at_far, at_shared, at_over, at_last = 0, 1, 2, 3, 7

    def go(block, peer, kind):
        remote(block, block, send.at[0], receive.at[kind], peer).start()

    def arrived(shards, kind):
        remote(many(shards), many(shards), send.at[0], receive.at[kind], partner).wait_recv()

    def share(at):
        go(whole(at), partner, at_shared)

    def spread_line(first):
        for peer in cross:
            go(whole(origin(first, 0)), peer, at_over + lines.index(first))
        share(origin(first, 0))

    def forward(first):
        arrived(2, at_over + lines.index(first))
        for way in range(2):
            go(half(origin(first, (-1, 1)[way]), way), cross[way], at_last + lines.index(first))
        for way in range(2):
            share(origin(first, (-1, 1)[way]))

    for peer in along:
        go(whole(origin(0, 0)), peer, at_line)
    spread_line(0)
    yield
    arrived(2, at_line)
    for way in range(2):
        go(half(origin((-1, 1)[way], 0), way), along[way], at_far)
    for way in range(2):
        spread_line((-1, 1)[way])
    yield
    forward(0)
    yield
    arrived(1, at_far)
    spread_line(2)
    yield
    forward(-1)
    yield
    forward(1)
    yield
    forward(2)
    yield
    for at, first in enumerate(lines):
        arrived(1, at_last + at)
        share(origin(first, 2))
    yield
    arrived(16, at_shared)
    yield
    remote(many(31), many(31), send.at[0], receive.at[at_line], partner).wait_send()
    yield


GATHER_WAITS = 11


def mixer_kernel(
    shift,
    x_ref,
    norm_gain_ref,
    gate_weights_ref,
    value_weights_ref,
    in_weights_ref,
    out_weights_ref,
    ahead_weights_ref,
    behind_weights_ref,
    offset_ref,
    speed_ref,
    taps_value_ref,
    taps_in_ref,
    taps_out_ref,
    gain_ref,
    w_out_ref,
    result_ref,
    tokens,
    weights,
    full_out,
    placed,
    paired,
    padded,
    gates,
    scale_ref,
    halo,
    signal_ref,
    inward_ref,
    outward_ref,
    within_ref,
    rows_ref,
    block_states_ref,
    block_logs_ref,
    sent,
    slices,
    log_tiles,
    all_logs,
    returned,
    incoming,
    total,
    staged,
    mixed,
    wide_gates,
    summed_ref,
    relay,
    raw_tokens,
    weights_send,
    weights_receive,
    out_send,
    out_receive,
    pair_send,
    pair_receive,
    cross_send,
    cross_receive,
    token_send,
    token_receive,
    onward_receive,
    halo_send,
    halo_receive,
    logs_send,
    logs_receive,
    scan_send,
    scan_receive,
    back_send,
    back_receive,
    mixed_send,
    mixed_receive,
    relay_receive,
    handed_receive,
    load,
):
    me, part = lax.axis_index("sp"), lax.axis_index("tp")
    core = me % 2
    stretches = slices.shape[0]
    parts, chunk, features = tokens.shape
    extent = parts * chunk
    depth = value_weights_ref.shape[0]
    content = value_weights_ref.shape[1]
    state_width = in_weights_ref.shape[1]
    heads = ahead_weights_ref.shape[0]
    groups = state_width // STATE
    ratio = heads // groups
    span = ratio * HEAD_DIM
    channels = content + 2 * state_width
    count = extent // BLOCK
    f32, bf16 = jnp.float32, jnp.bfloat16

    peers = [((me + hop) % stretches, part) for hop in range(1, stretches)]
    across = [(me, (part + hop) % parts) for hop in range(1, parts)]
    settle = greet(peers + across)

    quarter = chunk // 4
    loads = []
    for at in (0, 3, 1, 2):
        here = pl.ds(at * quarter, quarter)
        copy = pltpu.make_async_copy(x_ref.at[here], raw_tokens.at[here], load.at[at])
        copy.start()
        loads.append(copy)
    rows = 16

    def normalize(at):
        for step in range(quarter // rows):
            here = pl.ds(at * quarter + step * rows, rows)
            normed = rms_rows(raw_tokens[here, :]) * norm_gain_ref[...]
            tokens[part, here, :] = normed.astype(bf16)

    own_rows = pl.ds(pl.multiple_of(me * depth, depth), depth)
    weights[own_rows, 0:content] = value_weights_ref[...]
    weights[own_rows, content : content + state_width] = in_weights_ref[...]
    weights[own_rows, content + state_width : channels] = out_weights_ref[...]
    weights[own_rows, channels : channels + content] = gate_weights_ref[...]

    def across_rows(left, right):
        return lax.dot_general(left, right, (((0,), (0,)), ((), ())), preferred_element_type=f32)

    head_row = lax.broadcasted_iota(jnp.int32, (heads, LANES), 0)
    head_lane = lax.broadcasted_iota(jnp.int32, (heads, LANES), 1)
    to_ahead = (head_row == head_lane).astype(bf16)
    to_behind = (head_row + heads == head_lane).astype(bf16)
    weights[own_rows, channels + content :] = (
        across_rows(ahead_weights_ref[...], to_ahead)
        + across_rows(behind_weights_ref[...], to_behind)
    ).astype(bf16)
    for at, copy in zip((0, 3), loads[:2]):
        copy.wait()
        normalize(at)
    settle()

    right, left = (me, (part + 1) % parts), (me, (part + parts - 1) % parts)
    before, after = (part + parts - 1) % parts, (part + 1) % parts
    opposite = (part + 2) % parts

    def piece(source, at):
        return tokens.at[source, pl.ds(at * quarter, quarter)]

    orders = ((0, 1, 2, 3), (3, 2, 1, 0))

    def arrived(block, semaphore):
        remote(block, block, semaphore, semaphore, right).wait_recv()

    def left_here(block, semaphore):
        remote(block, block, semaphore, semaphore, right).wait_send()

    def send_own(step):
        for way, peer in enumerate((right, left)):
            block = piece(part, orders[way][step])
            received = token_receive.at[way, min(step, 2)]
            remote(block, block, token_send.at[0], received, peer).start()

    def pass_on(step):
        for way, peer in enumerate((right, left)):
            block = piece((before, after)[way], orders[way][step])
            arrived(block, token_receive.at[way, step])
            remote(block, block, token_send.at[0], onward_receive.at[0], peer).start()

    weights_steps = plane_gather(
        lambda at: weights.at[pl.ds(pl.multiple_of(at * depth, depth), depth)],
        lambda at, side: weights.at[
            pl.ds(pl.multiple_of(at * depth + side * (depth // 2), depth // 2), depth // 2)
        ],
        lambda shards: weights.at[pl.ds(0, shards * depth)],
        weights_send,
        weights_receive,
    )
    out_steps = plane_gather(
        lambda at: full_out.at[at],
        lambda at, side: full_out.at[at, pl.ds(side * (parts // 2), parts // 2)],
        lambda shards: full_out.at[pl.ds(0, shards)],
        out_send,
        out_receive,
    )

    z, y, _ = place()
    partner = ((z * SIDE + y) * 2 + 1 - core, part)
    pair = remote(placed.at[1 - core], paired, pair_send.at[0], pair_receive.at[0], partner)
    send_own(0)
    next(weights_steps)
    width = w_out_ref.shape[0]
    move_row = lax.broadcasted_iota(jnp.int32, (width, LANES), 0)
    move_lane = lax.broadcasted_iota(jnp.int32, (width, LANES), 1)
    to_half = (move_row + core * width == move_lane).astype(bf16)
    half_rows = w_out_ref.shape[1] // 2
    for side in range(2):
        placed[side] = across_rows(
            w_out_ref[:, side * half_rows : (side + 1) * half_rows], to_half
        ).astype(bf16)
    pair.start()
    loads[2].wait()
    normalize(1)
    pair.wait_recv()
    full_out[me, part] = placed[core] + paired[...]
    loads[3].wait()
    normalize(2)
    for peer in (right, left):
        block = full_out.at[me, part]
        remote(block, block, cross_send.at[0], cross_receive.at[0], peer).start()
    send_own(1)
    next(weights_steps)
    next(weights_steps)
    both = full_out.at[me, pl.ds(0, 2)]
    arrived(both, cross_receive.at[0])
    block = full_out.at[me, (part + 3 + 2 * core) % parts]
    onward_peer = (me, (part + 1 + 2 * core) % parts)
    remote(block, block, cross_send.at[0], cross_receive.at[1], onward_peer).start()
    send_own(2)
    send_own(3)
    next(weights_steps)
    pass_on(0)
    next(weights_steps)
    next(weights_steps)
    pass_on(1)
    next(weights_steps)
    arrived(full_out.at[me, 0], cross_receive.at[1])
    next(out_steps)
    next(weights_steps)
    next(weights_steps)

    wide_tile = 2 * LANES

    def product(source, columns):
        return jnp.dot(tokens[source], weights[:, columns], preferred_element_type=f32)

    row = lax.broadcasted_iota(jnp.int32, (BLOCK, BLOCK), 0)
    column = lax.broadcasted_iota(jnp.int32, (BLOCK, BLOCK), 1)
    triangles = jnp.concatenate([row >= column, row <= column], axis=0).astype(bf16)
    lane = lax.broadcasted_iota(jnp.int32, (1, LANES), 1)
    spare = jnp.zeros((1, LANES - 2 * heads), f32)
    offset = jnp.concatenate([offset_ref[0:1, :], offset_ref[1:2, :], spare], axis=1)
    rate = jnp.concatenate([speed_ref[0:1, :], speed_ref[1:2, :], spare], axis=1)

    def decays_of(source, raw):
        steps = softplus(raw + offset - shift)
        logs = -steps * rate
        logs = jnp.concatenate([logs[:BLOCK], logs[BLOCK:]], axis=1)
        high = logs.astype(bf16)
        rest = logs - high.astype(f32)
        middle = rest.astype(bf16)
        low = (rest - middle.astype(f32)).astype(bf16)
        sums = jnp.dot(
            triangles,
            jnp.concatenate([high, middle, low], axis=1),
            preferred_element_type=f32,
        )
        sums = sums[:, : 2 * LANES] + (
            sums[:, 2 * LANES : 4 * LANES] + sums[:, 4 * LANES : 6 * LANES]
        )
        for inner in range(2):
            at = 2 * source + inner
            here = pl.ds(pl.multiple_of(at * BLOCK, BLOCK), BLOCK)
            lanes_of = slice(inner * LANES, (inner + 1) * LANES)
            within = jnp.where(lane < heads, sums[:BLOCK, lanes_of], sums[BLOCK:, lanes_of])
            final = jnp.where(lane < heads, within[BLOCK - 1 : BLOCK], within[0:1])
            step = steps[inner * BLOCK : (inner + 1) * BLOCK]
            within_ref[here, :] = within
            rows_ref[0 : 2 * heads, here] = within.T[0 : 2 * heads]
            rows_ref[2 * heads : 4 * heads, here] = step.T[0 : 2 * heads]
            scale_ref[here, :] = jnp.exp(final - within) * step
            for group in range(groups):
                block_logs_ref[group, at] = jnp.concatenate(
                    [spread(final, way * heads + group * ratio, ratio) for way in range(2)],
                    axis=1,
                )

    def project(source):
        start = pl.multiple_of(source * chunk, chunk)
        raw = product(source, slice(channels + content, channels + content + LANES))
        decays_of(source, raw.astype(bf16).astype(f32))

        for first in range(0, channels, wide_tile):
            columns = slice(first, first + wide_tile)
            padded[pl.ds(start + 8, chunk), columns] = (
                product(source, columns).astype(bf16).astype(f32)
            )
    def project_gate(source):
        start = pl.multiple_of(source * chunk, chunk)

        for first in range(0, content, wide_tile):
            gates[pl.ds(start, chunk), first : first + wide_tile] = product(
                source, slice(channels + first, channels + first + wide_tile)
            ).astype(bf16)

    has_next, has_last = me < stretches - 1, me > 0
    sends_to, takes_from = (has_next, has_last), (has_last, has_next)

    def edge_copy(way):
        peer = ((me + (1, stretches - 1)[way]) % stretches, part)
        block = padded.at[pl.ds((extent, 8)[way], 8)]
        return remote(block, halo.at[way], halo_send.at[way], halo_receive.at[way], peer)

    def send_edge(way, when):
        @pl.when(jnp.logical_and(when, sends_to[way]))
        def _():
            edge_copy(way).start()

    def take_edges():
        for way in range(2):
            beyond = pl.ds((0, extent + 8)[way], 8)

            @pl.when(takes_from[way])
            def _():
                edge_copy(way).wait_recv()
                padded[beyond, :] = halo[way]

            @pl.when(jnp.logical_not(takes_from[way]))
            def _():
                padded[beyond, :] = jnp.zeros((8, channels), f32)

            @pl.when(sends_to[way])
            def _():
                edge_copy(way).wait_send()

    def filter_columns(start, first, width):
        part_rows = padded[pl.ds(start, BLOCK + 16), first : first + width]
        if first < content:
            taps = taps_value_ref[:, first : first + width]
        elif first < content + state_width:
            taps = taps_in_ref[:, first - content : first - content + width]
        else:
            base = first - content - state_width
            taps = taps_out_ref[:, base : base + width]
        mixed_rows = (
            taps[0:1] * part_rows[7 : 7 + BLOCK]
            + taps[1:2] * part_rows[8 : 8 + BLOCK]
            + taps[2:3] * part_rows[9 : 9 + BLOCK]
        )
        return silu(mixed_rows).astype(bf16)

    def filter_outward(at):
        start = pl.multiple_of(at * BLOCK, BLOCK)
        for first in range(0, state_width, wide_tile):
            outward_ref[pl.ds(start, BLOCK), first : first + wide_tile] = filter_columns(
                start, content + state_width + first, wide_tile
            )

    def block(at, group):
        start = pl.multiple_of(at * BLOCK, BLOCK)
        here = pl.ds(start, BLOCK)
        signal = filter_columns(start, group * span, span)
        inward = filter_columns(start, content + group * STATE, STATE)
        signal_ref[here, group * span : (group + 1) * span] = signal
        inward_ref[here, group * STATE : (group + 1) * STATE] = inward
        scale = scale_ref[here, :]
        wide = signal.astype(f32)
        scaled = jnp.concatenate(
            [wide * spread(scale, way * heads + group * ratio, ratio) for way in range(2)],
            axis=1,
        ).astype(bf16)
        block_states_ref[group, at] = lax.dot_general(
            inward, scaled, (((0,), (0,)), ((), ())), preferred_element_type=f32
        )

    project(part)
    project_gate(part)
    next(out_steps)
    next(out_steps)
    arrived(tokens.at[0, pl.ds(0, 2 * quarter)], token_receive.at[0, 2])
    project(before)
    project_gate(before)
    arrived(tokens.at[0, pl.ds(0, 2 * quarter)], token_receive.at[1, 2])
    project(after)

    early = part % 3 == 0

    send_edge(0, part != 1)
    send_edge(1, part != 2)
    project_gate(after)
    next(out_steps)
    ahead_of_last = 2 * opposite + 3
    turn = 2 - 2 * (part // 3)

    def early_block(step, _):
        at = (ahead_of_last + (step + turn) % 4) % count
        for group in range(groups):
            block(at, group)
        filter_outward(at)
        return 0

    early_block(0, 0)
    early_block(1, 0)
    @pl.when(part % 3 != 0)
    def _():
        early_block(2, 0)
        early_block(3, 0)

    arrived(tokens.at[0], onward_receive.at[0])
    project(opposite)

    send_edge(0, part == 1)
    send_edge(1, part == 2)

    summed_logs = [
        functools.reduce(jnp.add, [block_logs_ref[group, at] for at in range(count)])
        for group in range(groups)
    ]
    for way in range(2):
        for group in range(groups):
            for lane_tile in range(span // LANES):
                first = way * span + lane_tile * LANES
                log_tiles[way * groups + group, lane_tile : lane_tile + 1, :] = summed_logs[group][
                    :, first : first + LANES
                ]
    handled = stretches // (2 * groups)
    for peer in peers:
        remote(
            log_tiles.at[peer[0] // handled],
            all_logs.at[me],
            logs_send.at[0],
            logs_receive.at[0],
            peer,
        ).start()
    all_logs[me] = log_tiles[me // handled]
    late_turn = 2 * (part // 2) * (1 - part % 2)

    def late_at(step):
        return (ahead_of_last + 4 + (step + late_turn) % 4) % count

    def late_block(step, group):
        block(late_at(step), group)

    slice_rows = sent.shape[1]
    per_state = STATE // slice_rows
    my_group = me // handled % groups
    my_index = me % handled + handled * (me // (groups * handled))

    def final_states(group):
        for way in range(2):
            order = range(count) if way == 0 else range(count - 1, -1, -1)
            for lane_tile in range(span // LANES):
                first = way * span + lane_tile * LANES
                state = jnp.zeros((STATE, LANES), f32)
                for at in order:
                    state = (
                        state * jnp.exp(block_logs_ref[group, at, :, first : first + LANES])
                        + block_states_ref[group, at, :, first : first + LANES]
                    )
                at_slice = (way * groups + group) * per_state
                here = slice(lane_tile * LANES, (lane_tile + 1) * LANES)
                sent[at_slice : at_slice + per_state, :, here] = state.astype(bf16).reshape(
                    per_state, slice_rows, LANES
                )

    def send_slices(group):
        scanners = 2 * handled
        for hop in range(scanners):
            index = (my_index + hop) % scanners
            target = index // handled * (groups * handled) + group * handled + index % handled

            def send():
                remote(
                    sent.at[target],
                    slices.at[me],
                    scan_send.at[0],
                    scan_receive.at[0],
                    (target, part),
                ).start()

            if hop:
                send()
            else:
                pl.when(my_group != group)(send)

        @pl.when(my_group == group)
        def _():
            slices[me] = sent[me]

    late_block(0, 0)
    late_block(1, 0)

    def early_at(step):
        return (ahead_of_last + (step + turn) % 4) % count

    @pl.when(early)
    def _():
        take_edges()
        block(early_at(2), 0)
        block(early_at(3), 0)

    @pl.when(part % 3 != 0)
    def _():
        late_block(0, 1)
        late_block(1, 1)
        take_edges()

    late_block(2, 0)
    late_block(3, 0)
    final_states(0)
    send_slices(0)
    @pl.when(early)
    def _():
        for step in range(2):
            late_block(step, 1)
        for step in range(2, 4):
            block(early_at(step), 1)
            filter_outward(early_at(step))

    late_block(2, 1)
    late_block(3, 1)
    final_states(1)
    send_slices(1)

    def keep_entries(group):
        def onward(at, carried):
            return enter(at, 0, *carried)

        def back(at, carried):
            return enter(count - 1 - at, span, *carried)

        def enter(at, base, state, logs):
            added = block_states_ref[group, at, :, base : base + span]
            decay = block_logs_ref[group, at, :, base : base + span]
            block_states_ref[group, at, :, base : base + span] = state
            block_logs_ref[group, at, :, base : base + span] = logs
            return state * jnp.exp(decay) + added, logs + decay

        empty = jnp.zeros((STATE, span), f32)
        still = jnp.zeros((1, span), f32)
        for body in (onward, back):
            lax.fori_loop(0, count, body, (empty, still))

    lanes = lax.broadcasted_iota(jnp.int32, (BLOCK, LANES), 1)

    def diagonal(at, _):
        here = pl.ds(pl.multiple_of(at * BLOCK, BLOCK), BLOCK)
        within = within_ref[here, :]
        wide_gates[here, :] = silu(gates[here, :].astype(f32))
        for group in range(groups):
            intersect = lax.dot_general(
                outward_ref[here, group * STATE : (group + 1) * STATE],
                inward_ref[here, group * STATE : (group + 1) * STATE],
                (((1,), (1,)), ((), ())),
                preferred_element_type=f32,
            )
            products = []
            for head in range(group * ratio, (group + 1) * ratio):
                other = heads + head
                gap_ahead = within[:, head : head + 1] - rows_ref[head : head + 1, here]
                gap_behind = within[:, other : other + 1] - rows_ref[other : other + 1, here]
                step_ahead = rows_ref[2 * heads + head : 2 * heads + head + 1, here]
                step_behind = rows_ref[2 * heads + other : 2 * heads + other + 1, here]
                gap = jnp.where(row >= column, gap_ahead, gap_behind)
                step = jnp.where(
                    row > column,
                    step_ahead,
                    jnp.where(row < column, step_behind, step_ahead + step_behind),
                )
                mixing = (intersect * jnp.exp(gap) * step).astype(bf16)
                tile = head // 2 * 2 * HEAD_DIM
                products.append(
                    jnp.dot(
                        mixing,
                        signal_ref[here, tile : tile + LANES],
                        preferred_element_type=f32,
                    )
                )
            for two in range(ratio // 2):
                at_tile = (group * ratio + 2 * two) * HEAD_DIM
                total[here, at_tile : at_tile + LANES] = jnp.where(
                    lanes < HEAD_DIM, products[2 * two], products[2 * two + 1]
                )
        return 0

    next(out_steps)
    next(out_steps)
    project_gate(opposite)

    def late_outward(step, _):
        filter_outward(late_at(step))
        return 0

    lax.fori_loop(0, 4, late_outward, 0)
    for group in range(groups):
        keep_entries(group)
    lax.fori_loop(0, count // 4, diagonal, 0)

    reverse = me // (stretches // 2)

    def scan_slices(group):
        arrived(all_logs.at[pl.ds(0, stretches - 1)], logs_receive.at[0])
        arrived(slices.at[pl.ds(0, stretches - 1)], scan_receive.at[0])

        def scan(step, state):
            for inner in range(4):
                at = 4 * step + inner
                source = at + reverse * (stretches - 1 - 2 * at)
                returned[source] = state.astype(bf16)
                logs = jnp.concatenate(
                    [all_logs[source, tile : tile + 1, :] for tile in range(span // LANES)],
                    axis=1,
                )
                state = state * jnp.exp(logs) + slices[source].astype(f32)
            return state

        lax.fori_loop(0, stretches // 4, scan, jnp.zeros((slice_rows, span), f32))
        for peer in peers:
            remote(
                returned.at[peer[0]],
                incoming.at[me],
                back_send.at[0],
                back_receive.at[group],
                peer,
            ).start()
        incoming[me] = returned[me]

    def take_incoming(group):
        scanners = 2 * handled

        @pl.when(my_group == group)
        def _():
            arrived(incoming.at[pl.ds(0, scanners - 1)], back_receive.at[group])

        @pl.when(my_group != group)
        def _():
            arrived(incoming.at[pl.ds(0, scanners)], back_receive.at[group])

    @pl.when(my_group == 0)
    def _():
        scan_slices(0)

    lax.fori_loop(count // 4, count // 2, diagonal, 0)

    @pl.when(my_group == 1)
    def _():
        scan_slices(1)

    lax.fori_loop(count // 2, count, diagonal, 0)
    take_incoming(0)
    next(out_steps)
    def carried_in(way, group):
        first = (way * groups + group) * per_state
        return incoming[first : first + per_state].reshape(STATE, span).astype(f32)

    def finish(source, inner, group):
        at = source * (chunk // BLOCK) + inner
        here = pl.ds(pl.multiple_of(at * BLOCK, BLOCK), BLOCK)
        decays = jnp.exp(within_ref[here, :])
        wide = slice(group * span, (group + 1) * span)
        summed = total[here, wide]
        for way in range(2):
            base = way * span
            state = block_states_ref[group, at, :, base : base + span] + jnp.exp(
                block_logs_ref[group, at, :, base : base + span]
            ) * carried_in(way, group)
            carried = jnp.dot(
                outward_ref[here, group * STATE : (group + 1) * STATE],
                state.astype(bf16),
                preferred_element_type=f32,
            )
            summed += carried * spread(decays, way * heads + group * ratio, ratio)
        gated = summed * wide_gates[here, wide]
        scale = lax.rsqrt(jnp.mean(gated * gated, axis=-1, keepdims=True) + EPSILON)
        staged[group, source, pl.ds(inner * BLOCK, BLOCK), :] = (
            gated * scale * gain_ref[:, wide]
        ).astype(bf16)

    sides = (right, left)
    half_chunk = chunk // 2

    def half_of(at):
        return pl.ds(at * half_chunk, half_chunk)

    def send_mixed(group):
        for way in range(2):
            finish(opposite, way, group)
            remote(
                staged.at[group, opposite, half_of(way)],
                relay.at[group, way],
                mixed_send.at[0],
                relay_receive.at[2 * group + way],
                sides[way],
            ).start()
        for at in range(2):
            for way, target in enumerate((after, before)):
                finish(target, at, group)
                remote(
                    staged.at[group, target, half_of(at)],
                    mixed.at[group, part, half_of(at)],
                    mixed_send.at[0],
                    mixed_receive.at[2 * group + way],
                    sides[way],
                ).start()

    def pass_mixed(group):
        for way in range(2):
            arrived(relay.at[group, way], relay_receive.at[2 * group + way])
            remote(
                relay.at[group, way],
                mixed.at[group, (before, after)[way], half_of(way)],
                mixed_send.at[0],
                handed_receive.at[group],
                sides[way],
            ).start()

    send_mixed(0)
    take_incoming(1)
    send_mixed(1)
    pass_mixed(0)
    for group in range(groups):
        for at in range(2):
            finish(part, at, group)
    next(out_steps)
    pass_mixed(1)
    next(out_steps)

    def output(terms, first, last):
        broad = 8 * LANES

        def tile(at, _):
            columns = pl.ds(pl.multiple_of(at * broad, broad), broad)
            summed = 0.0 if first else summed_ref[:, columns]
            for block_of, group, source in terms:
                weight = jnp.concatenate(
                    [full_out[16 * at + 2 * place + group, source] for place in range(8)], axis=1
                )
                summed += jnp.dot(
                    block_of[group, source], weight, preferred_element_type=f32
                )
            if last:
                result_ref[:, columns] = summed.astype(bf16)
            else:
                summed_ref[:, columns] = summed
            return 0

        lax.fori_loop(0, features // broad, tile, 0)

    def take_sides(group):
        arrived(mixed.at[group, before], mixed_receive.at[2 * group])
        arrived(mixed.at[group, after], mixed_receive.at[2 * group + 1])

    take_sides(0)
    output(
        [(staged, 0, part), (staged, 1, part), (mixed, 0, before), (mixed, 0, after)],
        True,
        False,
    )
    take_sides(1)
    arrived(mixed.at[0, opposite], handed_receive.at[0])
    output([(mixed, 1, before), (mixed, 1, after), (mixed, 0, opposite)], False, False)
    arrived(mixed.at[1, opposite], handed_receive.at[1])
    output([(mixed, 1, opposite)], False, True)
    next(weights_steps)
    next(out_steps)
    pair.wait_send()
    left_here(full_out.at[0, pl.ds(0, 3)], cross_send.at[0])
    left_here(tokens.at[pl.ds(0, 3)], token_send.at[0])
    left_here(all_logs.at[pl.ds(0, stretches - 1)], logs_send.at[0])
    left_here(slices.at[pl.ds(0, stretches - 1)], scan_send.at[0])
    left_here(incoming.at[pl.ds(0, stretches - 1)], back_send.at[0])
    left_here(mixed, mixed_send.at[0])


def on_device(
    input_activations,
    norm_gain,
    w_gate,
    w_value,
    w_state_in,
    w_state_out,
    w_step_forward,
    w_step_backward,
    step_offset,
    fading_speed,
    conv_value,
    conv_state_in,
    conv_state_out,
    out_gain,
    w_out,
):
    stretches = lax.axis_size("sp")
    parts = lax.axis_size("tp")
    chunk, features = input_activations.shape
    extent = parts * chunk
    depth = w_gate.shape[0]
    content = w_value.shape[1]
    state_width = w_state_in.shape[1]
    heads = w_step_forward.shape[1]
    groups = state_width // STATE
    span = heads // groups * HEAD_DIM
    channels = content + 2 * state_width
    count = extent // BLOCK
    slice_rows = 2 * groups * STATE // stretches
    shift = math.log(extent * stretches)
    bf16, f32 = jnp.bfloat16, jnp.float32
    vmem, dma = pltpu.VMEM, pltpu.SemaphoreType.DMA
    space = pl.BlockSpec(memory_space=pltpu.VMEM)
    half_rows = w_out.shape[0] // 2
    return pl.pallas_call(
        functools.partial(mixer_kernel, shift),
        out_shape=pltpu.VMEM((chunk, features), bf16),
        in_specs=[pl.BlockSpec(memory_space=pl.ANY)] + [space] * 14,
        out_specs=space,
        scratch_shapes=[
            vmem((parts, chunk, features), bf16),
            vmem((stretches * depth, channels + content + LANES), bf16),
            vmem((stretches, parts, half_rows, LANES), bf16),
            vmem((2, half_rows, LANES), bf16),
            vmem((half_rows, LANES), bf16),
            vmem((extent + 16, channels), f32),
            vmem((extent, content), bf16),
            vmem((extent, LANES), f32),
            vmem((2, 8, channels), f32),
            vmem((extent, content), bf16),
            vmem((extent, state_width), bf16),
            vmem((extent, state_width), bf16),
            vmem((extent, LANES), f32),
            vmem((4 * heads, extent), f32),
            vmem((groups, count, STATE, 2 * span), f32),
            vmem((groups, count, 1, 2 * span), f32),
            vmem((stretches, slice_rows, span), bf16),
            vmem((stretches, slice_rows, span), bf16),
            vmem((2 * groups, 8, LANES), f32),
            vmem((stretches, 8, LANES), f32),
            vmem((stretches, slice_rows, span), bf16),
            vmem((stretches, slice_rows, span), bf16),
            vmem((extent, content), f32),
            vmem((groups, parts, chunk, span), bf16),
            vmem((groups, parts, chunk, span), bf16),
            vmem((extent, content), f32),
            vmem((chunk, features), f32),
            vmem((groups, 2, chunk // 2, span), bf16),
            vmem((chunk, features), bf16),
            dma((1,)),
            dma((GATHER_WAITS,)),
            dma((1,)),
            dma((GATHER_WAITS,)),
            dma((1,)),
            dma((1,)),
            dma((1,)),
            dma((2,)),
            dma((1,)),
            dma((2, 3)),
            dma((1,)),
            dma((2,)),
            dma((2,)),
            dma((1,)),
            dma((1,)),
            dma((1,)),
            dma((1,)),
            dma((1,)),
            dma((2,)),
            dma((1,)),
            dma((4,)),
            dma((4,)),
            dma((2,)),
            dma((4,)),
        ],
        cost_estimate=pl.CostEstimate(
            flops=int(3e10), bytes_accessed=1 << 20, transcendentals=0
        ),
        compiler_params=pltpu.CompilerParams(
            collective_id=1, has_side_effects=True, vmem_limit_bytes=VMEM_LIMIT
        ),
    )(
        input_activations,
        norm_gain.reshape(1, features),
        w_gate,
        w_value,
        w_state_in,
        w_state_out,
        w_step_forward.T,
        w_step_backward.T,
        step_offset,
        fading_speed,
        conv_value,
        conv_state_in,
        conv_state_out,
        out_gain.reshape(1, content),
        w_out.T,
    )


def solution(mesh):
    return jax.shard_map(
        on_device,
        mesh=mesh,
        in_specs=(
            P(("sp", "tp"), None),
            P(),
            P("sp", "tp"),
            P("sp", "tp"),
            P("sp", "tp"),
            P("sp", "tp"),
            P("sp", "tp"),
            P("sp", "tp"),
            P(None, "tp"),
            P(None, "tp"),
            P(None, "tp"),
            P(None, "tp"),
            P(None, "tp"),
            P("tp"),
            P("tp", "sp"),
        ),
        out_specs=P(("sp", "tp"), None),
        check_vma=False,
    )
```

```python
import functools
import math

import jax
import jax.numpy as jnp
from jax import lax
from jax.experimental import pallas as pl
from jax.experimental.pallas import tpu as pltpu
from jax.sharding import PartitionSpec as P

HEAD_DIM = 64
STATE = 128
BLOCK = 128
LANES = 128
EPSILON = 1e-06
HIGHEST = lax.Precision.HIGHEST
VMEM_LIMIT = 60 * 1024 * 1024
SIDE = 4


def rms_rows(values):
    wide = values.astype(jnp.float32)
    return wide * lax.rsqrt(jnp.mean(wide * wide, axis=-1, keepdims=True) + EPSILON)


def softplus(values):
    return jnp.maximum(values, 0.0) + jnp.log1p(jnp.exp(-jnp.abs(values)))


def spread(columns, first, count):
    rows = columns.shape[0]
    lane = lax.broadcasted_iota(jnp.int32, (rows, LANES), 1)
    tiles = []
    for at in range(first, first + count, 2):
        low = jnp.broadcast_to(columns[:, at : at + 1], (rows, LANES))
        high = jnp.broadcast_to(columns[:, at + 1 : at + 2], (rows, LANES))
        tiles.append(jnp.where(lane < HEAD_DIM, low, high))
    return jnp.concatenate(tiles, axis=1)


def silu(values):
    half = 0.5 * values
    return half + half * jnp.tanh(half)


def greet(peers):
    barrier = pltpu.get_barrier_semaphore()
    for peer in peers:
        pl.semaphore_signal(
            barrier, inc=1, device_id=peer, device_id_type=pl.DeviceIdType.MESH
        )
    return lambda: pl.semaphore_wait(barrier, len(peers))


def remote(source, target, send, receive, peer):
    return pltpu.make_async_remote_copy(
        src_ref=source,
        dst_ref=target,
        send_sem=send,
        recv_sem=receive,
        device_id=peer,
        device_id_type=pl.DeviceIdType.MESH,
    )


def place():
    me = lax.axis_index("sp")
    return me // (2 * SIDE), me // 2 % SIDE, me % 2


def plane_gather(whole, half, many, send, receive):
    z, y, c = place()
    part = lax.axis_index("tp")

    def origin(first, second):
        over_z = (z + c * first + (1 - c) * second + 2 * SIDE) % SIDE
        over_y = (y + (1 - c) * first + c * second + 2 * SIDE) % SIDE
        return (over_z * SIDE + over_y) * 2 + c

    along = [(origin(1, 0), part), (origin(-1, 0), part)]
    cross = [(origin(0, 1), part), (origin(0, -1), part)]
    partner = ((z * SIDE + y) * 2 + 1 - c, part)
    lines = (0, -1, 1, 2)
    at_line, at_far, at_shared, at_over, at_last = 0, 1, 2, 3, 7

    def go(block, peer, kind):
        remote(block, block, send.at[0], receive.at[kind], peer).start()

    def arrived(shards, kind):
        remote(many(shards), many(shards), send.at[0], receive.at[kind], partner).wait_recv()

    def share(at):
        go(whole(at), partner, at_shared)

    def spread_line(first):
        for peer in cross:
            go(whole(origin(first, 0)), peer, at_over + lines.index(first))
        share(origin(first, 0))

    def forward(first):
        arrived(2, at_over + lines.index(first))
        for way in range(2):
            go(half(origin(first, (-1, 1)[way]), way), cross[way], at_last + lines.index(first))
        for way in range(2):
            share(origin(first, (-1, 1)[way]))

    for peer in along:
        go(whole(origin(0, 0)), peer, at_line)
    spread_line(0)
    yield
    arrived(2, at_line)
    for way in range(2):
        go(half(origin((-1, 1)[way], 0), way), along[way], at_far)
    for way in range(2):
        spread_line((-1, 1)[way])
    yield
    forward(0)
    yield
    arrived(1, at_far)
    spread_line(2)
    yield
    forward(-1)
    yield
    forward(1)
    yield
    forward(2)
    yield
    for at, first in enumerate(lines):
        arrived(1, at_last + at)
        share(origin(first, 2))
    yield
    arrived(16, at_shared)
    yield
    remote(many(31), many(31), send.at[0], receive.at[at_line], partner).wait_send()
    yield


GATHER_WAITS = 11


def mixer_kernel(
    shift,
    x_ref,
    norm_gain_ref,
    gate_weights_ref,
    value_weights_ref,
    in_weights_ref,
    out_weights_ref,
    ahead_weights_ref,
    behind_weights_ref,
    offset_ref,
    speed_ref,
    taps_value_ref,
    taps_in_ref,
    taps_out_ref,
    gain_ref,
    w_out_ref,
    result_ref,
    tokens,
    weights,
    full_out,
    placed,
    paired,
    padded,
    gates,
    scale_ref,
    outer_steps,
    halo,
    signal_ref,
    inward_ref,
    outward_ref,
    within_ref,
    rows_ref,
    block_states_ref,
    block_logs_ref,
    sent,
    slices,
    log_tiles,
    all_logs,
    returned,
    incoming,
    total,
    staged,
    mixed,
    wide_gates,
    summed_ref,
    relay,
    raw_tokens,
    weights_send,
    weights_receive,
    out_send,
    out_receive,
    pair_send,
    pair_receive,
    cross_send,
    cross_receive,
    token_send,
    token_receive,
    onward_receive,
    halo_send,
    halo_receive,
    logs_send,
    logs_receive,
    scan_send,
    scan_receive,
    back_send,
    back_receive,
    mixed_send,
    mixed_receive,
    relay_receive,
    handed_receive,
    load,
):
    me, part = lax.axis_index("sp"), lax.axis_index("tp")
    core = me % 2
    stretches = slices.shape[0]
    parts, chunk, features = tokens.shape
    extent = parts * chunk
    depth = value_weights_ref.shape[0]
    content = value_weights_ref.shape[1]
    state_width = in_weights_ref.shape[1]
    heads = ahead_weights_ref.shape[0]
    groups = state_width // STATE
    ratio = heads // groups
    span = ratio * HEAD_DIM
    channels = content + 2 * state_width
    count = extent // BLOCK
    f32, bf16 = jnp.float32, jnp.bfloat16

    peers = [((me + hop) % stretches, part) for hop in range(1, stretches)]
    across = [(me, (part + hop) % parts) for hop in range(1, parts)]
    settle = greet(peers + across)

    quarter = chunk // 4
    loads = []
    for at in (0, 3, 1, 2):
        here = pl.ds(at * quarter, quarter)
        copy = pltpu.make_async_copy(x_ref.at[here], raw_tokens.at[here], load.at[at])
        copy.start()
        loads.append(copy)
    rows = 16

    def normalize(at):
        for step in range(quarter // rows):
            here = pl.ds(at * quarter + step * rows, rows)
            normed = rms_rows(raw_tokens[here, :]) * norm_gain_ref[...]
            tokens[part, here, :] = normed.astype(bf16)

    own_rows = pl.ds(pl.multiple_of(me * depth, depth), depth)
    weights[own_rows, 0:content] = value_weights_ref[...]
    weights[own_rows, content : content + state_width] = in_weights_ref[...]
    weights[own_rows, content + state_width : channels] = out_weights_ref[...]
    weights[own_rows, channels : channels + content] = gate_weights_ref[...]

    def across_rows(left, right):
        return lax.dot_general(left, right, (((0,), (0,)), ((), ())), preferred_element_type=f32)

    head_row = lax.broadcasted_iota(jnp.int32, (heads, LANES), 0)
    head_lane = lax.broadcasted_iota(jnp.int32, (heads, LANES), 1)
    to_ahead = (head_row == head_lane).astype(bf16)
    to_behind = (head_row + heads == head_lane).astype(bf16)
    weights[own_rows, channels + content :] = (
        across_rows(ahead_weights_ref[...], to_ahead)
        + across_rows(behind_weights_ref[...], to_behind)
    ).astype(bf16)
    for at, copy in zip((0, 3), loads[:2]):
        copy.wait()
        normalize(at)
    settle()

    right, left = (me, (part + 1) % parts), (me, (part + parts - 1) % parts)
    before, after = (part + parts - 1) % parts, (part + 1) % parts
    opposite = (part + 2) % parts

    def piece(source, at):
        return tokens.at[source, pl.ds(at * quarter, quarter)]

    orders = ((0, 1, 2, 3), (3, 2, 1, 0))

    def arrived(block, semaphore):
        remote(block, block, semaphore, semaphore, right).wait_recv()

    def left_here(block, semaphore):
        remote(block, block, semaphore, semaphore, right).wait_send()

    def send_own(step):
        for way, peer in enumerate((right, left)):
            block = piece(part, orders[way][step])
            received = token_receive.at[way, min(step, 2)]
            remote(block, block, token_send.at[0], received, peer).start()

    def pass_on(step):
        for way, peer in enumerate((right, left)):
            block = piece((before, after)[way], orders[way][step])
            arrived(block, token_receive.at[way, step])
            remote(block, block, token_send.at[0], onward_receive.at[step], peer).start()

    weights_steps = plane_gather(
        lambda at: weights.at[pl.ds(pl.multiple_of(at * depth, depth), depth)],
        lambda at, side: weights.at[
            pl.ds(pl.multiple_of(at * depth + side * (depth // 2), depth // 2), depth // 2)
        ],
        lambda shards: weights.at[pl.ds(0, shards * depth)],
        weights_send,
        weights_receive,
    )
    out_steps = plane_gather(
        lambda at: full_out.at[at],
        lambda at, side: full_out.at[at, pl.ds(side * (parts // 2), parts // 2)],
        lambda shards: full_out.at[pl.ds(0, shards)],
        out_send,
        out_receive,
    )

    z, y, _ = place()
    partner = ((z * SIDE + y) * 2 + 1 - core, part)
    pair = remote(placed.at[1 - core], paired, pair_send.at[0], pair_receive.at[0], partner)
    send_own(0)
    next(weights_steps)
    width = w_out_ref.shape[0]
    move_row = lax.broadcasted_iota(jnp.int32, (width, LANES), 0)
    move_lane = lax.broadcasted_iota(jnp.int32, (width, LANES), 1)
    to_half = (move_row + core * width == move_lane).astype(bf16)
    half_rows = w_out_ref.shape[1] // 2
    for side in range(2):
        placed[side] = across_rows(
            w_out_ref[:, side * half_rows : (side + 1) * half_rows], to_half
        ).astype(bf16)
    pair.start()
    loads[2].wait()
    normalize(1)
    pair.wait_recv()
    full_out[me, part] = placed[core] + paired[...]
    loads[3].wait()
    normalize(2)
    for peer in (right, left):
        block = full_out.at[me, part]
        remote(block, block, cross_send.at[0], cross_receive.at[0], peer).start()
    send_own(1)
    next(weights_steps)
    next(weights_steps)
    both = full_out.at[me, pl.ds(0, 2)]
    arrived(both, cross_receive.at[0])
    block = full_out.at[me, (part + 3 + 2 * core) % parts]
    onward_peer = (me, (part + 1 + 2 * core) % parts)
    remote(block, block, cross_send.at[0], cross_receive.at[1], onward_peer).start()
    send_own(2)
    send_own(3)
    next(weights_steps)
    pass_on(0)
    next(weights_steps)
    next(weights_steps)
    pass_on(1)
    next(weights_steps)
    arrived(full_out.at[me, 0], cross_receive.at[1])
    next(out_steps)
    next(weights_steps)
    next(weights_steps)

    wide_tile = 2 * LANES

    def product(source, columns):
        return jnp.dot(tokens[source], weights[:, columns], preferred_element_type=f32)

    row = lax.broadcasted_iota(jnp.int32, (BLOCK, BLOCK), 0)
    column = lax.broadcasted_iota(jnp.int32, (BLOCK, BLOCK), 1)
    triangles = jnp.concatenate([row >= column, row <= column], axis=0).astype(bf16)
    lane = lax.broadcasted_iota(jnp.int32, (1, LANES), 1)
    spare = jnp.zeros((1, LANES - 2 * heads), f32)
    offset = jnp.concatenate([offset_ref[0:1, :], offset_ref[1:2, :], spare], axis=1)
    rate = jnp.concatenate([speed_ref[0:1, :], speed_ref[1:2, :], spare], axis=1)

    def decays_of(source, raw):
        steps = softplus(raw + offset - shift)
        logs = -steps * rate
        logs = jnp.concatenate([logs[:BLOCK], logs[BLOCK:]], axis=1)
        high = logs.astype(bf16)
        rest = logs - high.astype(f32)
        middle = rest.astype(bf16)
        low = (rest - middle.astype(f32)).astype(bf16)
        sums = jnp.dot(
            triangles,
            jnp.concatenate([high, middle, low], axis=1),
            preferred_element_type=f32,
        )
        sums = sums[:, : 2 * LANES] + (
            sums[:, 2 * LANES : 4 * LANES] + sums[:, 4 * LANES : 6 * LANES]
        )
        for inner in range(2):
            at = 2 * source + inner
            here = pl.ds(pl.multiple_of(at * BLOCK, BLOCK), BLOCK)
            lanes_of = slice(inner * LANES, (inner + 1) * LANES)
            within = jnp.where(lane < heads, sums[:BLOCK, lanes_of], sums[BLOCK:, lanes_of])
            final = jnp.where(lane < heads, within[BLOCK - 1 : BLOCK], within[0:1])
            step = steps[inner * BLOCK : (inner + 1) * BLOCK]
            within_ref[here, :] = within
            rows_ref[0 : 2 * heads, here] = within.T[0 : 2 * heads]
            rows_ref[2 * heads : 4 * heads, here] = step.T[0 : 2 * heads]
            scale_ref[here, :] = jnp.exp(final - within) * step
            for group in range(groups):
                block_logs_ref[group, at] = jnp.concatenate(
                    [spread(final, way * heads + group * ratio, ratio) for way in range(2)],
                    axis=1,
                )

    def project(source):
        start = pl.multiple_of(source * chunk, chunk)
        raw = product(source, slice(channels + content, channels + content + LANES))
        decays_of(source, raw.astype(bf16).astype(f32))

        for first in range(0, channels, wide_tile):
            columns = slice(first, first + wide_tile)
            padded[pl.ds(start + 8, chunk), columns] = (
                product(source, columns).astype(bf16).astype(f32)
            )
    def project_quarters(source, at, rest=None):
        start = pl.multiple_of(source * chunk, chunk)
        halves = [tokens[source, place * quarter : (place + 1) * quarter] for place in at]
        left_side = jnp.concatenate(halves, axis=0)

        def some(columns):
            made = jnp.dot(left_side, weights[:, columns], preferred_element_type=f32)
            return made.astype(bf16).astype(f32)

        raw = some(slice(channels + content, channels + content + LANES))
        if rest is None:
            outer_steps[...] = raw
        else:
            outer = rest[...]
            decays_of(source, jnp.concatenate([outer[:quarter], raw, outer[quarter:]], axis=0))
        for first in range(0, channels, wide_tile):
            columns = slice(first, first + wide_tile)
            made = some(columns)
            for half_at, place in enumerate(at):
                padded[pl.ds(start + 8 + place * quarter, quarter), columns] = made[
                    half_at * quarter : (half_at + 1) * quarter
                ]

    def project_gate(source):
        start = pl.multiple_of(source * chunk, chunk)

        for first in range(0, content, wide_tile):
            gates[pl.ds(start, chunk), first : first + wide_tile] = product(
                source, slice(channels + first, channels + first + wide_tile)
            ).astype(bf16)

    has_next, has_last = me < stretches - 1, me > 0
    sends_to, takes_from = (has_next, has_last), (has_last, has_next)

    def edge_copy(way):
        peer = ((me + (1, stretches - 1)[way]) % stretches, part)
        block = padded.at[pl.ds((extent, 8)[way], 8)]
        return remote(block, halo.at[way], halo_send.at[way], halo_receive.at[way], peer)

    def send_edge(way, when):
        @pl.when(jnp.logical_and(when, sends_to[way]))
        def _():
            edge_copy(way).start()

    def take_edges():
        for way in range(2):
            beyond = pl.ds((0, extent + 8)[way], 8)

            @pl.when(takes_from[way])
            def _():
                edge_copy(way).wait_recv()
                padded[beyond, :] = halo[way]

            @pl.when(jnp.logical_not(takes_from[way]))
            def _():
                padded[beyond, :] = jnp.zeros((8, channels), f32)

            @pl.when(sends_to[way])
            def _():
                edge_copy(way).wait_send()

    def filter_columns(start, first, width):
        part_rows = padded[pl.ds(start, BLOCK + 16), first : first + width]
        if first < content:
            taps = taps_value_ref[:, first : first + width]
        elif first < content + state_width:
            taps = taps_in_ref[:, first - content : first - content + width]
        else:
            base = first - content - state_width
            taps = taps_out_ref[:, base : base + width]
        mixed_rows = (
            taps[0:1] * part_rows[7 : 7 + BLOCK]
            + taps[1:2] * part_rows[8 : 8 + BLOCK]
            + taps[2:3] * part_rows[9 : 9 + BLOCK]
        )
        return silu(mixed_rows).astype(bf16)

    def filter_outward(at):
        start = pl.multiple_of(at * BLOCK, BLOCK)
        for first in range(0, state_width, wide_tile):
            outward_ref[pl.ds(start, BLOCK), first : first + wide_tile] = filter_columns(
                start, content + state_width + first, wide_tile
            )

    def block(at, group):
        start = pl.multiple_of(at * BLOCK, BLOCK)
        here = pl.ds(start, BLOCK)
        signal = filter_columns(start, group * span, span)
        inward = filter_columns(start, content + group * STATE, STATE)
        signal_ref[here, group * span : (group + 1) * span] = signal
        inward_ref[here, group * STATE : (group + 1) * STATE] = inward
        scale = scale_ref[here, :]
        wide = signal.astype(f32)
        scaled = jnp.concatenate(
            [wide * spread(scale, way * heads + group * ratio, ratio) for way in range(2)],
            axis=1,
        ).astype(bf16)
        block_states_ref[group, at] = lax.dot_general(
            inward, scaled, (((0,), (0,)), ((), ())), preferred_element_type=f32
        )

    project(part)
    project_gate(part)
    next(out_steps)
    next(out_steps)
    arrived(tokens.at[0, pl.ds(0, 2 * quarter)], token_receive.at[0, 2])
    project(before)
    project_gate(before)
    arrived(tokens.at[0, pl.ds(0, 2 * quarter)], token_receive.at[1, 2])
    project(after)

    early = part % 3 == 0

    send_edge(0, part != 1)
    send_edge(1, part != 2)
    project_gate(after)
    arrived(tokens.at[0, pl.ds(0, 2 * quarter)], onward_receive.at[0])
    project_quarters(opposite, (0, 3))
    send_edge(0, part == 1)
    send_edge(1, part == 2)
    next(out_steps)
    ahead_of_last = 2 * opposite + 3
    turn = 2 - 2 * (part // 3)

    def early_block(step, _):
        at = (ahead_of_last + (step + turn) % 4) % count
        for group in range(groups):
            block(at, group)
        filter_outward(at)
        return 0

    early_block(0, 0)
    early_block(1, 0)
    @pl.when(part % 3 != 0)
    def _():
        early_block(2, 0)
        early_block(3, 0)

    arrived(tokens.at[0, pl.ds(0, 2 * quarter)], onward_receive.at[1])
    project_quarters(opposite, (1, 2), outer_steps)
    summed_logs = [
        functools.reduce(jnp.add, [block_logs_ref[group, at] for at in range(count)])
        for group in range(groups)
    ]
    for way in range(2):
        for group in range(groups):
            for lane_tile in range(span // LANES):
                first = way * span + lane_tile * LANES
                log_tiles[way * groups + group, lane_tile : lane_tile + 1, :] = summed_logs[group][
                    :, first : first + LANES
                ]
    handled = stretches // (2 * groups)
    for peer in peers:
        remote(
            log_tiles.at[peer[0] // handled],
            all_logs.at[me],
            logs_send.at[0],
            logs_receive.at[0],
            peer,
        ).start()
    all_logs[me] = log_tiles[me // handled]
    late_turn = 2 * (part // 2) * (1 - part % 2)

    def late_at(step):
        return (ahead_of_last + 4 + (step + late_turn) % 4) % count

    def late_block(step, group):
        block(late_at(step), group)

    slice_rows = sent.shape[1]
    per_state = STATE // slice_rows
    my_group = me // handled % groups
    my_index = me % handled + handled * (me // (groups * handled))

    def final_states(group):
        for way in range(2):
            order = range(count) if way == 0 else range(count - 1, -1, -1)
            for lane_tile in range(span // LANES):
                first = way * span + lane_tile * LANES
                state = jnp.zeros((STATE, LANES), f32)
                for at in order:
                    state = (
                        state * jnp.exp(block_logs_ref[group, at, :, first : first + LANES])
                        + block_states_ref[group, at, :, first : first + LANES]
                    )
                at_slice = (way * groups + group) * per_state
                here = slice(lane_tile * LANES, (lane_tile + 1) * LANES)
                sent[at_slice : at_slice + per_state, :, here] = state.astype(bf16).reshape(
                    per_state, slice_rows, LANES
                )

    def send_slices(group):
        scanners = 2 * handled
        for hop in range(scanners):
            index = (my_index + hop) % scanners
            target = index // handled * (groups * handled) + group * handled + index % handled

            def send():
                remote(
                    sent.at[target],
                    slices.at[me],
                    scan_send.at[0],
                    scan_receive.at[0],
                    (target, part),
                ).start()

            if hop:
                send()
            else:
                pl.when(my_group != group)(send)

        @pl.when(my_group == group)
        def _():
            slices[me] = sent[me]

    late_block(0, 0)
    late_block(1, 0)

    def early_at(step):
        return (ahead_of_last + (step + turn) % 4) % count

    @pl.when(early)
    def _():
        take_edges()
        block(early_at(2), 0)
        block(early_at(3), 0)

    @pl.when(part % 3 != 0)
    def _():
        late_block(0, 1)
        late_block(1, 1)
        take_edges()

    late_block(2, 0)
    late_block(3, 0)
    final_states(0)
    send_slices(0)
    @pl.when(early)
    def _():
        for step in range(2):
            late_block(step, 1)
        for step in range(2, 4):
            block(early_at(step), 1)
            filter_outward(early_at(step))

    late_block(2, 1)
    late_block(3, 1)
    final_states(1)
    send_slices(1)

    def keep_entries(group):
        def onward(at, carried):
            return enter(at, 0, *carried)

        def back(at, carried):
            return enter(count - 1 - at, span, *carried)

        def enter(at, base, state, logs):
            added = block_states_ref[group, at, :, base : base + span]
            decay = block_logs_ref[group, at, :, base : base + span]
            block_states_ref[group, at, :, base : base + span] = state
            block_logs_ref[group, at, :, base : base + span] = logs
            return state * jnp.exp(decay) + added, logs + decay

        empty = jnp.zeros((STATE, span), f32)
        still = jnp.zeros((1, span), f32)
        for body in (onward, back):
            lax.fori_loop(0, count, body, (empty, still))

    lanes = lax.broadcasted_iota(jnp.int32, (BLOCK, LANES), 1)

    def diagonal(at, _):
        here = pl.ds(pl.multiple_of(at * BLOCK, BLOCK), BLOCK)
        within = within_ref[here, :]
        wide_gates[here, :] = silu(gates[here, :].astype(f32))
        for group in range(groups):
            intersect = lax.dot_general(
                outward_ref[here, group * STATE : (group + 1) * STATE],
                inward_ref[here, group * STATE : (group + 1) * STATE],
                (((1,), (1,)), ((), ())),
                preferred_element_type=f32,
            )
            products = []
            for head in range(group * ratio, (group + 1) * ratio):
                other = heads + head
                gap_ahead = within[:, head : head + 1] - rows_ref[head : head + 1, here]
                gap_behind = within[:, other : other + 1] - rows_ref[other : other + 1, here]
                step_ahead = rows_ref[2 * heads + head : 2 * heads + head + 1, here]
                step_behind = rows_ref[2 * heads + other : 2 * heads + other + 1, here]
                gap = jnp.where(row >= column, gap_ahead, gap_behind)
                step = jnp.where(
                    row > column,
                    step_ahead,
                    jnp.where(row < column, step_behind, step_ahead + step_behind),
                )
                mixing = (intersect * jnp.exp(gap) * step).astype(bf16)
                tile = head // 2 * 2 * HEAD_DIM
                products.append(
                    jnp.dot(
                        mixing,
                        signal_ref[here, tile : tile + LANES],
                        preferred_element_type=f32,
                    )
                )
            for two in range(ratio // 2):
                at_tile = (group * ratio + 2 * two) * HEAD_DIM
                total[here, at_tile : at_tile + LANES] = jnp.where(
                    lanes < HEAD_DIM, products[2 * two], products[2 * two + 1]
                )
        return 0

    next(out_steps)
    next(out_steps)
    project_gate(opposite)

    def late_outward(step, _):
        filter_outward(late_at(step))
        return 0

    lax.fori_loop(0, 4, late_outward, 0)
    for group in range(groups):
        keep_entries(group)
    lax.fori_loop(0, count // 4, diagonal, 0)

    reverse = me // (stretches // 2)

    def scan_slices(group):
        arrived(all_logs.at[pl.ds(0, stretches - 1)], logs_receive.at[0])
        arrived(slices.at[pl.ds(0, stretches - 1)], scan_receive.at[0])

        def scan(step, state):
            for inner in range(4):
                at = 4 * step + inner
                source = at + reverse * (stretches - 1 - 2 * at)
                returned[source] = state.astype(bf16)
                logs = jnp.concatenate(
                    [all_logs[source, tile : tile + 1, :] for tile in range(span // LANES)],
                    axis=1,
                )
                state = state * jnp.exp(logs) + slices[source].astype(f32)
            return state

        lax.fori_loop(0, stretches // 4, scan, jnp.zeros((slice_rows, span), f32))
        for peer in peers:
            remote(
                returned.at[peer[0]],
                incoming.at[me],
                back_send.at[0],
                back_receive.at[group],
                peer,
            ).start()
        incoming[me] = returned[me]

    def take_incoming(group):
        scanners = 2 * handled

        @pl.when(my_group == group)
        def _():
            arrived(incoming.at[pl.ds(0, scanners - 1)], back_receive.at[group])

        @pl.when(my_group != group)
        def _():
            arrived(incoming.at[pl.ds(0, scanners)], back_receive.at[group])

    @pl.when(my_group == 0)
    def _():
        scan_slices(0)

    lax.fori_loop(count // 4, count // 2, diagonal, 0)

    @pl.when(my_group == 1)
    def _():
        scan_slices(1)

    lax.fori_loop(count // 2, count, diagonal, 0)
    take_incoming(0)
    next(out_steps)
    def carried_in(way, group):
        first = (way * groups + group) * per_state
        return incoming[first : first + per_state].reshape(STATE, span).astype(f32)

    def finish(source, inner, group):
        at = source * (chunk // BLOCK) + inner
        here = pl.ds(pl.multiple_of(at * BLOCK, BLOCK), BLOCK)
        decays = jnp.exp(within_ref[here, :])
        wide = slice(group * span, (group + 1) * span)
        summed = total[here, wide]
        for way in range(2):
            base = way * span
            state = block_states_ref[group, at, :, base : base + span] + jnp.exp(
                block_logs_ref[group, at, :, base : base + span]
            ) * carried_in(way, group)
            carried = jnp.dot(
                outward_ref[here, group * STATE : (group + 1) * STATE],
                state.astype(bf16),
                preferred_element_type=f32,
            )
            summed += carried * spread(decays, way * heads + group * ratio, ratio)
        gated = summed * wide_gates[here, wide]
        scale = lax.rsqrt(jnp.mean(gated * gated, axis=-1, keepdims=True) + EPSILON)
        staged[group, source, pl.ds(inner * BLOCK, BLOCK), :] = (
            gated * scale * gain_ref[:, wide]
        ).astype(bf16)

    sides = (right, left)
    half_chunk = chunk // 2

    def half_of(at):
        return pl.ds(at * half_chunk, half_chunk)

    def send_mixed(group):
        for way in range(2):
            finish(opposite, way, group)
            remote(
                staged.at[group, opposite, half_of(way)],
                relay.at[group, way],
                mixed_send.at[0],
                relay_receive.at[2 * group + way],
                sides[way],
            ).start()
        for at in range(2):
            for way, target in enumerate((after, before)):
                finish(target, at, group)
                remote(
                    staged.at[group, target, half_of(at)],
                    mixed.at[group, part, half_of(at)],
                    mixed_send.at[0],
                    mixed_receive.at[2 * group + way],
                    sides[way],
                ).start()

    def pass_mixed(group):
        for way in range(2):
            arrived(relay.at[group, way], relay_receive.at[2 * group + way])
            remote(
                relay.at[group, way],
                mixed.at[group, (before, after)[way], half_of(way)],
                mixed_send.at[0],
                handed_receive.at[group],
                sides[way],
            ).start()

    send_mixed(0)
    take_incoming(1)
    send_mixed(1)
    pass_mixed(0)
    for group in range(groups):
        for at in range(2):
            finish(part, at, group)
    next(out_steps)
    pass_mixed(1)
    next(out_steps)

    def output(terms, first, last):
        broad = 8 * LANES

        def tile(at, _):
            columns = pl.ds(pl.multiple_of(at * broad, broad), broad)
            summed = 0.0 if first else summed_ref[:, columns]
            for block_of, group, source in terms:
                weight = jnp.concatenate(
                    [full_out[16 * at + 2 * place + group, source] for place in range(8)], axis=1
                )
                summed += jnp.dot(
                    block_of[group, source], weight, preferred_element_type=f32
                )
            if last:
                result_ref[:, columns] = summed.astype(bf16)
            else:
                summed_ref[:, columns] = summed
            return 0

        lax.fori_loop(0, features // broad, tile, 0)

    def take_sides(group):
        arrived(mixed.at[group, before], mixed_receive.at[2 * group])
        arrived(mixed.at[group, after], mixed_receive.at[2 * group + 1])

    take_sides(0)
    output(
        [(staged, 0, part), (staged, 1, part), (mixed, 0, before), (mixed, 0, after)],
        True,
        False,
    )
    take_sides(1)
    arrived(mixed.at[0, opposite], handed_receive.at[0])
    output([(mixed, 1, before), (mixed, 1, after), (mixed, 0, opposite)], False, False)
    arrived(mixed.at[1, opposite], handed_receive.at[1])
    output([(mixed, 1, opposite)], False, True)
    next(weights_steps)
    next(out_steps)
    pair.wait_send()
    left_here(full_out.at[0, pl.ds(0, 3)], cross_send.at[0])
    left_here(tokens.at[pl.ds(0, 3)], token_send.at[0])
    left_here(all_logs.at[pl.ds(0, stretches - 1)], logs_send.at[0])
    left_here(slices.at[pl.ds(0, stretches - 1)], scan_send.at[0])
    left_here(incoming.at[pl.ds(0, stretches - 1)], back_send.at[0])
    left_here(mixed, mixed_send.at[0])


def on_device(
    input_activations,
    norm_gain,
    w_gate,
    w_value,
    w_state_in,
    w_state_out,
    w_step_forward,
    w_step_backward,
    step_offset,
    fading_speed,
    conv_value,
    conv_state_in,
    conv_state_out,
    out_gain,
    w_out,
):
    stretches = lax.axis_size("sp")
    parts = lax.axis_size("tp")
    chunk, features = input_activations.shape
    extent = parts * chunk
    depth = w_gate.shape[0]
    content = w_value.shape[1]
    state_width = w_state_in.shape[1]
    heads = w_step_forward.shape[1]
    groups = state_width // STATE
    span = heads // groups * HEAD_DIM
    channels = content + 2 * state_width
    count = extent // BLOCK
    slice_rows = 2 * groups * STATE // stretches
    shift = math.log(extent * stretches)
    bf16, f32 = jnp.bfloat16, jnp.float32
    vmem, dma = pltpu.VMEM, pltpu.SemaphoreType.DMA
    space = pl.BlockSpec(memory_space=pltpu.VMEM)
    half_rows = w_out.shape[0] // 2
    return pl.pallas_call(
        functools.partial(mixer_kernel, shift),
        out_shape=pltpu.VMEM((chunk, features), bf16),
        in_specs=[pl.BlockSpec(memory_space=pl.ANY)] + [space] * 14,
        out_specs=space,
        scratch_shapes=[
            vmem((parts, chunk, features), bf16),
            vmem((stretches * depth, channels + content + LANES), bf16),
            vmem((stretches, parts, half_rows, LANES), bf16),
            vmem((2, half_rows, LANES), bf16),
            vmem((half_rows, LANES), bf16),
            vmem((extent + 16, channels), f32),
            vmem((extent, content), bf16),
            vmem((extent, LANES), f32),
            vmem((chunk // 2, LANES), f32),
            vmem((2, 8, channels), f32),
            vmem((extent, content), bf16),
            vmem((extent, state_width), bf16),
            vmem((extent, state_width), bf16),
            vmem((extent, LANES), f32),
            vmem((4 * heads, extent), f32),
            vmem((groups, count, STATE, 2 * span), f32),
            vmem((groups, count, 1, 2 * span), f32),
            vmem((stretches, slice_rows, span), bf16),
            vmem((stretches, slice_rows, span), bf16),
            vmem((2 * groups, 8, LANES), f32),
            vmem((stretches, 8, LANES), f32),
            vmem((stretches, slice_rows, span), bf16),
            vmem((stretches, slice_rows, span), bf16),
            vmem((extent, content), f32),
            vmem((groups, parts, chunk, span), bf16),
            vmem((groups, parts, chunk, span), bf16),
            vmem((extent, content), f32),
            vmem((chunk, features), f32),
            vmem((groups, 2, chunk // 2, span), bf16),
            vmem((chunk, features), bf16),
            dma((1,)),
            dma((GATHER_WAITS,)),
            dma((1,)),
            dma((GATHER_WAITS,)),
            dma((1,)),
            dma((1,)),
            dma((1,)),
            dma((2,)),
            dma((1,)),
            dma((2, 3)),
            dma((2,)),
            dma((2,)),
            dma((2,)),
            dma((1,)),
            dma((1,)),
            dma((1,)),
            dma((1,)),
            dma((1,)),
            dma((2,)),
            dma((1,)),
            dma((4,)),
            dma((4,)),
            dma((2,)),
            dma((4,)),
        ],
        cost_estimate=pl.CostEstimate(
            flops=int(3e10), bytes_accessed=1 << 20, transcendentals=0
        ),
        compiler_params=pltpu.CompilerParams(
            collective_id=1, has_side_effects=True, vmem_limit_bytes=VMEM_LIMIT
        ),
    )(
        input_activations,
        norm_gain.reshape(1, features),
        w_gate,
        w_value,
        w_state_in,
        w_state_out,
        w_step_forward.T,
        w_step_backward.T,
        step_offset,
        fading_speed,
        conv_value,
        conv_state_in,
        conv_state_out,
        out_gain.reshape(1, content),
        w_out.T,
    )


def solution(mesh):
    return jax.shard_map(
        on_device,
        mesh=mesh,
        in_specs=(
            P(("sp", "tp"), None),
            P(),
            P("sp", "tp"),
            P("sp", "tp"),
            P("sp", "tp"),
            P("sp", "tp"),
            P("sp", "tp"),
            P("sp", "tp"),
            P(None, "tp"),
            P(None, "tp"),
            P(None, "tp"),
            P(None, "tp"),
            P(None, "tp"),
            P("tp"),
            P("tp", "sp"),
        ),
        out_specs=P(("sp", "tp"), None),
        check_vma=False,
    )
```

```python
import functools
import math

import jax
import jax.numpy as jnp
from jax import lax
from jax.experimental import pallas as pl
from jax.experimental.pallas import tpu as pltpu
from jax.sharding import PartitionSpec as P

HEAD_DIM = 64
STATE = 128
BLOCK = 128
LANES = 128
EPSILON = 1e-06
HIGHEST = lax.Precision.HIGHEST
VMEM_LIMIT = 60 * 1024 * 1024
SIDE = 4


def rms_rows(values):
    wide = values.astype(jnp.float32)
    return wide * lax.rsqrt(jnp.mean(wide * wide, axis=-1, keepdims=True) + EPSILON)


def softplus(values):
    return jnp.maximum(values, 0.0) + jnp.log1p(jnp.exp(-jnp.abs(values)))


def spread(columns, first, count):
    rows = columns.shape[0]
    lane = lax.broadcasted_iota(jnp.int32, (rows, LANES), 1)
    tiles = []
    for at in range(first, first + count, 2):
        low = jnp.broadcast_to(columns[:, at : at + 1], (rows, LANES))
        high = jnp.broadcast_to(columns[:, at + 1 : at + 2], (rows, LANES))
        tiles.append(jnp.where(lane < HEAD_DIM, low, high))
    return jnp.concatenate(tiles, axis=1)


def silu(values):
    half = 0.5 * values
    return half + half * jnp.tanh(half)


def greet(peers):
    barrier = pltpu.get_barrier_semaphore()
    for peer in peers:
        pl.semaphore_signal(
            barrier, inc=1, device_id=peer, device_id_type=pl.DeviceIdType.MESH
        )
    return lambda: pl.semaphore_wait(barrier, len(peers))


def remote(source, target, send, receive, peer):
    return pltpu.make_async_remote_copy(
        src_ref=source,
        dst_ref=target,
        send_sem=send,
        recv_sem=receive,
        device_id=peer,
        device_id_type=pl.DeviceIdType.MESH,
    )


def place():
    me = lax.axis_index("sp")
    return me // (2 * SIDE), me // 2 % SIDE, me % 2


def plane_gather(whole, half, many, send, receive):
    z, y, c = place()
    part = lax.axis_index("tp")

    def origin(first, second):
        over_z = (z + c * first + (1 - c) * second + 2 * SIDE) % SIDE
        over_y = (y + (1 - c) * first + c * second + 2 * SIDE) % SIDE
        return (over_z * SIDE + over_y) * 2 + c

    along = [(origin(1, 0), part), (origin(-1, 0), part)]
    cross = [(origin(0, 1), part), (origin(0, -1), part)]
    partner = ((z * SIDE + y) * 2 + 1 - c, part)
    lines = (0, -1, 1, 2)
    at_line, at_far, at_shared, at_over, at_last = 0, 1, 2, 3, 7

    def go(block, peer, kind):
        remote(block, block, send.at[0], receive.at[kind], peer).start()

    def arrived(shards, kind):
        remote(many(shards), many(shards), send.at[0], receive.at[kind], partner).wait_recv()

    def share(at):
        go(whole(at), partner, at_shared)

    def spread_line(first):
        for peer in cross:
            go(whole(origin(first, 0)), peer, at_over + lines.index(first))
        share(origin(first, 0))

    def forward(first):
        arrived(2, at_over + lines.index(first))
        for way in range(2):
            go(half(origin(first, (-1, 1)[way]), way), cross[way], at_last + lines.index(first))
        for way in range(2):
            share(origin(first, (-1, 1)[way]))

    for peer in along:
        go(whole(origin(0, 0)), peer, at_line)
    spread_line(0)
    yield
    arrived(2, at_line)
    for way in range(2):
        go(half(origin((-1, 1)[way], 0), way), along[way], at_far)
    for way in range(2):
        spread_line((-1, 1)[way])
    yield
    forward(0)
    yield
    arrived(1, at_far)
    spread_line(2)
    yield
    forward(-1)
    yield
    forward(1)
    yield
    forward(2)
    yield
    for at, first in enumerate(lines):
        arrived(1, at_last + at)
        share(origin(first, 2))
    yield
    arrived(16, at_shared)
    yield
    remote(many(31), many(31), send.at[0], receive.at[at_line], partner).wait_send()
    yield


GATHER_WAITS = 11


def mixer_kernel(
    shift,
    x_ref,
    norm_gain_from,
    gate_weights_from,
    value_weights_from,
    in_weights_from,
    out_weights_from,
    ahead_weights_from,
    behind_weights_from,
    offset_from,
    speed_from,
    taps_value_from,
    taps_in_from,
    taps_out_from,
    gain_from,
    w_out_from,
    result_ref,
    tokens,
    weights,
    full_out,
    placed,
    paired,
    padded,
    gates,
    scale_ref,
    outer_steps,
    halo,
    signal_ref,
    inward_ref,
    outward_ref,
    within_ref,
    rows_ref,
    block_states_ref,
    block_logs_ref,
    sent,
    slices,
    log_tiles,
    all_logs,
    returned,
    incoming,
    total,
    staged,
    mixed,
    wide_gates,
    summed_ref,
    relay,
    raw_tokens,
    norm_gain_ref,
    gate_weights_ref,
    value_weights_ref,
    in_weights_ref,
    out_weights_ref,
    ahead_weights_ref,
    behind_weights_ref,
    offset_ref,
    speed_ref,
    taps_value_ref,
    taps_in_ref,
    taps_out_ref,
    gain_ref,
    w_out_ref,
    weights_send,
    weights_receive,
    out_send,
    out_receive,
    pair_send,
    pair_receive,
    cross_send,
    cross_receive,
    token_send,
    token_receive,
    onward_receive,
    halo_send,
    halo_receive,
    logs_send,
    logs_receive,
    scan_send,
    scan_receive,
    back_send,
    back_receive,
    mixed_send,
    mixed_receive,
    relay_receive,
    handed_receive,
    load,
    inputs_load,
):
    me, part = lax.axis_index("sp"), lax.axis_index("tp")
    core = me % 2
    stretches = slices.shape[0]
    parts, chunk, features = tokens.shape
    extent = parts * chunk
    depth = value_weights_ref.shape[0]
    content = value_weights_ref.shape[1]
    state_width = in_weights_ref.shape[1]
    heads = ahead_weights_ref.shape[0]
    groups = state_width // STATE
    ratio = heads // groups
    span = ratio * HEAD_DIM
    channels = content + 2 * state_width
    count = extent // BLOCK
    f32, bf16 = jnp.float32, jnp.bfloat16

    peers = [((me + hop) % stretches, part) for hop in range(1, stretches)]
    across = [(me, (part + hop) % parts) for hop in range(1, parts)]
    settle = greet(peers + across)

    quarter = chunk // 4
    loads = []
    for at in (0, 3, 1, 2):
        here = pl.ds(at * quarter, quarter)
        copy = pltpu.make_async_copy(x_ref.at[here], raw_tokens.at[here], load.at[at])
        copy.start()
        loads.append(copy)
    fetched = []
    for at, (source, target) in enumerate(
        (
            (norm_gain_from, norm_gain_ref),
            (gate_weights_from, gate_weights_ref),
            (value_weights_from, value_weights_ref),
            (in_weights_from, in_weights_ref),
            (out_weights_from, out_weights_ref),
            (ahead_weights_from, ahead_weights_ref),
            (behind_weights_from, behind_weights_ref),
            (offset_from, offset_ref),
            (speed_from, speed_ref),
            (taps_value_from, taps_value_ref),
            (taps_in_from, taps_in_ref),
            (taps_out_from, taps_out_ref),
            (gain_from, gain_ref),
            (w_out_from, w_out_ref),
        )
    ):
        copy = pltpu.make_async_copy(source, target, inputs_load.at[at])
        copy.start()
        fetched.append(copy)
    rows = 16

    def normalize(at):
        for step in range(quarter // rows):
            here = pl.ds(at * quarter + step * rows, rows)
            normed = rms_rows(raw_tokens[here, :]) * norm_gain_ref[...]
            tokens[part, here, :] = normed.astype(bf16)

    fetched[0].wait()
    for at, copy in zip((0, 3), loads[:2]):
        copy.wait()
        normalize(at)
    settle()

    right, left = (me, (part + 1) % parts), (me, (part + parts - 1) % parts)
    before, after = (part + parts - 1) % parts, (part + 1) % parts
    opposite = (part + 2) % parts

    def piece(source, at):
        return tokens.at[source, pl.ds(at * quarter, quarter)]

    orders = ((0, 1, 2, 3), (3, 2, 1, 0))

    def arrived(block, semaphore):
        remote(block, block, semaphore, semaphore, right).wait_recv()

    def left_here(block, semaphore):
        remote(block, block, semaphore, semaphore, right).wait_send()

    def send_own(step):
        for way, peer in enumerate((right, left)):
            block = piece(part, orders[way][step])
            received = token_receive.at[way, min(step, 2)]
            remote(block, block, token_send.at[0], received, peer).start()

    def pass_on(step):
        for way, peer in enumerate((right, left)):
            block = piece((before, after)[way], orders[way][step])
            arrived(block, token_receive.at[way, step])
            remote(block, block, token_send.at[0], onward_receive.at[step], peer).start()

    weights_steps = plane_gather(
        lambda at: weights.at[pl.ds(pl.multiple_of(at * depth, depth), depth)],
        lambda at, side: weights.at[
            pl.ds(pl.multiple_of(at * depth + side * (depth // 2), depth // 2), depth // 2)
        ],
        lambda shards: weights.at[pl.ds(0, shards * depth)],
        weights_send,
        weights_receive,
    )
    out_steps = plane_gather(
        lambda at: full_out.at[at],
        lambda at, side: full_out.at[at, pl.ds(side * (parts // 2), parts // 2)],
        lambda shards: full_out.at[pl.ds(0, shards)],
        out_send,
        out_receive,
    )

    z, y, _ = place()
    partner = ((z * SIDE + y) * 2 + 1 - core, part)
    pair = remote(placed.at[1 - core], paired, pair_send.at[0], pair_receive.at[0], partner)
    send_own(0)
    for copy in fetched[1:7]:
        copy.wait()
    own_rows = pl.ds(pl.multiple_of(me * depth, depth), depth)
    weights[own_rows, 0:content] = value_weights_ref[...]
    weights[own_rows, content : content + state_width] = in_weights_ref[...]
    weights[own_rows, content + state_width : channels] = out_weights_ref[...]
    weights[own_rows, channels : channels + content] = gate_weights_ref[...]

    def across_rows(left, right):
        return lax.dot_general(left, right, (((0,), (0,)), ((), ())), preferred_element_type=f32)

    head_row = lax.broadcasted_iota(jnp.int32, (heads, LANES), 0)
    head_lane = lax.broadcasted_iota(jnp.int32, (heads, LANES), 1)
    to_ahead = (head_row == head_lane).astype(bf16)
    to_behind = (head_row + heads == head_lane).astype(bf16)
    weights[own_rows, channels + content :] = (
        across_rows(ahead_weights_ref[...], to_ahead)
        + across_rows(behind_weights_ref[...], to_behind)
    ).astype(bf16)
    next(weights_steps)
    width = w_out_ref.shape[0]
    move_row = lax.broadcasted_iota(jnp.int32, (width, LANES), 0)
    move_lane = lax.broadcasted_iota(jnp.int32, (width, LANES), 1)
    to_half = (move_row + core * width == move_lane).astype(bf16)
    half_rows = w_out_ref.shape[1] // 2
    fetched[13].wait()
    for side in range(2):
        placed[side] = across_rows(
            w_out_ref[:, side * half_rows : (side + 1) * half_rows], to_half
        ).astype(bf16)
    pair.start()
    loads[2].wait()
    normalize(1)
    pair.wait_recv()
    full_out[me, part] = placed[core] + paired[...]
    loads[3].wait()
    normalize(2)
    for peer in (right, left):
        block = full_out.at[me, part]
        remote(block, block, cross_send.at[0], cross_receive.at[0], peer).start()
    send_own(1)
    next(weights_steps)
    next(weights_steps)
    both = full_out.at[me, pl.ds(0, 2)]
    arrived(both, cross_receive.at[0])
    block = full_out.at[me, (part + 3 + 2 * core) % parts]
    onward_peer = (me, (part + 1 + 2 * core) % parts)
    remote(block, block, cross_send.at[0], cross_receive.at[1], onward_peer).start()
    send_own(2)
    send_own(3)
    next(weights_steps)
    pass_on(0)
    next(weights_steps)
    next(weights_steps)
    pass_on(1)
    next(weights_steps)
    arrived(full_out.at[me, 0], cross_receive.at[1])
    next(out_steps)
    next(weights_steps)
    next(weights_steps)

    wide_tile = 2 * LANES

    def product(source, columns):
        return jnp.dot(tokens[source], weights[:, columns], preferred_element_type=f32)

    row = lax.broadcasted_iota(jnp.int32, (BLOCK, BLOCK), 0)
    column = lax.broadcasted_iota(jnp.int32, (BLOCK, BLOCK), 1)
    for copy in fetched[7:13]:
        copy.wait()
    triangles = jnp.concatenate([row >= column, row <= column], axis=0).astype(bf16)
    lane = lax.broadcasted_iota(jnp.int32, (1, LANES), 1)
    spare = jnp.zeros((1, LANES - 2 * heads), f32)
    offset = jnp.concatenate([offset_ref[0:1, :], offset_ref[1:2, :], spare], axis=1)
    rate = jnp.concatenate([speed_ref[0:1, :], speed_ref[1:2, :], spare], axis=1)

    def decays_of(source, raw):
        steps = softplus(raw + offset - shift)
        logs = -steps * rate
        logs = jnp.concatenate([logs[:BLOCK], logs[BLOCK:]], axis=1)
        high = logs.astype(bf16)
        rest = logs - high.astype(f32)
        middle = rest.astype(bf16)
        low = (rest - middle.astype(f32)).astype(bf16)
        sums = jnp.dot(
            triangles,
            jnp.concatenate([high, middle, low], axis=1),
            preferred_element_type=f32,
        )
        sums = sums[:, : 2 * LANES] + (
            sums[:, 2 * LANES : 4 * LANES] + sums[:, 4 * LANES : 6 * LANES]
        )
        for inner in range(2):
            at = 2 * source + inner
            here = pl.ds(pl.multiple_of(at * BLOCK, BLOCK), BLOCK)
            lanes_of = slice(inner * LANES, (inner + 1) * LANES)
            within = jnp.where(lane < heads, sums[:BLOCK, lanes_of], sums[BLOCK:, lanes_of])
            final = jnp.where(lane < heads, within[BLOCK - 1 : BLOCK], within[0:1])
            step = steps[inner * BLOCK : (inner + 1) * BLOCK]
            within_ref[here, :] = within
            rows_ref[0 : 2 * heads, here] = within.T[0 : 2 * heads]
            rows_ref[2 * heads : 4 * heads, here] = step.T[0 : 2 * heads]
            scale_ref[here, :] = jnp.exp(final - within) * step
            for group in range(groups):
                block_logs_ref[group, at] = jnp.concatenate(
                    [spread(final, way * heads + group * ratio, ratio) for way in range(2)],
                    axis=1,
                )

    def project(source):
        start = pl.multiple_of(source * chunk, chunk)
        raw = product(source, slice(channels + content, channels + content + LANES))
        decays_of(source, raw.astype(bf16).astype(f32))

        for first in range(0, channels, wide_tile):
            columns = slice(first, first + wide_tile)
            padded[pl.ds(start + 8, chunk), columns] = (
                product(source, columns).astype(bf16).astype(f32)
            )
    def project_quarters(source, at, firsts, rest=None):
        start = pl.multiple_of(source * chunk, chunk)
        halves = [tokens[source, place * quarter : (place + 1) * quarter] for place in at]
        left_side = jnp.concatenate(halves, axis=0)

        def some(columns):
            made = jnp.dot(left_side, weights[:, columns], preferred_element_type=f32)
            return made.astype(bf16).astype(f32)

        if rest is not False:
            raw = some(slice(channels + content, channels + content + LANES))
        if rest is None:
            outer_steps[...] = raw
        elif rest is not False:
            outer = rest[...]
            decays_of(source, jnp.concatenate([outer[:quarter], raw, outer[quarter:]], axis=0))
        for first in firsts:
            columns = slice(first, first + wide_tile)
            made = some(columns)
            for half_at, place in enumerate(at):
                padded[pl.ds(start + 8 + place * quarter, quarter), columns] = made[
                    half_at * quarter : (half_at + 1) * quarter
                ]

    def project_gate(source):
        start = pl.multiple_of(source * chunk, chunk)

        for first in range(0, content, wide_tile):
            gates[pl.ds(start, chunk), first : first + wide_tile] = product(
                source, slice(channels + first, channels + first + wide_tile)
            ).astype(bf16)

    has_next, has_last = me < stretches - 1, me > 0
    sends_to, takes_from = (has_next, has_last), (has_last, has_next)

    def edge_copy(way):
        peer = ((me + (1, stretches - 1)[way]) % stretches, part)
        block = padded.at[pl.ds((extent, 8)[way], 8)]
        return remote(block, halo.at[way], halo_send.at[way], halo_receive.at[way], peer)

    def send_edge(way, when):
        @pl.when(jnp.logical_and(when, sends_to[way]))
        def _():
            edge_copy(way).start()

    def take_edges():
        for way in range(2):
            beyond = pl.ds((0, extent + 8)[way], 8)

            @pl.when(takes_from[way])
            def _():
                edge_copy(way).wait_recv()
                padded[beyond, :] = halo[way]

            @pl.when(jnp.logical_not(takes_from[way]))
            def _():
                padded[beyond, :] = jnp.zeros((8, channels), f32)

            @pl.when(sends_to[way])
            def _():
                edge_copy(way).wait_send()

    def filter_columns(start, first, width):
        part_rows = padded[pl.ds(start, BLOCK + 16), first : first + width]
        if first < content:
            taps = taps_value_ref[:, first : first + width]
        elif first < content + state_width:
            taps = taps_in_ref[:, first - content : first - content + width]
        else:
            base = first - content - state_width
            taps = taps_out_ref[:, base : base + width]
        mixed_rows = (
            taps[0:1] * part_rows[7 : 7 + BLOCK]
            + taps[1:2] * part_rows[8 : 8 + BLOCK]
            + taps[2:3] * part_rows[9 : 9 + BLOCK]
        )
        return silu(mixed_rows).astype(bf16)

    def filter_outward(at):
        start = pl.multiple_of(at * BLOCK, BLOCK)
        for first in range(0, state_width, wide_tile):
            outward_ref[pl.ds(start, BLOCK), first : first + wide_tile] = filter_columns(
                start, content + state_width + first, wide_tile
            )

    def block(at, group):
        start = pl.multiple_of(at * BLOCK, BLOCK)
        here = pl.ds(start, BLOCK)
        signal = filter_columns(start, group * span, span)
        inward = filter_columns(start, content + group * STATE, STATE)
        signal_ref[here, group * span : (group + 1) * span] = signal
        inward_ref[here, group * STATE : (group + 1) * STATE] = inward
        scale = scale_ref[here, :]
        wide = signal.astype(f32)
        scaled = jnp.concatenate(
            [wide * spread(scale, way * heads + group * ratio, ratio) for way in range(2)],
            axis=1,
        ).astype(bf16)
        block_states_ref[group, at] = lax.dot_general(
            inward, scaled, (((0,), (0,)), ((), ())), preferred_element_type=f32
        )

    project(part)
    project_gate(part)
    next(out_steps)
    next(out_steps)
    arrived(tokens.at[0, pl.ds(0, 2 * quarter)], token_receive.at[0, 2])
    project(before)
    project_gate(before)
    arrived(tokens.at[0, pl.ds(0, 2 * quarter)], token_receive.at[1, 2])
    project(after)

    early = part % 3 == 0

    send_edge(0, part != 1)
    send_edge(1, part != 2)
    project_gate(after)
    arrived(tokens.at[0, pl.ds(0, 2 * quarter)], onward_receive.at[0])
    project_quarters(opposite, (0, 3), range(0, channels, wide_tile))
    send_edge(0, part == 1)
    send_edge(1, part == 2)
    next(out_steps)
    ahead_of_last = 2 * opposite + 3
    turn = 2 - 2 * (part // 3)

    def early_block(step, _):
        at = (ahead_of_last + (step + turn) % 4) % count
        for group in range(groups):
            block(at, group)
        filter_outward(at)
        return 0

    early_block(0, 0)
    early_block(1, 0)
    @pl.when(part % 3 != 0)
    def _():
        early_block(2, 0)
        early_block(3, 0)

    arrived(tokens.at[0, pl.ds(0, 2 * quarter)], onward_receive.at[1])
    project_quarters(opposite, (1, 2), (0, content), outer_steps)
    summed_logs = [
        functools.reduce(jnp.add, [block_logs_ref[group, at] for at in range(count)])
        for group in range(groups)
    ]
    for way in range(2):
        for group in range(groups):
            for lane_tile in range(span // LANES):
                first = way * span + lane_tile * LANES
                log_tiles[way * groups + group, lane_tile : lane_tile + 1, :] = summed_logs[group][
                    :, first : first + LANES
                ]
    handled = stretches // (2 * groups)
    for peer in peers:
        remote(
            log_tiles.at[peer[0] // handled],
            all_logs.at[me],
            logs_send.at[0],
            logs_receive.at[0],
            peer,
        ).start()
    all_logs[me] = log_tiles[me // handled]
    late_turn = 2 * (part // 2) * (1 - part % 2)

    def late_at(step):
        return (ahead_of_last + 4 + (step + late_turn) % 4) % count

    def late_block(step, group):
        block(late_at(step), group)

    slice_rows = sent.shape[1]
    per_state = STATE // slice_rows
    my_group = me // handled % groups
    my_index = me % handled + handled * (me // (groups * handled))

    def final_states(group):
        for way in range(2):
            order = range(count) if way == 0 else range(count - 1, -1, -1)
            for lane_tile in range(span // LANES):
                first = way * span + lane_tile * LANES
                state = jnp.zeros((STATE, LANES), f32)
                for at in order:
                    state = (
                        state * jnp.exp(block_logs_ref[group, at, :, first : first + LANES])
                        + block_states_ref[group, at, :, first : first + LANES]
                    )
                at_slice = (way * groups + group) * per_state
                here = slice(lane_tile * LANES, (lane_tile + 1) * LANES)
                sent[at_slice : at_slice + per_state, :, here] = state.astype(bf16).reshape(
                    per_state, slice_rows, LANES
                )

    def send_slices(group):
        scanners = 2 * handled
        for hop in range(scanners):
            index = (my_index + hop) % scanners
            target = index // handled * (groups * handled) + group * handled + index % handled

            def send():
                remote(
                    sent.at[target],
                    slices.at[me],
                    scan_send.at[0],
                    scan_receive.at[0],
                    (target, part),
                ).start()

            if hop:
                send()
            else:
                pl.when(my_group != group)(send)

        @pl.when(my_group == group)
        def _():
            slices[me] = sent[me]

    late_block(0, 0)
    late_block(1, 0)

    def early_at(step):
        return (ahead_of_last + (step + turn) % 4) % count

    @pl.when(early)
    def _():
        take_edges()
        block(early_at(2), 0)
        block(early_at(3), 0)

    @pl.when(part % 3 != 0)
    def _():
        take_edges()

    late_block(2, 0)
    late_block(3, 0)
    final_states(0)
    send_slices(0)
    project_quarters(opposite, (1, 2), (span, content + state_width), False)
    @pl.when(early)
    def _():
        for step in range(2, 4):
            block(early_at(step), 1)
            filter_outward(early_at(step))

    for step in range(4):
        late_block(step, 1)
    final_states(1)
    send_slices(1)

    def keep_entries(group):
        def onward(at, carried):
            return enter(at, 0, *carried)

        def back(at, carried):
            return enter(count - 1 - at, span, *carried)

        def enter(at, base, state, logs):
            added = block_states_ref[group, at, :, base : base + span]
            decay = block_logs_ref[group, at, :, base : base + span]
            block_states_ref[group, at, :, base : base + span] = state
            block_logs_ref[group, at, :, base : base + span] = logs
            return state * jnp.exp(decay) + added, logs + decay

        empty = jnp.zeros((STATE, span), f32)
        still = jnp.zeros((1, span), f32)
        for body in (onward, back):
            lax.fori_loop(0, count, body, (empty, still))

    lanes = lax.broadcasted_iota(jnp.int32, (BLOCK, LANES), 1)

    def diagonal(at, _):
        here = pl.ds(pl.multiple_of(at * BLOCK, BLOCK), BLOCK)
        within = within_ref[here, :]
        wide_gates[here, :] = silu(gates[here, :].astype(f32))
        for group in range(groups):
            intersect = lax.dot_general(
                outward_ref[here, group * STATE : (group + 1) * STATE],
                inward_ref[here, group * STATE : (group + 1) * STATE],
                (((1,), (1,)), ((), ())),
                preferred_element_type=f32,
            )
            products = []
            for head in range(group * ratio, (group + 1) * ratio):
                other = heads + head
                gap_ahead = within[:, head : head + 1] - rows_ref[head : head + 1, here]
                gap_behind = within[:, other : other + 1] - rows_ref[other : other + 1, here]
                step_ahead = rows_ref[2 * heads + head : 2 * heads + head + 1, here]
                step_behind = rows_ref[2 * heads + other : 2 * heads + other + 1, here]
                gap = jnp.where(row >= column, gap_ahead, gap_behind)
                step = jnp.where(
                    row > column,
                    step_ahead,
                    jnp.where(row < column, step_behind, step_ahead + step_behind),
                )
                mixing = (intersect * jnp.exp(gap) * step).astype(bf16)
                tile = head // 2 * 2 * HEAD_DIM
                products.append(
                    jnp.dot(
                        mixing,
                        signal_ref[here, tile : tile + LANES],
                        preferred_element_type=f32,
                    )
                )
            for two in range(ratio // 2):
                at_tile = (group * ratio + 2 * two) * HEAD_DIM
                total[here, at_tile : at_tile + LANES] = jnp.where(
                    lanes < HEAD_DIM, products[2 * two], products[2 * two + 1]
                )
        return 0

    project_gate(opposite)

    def late_outward(step, _):
        filter_outward(late_at(step))
        return 0

    lax.fori_loop(0, 4, late_outward, 0)
    for group in range(groups):
        keep_entries(group)
    reverse = me // (stretches // 2)

    def scan_slices(group):
        arrived(all_logs.at[pl.ds(0, stretches - 1)], logs_receive.at[0])
        arrived(slices.at[pl.ds(0, stretches - 1)], scan_receive.at[0])

        def scan(step, state):
            for inner in range(4):
                at = 4 * step + inner
                source = at + reverse * (stretches - 1 - 2 * at)
                returned[source] = state.astype(bf16)
                logs = jnp.concatenate(
                    [all_logs[source, tile : tile + 1, :] for tile in range(span // LANES)],
                    axis=1,
                )
                state = state * jnp.exp(logs) + slices[source].astype(f32)
            return state

        lax.fori_loop(0, stretches // 4, scan, jnp.zeros((slice_rows, span), f32))
        for peer in peers:
            remote(
                returned.at[peer[0]],
                incoming.at[me],
                back_send.at[0],
                back_receive.at[group],
                peer,
            ).start()
        incoming[me] = returned[me]

    def take_incoming(group):
        scanners = 2 * handled

        @pl.when(my_group == group)
        def _():
            arrived(incoming.at[pl.ds(0, scanners - 1)], back_receive.at[group])

        @pl.when(my_group != group)
        def _():
            arrived(incoming.at[pl.ds(0, scanners)], back_receive.at[group])

    @pl.when(my_group == 0)
    def _():
        scan_slices(0)

    lax.fori_loop(0, count // 2, diagonal, 0)

    @pl.when(my_group == 1)
    def _():
        scan_slices(1)

    lax.fori_loop(count // 2, count, diagonal, 0)
    take_incoming(0)
    for _ in range(3):
        next(out_steps)
    def carried_in(way, group):
        first = (way * groups + group) * per_state
        return incoming[first : first + per_state].reshape(STATE, span).astype(f32)

    def finish(source, inner, group):
        at = source * (chunk // BLOCK) + inner
        here = pl.ds(pl.multiple_of(at * BLOCK, BLOCK), BLOCK)
        decays = jnp.exp(within_ref[here, :])
        wide = slice(group * span, (group + 1) * span)
        summed = total[here, wide]
        for way in range(2):
            base = way * span
            state = block_states_ref[group, at, :, base : base + span] + jnp.exp(
                block_logs_ref[group, at, :, base : base + span]
            ) * carried_in(way, group)
            carried = jnp.dot(
                outward_ref[here, group * STATE : (group + 1) * STATE],
                state.astype(bf16),
                preferred_element_type=f32,
            )
            summed += carried * spread(decays, way * heads + group * ratio, ratio)
        gated = summed * wide_gates[here, wide]
        scale = lax.rsqrt(jnp.mean(gated * gated, axis=-1, keepdims=True) + EPSILON)
        staged[group, source, pl.ds(inner * BLOCK, BLOCK), :] = (
            gated * scale * gain_ref[:, wide]
        ).astype(bf16)

    sides = (right, left)
    half_chunk = chunk // 2

    def half_of(at):
        return pl.ds(at * half_chunk, half_chunk)

    def send_mixed(group):
        for way in range(2):
            finish(opposite, way, group)
            remote(
                staged.at[group, opposite, half_of(way)],
                relay.at[group, way],
                mixed_send.at[0],
                relay_receive.at[2 * group + way],
                sides[way],
            ).start()
        for at in range(2):
            for way, target in enumerate((after, before)):
                finish(target, at, group)
                remote(
                    staged.at[group, target, half_of(at)],
                    mixed.at[group, part, half_of(at)],
                    mixed_send.at[0],
                    mixed_receive.at[2 * group + way],
                    sides[way],
                ).start()

    def pass_mixed(group):
        for way in range(2):
            arrived(relay.at[group, way], relay_receive.at[2 * group + way])
            remote(
                relay.at[group, way],
                mixed.at[group, (before, after)[way], half_of(way)],
                mixed_send.at[0],
                handed_receive.at[group],
                sides[way],
            ).start()

    send_mixed(0)
    take_incoming(1)
    send_mixed(1)
    pass_mixed(0)
    for group in range(groups):
        for at in range(2):
            finish(part, at, group)
    next(out_steps)
    pass_mixed(1)
    next(out_steps)

    def output(terms, first, last):
        broad = 8 * LANES

        def tile(at, _):
            columns = pl.ds(pl.multiple_of(at * broad, broad), broad)
            summed = 0.0 if first else summed_ref[:, columns]
            for block_of, group, source in terms:
                weight = jnp.concatenate(
                    [full_out[16 * at + 2 * place + group, source] for place in range(8)], axis=1
                )
                summed += jnp.dot(
                    block_of[group, source], weight, preferred_element_type=f32
                )
            if last:
                result_ref[:, columns] = summed.astype(bf16)
            else:
                summed_ref[:, columns] = summed
            return 0

        lax.fori_loop(0, features // broad, tile, 0)

    def take_sides(group):
        arrived(mixed.at[group, before], mixed_receive.at[2 * group])
        arrived(mixed.at[group, after], mixed_receive.at[2 * group + 1])

    take_sides(0)
    output(
        [(staged, 0, part), (staged, 1, part), (mixed, 0, before), (mixed, 0, after)],
        True,
        False,
    )
    take_sides(1)
    arrived(mixed.at[0, opposite], handed_receive.at[0])
    output([(mixed, 1, before), (mixed, 1, after), (mixed, 0, opposite)], False, False)
    arrived(mixed.at[1, opposite], handed_receive.at[1])
    output([(mixed, 1, opposite)], False, True)
    next(weights_steps)
    next(out_steps)
    pair.wait_send()
    left_here(full_out.at[0, pl.ds(0, 3)], cross_send.at[0])
    left_here(tokens.at[pl.ds(0, 3)], token_send.at[0])
    left_here(all_logs.at[pl.ds(0, stretches - 1)], logs_send.at[0])
    left_here(slices.at[pl.ds(0, stretches - 1)], scan_send.at[0])
    left_here(incoming.at[pl.ds(0, stretches - 1)], back_send.at[0])
    left_here(mixed, mixed_send.at[0])


def on_device(
    input_activations,
    norm_gain,
    w_gate,
    w_value,
    w_state_in,
    w_state_out,
    w_step_forward,
    w_step_backward,
    step_offset,
    fading_speed,
    conv_value,
    conv_state_in,
    conv_state_out,
    out_gain,
    w_out,
):
    stretches = lax.axis_size("sp")
    parts = lax.axis_size("tp")
    chunk, features = input_activations.shape
    extent = parts * chunk
    depth = w_gate.shape[0]
    content = w_value.shape[1]
    state_width = w_state_in.shape[1]
    heads = w_step_forward.shape[1]
    groups = state_width // STATE
    span = heads // groups * HEAD_DIM
    channels = content + 2 * state_width
    count = extent // BLOCK
    slice_rows = 2 * groups * STATE // stretches
    shift = math.log(extent * stretches)
    bf16, f32 = jnp.bfloat16, jnp.float32
    vmem, dma = pltpu.VMEM, pltpu.SemaphoreType.DMA
    space = pl.BlockSpec(memory_space=pltpu.VMEM)
    half_rows = w_out.shape[0] // 2
    inputs = (
        input_activations,
        norm_gain.reshape(1, features),
        w_gate,
        w_value,
        w_state_in,
        w_state_out,
        w_step_forward.T,
        w_step_backward.T,
        step_offset,
        fading_speed,
        conv_value,
        conv_state_in,
        conv_state_out,
        out_gain.reshape(1, content),
        w_out.T,
    )
    return pl.pallas_call(
        functools.partial(mixer_kernel, shift),
        out_shape=pltpu.VMEM((chunk, features), bf16),
        in_specs=[pl.BlockSpec(memory_space=pl.ANY)] * 15,
        out_specs=space,
        scratch_shapes=[
            vmem((parts, chunk, features), bf16),
            vmem((stretches * depth, channels + content + LANES), bf16),
            vmem((stretches, parts, half_rows, LANES), bf16),
            vmem((2, half_rows, LANES), bf16),
            vmem((half_rows, LANES), bf16),
            vmem((extent + 16, channels), f32),
            vmem((extent, content), bf16),
            vmem((extent, LANES), f32),
            vmem((chunk // 2, LANES), f32),
            vmem((2, 8, channels), f32),
            vmem((extent, content), bf16),
            vmem((extent, state_width), bf16),
            vmem((extent, state_width), bf16),
            vmem((extent, LANES), f32),
            vmem((4 * heads, extent), f32),
            vmem((groups, count, STATE, 2 * span), f32),
            vmem((groups, count, 1, 2 * span), f32),
            vmem((stretches, slice_rows, span), bf16),
            vmem((stretches, slice_rows, span), bf16),
            vmem((2 * groups, 8, LANES), f32),
            vmem((stretches, 8, LANES), f32),
            vmem((stretches, slice_rows, span), bf16),
            vmem((stretches, slice_rows, span), bf16),
            vmem((extent, content), f32),
            vmem((groups, parts, chunk, span), bf16),
            vmem((groups, parts, chunk, span), bf16),
            vmem((extent, content), f32),
            vmem((chunk, features), f32),
            vmem((groups, 2, chunk // 2, span), bf16),
            vmem((chunk, features), bf16),
            *[vmem(value.shape, value.dtype) for value in inputs[1:]],
            dma((1,)),
            dma((GATHER_WAITS,)),
            dma((1,)),
            dma((GATHER_WAITS,)),
            dma((1,)),
            dma((1,)),
            dma((1,)),
            dma((2,)),
            dma((1,)),
            dma((2, 3)),
            dma((2,)),
            dma((2,)),
            dma((2,)),
            dma((1,)),
            dma((1,)),
            dma((1,)),
            dma((1,)),
            dma((1,)),
            dma((2,)),
            dma((1,)),
            dma((4,)),
            dma((4,)),
            dma((2,)),
            dma((4,)),
            dma((14,)),
        ],
        cost_estimate=pl.CostEstimate(
            flops=int(3e10), bytes_accessed=1 << 20, transcendentals=0
        ),
        compiler_params=pltpu.CompilerParams(
            collective_id=1, has_side_effects=True, vmem_limit_bytes=VMEM_LIMIT
        ),
    )(*inputs)


def solution(mesh):
    return jax.shard_map(
        on_device,
        mesh=mesh,
        in_specs=(
            P(("sp", "tp"), None),
            P(),
            P("sp", "tp"),
            P("sp", "tp"),
            P("sp", "tp"),
            P("sp", "tp"),
            P("sp", "tp"),
            P("sp", "tp"),
            P(None, "tp"),
            P(None, "tp"),
            P(None, "tp"),
            P(None, "tp"),
            P(None, "tp"),
            P("tp"),
            P("tp", "sp"),
        ),
        out_specs=P(("sp", "tp"), None),
        check_vma=False,
    )
```

```python
import functools
import math

import jax
import jax.numpy as jnp
from jax import lax
from jax.experimental import pallas as pl
from jax.experimental.pallas import tpu as pltpu
from jax.sharding import PartitionSpec as P

HEAD_DIM = 64
STATE = 128
BLOCK = 128
LANES = 128
EPSILON = 1e-06
HIGHEST = lax.Precision.HIGHEST
VMEM_LIMIT = 60 * 1024 * 1024
SIDE = 4


def rms_rows(values):
    wide = values.astype(jnp.float32)
    return wide * lax.rsqrt(jnp.mean(wide * wide, axis=-1, keepdims=True) + EPSILON)


def softplus(values):
    return jnp.maximum(values, 0.0) + jnp.log1p(jnp.exp(-jnp.abs(values)))


def spread(columns, first, count):
    rows = columns.shape[0]
    lane = lax.broadcasted_iota(jnp.int32, (rows, LANES), 1)
    tiles = []
    for at in range(first, first + count, 2):
        low = jnp.broadcast_to(columns[:, at : at + 1], (rows, LANES))
        high = jnp.broadcast_to(columns[:, at + 1 : at + 2], (rows, LANES))
        tiles.append(jnp.where(lane < HEAD_DIM, low, high))
    return jnp.concatenate(tiles, axis=1)


def silu(values):
    half = 0.5 * values
    return half + half * jnp.tanh(half)


def greet(peers):
    barrier = pltpu.get_barrier_semaphore()
    for peer in peers:
        pl.semaphore_signal(
            barrier, inc=1, device_id=peer, device_id_type=pl.DeviceIdType.MESH
        )
    return lambda: pl.semaphore_wait(barrier, len(peers))


def remote(source, target, send, receive, peer):
    return pltpu.make_async_remote_copy(
        src_ref=source,
        dst_ref=target,
        send_sem=send,
        recv_sem=receive,
        device_id=peer,
        device_id_type=pl.DeviceIdType.MESH,
    )


def place():
    me = lax.axis_index("sp")
    return me // (2 * SIDE), me // 2 % SIDE, me % 2


def plane_gather(whole, half, many, send, receive):
    z, y, c = place()
    part = lax.axis_index("tp")

    def origin(first, second):
        over_z = (z + c * first + (1 - c) * second + 2 * SIDE) % SIDE
        over_y = (y + (1 - c) * first + c * second + 2 * SIDE) % SIDE
        return (over_z * SIDE + over_y) * 2 + c

    along = [(origin(1, 0), part), (origin(-1, 0), part)]
    cross = [(origin(0, 1), part), (origin(0, -1), part)]
    partner = ((z * SIDE + y) * 2 + 1 - c, part)
    lines = (0, -1, 1, 2)
    at_line, at_far, at_shared, at_over, at_last = 0, 1, 2, 3, 7

    def go(block, peer, kind):
        remote(block, block, send.at[0], receive.at[kind], peer).start()

    def arrived(shards, kind):
        remote(many(shards), many(shards), send.at[0], receive.at[kind], partner).wait_recv()

    def share(at):
        go(whole(at), partner, at_shared)

    def spread_line(first):
        for peer in cross:
            go(whole(origin(first, 0)), peer, at_over + lines.index(first))
        share(origin(first, 0))

    def forward(first):
        arrived(2, at_over + lines.index(first))
        for way in range(2):
            go(half(origin(first, (-1, 1)[way]), way), cross[way], at_last + lines.index(first))
        for way in range(2):
            share(origin(first, (-1, 1)[way]))

    for peer in along:
        go(whole(origin(0, 0)), peer, at_line)
    spread_line(0)
    yield
    arrived(2, at_line)
    for way in range(2):
        go(half(origin((-1, 1)[way], 0), way), along[way], at_far)
    for way in range(2):
        spread_line((-1, 1)[way])
    yield
    forward(0)
    yield
    arrived(1, at_far)
    spread_line(2)
    yield
    forward(-1)
    yield
    forward(1)
    yield
    forward(2)
    yield
    for at, first in enumerate(lines):
        arrived(1, at_last + at)
        share(origin(first, 2))
    yield
    arrived(16, at_shared)
    yield
    remote(many(31), many(31), send.at[0], receive.at[at_line], partner).wait_send()
    yield


GATHER_WAITS = 11


def mixer_kernel(
    shift,
    x_ref,
    norm_gain_from,
    gate_weights_from,
    value_weights_from,
    in_weights_from,
    out_weights_from,
    ahead_weights_from,
    behind_weights_from,
    offset_from,
    speed_from,
    taps_value_from,
    taps_in_from,
    taps_out_from,
    gain_from,
    w_out_from,
    result_ref,
    tokens,
    weights,
    full_out,
    placed,
    paired,
    padded,
    gates,
    scale_ref,
    outer_steps,
    halo,
    signal_ref,
    inward_ref,
    outward_ref,
    within_ref,
    rows_ref,
    block_states_ref,
    block_logs_ref,
    sent,
    slices,
    log_tiles,
    all_logs,
    returned,
    incoming,
    total,
    staged,
    mixed,
    wide_gates,
    summed_ref,
    relay,
    raw_tokens,
    norm_gain_ref,
    gate_weights_ref,
    value_weights_ref,
    in_weights_ref,
    out_weights_ref,
    ahead_weights_ref,
    behind_weights_ref,
    offset_ref,
    speed_ref,
    taps_value_ref,
    taps_in_ref,
    taps_out_ref,
    gain_ref,
    w_out_ref,
    weights_send,
    weights_receive,
    out_send,
    out_receive,
    pair_send,
    pair_receive,
    cross_send,
    cross_receive,
    token_send,
    token_receive,
    onward_receive,
    halo_send,
    halo_receive,
    logs_send,
    logs_receive,
    scan_send,
    scan_receive,
    back_send,
    back_receive,
    mixed_send,
    mixed_receive,
    relay_receive,
    handed_receive,
    load,
    inputs_load,
):
    me, part = lax.axis_index("sp"), lax.axis_index("tp")
    core = me % 2
    stretches = slices.shape[0]
    parts, chunk, features = tokens.shape
    extent = parts * chunk
    depth = value_weights_ref.shape[0]
    content = value_weights_ref.shape[1]
    state_width = in_weights_ref.shape[1]
    heads = ahead_weights_ref.shape[0]
    groups = state_width // STATE
    ratio = heads // groups
    span = ratio * HEAD_DIM
    channels = content + 2 * state_width
    count = extent // BLOCK
    f32, bf16 = jnp.float32, jnp.bfloat16

    peers = [((me + hop) % stretches, part) for hop in range(1, stretches)]
    across = [(me, (part + hop) % parts) for hop in range(1, parts)]
    settle = greet(peers + across)

    quarter = chunk // 4
    loads = []
    for at in (0, 3, 1, 2):
        here = pl.ds(at * quarter, quarter)
        copy = pltpu.make_async_copy(x_ref.at[here], raw_tokens.at[here], load.at[at])
        copy.start()
        loads.append(copy)
    fetched = []
    for at, (source, target) in enumerate(
        (
            (norm_gain_from, norm_gain_ref),
            (gate_weights_from, gate_weights_ref),
            (value_weights_from, value_weights_ref),
            (in_weights_from, in_weights_ref),
            (out_weights_from, out_weights_ref),
            (ahead_weights_from, ahead_weights_ref),
            (behind_weights_from, behind_weights_ref),
            (offset_from, offset_ref),
            (speed_from, speed_ref),
            (taps_value_from, taps_value_ref),
            (taps_in_from, taps_in_ref),
            (taps_out_from, taps_out_ref),
            (gain_from, gain_ref),
            (w_out_from, w_out_ref),
        )
    ):
        copy = pltpu.make_async_copy(source, target, inputs_load.at[at])
        copy.start()
        fetched.append(copy)
    rows = 16

    def normalize(at):
        for step in range(quarter // rows):
            here = pl.ds(at * quarter + step * rows, rows)
            normed = rms_rows(raw_tokens[here, :]) * norm_gain_ref[...]
            tokens[part, here, :] = normed.astype(bf16)

    fetched[0].wait()
    for at, copy in zip((0, 3), loads[:2]):
        copy.wait()
        normalize(at)
    settle()

    right, left = (me, (part + 1) % parts), (me, (part + parts - 1) % parts)
    before, after = (part + parts - 1) % parts, (part + 1) % parts
    opposite = (part + 2) % parts

    def piece(source, at):
        return tokens.at[source, pl.ds(at * quarter, quarter)]

    orders = ((0, 1, 2, 3), (3, 2, 1, 0))

    def arrived(block, semaphore):
        remote(block, block, semaphore, semaphore, right).wait_recv()

    def left_here(block, semaphore):
        remote(block, block, semaphore, semaphore, right).wait_send()

    def send_own(step):
        for way, peer in enumerate((right, left)):
            block = piece(part, orders[way][step])
            received = token_receive.at[way, min(step, 2)]
            remote(block, block, token_send.at[0], received, peer).start()

    def pass_on(step):
        for way, peer in enumerate((right, left)):
            block = piece((before, after)[way], orders[way][step])
            arrived(block, token_receive.at[way, step])
            remote(block, block, token_send.at[0], onward_receive.at[step], peer).start()

    weights_steps = plane_gather(
        lambda at: weights.at[pl.ds(pl.multiple_of(at * depth, depth), depth)],
        lambda at, side: weights.at[
            pl.ds(pl.multiple_of(at * depth + side * (depth // 2), depth // 2), depth // 2)
        ],
        lambda shards: weights.at[pl.ds(0, shards * depth)],
        weights_send,
        weights_receive,
    )
    out_steps = plane_gather(
        lambda at: full_out.at[at],
        lambda at, side: full_out.at[at, pl.ds(side * (parts // 2), parts // 2)],
        lambda shards: full_out.at[pl.ds(0, shards)],
        out_send,
        out_receive,
    )

    z, y, _ = place()
    partner = ((z * SIDE + y) * 2 + 1 - core, part)
    pair = remote(placed.at[1 - core], paired, pair_send.at[0], pair_receive.at[0], partner)
    send_own(0)
    for copy in fetched[1:7]:
        copy.wait()
    own_rows = pl.ds(pl.multiple_of(me * depth, depth), depth)
    weights[own_rows, 0:content] = value_weights_ref[...]
    weights[own_rows, content : content + state_width] = in_weights_ref[...]
    weights[own_rows, content + state_width : channels] = out_weights_ref[...]
    weights[own_rows, channels : channels + content] = gate_weights_ref[...]

    def across_rows(left, right):
        return lax.dot_general(left, right, (((0,), (0,)), ((), ())), preferred_element_type=f32)

    head_row = lax.broadcasted_iota(jnp.int32, (heads, LANES), 0)
    head_lane = lax.broadcasted_iota(jnp.int32, (heads, LANES), 1)
    to_ahead = (head_row == head_lane).astype(bf16)
    to_behind = (head_row + heads == head_lane).astype(bf16)
    weights[own_rows, channels + content :] = (
        across_rows(ahead_weights_ref[...], to_ahead)
        + across_rows(behind_weights_ref[...], to_behind)
    ).astype(bf16)
    next(weights_steps)
    width = w_out_ref.shape[0]
    move_row = lax.broadcasted_iota(jnp.int32, (width, LANES), 0)
    move_lane = lax.broadcasted_iota(jnp.int32, (width, LANES), 1)
    to_half = (move_row + core * width == move_lane).astype(bf16)
    half_rows = w_out_ref.shape[1] // 2
    fetched[13].wait()
    for side in range(2):
        placed[side] = across_rows(
            w_out_ref[:, side * half_rows : (side + 1) * half_rows], to_half
        ).astype(bf16)
    pair.start()
    loads[2].wait()
    normalize(1)
    pair.wait_recv()
    full_out[me, part] = placed[core] + paired[...]
    loads[3].wait()
    normalize(2)
    for peer in (right, left):
        block = full_out.at[me, part]
        remote(block, block, cross_send.at[0], cross_receive.at[0], peer).start()
    send_own(1)
    next(weights_steps)
    next(weights_steps)
    both = full_out.at[me, pl.ds(0, 2)]
    arrived(both, cross_receive.at[0])
    block = full_out.at[me, (part + 3 + 2 * core) % parts]
    onward_peer = (me, (part + 1 + 2 * core) % parts)
    remote(block, block, cross_send.at[0], cross_receive.at[1], onward_peer).start()
    send_own(2)
    send_own(3)
    next(weights_steps)
    pass_on(0)
    next(weights_steps)
    next(weights_steps)
    pass_on(1)
    next(weights_steps)
    arrived(full_out.at[me, 0], cross_receive.at[1])
    next(out_steps)
    next(weights_steps)
    next(weights_steps)

    wide_tile = 2 * LANES

    def product(source, columns):
        return jnp.dot(tokens[source], weights[:, columns], preferred_element_type=f32)

    row = lax.broadcasted_iota(jnp.int32, (BLOCK, BLOCK), 0)
    column = lax.broadcasted_iota(jnp.int32, (BLOCK, BLOCK), 1)
    for copy in fetched[7:13]:
        copy.wait()
    triangles = jnp.concatenate([row >= column, row <= column], axis=0).astype(bf16)
    lane = lax.broadcasted_iota(jnp.int32, (1, LANES), 1)
    spare = jnp.zeros((1, LANES - 2 * heads), f32)
    offset = jnp.concatenate([offset_ref[0:1, :], offset_ref[1:2, :], spare], axis=1)
    rate = jnp.concatenate([speed_ref[0:1, :], speed_ref[1:2, :], spare], axis=1)

    def decays_of(source, raw):
        steps = softplus(raw + offset - shift)
        logs = -steps * rate
        logs = jnp.concatenate([logs[:BLOCK], logs[BLOCK:]], axis=1)
        high = logs.astype(bf16)
        rest = logs - high.astype(f32)
        middle = rest.astype(bf16)
        low = (rest - middle.astype(f32)).astype(bf16)
        sums = jnp.dot(
            triangles,
            jnp.concatenate([high, middle, low], axis=1),
            preferred_element_type=f32,
        )
        sums = sums[:, : 2 * LANES] + (
            sums[:, 2 * LANES : 4 * LANES] + sums[:, 4 * LANES : 6 * LANES]
        )
        for inner in range(2):
            at = 2 * source + inner
            here = pl.ds(pl.multiple_of(at * BLOCK, BLOCK), BLOCK)
            lanes_of = slice(inner * LANES, (inner + 1) * LANES)
            within = jnp.where(lane < heads, sums[:BLOCK, lanes_of], sums[BLOCK:, lanes_of])
            final = jnp.where(lane < heads, within[BLOCK - 1 : BLOCK], within[0:1])
            step = steps[inner * BLOCK : (inner + 1) * BLOCK]
            within_ref[here, :] = within
            rows_ref[0 : 2 * heads, here] = within.T[0 : 2 * heads]
            rows_ref[2 * heads : 4 * heads, here] = step.T[0 : 2 * heads]
            scale_ref[here, :] = jnp.exp(final - within) * step
            for group in range(groups):
                block_logs_ref[group, at] = jnp.concatenate(
                    [spread(final, way * heads + group * ratio, ratio) for way in range(2)],
                    axis=1,
                )

    def project(source):
        start = pl.multiple_of(source * chunk, chunk)
        raw = product(source, slice(channels + content, channels + content + LANES))
        decays_of(source, raw.astype(bf16).astype(f32))

        for first in range(0, channels, wide_tile):
            columns = slice(first, first + wide_tile)
            padded[pl.ds(start + 8, chunk), columns] = (
                product(source, columns).astype(bf16).astype(f32)
            )
    def project_quarters(source, at, firsts, rest=None):
        start = pl.multiple_of(source * chunk, chunk)
        halves = [tokens[source, place * quarter : (place + 1) * quarter] for place in at]
        left_side = jnp.concatenate(halves, axis=0)

        def some(columns):
            made = jnp.dot(left_side, weights[:, columns], preferred_element_type=f32)
            return made.astype(bf16).astype(f32)

        if rest is not False:
            raw = some(slice(channels + content, channels + content + LANES))
        if rest is None:
            outer_steps[...] = raw
        elif rest is not False:
            outer = rest[...]
            decays_of(source, jnp.concatenate([outer[:quarter], raw, outer[quarter:]], axis=0))
        for first in firsts:
            columns = slice(first, first + wide_tile)
            made = some(columns)
            for half_at, place in enumerate(at):
                padded[pl.ds(start + 8 + place * quarter, quarter), columns] = made[
                    half_at * quarter : (half_at + 1) * quarter
                ]

    def project_gate(source):
        start = pl.multiple_of(source * chunk, chunk)

        for first in range(0, content, wide_tile):
            gates[pl.ds(start, chunk), first : first + wide_tile] = product(
                source, slice(channels + first, channels + first + wide_tile)
            ).astype(bf16)

    has_next, has_last = me < stretches - 1, me > 0
    sends_to, takes_from = (has_next, has_last), (has_last, has_next)

    def edge_copy(way):
        peer = ((me + (1, stretches - 1)[way]) % stretches, part)
        block = padded.at[pl.ds((extent, 8)[way], 8)]
        return remote(block, halo.at[way], halo_send.at[way], halo_receive.at[way], peer)

    def send_edge(way, when):
        @pl.when(jnp.logical_and(when, sends_to[way]))
        def _():
            edge_copy(way).start()

    def take_edges():
        for way in range(2):
            beyond = pl.ds((0, extent + 8)[way], 8)

            @pl.when(takes_from[way])
            def _():
                edge_copy(way).wait_recv()
                padded[beyond, :] = halo[way]

            @pl.when(jnp.logical_not(takes_from[way]))
            def _():
                padded[beyond, :] = jnp.zeros((8, channels), f32)

            @pl.when(sends_to[way])
            def _():
                edge_copy(way).wait_send()

    def filter_columns(start, first, width):
        part_rows = padded[pl.ds(start, BLOCK + 16), first : first + width]
        if first < content:
            taps = taps_value_ref[:, first : first + width]
        elif first < content + state_width:
            taps = taps_in_ref[:, first - content : first - content + width]
        else:
            base = first - content - state_width
            taps = taps_out_ref[:, base : base + width]
        mixed_rows = (
            taps[0:1] * part_rows[7 : 7 + BLOCK]
            + taps[1:2] * part_rows[8 : 8 + BLOCK]
            + taps[2:3] * part_rows[9 : 9 + BLOCK]
        )
        return silu(mixed_rows).astype(bf16)

    def filter_outward(at):
        start = pl.multiple_of(at * BLOCK, BLOCK)
        for first in range(0, state_width, wide_tile):
            outward_ref[pl.ds(start, BLOCK), first : first + wide_tile] = filter_columns(
                start, content + state_width + first, wide_tile
            )

    def block(at, group):
        start = pl.multiple_of(at * BLOCK, BLOCK)
        here = pl.ds(start, BLOCK)
        signal = filter_columns(start, group * span, span)
        inward = filter_columns(start, content + group * STATE, STATE)
        signal_ref[here, group * span : (group + 1) * span] = signal
        inward_ref[here, group * STATE : (group + 1) * STATE] = inward
        scale = scale_ref[here, :]
        wide = signal.astype(f32)
        scaled = jnp.concatenate(
            [wide * spread(scale, way * heads + group * ratio, ratio) for way in range(2)],
            axis=1,
        ).astype(bf16)
        block_states_ref[group, at] = lax.dot_general(
            inward, scaled, (((0,), (0,)), ((), ())), preferred_element_type=f32
        )

    project(part)
    project_gate(part)
    next(out_steps)
    next(out_steps)
    arrived(tokens.at[0, pl.ds(0, 2 * quarter)], token_receive.at[0, 2])
    project(before)
    project_gate(before)
    arrived(tokens.at[0, pl.ds(0, 2 * quarter)], token_receive.at[1, 2])
    project(after)

    early = part % 3 == 0

    send_edge(0, part != 1)
    send_edge(1, part != 2)
    project_gate(after)
    arrived(tokens.at[0, pl.ds(0, 2 * quarter)], onward_receive.at[0])
    project_quarters(opposite, (0, 3), range(0, channels, wide_tile))
    send_edge(0, part == 1)
    send_edge(1, part == 2)
    next(out_steps)
    ahead_of_last = 2 * opposite + 3
    turn = 2 - 2 * (part // 3)

    def early_block(step, _):
        at = (ahead_of_last + (step + turn) % 4) % count
        for group in range(groups):
            block(at, group)
        filter_outward(at)
        return 0

    early_block(0, 0)
    early_block(1, 0)
    @pl.when(part % 3 != 0)
    def _():
        early_block(2, 0)
        early_block(3, 0)

    arrived(tokens.at[0, pl.ds(0, 2 * quarter)], onward_receive.at[1])
    project_quarters(opposite, (1, 2), (0, content), outer_steps)
    summed_logs = [
        functools.reduce(jnp.add, [block_logs_ref[group, at] for at in range(count)])
        for group in range(groups)
    ]
    for way in range(2):
        for group in range(groups):
            for lane_tile in range(span // LANES):
                first = way * span + lane_tile * LANES
                log_tiles[way * groups + group, lane_tile : lane_tile + 1, :] = summed_logs[group][
                    :, first : first + LANES
                ]
    handled = stretches // (2 * groups)
    for peer in peers:
        remote(
            log_tiles.at[peer[0] // handled],
            all_logs.at[me],
            logs_send.at[0],
            logs_receive.at[0],
            peer,
        ).start()
    all_logs[me] = log_tiles[me // handled]
    late_turn = 2 * (part // 2) * (1 - part % 2)

    def late_at(step):
        return (ahead_of_last + 4 + (step + late_turn) % 4) % count

    def late_block(step, group):
        block(late_at(step), group)

    slice_rows = sent.shape[1]
    per_state = STATE // slice_rows
    my_group = me // handled % groups
    my_index = me % handled + handled * (me // (groups * handled))

    def final_states(group):
        for way in range(2):
            order = range(count) if way == 0 else range(count - 1, -1, -1)
            for lane_tile in range(span // LANES):
                first = way * span + lane_tile * LANES
                state = jnp.zeros((STATE, LANES), f32)
                for at in order:
                    state = (
                        state * jnp.exp(block_logs_ref[group, at, :, first : first + LANES])
                        + block_states_ref[group, at, :, first : first + LANES]
                    )
                at_slice = (way * groups + group) * per_state
                here = slice(lane_tile * LANES, (lane_tile + 1) * LANES)
                sent[at_slice : at_slice + per_state, :, here] = state.astype(bf16).reshape(
                    per_state, slice_rows, LANES
                )

    def send_slices(group):
        scanners = 2 * handled
        for hop in range(scanners):
            index = (my_index + hop) % scanners
            target = index // handled * (groups * handled) + group * handled + index % handled

            def send():
                remote(
                    sent.at[target],
                    slices.at[me],
                    scan_send.at[0],
                    scan_receive.at[0],
                    (target, part),
                ).start()

            if hop:
                send()
            else:
                pl.when(my_group != group)(send)

        @pl.when(my_group == group)
        def _():
            slices[me] = sent[me]

    late_block(0, 0)
    late_block(1, 0)

    def early_at(step):
        return (ahead_of_last + (step + turn) % 4) % count

    @pl.when(early)
    def _():
        take_edges()
        block(early_at(2), 0)
        block(early_at(3), 0)

    @pl.when(part % 3 != 0)
    def _():
        take_edges()

    late_block(2, 0)
    late_block(3, 0)
    final_states(0)
    send_slices(0)
    project_quarters(opposite, (1, 2), (span, content + state_width), False)
    @pl.when(early)
    def _():
        for step in range(2, 4):
            block(early_at(step), 1)
            filter_outward(early_at(step))

    for step in range(4):
        late_block(step, 1)
    final_states(1)
    send_slices(1)

    def keep_entries(group):
        def onward(at, carried):
            return enter(at, 0, *carried)

        def back(at, carried):
            return enter(count - 1 - at, span, *carried)

        def enter(at, base, state, logs):
            added = block_states_ref[group, at, :, base : base + span]
            decay = block_logs_ref[group, at, :, base : base + span]
            block_states_ref[group, at, :, base : base + span] = state
            block_logs_ref[group, at, :, base : base + span] = logs
            return state * jnp.exp(decay) + added, logs + decay

        empty = jnp.zeros((STATE, span), f32)
        still = jnp.zeros((1, span), f32)
        for body in (onward, back):
            lax.fori_loop(0, count, body, (empty, still))

    lanes = lax.broadcasted_iota(jnp.int32, (BLOCK, LANES), 1)

    def diagonal(at, _):
        here = pl.ds(pl.multiple_of(at * BLOCK, BLOCK), BLOCK)
        within = within_ref[here, :]
        wide_gates[here, :] = silu(gates[here, :].astype(f32))
        for group in range(groups):
            intersect = lax.dot_general(
                outward_ref[here, group * STATE : (group + 1) * STATE],
                inward_ref[here, group * STATE : (group + 1) * STATE],
                (((1,), (1,)), ((), ())),
                preferred_element_type=f32,
            )
            products = []
            for head in range(group * ratio, (group + 1) * ratio):
                other = heads + head
                gap_ahead = within[:, head : head + 1] - rows_ref[head : head + 1, here]
                gap_behind = within[:, other : other + 1] - rows_ref[other : other + 1, here]
                step_ahead = rows_ref[2 * heads + head : 2 * heads + head + 1, here]
                step_behind = rows_ref[2 * heads + other : 2 * heads + other + 1, here]
                gap = jnp.where(row >= column, gap_ahead, gap_behind)
                step = jnp.where(
                    row > column,
                    step_ahead,
                    jnp.where(row < column, step_behind, step_ahead + step_behind),
                )
                mixing = (intersect * jnp.exp(gap) * step).astype(bf16)
                tile = head // 2 * 2 * HEAD_DIM
                products.append(
                    jnp.dot(
                        mixing,
                        signal_ref[here, tile : tile + LANES],
                        preferred_element_type=f32,
                    )
                )
            for two in range(ratio // 2):
                at_tile = (group * ratio + 2 * two) * HEAD_DIM
                total[here, at_tile : at_tile + LANES] = jnp.where(
                    lanes < HEAD_DIM, products[2 * two], products[2 * two + 1]
                )
        return 0

    project_gate(opposite)

    def late_outward(step, _):
        filter_outward(late_at(step))
        return 0

    lax.fori_loop(0, 4, late_outward, 0)
    for group in range(groups):
        keep_entries(group)
    reverse = me // (stretches // 2)

    def scan_slices(group):
        arrived(all_logs.at[pl.ds(0, stretches - 1)], logs_receive.at[0])
        arrived(slices.at[pl.ds(0, stretches - 1)], scan_receive.at[0])

        def scan(step, state):
            for inner in range(4):
                at = 4 * step + inner
                source = at + reverse * (stretches - 1 - 2 * at)
                returned[source] = state.astype(bf16)
                logs = jnp.concatenate(
                    [all_logs[source, tile : tile + 1, :] for tile in range(span // LANES)],
                    axis=1,
                )
                state = state * jnp.exp(logs) + slices[source].astype(f32)
            return state

        lax.fori_loop(0, stretches // 4, scan, jnp.zeros((slice_rows, span), f32))
        for peer in peers:
            remote(
                returned.at[peer[0]],
                incoming.at[me],
                back_send.at[0],
                back_receive.at[group],
                peer,
            ).start()
        incoming[me] = returned[me]

    def take_incoming(group):
        scanners = 2 * handled

        @pl.when(my_group == group)
        def _():
            arrived(incoming.at[pl.ds(0, scanners - 1)], back_receive.at[group])

        @pl.when(my_group != group)
        def _():
            arrived(incoming.at[pl.ds(0, scanners)], back_receive.at[group])

    @pl.when(my_group == 0)
    def _():
        scan_slices(0)

    lax.fori_loop(0, 3 * count // 4, diagonal, 0)

    @pl.when(my_group == 1)
    def _():
        scan_slices(1)

    lax.fori_loop(3 * count // 4, count, diagonal, 0)
    take_incoming(0)
    for _ in range(3):
        next(out_steps)
    def carried_in(way, group):
        first = (way * groups + group) * per_state
        return incoming[first : first + per_state].reshape(STATE, span).astype(f32)

    def finish(source, inner, group):
        at = source * (chunk // BLOCK) + inner
        here = pl.ds(pl.multiple_of(at * BLOCK, BLOCK), BLOCK)
        decays = jnp.exp(within_ref[here, :])
        wide = slice(group * span, (group + 1) * span)
        summed = total[here, wide]
        for way in range(2):
            base = way * span
            state = block_states_ref[group, at, :, base : base + span] + jnp.exp(
                block_logs_ref[group, at, :, base : base + span]
            ) * carried_in(way, group)
            carried = jnp.dot(
                outward_ref[here, group * STATE : (group + 1) * STATE],
                state.astype(bf16),
                preferred_element_type=f32,
            )
            summed += carried * spread(decays, way * heads + group * ratio, ratio)
        gated = summed * wide_gates[here, wide]
        scale = lax.rsqrt(jnp.mean(gated * gated, axis=-1, keepdims=True) + EPSILON)
        staged[group, source, pl.ds(inner * BLOCK, BLOCK), :] = (
            gated * scale * gain_ref[:, wide]
        ).astype(bf16)

    sides = (right, left)
    half_chunk = chunk // 2

    def half_of(at):
        return pl.ds(at * half_chunk, half_chunk)

    def send_mixed(group):
        for way in range(2):
            finish(opposite, way, group)
            remote(
                staged.at[group, opposite, half_of(way)],
                relay.at[group, way],
                mixed_send.at[0],
                relay_receive.at[2 * group + way],
                sides[way],
            ).start()
        for at in range(2):
            for way, target in enumerate((after, before)):
                finish(target, at, group)
                remote(
                    staged.at[group, target, half_of(at)],
                    mixed.at[group, part, half_of(at)],
                    mixed_send.at[0],
                    mixed_receive.at[2 * group + way],
                    sides[way],
                ).start()

    def pass_mixed(group):
        for way in range(2):
            arrived(relay.at[group, way], relay_receive.at[2 * group + way])
            remote(
                relay.at[group, way],
                mixed.at[group, (before, after)[way], half_of(way)],
                mixed_send.at[0],
                handed_receive.at[group],
                sides[way],
            ).start()

    send_mixed(0)
    take_incoming(1)
    send_mixed(1)
    pass_mixed(0)
    for group in range(groups):
        for at in range(2):
            finish(part, at, group)
    next(out_steps)
    pass_mixed(1)
    next(out_steps)

    def output(terms, first, last):
        broad = 8 * LANES

        def tile(at, _):
            columns = pl.ds(pl.multiple_of(at * broad, broad), broad)
            summed = 0.0 if first else summed_ref[:, columns]
            for block_of, group, source in terms:
                weight = jnp.concatenate(
                    [full_out[16 * at + 2 * place + group, source] for place in range(8)], axis=1
                )
                summed += jnp.dot(
                    block_of[group, source], weight, preferred_element_type=f32
                )
            if last:
                result_ref[:, columns] = summed.astype(bf16)
            else:
                summed_ref[:, columns] = summed
            return 0

        lax.fori_loop(0, features // broad, tile, 0)

    def take_sides(group):
        arrived(mixed.at[group, before], mixed_receive.at[2 * group])
        arrived(mixed.at[group, after], mixed_receive.at[2 * group + 1])

    take_sides(0)
    output(
        [(staged, 0, part), (staged, 1, part), (mixed, 0, before), (mixed, 0, after)],
        True,
        False,
    )
    take_sides(1)
    arrived(mixed.at[0, opposite], handed_receive.at[0])
    output([(mixed, 1, before), (mixed, 1, after), (mixed, 0, opposite)], False, False)
    arrived(mixed.at[1, opposite], handed_receive.at[1])
    output([(mixed, 1, opposite)], False, True)
    next(weights_steps)
    next(out_steps)
    pair.wait_send()
    left_here(full_out.at[0, pl.ds(0, 3)], cross_send.at[0])
    left_here(tokens.at[pl.ds(0, 3)], token_send.at[0])
    left_here(all_logs.at[pl.ds(0, stretches - 1)], logs_send.at[0])
    left_here(slices.at[pl.ds(0, stretches - 1)], scan_send.at[0])
    left_here(incoming.at[pl.ds(0, stretches - 1)], back_send.at[0])
    left_here(mixed, mixed_send.at[0])


def on_device(
    input_activations,
    norm_gain,
    w_gate,
    w_value,
    w_state_in,
    w_state_out,
    w_step_forward,
    w_step_backward,
    step_offset,
    fading_speed,
    conv_value,
    conv_state_in,
    conv_state_out,
    out_gain,
    w_out,
):
    stretches = lax.axis_size("sp")
    parts = lax.axis_size("tp")
    chunk, features = input_activations.shape
    extent = parts * chunk
    depth = w_gate.shape[0]
    content = w_value.shape[1]
    state_width = w_state_in.shape[1]
    heads = w_step_forward.shape[1]
    groups = state_width // STATE
    span = heads // groups * HEAD_DIM
    channels = content + 2 * state_width
    count = extent // BLOCK
    slice_rows = 2 * groups * STATE // stretches
    shift = math.log(extent * stretches)
    bf16, f32 = jnp.bfloat16, jnp.float32
    vmem, dma = pltpu.VMEM, pltpu.SemaphoreType.DMA
    space = pl.BlockSpec(memory_space=pltpu.VMEM)
    half_rows = w_out.shape[0] // 2
    inputs = (
        input_activations,
        norm_gain.reshape(1, features),
        w_gate,
        w_value,
        w_state_in,
        w_state_out,
        w_step_forward.T,
        w_step_backward.T,
        step_offset,
        fading_speed,
        conv_value,
        conv_state_in,
        conv_state_out,
        out_gain.reshape(1, content),
        w_out.T,
    )
    return pl.pallas_call(
        functools.partial(mixer_kernel, shift),
        out_shape=pltpu.VMEM((chunk, features), bf16),
        in_specs=[pl.BlockSpec(memory_space=pl.ANY)] * 15,
        out_specs=space,
        scratch_shapes=[
            vmem((parts, chunk, features), bf16),
            vmem((stretches * depth, channels + content + LANES), bf16),
            vmem((stretches, parts, half_rows, LANES), bf16),
            vmem((2, half_rows, LANES), bf16),
            vmem((half_rows, LANES), bf16),
            vmem((extent + 16, channels), f32),
            vmem((extent, content), bf16),
            vmem((extent, LANES), f32),
            vmem((chunk // 2, LANES), f32),
            vmem((2, 8, channels), f32),
            vmem((extent, content), bf16),
            vmem((extent, state_width), bf16),
            vmem((extent, state_width), bf16),
            vmem((extent, LANES), f32),
            vmem((4 * heads, extent), f32),
            vmem((groups, count, STATE, 2 * span), f32),
            vmem((groups, count, 1, 2 * span), f32),
            vmem((stretches, slice_rows, span), bf16),
            vmem((stretches, slice_rows, span), bf16),
            vmem((2 * groups, 8, LANES), f32),
            vmem((stretches, 8, LANES), f32),
            vmem((stretches, slice_rows, span), bf16),
            vmem((stretches, slice_rows, span), bf16),
            vmem((extent, content), f32),
            vmem((groups, parts, chunk, span), bf16),
            vmem((groups, parts, chunk, span), bf16),
            vmem((extent, content), f32),
            vmem((chunk, features), f32),
            vmem((groups, 2, chunk // 2, span), bf16),
            vmem((chunk, features), bf16),
            *[vmem(value.shape, value.dtype) for value in inputs[1:]],
            dma((1,)),
            dma((GATHER_WAITS,)),
            dma((1,)),
            dma((GATHER_WAITS,)),
            dma((1,)),
            dma((1,)),
            dma((1,)),
            dma((2,)),
            dma((1,)),
            dma((2, 3)),
            dma((2,)),
            dma((2,)),
            dma((2,)),
            dma((1,)),
            dma((1,)),
            dma((1,)),
            dma((1,)),
            dma((1,)),
            dma((2,)),
            dma((1,)),
            dma((4,)),
            dma((4,)),
            dma((2,)),
            dma((4,)),
            dma((14,)),
        ],
        cost_estimate=pl.CostEstimate(
            flops=int(3e10), bytes_accessed=1 << 20, transcendentals=0
        ),
        compiler_params=pltpu.CompilerParams(
            collective_id=1, has_side_effects=True, vmem_limit_bytes=VMEM_LIMIT
        ),
    )(*inputs)


def solution(mesh):
    return jax.shard_map(
        on_device,
        mesh=mesh,
        in_specs=(
            P(("sp", "tp"), None),
            P(),
            P("sp", "tp"),
            P("sp", "tp"),
            P("sp", "tp"),
            P("sp", "tp"),
            P("sp", "tp"),
            P("sp", "tp"),
            P(None, "tp"),
            P(None, "tp"),
            P(None, "tp"),
            P(None, "tp"),
            P(None, "tp"),
            P("tp"),
            P("tp", "sp"),
        ),
        out_specs=P(("sp", "tp"), None),
        check_vma=False,
    )
```

```python
import functools
import math

import jax
import jax.numpy as jnp
from jax import lax
from jax.experimental import pallas as pl
from jax.experimental.pallas import tpu as pltpu
from jax.sharding import PartitionSpec as P

HEAD_DIM = 64
STATE = 128
BLOCK = 128
LANES = 128
EPSILON = 1e-06
HIGHEST = lax.Precision.HIGHEST
VMEM_LIMIT = 60 * 1024 * 1024
SIDE = 4


def rms_rows(values):
    wide = values.astype(jnp.float32)
    return wide * lax.rsqrt(jnp.mean(wide * wide, axis=-1, keepdims=True) + EPSILON)


def softplus(values):
    return jnp.maximum(values, 0.0) + jnp.log1p(jnp.exp(-jnp.abs(values)))


def spread(columns, first, count):
    rows = columns.shape[0]
    lane = lax.broadcasted_iota(jnp.int32, (rows, LANES), 1)
    tiles = []
    for at in range(first, first + count, 2):
        low = jnp.broadcast_to(columns[:, at : at + 1], (rows, LANES))
        high = jnp.broadcast_to(columns[:, at + 1 : at + 2], (rows, LANES))
        tiles.append(jnp.where(lane < HEAD_DIM, low, high))
    return jnp.concatenate(tiles, axis=1)


def silu(values):
    half = 0.5 * values
    return half + half * jnp.tanh(half)


def greet(peers):
    barrier = pltpu.get_barrier_semaphore()
    for peer in peers:
        pl.semaphore_signal(
            barrier, inc=1, device_id=peer, device_id_type=pl.DeviceIdType.MESH
        )
    return lambda: pl.semaphore_wait(barrier, len(peers))


def remote(source, target, send, receive, peer):
    return pltpu.make_async_remote_copy(
        src_ref=source,
        dst_ref=target,
        send_sem=send,
        recv_sem=receive,
        device_id=peer,
        device_id_type=pl.DeviceIdType.MESH,
    )


def place():
    me = lax.axis_index("sp")
    return me // (2 * SIDE), me // 2 % SIDE, me % 2


def plane_gather(whole, half, many, send, receive):
    z, y, c = place()
    part = lax.axis_index("tp")

    def origin(first, second):
        over_z = (z + c * first + (1 - c) * second + 2 * SIDE) % SIDE
        over_y = (y + (1 - c) * first + c * second + 2 * SIDE) % SIDE
        return (over_z * SIDE + over_y) * 2 + c

    along = [(origin(1, 0), part), (origin(-1, 0), part)]
    cross = [(origin(0, 1), part), (origin(0, -1), part)]
    partner = ((z * SIDE + y) * 2 + 1 - c, part)
    lines = (0, -1, 1, 2)
    at_line, at_far, at_shared, at_over, at_last = 0, 1, 2, 3, 7

    def go(block, peer, kind):
        remote(block, block, send.at[0], receive.at[kind], peer).start()

    def arrived(shards, kind):
        remote(many(shards), many(shards), send.at[0], receive.at[kind], partner).wait_recv()

    def share(at):
        go(whole(at), partner, at_shared)

    def spread_line(first):
        for peer in cross:
            go(whole(origin(first, 0)), peer, at_over + lines.index(first))
        share(origin(first, 0))

    def forward(first):
        arrived(2, at_over + lines.index(first))
        for way in range(2):
            go(half(origin(first, (-1, 1)[way]), way), cross[way], at_last + lines.index(first))
        for way in range(2):
            share(origin(first, (-1, 1)[way]))

    for peer in along:
        go(whole(origin(0, 0)), peer, at_line)
    spread_line(0)
    yield
    arrived(2, at_line)
    for way in range(2):
        go(half(origin((-1, 1)[way], 0), way), along[way], at_far)
    for way in range(2):
        spread_line((-1, 1)[way])
    yield
    forward(0)
    yield
    arrived(1, at_far)
    spread_line(2)
    yield
    forward(-1)
    yield
    forward(1)
    yield
    forward(2)
    yield
    for at, first in enumerate(lines):
        arrived(1, at_last + at)
        share(origin(first, 2))
    yield
    arrived(16, at_shared)
    yield
    remote(many(31), many(31), send.at[0], receive.at[at_line], partner).wait_send()
    yield


GATHER_WAITS = 11


def mixer_kernel(
    shift,
    x_ref,
    norm_gain_from,
    gate_weights_from,
    value_weights_from,
    in_weights_from,
    out_weights_from,
    ahead_weights_from,
    behind_weights_from,
    offset_from,
    speed_from,
    taps_value_from,
    taps_in_from,
    taps_out_from,
    gain_from,
    w_out_from,
    result_ref,
    tokens,
    weights,
    full_out,
    placed,
    paired,
    padded,
    gates,
    scale_ref,
    outer_steps,
    halo,
    signal_ref,
    inward_ref,
    outward_ref,
    within_ref,
    rows_ref,
    block_states_ref,
    block_logs_ref,
    sent,
    slices,
    log_tiles,
    all_logs,
    returned,
    incoming,
    total,
    staged,
    mixed,
    wide_gates,
    summed_ref,
    relay,
    raw_tokens,
    norm_gain_ref,
    gate_weights_ref,
    value_weights_ref,
    in_weights_ref,
    out_weights_ref,
    ahead_weights_ref,
    behind_weights_ref,
    offset_ref,
    speed_ref,
    taps_value_ref,
    taps_in_ref,
    taps_out_ref,
    gain_ref,
    w_out_ref,
    weights_send,
    weights_receive,
    out_send,
    out_receive,
    pair_send,
    pair_receive,
    cross_send,
    cross_receive,
    token_send,
    token_receive,
    onward_receive,
    halo_send,
    halo_receive,
    logs_send,
    logs_receive,
    scan_send,
    scan_receive,
    back_send,
    back_receive,
    mixed_send,
    mixed_receive,
    relay_receive,
    handed_receive,
    load,
    inputs_load,
):
    me, part = lax.axis_index("sp"), lax.axis_index("tp")
    core = me % 2
    stretches = slices.shape[0]
    parts, chunk, features = tokens.shape
    extent = parts * chunk
    depth = value_weights_ref.shape[0]
    content = value_weights_ref.shape[1]
    state_width = in_weights_ref.shape[1]
    heads = ahead_weights_ref.shape[0]
    groups = state_width // STATE
    ratio = heads // groups
    span = ratio * HEAD_DIM
    channels = content + 2 * state_width
    count = extent // BLOCK
    f32, bf16 = jnp.float32, jnp.bfloat16

    peers = [((me + hop) % stretches, part) for hop in range(1, stretches)]
    across = [(me, (part + hop) % parts) for hop in range(1, parts)]
    settle = greet(peers + across)

    quarter = chunk // 4
    loads = []
    for at in (0, 3, 1, 2):
        here = pl.ds(at * quarter, quarter)
        copy = pltpu.make_async_copy(x_ref.at[here], raw_tokens.at[here], load.at[at])
        copy.start()
        loads.append(copy)
    fetched = []
    for at, (source, target) in enumerate(
        (
            (norm_gain_from, norm_gain_ref),
            (gate_weights_from, gate_weights_ref),
            (value_weights_from, value_weights_ref),
            (in_weights_from, in_weights_ref),
            (out_weights_from, out_weights_ref),
            (ahead_weights_from, ahead_weights_ref),
            (behind_weights_from, behind_weights_ref),
            (offset_from, offset_ref),
            (speed_from, speed_ref),
            (taps_value_from, taps_value_ref),
            (taps_in_from, taps_in_ref),
            (taps_out_from, taps_out_ref),
            (gain_from, gain_ref),
            (w_out_from, w_out_ref),
        )
    ):
        copy = pltpu.make_async_copy(source, target, inputs_load.at[at])
        copy.start()
        fetched.append(copy)
    rows = 16

    def normalize(at):
        for step in range(quarter // rows):
            here = pl.ds(at * quarter + step * rows, rows)
            normed = rms_rows(raw_tokens[here, :]) * norm_gain_ref[...]
            tokens[part, here, :] = normed.astype(bf16)

    fetched[0].wait()
    for at, copy in zip((0, 3), loads[:2]):
        copy.wait()
        normalize(at)
    settle()

    right, left = (me, (part + 1) % parts), (me, (part + parts - 1) % parts)
    before, after = (part + parts - 1) % parts, (part + 1) % parts
    opposite = (part + 2) % parts

    def piece(source, at):
        return tokens.at[source, pl.ds(at * quarter, quarter)]

    orders = ((0, 1, 2, 3), (3, 2, 1, 0))

    def arrived(block, semaphore):
        remote(block, block, semaphore, semaphore, right).wait_recv()

    def left_here(block, semaphore):
        remote(block, block, semaphore, semaphore, right).wait_send()

    def send_own(step):
        for way, peer in enumerate((right, left)):
            block = piece(part, orders[way][step])
            received = token_receive.at[way, min(step, 2)]
            remote(block, block, token_send.at[0], received, peer).start()

    def pass_on(step):
        for way, peer in enumerate((right, left)):
            block = piece((before, after)[way], orders[way][step])
            arrived(block, token_receive.at[way, step])
            remote(block, block, token_send.at[0], onward_receive.at[step], peer).start()

    weights_steps = plane_gather(
        lambda at: weights.at[pl.ds(pl.multiple_of(at * depth, depth), depth)],
        lambda at, side: weights.at[
            pl.ds(pl.multiple_of(at * depth + side * (depth // 2), depth // 2), depth // 2)
        ],
        lambda shards: weights.at[pl.ds(0, shards * depth)],
        weights_send,
        weights_receive,
    )
    out_steps = plane_gather(
        lambda at: full_out.at[at],
        lambda at, side: full_out.at[at, pl.ds(side * (parts // 2), parts // 2)],
        lambda shards: full_out.at[pl.ds(0, shards)],
        out_send,
        out_receive,
    )

    z, y, _ = place()
    partner = ((z * SIDE + y) * 2 + 1 - core, part)
    pair = remote(placed.at[1 - core], paired, pair_send.at[0], pair_receive.at[0], partner)
    send_own(0)
    for copy in fetched[1:7]:
        copy.wait()
    own_rows = pl.ds(pl.multiple_of(me * depth, depth), depth)
    weights[own_rows, 0:content] = value_weights_ref[...]
    weights[own_rows, content : content + state_width] = in_weights_ref[...]
    weights[own_rows, content + state_width : channels] = out_weights_ref[...]
    weights[own_rows, channels : channels + content] = gate_weights_ref[...]

    def across_rows(left, right):
        return lax.dot_general(left, right, (((0,), (0,)), ((), ())), preferred_element_type=f32)

    head_row = lax.broadcasted_iota(jnp.int32, (heads, LANES), 0)
    head_lane = lax.broadcasted_iota(jnp.int32, (heads, LANES), 1)
    to_ahead = (head_row == head_lane).astype(bf16)
    to_behind = (head_row + heads == head_lane).astype(bf16)
    weights[own_rows, channels + content :] = (
        across_rows(ahead_weights_ref[...], to_ahead)
        + across_rows(behind_weights_ref[...], to_behind)
    ).astype(bf16)
    next(weights_steps)
    width = w_out_ref.shape[0]
    move_row = lax.broadcasted_iota(jnp.int32, (width, LANES), 0)
    move_lane = lax.broadcasted_iota(jnp.int32, (width, LANES), 1)
    to_half = (move_row + core * width == move_lane).astype(bf16)
    half_rows = w_out_ref.shape[1] // 2
    fetched[13].wait()
    for side in range(2):
        placed[side] = across_rows(
            w_out_ref[:, side * half_rows : (side + 1) * half_rows], to_half
        ).astype(bf16)
    pair.start()
    loads[2].wait()
    normalize(1)
    pair.wait_recv()
    full_out[me, part] = placed[core] + paired[...]
    loads[3].wait()
    normalize(2)
    for peer in (right, left):
        block = full_out.at[me, part]
        remote(block, block, cross_send.at[0], cross_receive.at[0], peer).start()
    send_own(1)
    next(weights_steps)
    next(weights_steps)
    both = full_out.at[me, pl.ds(0, 2)]
    arrived(both, cross_receive.at[0])
    block = full_out.at[me, (part + 3 + 2 * core) % parts]
    onward_peer = (me, (part + 1 + 2 * core) % parts)
    remote(block, block, cross_send.at[0], cross_receive.at[1], onward_peer).start()
    send_own(2)
    send_own(3)
    next(weights_steps)
    pass_on(0)
    next(weights_steps)
    next(weights_steps)
    pass_on(1)
    next(weights_steps)
    arrived(full_out.at[me, 0], cross_receive.at[1])
    next(out_steps)
    next(weights_steps)
    next(weights_steps)

    wide_tile = 2 * LANES

    def product(source, columns):
        return jnp.dot(tokens[source], weights[:, columns], preferred_element_type=f32)

    row = lax.broadcasted_iota(jnp.int32, (BLOCK, BLOCK), 0)
    column = lax.broadcasted_iota(jnp.int32, (BLOCK, BLOCK), 1)
    for copy in fetched[7:13]:
        copy.wait()
    triangles = jnp.concatenate([row >= column, row <= column], axis=0).astype(bf16)
    lane = lax.broadcasted_iota(jnp.int32, (1, LANES), 1)
    spare = jnp.zeros((1, LANES - 2 * heads), f32)
    offset = jnp.concatenate([offset_ref[0:1, :], offset_ref[1:2, :], spare], axis=1)
    rate = jnp.concatenate([speed_ref[0:1, :], speed_ref[1:2, :], spare], axis=1)

    def decays_of(source, raw):
        steps = softplus(raw + offset - shift)
        logs = -steps * rate
        logs = jnp.concatenate([logs[:BLOCK], logs[BLOCK:]], axis=1)
        high = logs.astype(bf16)
        rest = logs - high.astype(f32)
        middle = rest.astype(bf16)
        low = (rest - middle.astype(f32)).astype(bf16)
        sums = jnp.dot(
            triangles,
            jnp.concatenate([high, middle, low], axis=1),
            preferred_element_type=f32,
        )
        sums = sums[:, : 2 * LANES] + (
            sums[:, 2 * LANES : 4 * LANES] + sums[:, 4 * LANES : 6 * LANES]
        )
        for inner in range(2):
            at = 2 * source + inner
            here = pl.ds(pl.multiple_of(at * BLOCK, BLOCK), BLOCK)
            lanes_of = slice(inner * LANES, (inner + 1) * LANES)
            within = jnp.where(lane < heads, sums[:BLOCK, lanes_of], sums[BLOCK:, lanes_of])
            final = jnp.where(lane < heads, within[BLOCK - 1 : BLOCK], within[0:1])
            step = steps[inner * BLOCK : (inner + 1) * BLOCK]
            within_ref[here, :] = within
            rows_ref[0 : 2 * heads, here] = within.T[0 : 2 * heads]
            rows_ref[2 * heads : 4 * heads, here] = step.T[0 : 2 * heads]
            scale_ref[here, :] = jnp.exp(final - within) * step
            for group in range(groups):
                block_logs_ref[group, at] = jnp.concatenate(
                    [spread(final, way * heads + group * ratio, ratio) for way in range(2)],
                    axis=1,
                )

    def project(source):
        start = pl.multiple_of(source * chunk, chunk)
        raw = product(source, slice(channels + content, channels + content + LANES))
        decays_of(source, raw.astype(bf16).astype(f32))

        for first in range(0, channels, wide_tile):
            columns = slice(first, first + wide_tile)
            padded[pl.ds(start + 8, chunk), columns] = (
                product(source, columns).astype(bf16).astype(f32)
            )
    def project_quarters(source, at, firsts, rest=None):
        start = pl.multiple_of(source * chunk, chunk)
        halves = [tokens[source, place * quarter : (place + 1) * quarter] for place in at]
        left_side = jnp.concatenate(halves, axis=0)

        def some(columns):
            made = jnp.dot(left_side, weights[:, columns], preferred_element_type=f32)
            return made.astype(bf16).astype(f32)

        if rest is not False:
            raw = some(slice(channels + content, channels + content + LANES))
        if rest is None:
            outer_steps[...] = raw
        elif rest is not False:
            outer = rest[...]
            decays_of(source, jnp.concatenate([outer[:quarter], raw, outer[quarter:]], axis=0))
        for first in firsts:
            columns = slice(first, first + wide_tile)
            made = some(columns)
            for half_at, place in enumerate(at):
                padded[pl.ds(start + 8 + place * quarter, quarter), columns] = made[
                    half_at * quarter : (half_at + 1) * quarter
                ]

    def project_gate(source):
        start = pl.multiple_of(source * chunk, chunk)

        for first in range(0, content, wide_tile):
            gates[pl.ds(start, chunk), first : first + wide_tile] = product(
                source, slice(channels + first, channels + first + wide_tile)
            ).astype(bf16)

    has_next, has_last = me < stretches - 1, me > 0
    sends_to, takes_from = (has_next, has_last), (has_last, has_next)

    def edge_copy(way):
        peer = ((me + (1, stretches - 1)[way]) % stretches, part)
        block = padded.at[pl.ds((extent, 8)[way], 8)]
        return remote(block, halo.at[way], halo_send.at[way], halo_receive.at[way], peer)

    def send_edge(way, when):
        @pl.when(jnp.logical_and(when, sends_to[way]))
        def _():
            edge_copy(way).start()

    def take_edges():
        for way in range(2):
            beyond = pl.ds((0, extent + 8)[way], 8)

            @pl.when(takes_from[way])
            def _():
                edge_copy(way).wait_recv()
                padded[beyond, :] = halo[way]

            @pl.when(jnp.logical_not(takes_from[way]))
            def _():
                padded[beyond, :] = jnp.zeros((8, channels), f32)

            @pl.when(sends_to[way])
            def _():
                edge_copy(way).wait_send()

    def filter_columns(start, first, width):
        part_rows = padded[pl.ds(start, BLOCK + 16), first : first + width]
        if first < content:
            taps = taps_value_ref[:, first : first + width]
        elif first < content + state_width:
            taps = taps_in_ref[:, first - content : first - content + width]
        else:
            base = first - content - state_width
            taps = taps_out_ref[:, base : base + width]
        mixed_rows = (
            taps[0:1] * part_rows[7 : 7 + BLOCK]
            + taps[1:2] * part_rows[8 : 8 + BLOCK]
            + taps[2:3] * part_rows[9 : 9 + BLOCK]
        )
        return silu(mixed_rows).astype(bf16)

    def filter_outward(at):
        start = pl.multiple_of(at * BLOCK, BLOCK)
        for first in range(0, state_width, wide_tile):
            outward_ref[pl.ds(start, BLOCK), first : first + wide_tile] = filter_columns(
                start, content + state_width + first, wide_tile
            )

    def block(at, group):
        start = pl.multiple_of(at * BLOCK, BLOCK)
        here = pl.ds(start, BLOCK)
        signal = filter_columns(start, group * span, span)
        inward = filter_columns(start, content + group * STATE, STATE)
        signal_ref[here, group * span : (group + 1) * span] = signal
        inward_ref[here, group * STATE : (group + 1) * STATE] = inward
        scale = scale_ref[here, :]
        wide = signal.astype(f32)
        scaled = jnp.concatenate(
            [wide * spread(scale, way * heads + group * ratio, ratio) for way in range(2)],
            axis=1,
        ).astype(bf16)
        block_states_ref[group, at] = lax.dot_general(
            inward, scaled, (((0,), (0,)), ((), ())), preferred_element_type=f32
        )

    project(part)
    project_gate(part)
    next(out_steps)
    next(out_steps)
    arrived(tokens.at[0, pl.ds(0, 2 * quarter)], token_receive.at[0, 2])
    project(before)
    project_gate(before)
    arrived(tokens.at[0, pl.ds(0, 2 * quarter)], token_receive.at[1, 2])
    project(after)

    early = part % 3 == 0

    send_edge(0, part != 1)
    send_edge(1, part != 2)
    project_gate(after)
    arrived(tokens.at[0, pl.ds(0, 2 * quarter)], onward_receive.at[0])
    project_quarters(opposite, (0, 3), range(0, channels, wide_tile))
    send_edge(0, part == 1)
    send_edge(1, part == 2)
    next(out_steps)
    ahead_of_last = 2 * opposite + 3
    turn = 2 - 2 * (part // 3)

    def early_block(step, _):
        at = (ahead_of_last + (step + turn) % 4) % count
        for group in range(groups):
            block(at, group)
        filter_outward(at)
        return 0

    early_block(0, 0)
    early_block(1, 0)
    @pl.when(part % 3 != 0)
    def _():
        early_block(2, 0)
        early_block(3, 0)

    arrived(tokens.at[0, pl.ds(0, 2 * quarter)], onward_receive.at[1])
    project_quarters(opposite, (1, 2), (0, content), outer_steps)
    summed_logs = [
        functools.reduce(jnp.add, [block_logs_ref[group, at] for at in range(count)])
        for group in range(groups)
    ]
    for way in range(2):
        for group in range(groups):
            for lane_tile in range(span // LANES):
                first = way * span + lane_tile * LANES
                log_tiles[way * groups + group, lane_tile : lane_tile + 1, :] = summed_logs[group][
                    :, first : first + LANES
                ]
    handled = stretches // (2 * groups)
    for peer in peers:
        remote(
            log_tiles.at[peer[0] // handled],
            all_logs.at[me],
            logs_send.at[0],
            logs_receive.at[0],
            peer,
        ).start()
    all_logs[me] = log_tiles[me // handled]
    late_turn = 2 * (part // 2) * (1 - part % 2)

    def late_at(step):
        return (ahead_of_last + 4 + (step + late_turn) % 4) % count

    def late_block(step, group):
        block(late_at(step), group)

    slice_rows = sent.shape[1]
    per_state = STATE // slice_rows
    my_group = me // handled % groups
    my_index = me % handled + handled * (me // (groups * handled))

    def final_states(group):
        for way in range(2):
            order = range(count) if way == 0 else range(count - 1, -1, -1)
            for lane_tile in range(span // LANES):
                first = way * span + lane_tile * LANES
                state = jnp.zeros((STATE, LANES), f32)
                for at in order:
                    state = (
                        state * jnp.exp(block_logs_ref[group, at, :, first : first + LANES])
                        + block_states_ref[group, at, :, first : first + LANES]
                    )
                at_slice = (way * groups + group) * per_state
                here = slice(lane_tile * LANES, (lane_tile + 1) * LANES)
                sent[at_slice : at_slice + per_state, :, here] = state.astype(bf16).reshape(
                    per_state, slice_rows, LANES
                )

    def send_slices(group):
        scanners = 2 * handled
        for hop in range(scanners):
            index = (my_index + hop) % scanners
            target = index // handled * (groups * handled) + group * handled + index % handled

            def send():
                remote(
                    sent.at[target],
                    slices.at[me],
                    scan_send.at[0],
                    scan_receive.at[0],
                    (target, part),
                ).start()

            if hop:
                send()
            else:
                pl.when(my_group != group)(send)

        @pl.when(my_group == group)
        def _():
            slices[me] = sent[me]

    late_block(0, 0)
    late_block(1, 0)

    def early_at(step):
        return (ahead_of_last + (step + turn) % 4) % count

    @pl.when(early)
    def _():
        take_edges()
        block(early_at(2), 0)
        block(early_at(3), 0)

    @pl.when(part % 3 != 0)
    def _():
        take_edges()

    late_block(2, 0)
    late_block(3, 0)
    final_states(0)
    send_slices(0)
    project_quarters(opposite, (1, 2), (span, content + state_width), False)
    @pl.when(early)
    def _():
        for step in range(2, 4):
            block(early_at(step), 1)
            filter_outward(early_at(step))

    for step in range(4):
        late_block(step, 1)
    final_states(1)
    send_slices(1)

    def keep_entries(group):
        def onward(at, carried):
            return enter(at, 0, *carried)

        def back(at, carried):
            return enter(count - 1 - at, span, *carried)

        def enter(at, base, state, logs):
            added = block_states_ref[group, at, :, base : base + span]
            decay = block_logs_ref[group, at, :, base : base + span]
            block_states_ref[group, at, :, base : base + span] = state
            block_logs_ref[group, at, :, base : base + span] = logs
            return state * jnp.exp(decay) + added, logs + decay

        empty = jnp.zeros((STATE, span), f32)
        still = jnp.zeros((1, span), f32)
        for body in (onward, back):
            lax.fori_loop(0, count, body, (empty, still))

    lanes = lax.broadcasted_iota(jnp.int32, (BLOCK, LANES), 1)

    def diagonal(at, _):
        here = pl.ds(pl.multiple_of(at * BLOCK, BLOCK), BLOCK)
        within = within_ref[here, :]
        wide_gates[here, :] = silu(gates[here, :].astype(f32))
        for group in range(groups):
            intersect = lax.dot_general(
                outward_ref[here, group * STATE : (group + 1) * STATE],
                inward_ref[here, group * STATE : (group + 1) * STATE],
                (((1,), (1,)), ((), ())),
                preferred_element_type=f32,
            )
            products = []
            for head in range(group * ratio, (group + 1) * ratio):
                other = heads + head
                gap_ahead = within[:, head : head + 1] - rows_ref[head : head + 1, here]
                gap_behind = within[:, other : other + 1] - rows_ref[other : other + 1, here]
                step_ahead = rows_ref[2 * heads + head : 2 * heads + head + 1, here]
                step_behind = rows_ref[2 * heads + other : 2 * heads + other + 1, here]
                gap = jnp.where(row >= column, gap_ahead, gap_behind)
                step = jnp.where(
                    row > column,
                    step_ahead,
                    jnp.where(row < column, step_behind, step_ahead + step_behind),
                )
                mixing = (intersect * jnp.exp(gap) * step).astype(bf16)
                tile = head // 2 * 2 * HEAD_DIM
                products.append(
                    jnp.dot(
                        mixing,
                        signal_ref[here, tile : tile + LANES],
                        preferred_element_type=f32,
                    )
                )
            for two in range(ratio // 2):
                at_tile = (group * ratio + 2 * two) * HEAD_DIM
                total[here, at_tile : at_tile + LANES] = jnp.where(
                    lanes < HEAD_DIM, products[2 * two], products[2 * two + 1]
                )
        return 0

    project_gate(opposite)

    def late_outward(step, _):
        filter_outward(late_at(step))
        return 0

    lax.fori_loop(0, 4, late_outward, 0)
    reverse = me // (stretches // 2)

    def scan_slices(group):
        arrived(all_logs.at[pl.ds(0, stretches - 1)], logs_receive.at[0])
        arrived(slices.at[pl.ds(0, stretches - 1)], scan_receive.at[0])

        def scan(step, state):
            for inner in range(4):
                at = 4 * step + inner
                source = at + reverse * (stretches - 1 - 2 * at)
                returned[source] = state.astype(bf16)
                logs = jnp.concatenate(
                    [all_logs[source, tile : tile + 1, :] for tile in range(span // LANES)],
                    axis=1,
                )
                state = state * jnp.exp(logs) + slices[source].astype(f32)
            return state

        lax.fori_loop(0, stretches // 4, scan, jnp.zeros((slice_rows, span), f32))
        for peer in peers:
            remote(
                returned.at[peer[0]],
                incoming.at[me],
                back_send.at[0],
                back_receive.at[group],
                peer,
            ).start()
        incoming[me] = returned[me]

    def take_incoming(group):
        scanners = 2 * handled

        @pl.when(my_group == group)
        def _():
            arrived(incoming.at[pl.ds(0, scanners - 1)], back_receive.at[group])

        @pl.when(my_group != group)
        def _():
            arrived(incoming.at[pl.ds(0, scanners)], back_receive.at[group])

    @pl.when(my_group == 0)
    def _():
        scan_slices(0)

    for group in range(groups):
        keep_entries(group)
    lax.fori_loop(0, 3 * count // 4, diagonal, 0)

    @pl.when(my_group == 1)
    def _():
        scan_slices(1)

    lax.fori_loop(3 * count // 4, count, diagonal, 0)
    take_incoming(0)
    for _ in range(3):
        next(out_steps)
    def carried_in(way, group):
        first = (way * groups + group) * per_state
        return incoming[first : first + per_state].reshape(STATE, span).astype(f32)

    def finish(source, inner, group):
        at = source * (chunk // BLOCK) + inner
        here = pl.ds(pl.multiple_of(at * BLOCK, BLOCK), BLOCK)
        decays = jnp.exp(within_ref[here, :])
        wide = slice(group * span, (group + 1) * span)
        summed = total[here, wide]
        for way in range(2):
            base = way * span
            state = block_states_ref[group, at, :, base : base + span] + jnp.exp(
                block_logs_ref[group, at, :, base : base + span]
            ) * carried_in(way, group)
            carried = jnp.dot(
                outward_ref[here, group * STATE : (group + 1) * STATE],
                state.astype(bf16),
                preferred_element_type=f32,
            )
            summed += carried * spread(decays, way * heads + group * ratio, ratio)
        gated = summed * wide_gates[here, wide]
        scale = lax.rsqrt(jnp.mean(gated * gated, axis=-1, keepdims=True) + EPSILON)
        staged[group, source, pl.ds(inner * BLOCK, BLOCK), :] = (
            gated * scale * gain_ref[:, wide]
        ).astype(bf16)

    sides = (right, left)
    half_chunk = chunk // 2

    def half_of(at):
        return pl.ds(at * half_chunk, half_chunk)

    def send_mixed(group):
        for way in range(2):
            finish(opposite, way, group)
            remote(
                staged.at[group, opposite, half_of(way)],
                relay.at[group, way],
                mixed_send.at[0],
                relay_receive.at[2 * group + way],
                sides[way],
            ).start()
        for at in range(2):
            for way, target in enumerate((after, before)):
                finish(target, at, group)
                remote(
                    staged.at[group, target, half_of(at)],
                    mixed.at[group, part, half_of(at)],
                    mixed_send.at[0],
                    mixed_receive.at[2 * group + way],
                    sides[way],
                ).start()

    def pass_mixed(group):
        for way in range(2):
            arrived(relay.at[group, way], relay_receive.at[2 * group + way])
            remote(
                relay.at[group, way],
                mixed.at[group, (before, after)[way], half_of(way)],
                mixed_send.at[0],
                handed_receive.at[group],
                sides[way],
            ).start()

    send_mixed(0)
    take_incoming(1)
    send_mixed(1)
    pass_mixed(0)
    for group in range(groups):
        for at in range(2):
            finish(part, at, group)
    next(out_steps)
    pass_mixed(1)
    next(out_steps)

    def output(terms, first, last):
        broad = 8 * LANES

        def tile(at, _):
            columns = pl.ds(pl.multiple_of(at * broad, broad), broad)
            summed = 0.0 if first else summed_ref[:, columns]
            for block_of, group, source in terms:
                weight = jnp.concatenate(
                    [full_out[16 * at + 2 * place + group, source] for place in range(8)], axis=1
                )
                summed += jnp.dot(
                    block_of[group, source], weight, preferred_element_type=f32
                )
            if last:
                result_ref[:, columns] = summed.astype(bf16)
            else:
                summed_ref[:, columns] = summed
            return 0

        lax.fori_loop(0, features // broad, tile, 0)

    def take_sides(group):
        arrived(mixed.at[group, before], mixed_receive.at[2 * group])
        arrived(mixed.at[group, after], mixed_receive.at[2 * group + 1])

    take_sides(0)
    output(
        [(staged, 0, part), (staged, 1, part), (mixed, 0, before), (mixed, 0, after)],
        True,
        False,
    )
    take_sides(1)
    arrived(mixed.at[0, opposite], handed_receive.at[0])
    output([(mixed, 1, before), (mixed, 1, after), (mixed, 0, opposite)], False, False)
    arrived(mixed.at[1, opposite], handed_receive.at[1])
    output([(mixed, 1, opposite)], False, True)
    next(weights_steps)
    next(out_steps)
    pair.wait_send()
    left_here(full_out.at[0, pl.ds(0, 3)], cross_send.at[0])
    left_here(tokens.at[pl.ds(0, 3)], token_send.at[0])
    left_here(all_logs.at[pl.ds(0, stretches - 1)], logs_send.at[0])
    left_here(slices.at[pl.ds(0, stretches - 1)], scan_send.at[0])
    left_here(incoming.at[pl.ds(0, stretches - 1)], back_send.at[0])
    left_here(mixed, mixed_send.at[0])


def on_device(
    input_activations,
    norm_gain,
    w_gate,
    w_value,
    w_state_in,
    w_state_out,
    w_step_forward,
    w_step_backward,
    step_offset,
    fading_speed,
    conv_value,
    conv_state_in,
    conv_state_out,
    out_gain,
    w_out,
):
    stretches = lax.axis_size("sp")
    parts = lax.axis_size("tp")
    chunk, features = input_activations.shape
    extent = parts * chunk
    depth = w_gate.shape[0]
    content = w_value.shape[1]
    state_width = w_state_in.shape[1]
    heads = w_step_forward.shape[1]
    groups = state_width // STATE
    span = heads // groups * HEAD_DIM
    channels = content + 2 * state_width
    count = extent // BLOCK
    slice_rows = 2 * groups * STATE // stretches
    shift = math.log(extent * stretches)
    bf16, f32 = jnp.bfloat16, jnp.float32
    vmem, dma = pltpu.VMEM, pltpu.SemaphoreType.DMA
    space = pl.BlockSpec(memory_space=pltpu.VMEM)
    half_rows = w_out.shape[0] // 2
    inputs = (
        input_activations,
        norm_gain.reshape(1, features),
        w_gate,
        w_value,
        w_state_in,
        w_state_out,
        w_step_forward.T,
        w_step_backward.T,
        step_offset,
        fading_speed,
        conv_value,
        conv_state_in,
        conv_state_out,
        out_gain.reshape(1, content),
        w_out.T,
    )
    return pl.pallas_call(
        functools.partial(mixer_kernel, shift),
        out_shape=pltpu.VMEM((chunk, features), bf16),
        in_specs=[pl.BlockSpec(memory_space=pl.ANY)] * 15,
        out_specs=space,
        scratch_shapes=[
            vmem((parts, chunk, features), bf16),
            vmem((stretches * depth, channels + content + LANES), bf16),
            vmem((stretches, parts, half_rows, LANES), bf16),
            vmem((2, half_rows, LANES), bf16),
            vmem((half_rows, LANES), bf16),
            vmem((extent + 16, channels), f32),
            vmem((extent, content), bf16),
            vmem((extent, LANES), f32),
            vmem((chunk // 2, LANES), f32),
            vmem((2, 8, channels), f32),
            vmem((extent, content), bf16),
            vmem((extent, state_width), bf16),
            vmem((extent, state_width), bf16),
            vmem((extent, LANES), f32),
            vmem((4 * heads, extent), f32),
            vmem((groups, count, STATE, 2 * span), f32),
            vmem((groups, count, 1, 2 * span), f32),
            vmem((stretches, slice_rows, span), bf16),
            vmem((stretches, slice_rows, span), bf16),
            vmem((2 * groups, 8, LANES), f32),
            vmem((stretches, 8, LANES), f32),
            vmem((stretches, slice_rows, span), bf16),
            vmem((stretches, slice_rows, span), bf16),
            vmem((extent, content), f32),
            vmem((groups, parts, chunk, span), bf16),
            vmem((groups, parts, chunk, span), bf16),
            vmem((extent, content), f32),
            vmem((chunk, features), f32),
            vmem((groups, 2, chunk // 2, span), bf16),
            vmem((chunk, features), bf16),
            *[vmem(value.shape, value.dtype) for value in inputs[1:]],
            dma((1,)),
            dma((GATHER_WAITS,)),
            dma((1,)),
            dma((GATHER_WAITS,)),
            dma((1,)),
            dma((1,)),
            dma((1,)),
            dma((2,)),
            dma((1,)),
            dma((2, 3)),
            dma((2,)),
            dma((2,)),
            dma((2,)),
            dma((1,)),
            dma((1,)),
            dma((1,)),
            dma((1,)),
            dma((1,)),
            dma((2,)),
            dma((1,)),
            dma((4,)),
            dma((4,)),
            dma((2,)),
            dma((4,)),
            dma((14,)),
        ],
        cost_estimate=pl.CostEstimate(
            flops=int(3e10), bytes_accessed=1 << 20, transcendentals=0
        ),
        compiler_params=pltpu.CompilerParams(
            collective_id=1, has_side_effects=True, vmem_limit_bytes=VMEM_LIMIT
        ),
    )(*inputs)


def solution(mesh):
    return jax.shard_map(
        on_device,
        mesh=mesh,
        in_specs=(
            P(("sp", "tp"), None),
            P(),
            P("sp", "tp"),
            P("sp", "tp"),
            P("sp", "tp"),
            P("sp", "tp"),
            P("sp", "tp"),
            P("sp", "tp"),
            P(None, "tp"),
            P(None, "tp"),
            P(None, "tp"),
            P(None, "tp"),
            P(None, "tp"),
            P("tp"),
            P("tp", "sp"),
        ),
        out_specs=P(("sp", "tp"), None),
        check_vma=False,
    )
```

```python
import functools
import math

import jax
import jax.numpy as jnp
from jax import lax
from jax.experimental import pallas as pl
from jax.experimental.pallas import tpu as pltpu
from jax.sharding import PartitionSpec as P

HEAD_DIM = 64
STATE = 128
BLOCK = 128
LANES = 128
EPSILON = 1e-06
HIGHEST = lax.Precision.HIGHEST
VMEM_LIMIT = 60 * 1024 * 1024
SIDE = 4


def rms_rows(values):
    wide = values.astype(jnp.float32)
    return wide * lax.rsqrt(jnp.mean(wide * wide, axis=-1, keepdims=True) + EPSILON)


def softplus(values):
    return jnp.maximum(values, 0.0) + jnp.log1p(jnp.exp(-jnp.abs(values)))


def spread(columns, first, count):
    rows = columns.shape[0]
    lane = lax.broadcasted_iota(jnp.int32, (rows, LANES), 1)
    tiles = []
    for at in range(first, first + count, 2):
        low = jnp.broadcast_to(columns[:, at : at + 1], (rows, LANES))
        high = jnp.broadcast_to(columns[:, at + 1 : at + 2], (rows, LANES))
        tiles.append(jnp.where(lane < HEAD_DIM, low, high))
    return jnp.concatenate(tiles, axis=1)


def silu(values):
    half = 0.5 * values
    return half + half * jnp.tanh(half)


def greet(peers):
    barrier = pltpu.get_barrier_semaphore()
    for peer in peers:
        pl.semaphore_signal(
            barrier, inc=1, device_id=peer, device_id_type=pl.DeviceIdType.MESH
        )
    return lambda: pl.semaphore_wait(barrier, len(peers))


def remote(source, target, send, receive, peer):
    return pltpu.make_async_remote_copy(
        src_ref=source,
        dst_ref=target,
        send_sem=send,
        recv_sem=receive,
        device_id=peer,
        device_id_type=pl.DeviceIdType.MESH,
    )


def place():
    me = lax.axis_index("sp")
    return me // (2 * SIDE), me // 2 % SIDE, me % 2


def plane_gather(whole, half, many, send, receive):
    z, y, c = place()
    part = lax.axis_index("tp")

    def origin(first, second):
        over_z = (z + c * first + (1 - c) * second + 2 * SIDE) % SIDE
        over_y = (y + (1 - c) * first + c * second + 2 * SIDE) % SIDE
        return (over_z * SIDE + over_y) * 2 + c

    along = [(origin(1, 0), part), (origin(-1, 0), part)]
    cross = [(origin(0, 1), part), (origin(0, -1), part)]
    partner = ((z * SIDE + y) * 2 + 1 - c, part)
    lines = (0, -1, 1, 2)
    at_line, at_far, at_shared, at_over, at_last = 0, 1, 2, 3, 7

    def go(block, peer, kind):
        remote(block, block, send.at[0], receive.at[kind], peer).start()

    def arrived(shards, kind):
        remote(many(shards), many(shards), send.at[0], receive.at[kind], partner).wait_recv()

    def share(at):
        go(whole(at), partner, at_shared)

    def spread_line(first):
        for peer in cross:
            go(whole(origin(first, 0)), peer, at_over + lines.index(first))
        share(origin(first, 0))

    def forward(first):
        arrived(2, at_over + lines.index(first))
        for way in range(2):
            go(half(origin(first, (-1, 1)[way]), way), cross[way], at_last + lines.index(first))
        for way in range(2):
            share(origin(first, (-1, 1)[way]))

    for peer in along:
        go(whole(origin(0, 0)), peer, at_line)
    spread_line(0)
    yield
    arrived(2, at_line)
    for way in range(2):
        go(half(origin((-1, 1)[way], 0), way), along[way], at_far)
    for way in range(2):
        spread_line((-1, 1)[way])
    yield
    forward(0)
    yield
    arrived(1, at_far)
    spread_line(2)
    yield
    forward(-1)
    yield
    forward(1)
    yield
    forward(2)
    yield
    for at, first in enumerate(lines):
        arrived(1, at_last + at)
        share(origin(first, 2))
    yield
    arrived(16, at_shared)
    yield
    remote(many(31), many(31), send.at[0], receive.at[at_line], partner).wait_send()
    yield


GATHER_WAITS = 11


def mixer_kernel(
    shift,
    x_ref,
    norm_gain_from,
    gate_weights_from,
    value_weights_from,
    in_weights_from,
    out_weights_from,
    ahead_weights_from,
    behind_weights_from,
    offset_from,
    speed_from,
    taps_value_from,
    taps_in_from,
    taps_out_from,
    gain_from,
    w_out_from,
    result_ref,
    tokens,
    weights,
    full_out,
    placed,
    paired,
    padded,
    gates,
    scale_ref,
    outer_steps,
    halo,
    signal_ref,
    inward_ref,
    outward_ref,
    within_ref,
    rows_ref,
    block_states_ref,
    block_logs_ref,
    sent,
    slices,
    log_tiles,
    all_logs,
    returned,
    incoming,
    total,
    staged,
    mixed,
    wide_gates,
    summed_ref,
    relay,
    raw_tokens,
    norm_gain_ref,
    gate_weights_ref,
    value_weights_ref,
    in_weights_ref,
    out_weights_ref,
    ahead_weights_ref,
    behind_weights_ref,
    offset_ref,
    speed_ref,
    taps_value_ref,
    taps_in_ref,
    taps_out_ref,
    gain_ref,
    w_out_ref,
    weights_send,
    weights_receive,
    out_send,
    out_receive,
    pair_send,
    pair_receive,
    cross_send,
    cross_receive,
    token_send,
    token_receive,
    onward_receive,
    halo_send,
    halo_receive,
    logs_send,
    logs_receive,
    scan_send,
    scan_receive,
    back_send,
    back_receive,
    mixed_send,
    mixed_receive,
    relay_receive,
    handed_receive,
    load,
    inputs_load,
):
    me, part = lax.axis_index("sp"), lax.axis_index("tp")
    core = me % 2
    stretches = slices.shape[0]
    parts, chunk, features = tokens.shape
    extent = parts * chunk
    depth = value_weights_ref.shape[0]
    content = value_weights_ref.shape[1]
    state_width = in_weights_ref.shape[1]
    heads = ahead_weights_ref.shape[0]
    groups = state_width // STATE
    ratio = heads // groups
    span = ratio * HEAD_DIM
    channels = content + 2 * state_width
    count = extent // BLOCK
    f32, bf16 = jnp.float32, jnp.bfloat16

    peers = [((me + hop) % stretches, part) for hop in range(1, stretches)]
    across = [(me, (part + hop) % parts) for hop in range(1, parts)]
    settle = greet(peers + across)

    quarter = chunk // 4
    loads = []
    for at in (0, 3, 1, 2):
        here = pl.ds(at * quarter, quarter)
        copy = pltpu.make_async_copy(x_ref.at[here], raw_tokens.at[here], load.at[at])
        copy.start()
        loads.append(copy)
    fetched = []
    for at, (source, target) in enumerate(
        (
            (norm_gain_from, norm_gain_ref),
            (gate_weights_from, gate_weights_ref),
            (value_weights_from, value_weights_ref),
            (in_weights_from, in_weights_ref),
            (out_weights_from, out_weights_ref),
            (ahead_weights_from, ahead_weights_ref),
            (behind_weights_from, behind_weights_ref),
            (offset_from, offset_ref),
            (speed_from, speed_ref),
            (taps_value_from, taps_value_ref),
            (taps_in_from, taps_in_ref),
            (taps_out_from, taps_out_ref),
            (gain_from, gain_ref),
            (w_out_from, w_out_ref),
        )
    ):
        copy = pltpu.make_async_copy(source, target, inputs_load.at[at])
        copy.start()
        fetched.append(copy)
    rows = 16

    def normalize(at):
        for step in range(quarter // rows):
            here = pl.ds(at * quarter + step * rows, rows)
            normed = rms_rows(raw_tokens[here, :]) * norm_gain_ref[...]
            tokens[part, here, :] = normed.astype(bf16)

    fetched[0].wait()
    for at, copy in zip((0, 3), loads[:2]):
        copy.wait()
        normalize(at)
    settle()

    right, left = (me, (part + 1) % parts), (me, (part + parts - 1) % parts)
    before, after = (part + parts - 1) % parts, (part + 1) % parts
    opposite = (part + 2) % parts

    def piece(source, at):
        return tokens.at[source, pl.ds(at * quarter, quarter)]

    orders = ((0, 1, 2, 3), (3, 2, 1, 0))

    def arrived(block, semaphore):
        remote(block, block, semaphore, semaphore, right).wait_recv()

    def left_here(block, semaphore):
        remote(block, block, semaphore, semaphore, right).wait_send()

    def send_own(step):
        for way, peer in enumerate((right, left)):
            block = piece(part, orders[way][step])
            received = token_receive.at[way, min(step, 2)]
            remote(block, block, token_send.at[0], received, peer).start()

    def pass_on(step):
        for way, peer in enumerate((right, left)):
            block = piece((before, after)[way], orders[way][step])
            arrived(block, token_receive.at[way, step])
            remote(block, block, token_send.at[0], onward_receive.at[step], peer).start()

    weights_steps = plane_gather(
        lambda at: weights.at[pl.ds(pl.multiple_of(at * depth, depth), depth)],
        lambda at, side: weights.at[
            pl.ds(pl.multiple_of(at * depth + side * (depth // 2), depth // 2), depth // 2)
        ],
        lambda shards: weights.at[pl.ds(0, shards * depth)],
        weights_send,
        weights_receive,
    )
    out_steps = plane_gather(
        lambda at: full_out.at[at],
        lambda at, side: full_out.at[at, pl.ds(side * (parts // 2), parts // 2)],
        lambda shards: full_out.at[pl.ds(0, shards)],
        out_send,
        out_receive,
    )

    z, y, _ = place()
    partner = ((z * SIDE + y) * 2 + 1 - core, part)
    pair = remote(placed.at[1 - core], paired, pair_send.at[0], pair_receive.at[0], partner)
    send_own(0)
    for copy in fetched[1:7]:
        copy.wait()
    own_rows = pl.ds(pl.multiple_of(me * depth, depth), depth)
    weights[own_rows, 0:content] = value_weights_ref[...]
    weights[own_rows, content : content + state_width] = in_weights_ref[...]
    weights[own_rows, content + state_width : channels] = out_weights_ref[...]
    weights[own_rows, channels : channels + content] = gate_weights_ref[...]

    def across_rows(left, right):
        return lax.dot_general(left, right, (((0,), (0,)), ((), ())), preferred_element_type=f32)

    head_row = lax.broadcasted_iota(jnp.int32, (heads, LANES), 0)
    head_lane = lax.broadcasted_iota(jnp.int32, (heads, LANES), 1)
    to_ahead = (head_row == head_lane).astype(bf16)
    to_behind = (head_row + heads == head_lane).astype(bf16)
    weights[own_rows, channels + content :] = (
        across_rows(ahead_weights_ref[...], to_ahead)
        + across_rows(behind_weights_ref[...], to_behind)
    ).astype(bf16)
    next(weights_steps)
    width = w_out_ref.shape[0]
    move_row = lax.broadcasted_iota(jnp.int32, (width, LANES), 0)
    move_lane = lax.broadcasted_iota(jnp.int32, (width, LANES), 1)
    to_half = (move_row + core * width == move_lane).astype(bf16)
    half_rows = w_out_ref.shape[1] // 2
    fetched[13].wait()
    for side in range(2):
        placed[side] = across_rows(
            w_out_ref[:, side * half_rows : (side + 1) * half_rows], to_half
        ).astype(bf16)
    pair.start()
    loads[2].wait()
    normalize(1)
    pair.wait_recv()
    full_out[me, part] = placed[core] + paired[...]
    loads[3].wait()
    normalize(2)
    for peer in (right, left):
        block = full_out.at[me, part]
        remote(block, block, cross_send.at[0], cross_receive.at[0], peer).start()
    send_own(1)
    next(weights_steps)
    next(weights_steps)
    both = full_out.at[me, pl.ds(0, 2)]
    arrived(both, cross_receive.at[0])
    block = full_out.at[me, (part + 3 + 2 * core) % parts]
    onward_peer = (me, (part + 1 + 2 * core) % parts)
    remote(block, block, cross_send.at[0], cross_receive.at[1], onward_peer).start()
    send_own(2)
    send_own(3)
    next(weights_steps)
    pass_on(0)
    next(weights_steps)
    next(weights_steps)
    pass_on(1)
    next(weights_steps)
    arrived(full_out.at[me, 0], cross_receive.at[1])
    next(out_steps)
    next(weights_steps)
    next(weights_steps)

    wide_tile = 2 * LANES

    def product(source, columns):
        return jnp.dot(tokens[source], weights[:, columns], preferred_element_type=f32)

    row = lax.broadcasted_iota(jnp.int32, (BLOCK, BLOCK), 0)
    column = lax.broadcasted_iota(jnp.int32, (BLOCK, BLOCK), 1)
    for copy in fetched[7:13]:
        copy.wait()
    triangles = jnp.concatenate([row >= column, row <= column], axis=0).astype(bf16)
    lane = lax.broadcasted_iota(jnp.int32, (1, LANES), 1)
    spare = jnp.zeros((1, LANES - 2 * heads), f32)
    offset = jnp.concatenate([offset_ref[0:1, :], offset_ref[1:2, :], spare], axis=1)
    rate = jnp.concatenate([speed_ref[0:1, :], speed_ref[1:2, :], spare], axis=1)

    def decays_of(source, raw):
        steps = softplus(raw + offset - shift)
        logs = -steps * rate
        logs = jnp.concatenate([logs[:BLOCK], logs[BLOCK:]], axis=1)
        high = logs.astype(bf16)
        rest = logs - high.astype(f32)
        middle = rest.astype(bf16)
        low = (rest - middle.astype(f32)).astype(bf16)
        sums = jnp.dot(
            triangles,
            jnp.concatenate([high, middle, low], axis=1),
            preferred_element_type=f32,
        )
        sums = sums[:, : 2 * LANES] + (
            sums[:, 2 * LANES : 4 * LANES] + sums[:, 4 * LANES : 6 * LANES]
        )
        for inner in range(2):
            at = 2 * source + inner
            here = pl.ds(pl.multiple_of(at * BLOCK, BLOCK), BLOCK)
            lanes_of = slice(inner * LANES, (inner + 1) * LANES)
            within = jnp.where(lane < heads, sums[:BLOCK, lanes_of], sums[BLOCK:, lanes_of])
            final = jnp.where(lane < heads, within[BLOCK - 1 : BLOCK], within[0:1])
            step = steps[inner * BLOCK : (inner + 1) * BLOCK]
            within_ref[here, :] = within
            rows_ref[0 : 2 * heads, here] = within.T[0 : 2 * heads]
            rows_ref[2 * heads : 4 * heads, here] = step.T[0 : 2 * heads]
            scale_ref[here, :] = jnp.exp(final - within) * step
            for group in range(groups):
                block_logs_ref[group, at] = jnp.concatenate(
                    [spread(final, way * heads + group * ratio, ratio) for way in range(2)],
                    axis=1,
                )

    def project(source):
        start = pl.multiple_of(source * chunk, chunk)
        raw = product(source, slice(channels + content, channels + content + LANES))
        decays_of(source, raw.astype(bf16).astype(f32))

        for first in range(0, channels, wide_tile):
            columns = slice(first, first + wide_tile)
            padded[pl.ds(start + 8, chunk), columns] = (
                product(source, columns).astype(bf16).astype(f32)
            )
    def project_quarters(source, at, firsts, rest=None):
        start = pl.multiple_of(source * chunk, chunk)
        halves = [tokens[source, place * quarter : (place + 1) * quarter] for place in at]
        left_side = jnp.concatenate(halves, axis=0)

        def some(columns):
            made = jnp.dot(left_side, weights[:, columns], preferred_element_type=f32)
            return made.astype(bf16).astype(f32)

        if rest is not False:
            raw = some(slice(channels + content, channels + content + LANES))
        if rest is None:
            outer_steps[...] = raw
        elif rest is not False:
            outer = rest[...]
            decays_of(source, jnp.concatenate([outer[:quarter], raw, outer[quarter:]], axis=0))
        for first in firsts:
            columns = slice(first, first + wide_tile)
            made = some(columns)
            for half_at, place in enumerate(at):
                padded[pl.ds(start + 8 + place * quarter, quarter), columns] = made[
                    half_at * quarter : (half_at + 1) * quarter
                ]

    def project_gate(source):
        start = pl.multiple_of(source * chunk, chunk)

        for first in range(0, content, wide_tile):
            gates[pl.ds(start, chunk), first : first + wide_tile] = product(
                source, slice(channels + first, channels + first + wide_tile)
            ).astype(bf16)

    has_next, has_last = me < stretches - 1, me > 0
    sends_to, takes_from = (has_next, has_last), (has_last, has_next)

    def edge_copy(way):
        peer = ((me + (1, stretches - 1)[way]) % stretches, part)
        block = padded.at[pl.ds((extent, 8)[way], 8)]
        return remote(block, halo.at[way], halo_send.at[way], halo_receive.at[way], peer)

    def send_edge(way, when):
        @pl.when(jnp.logical_and(when, sends_to[way]))
        def _():
            edge_copy(way).start()

    def take_edges():
        for way in range(2):
            beyond = pl.ds((0, extent + 8)[way], 8)

            @pl.when(takes_from[way])
            def _():
                edge_copy(way).wait_recv()
                padded[beyond, :] = halo[way]

            @pl.when(jnp.logical_not(takes_from[way]))
            def _():
                padded[beyond, :] = jnp.zeros((8, channels), f32)

            @pl.when(sends_to[way])
            def _():
                edge_copy(way).wait_send()

    def filter_columns(start, first, width):
        part_rows = padded[pl.ds(start, BLOCK + 16), first : first + width]
        if first < content:
            taps = taps_value_ref[:, first : first + width]
        elif first < content + state_width:
            taps = taps_in_ref[:, first - content : first - content + width]
        else:
            base = first - content - state_width
            taps = taps_out_ref[:, base : base + width]
        mixed_rows = (
            taps[0:1] * part_rows[7 : 7 + BLOCK]
            + taps[1:2] * part_rows[8 : 8 + BLOCK]
            + taps[2:3] * part_rows[9 : 9 + BLOCK]
        )
        return silu(mixed_rows).astype(bf16)

    def filter_outward(at):
        start = pl.multiple_of(at * BLOCK, BLOCK)
        for first in range(0, state_width, wide_tile):
            outward_ref[pl.ds(start, BLOCK), first : first + wide_tile] = filter_columns(
                start, content + state_width + first, wide_tile
            )

    def block(at, group):
        start = pl.multiple_of(at * BLOCK, BLOCK)
        here = pl.ds(start, BLOCK)
        signal = filter_columns(start, group * span, span)
        inward = filter_columns(start, content + group * STATE, STATE)
        signal_ref[here, group * span : (group + 1) * span] = signal
        inward_ref[here, group * STATE : (group + 1) * STATE] = inward
        scale = scale_ref[here, :]
        wide = signal.astype(f32)
        scaled = jnp.concatenate(
            [wide * spread(scale, way * heads + group * ratio, ratio) for way in range(2)],
            axis=1,
        ).astype(bf16)
        block_states_ref[group, at] = lax.dot_general(
            inward, scaled, (((0,), (0,)), ((), ())), preferred_element_type=f32
        )

    project(part)
    project_gate(part)
    next(out_steps)
    next(out_steps)
    arrived(tokens.at[0, pl.ds(0, 2 * quarter)], token_receive.at[0, 2])
    project(before)
    project_gate(before)
    arrived(tokens.at[0, pl.ds(0, 2 * quarter)], token_receive.at[1, 2])
    project(after)

    early = part % 3 == 0

    send_edge(0, part != 1)
    send_edge(1, part != 2)
    project_gate(after)
    arrived(tokens.at[0, pl.ds(0, 2 * quarter)], onward_receive.at[0])
    project_quarters(opposite, (0, 3), range(0, channels, wide_tile))
    send_edge(0, part == 1)
    send_edge(1, part == 2)
    next(out_steps)
    ahead_of_last = 2 * opposite + 3
    turn = 2 - 2 * (part // 3)

    def early_block(step, _):
        at = (ahead_of_last + (step + turn) % 4) % count
        for group in range(groups):
            block(at, group)
        filter_outward(at)
        return 0

    early_block(0, 0)
    early_block(1, 0)
    @pl.when(part % 3 != 0)
    def _():
        early_block(2, 0)
        early_block(3, 0)

    arrived(tokens.at[0, pl.ds(0, 2 * quarter)], onward_receive.at[1])
    project_quarters(opposite, (1, 2), (0, content), outer_steps)
    summed_logs = [
        functools.reduce(jnp.add, [block_logs_ref[group, at] for at in range(count)])
        for group in range(groups)
    ]
    for way in range(2):
        for group in range(groups):
            for lane_tile in range(span // LANES):
                first = way * span + lane_tile * LANES
                log_tiles[way * groups + group, lane_tile : lane_tile + 1, :] = summed_logs[group][
                    :, first : first + LANES
                ]
    handled = stretches // (2 * groups)
    for peer in peers:
        remote(
            log_tiles.at[peer[0] // handled],
            all_logs.at[me],
            logs_send.at[0],
            logs_receive.at[0],
            peer,
        ).start()
    all_logs[me] = log_tiles[me // handled]
    late_turn = 2 * (part // 2) * (1 - part % 2)

    def late_at(step):
        return (ahead_of_last + 4 + (step + late_turn) % 4) % count

    def late_block(step, group):
        block(late_at(step), group)

    slice_rows = sent.shape[1]
    per_state = STATE // slice_rows
    my_group = me // handled % groups
    my_index = me % handled + handled * (me // (groups * handled))

    def final_states(group):
        for way in range(2):
            order = range(count) if way == 0 else range(count - 1, -1, -1)
            for lane_tile in range(span // LANES):
                first = way * span + lane_tile * LANES
                state = jnp.zeros((STATE, LANES), f32)
                for at in order:
                    state = (
                        state * jnp.exp(block_logs_ref[group, at, :, first : first + LANES])
                        + block_states_ref[group, at, :, first : first + LANES]
                    )
                at_slice = (way * groups + group) * per_state
                here = slice(lane_tile * LANES, (lane_tile + 1) * LANES)
                sent[at_slice : at_slice + per_state, :, here] = state.astype(bf16).reshape(
                    per_state, slice_rows, LANES
                )

    def send_slices(group):
        scanners = 2 * handled
        for hop in range(scanners):
            index = (my_index + hop) % scanners
            target = index // handled * (groups * handled) + group * handled + index % handled

            def send():
                remote(
                    sent.at[target],
                    slices.at[me],
                    scan_send.at[0],
                    scan_receive.at[0],
                    (target, part),
                ).start()

            if hop:
                send()
            else:
                pl.when(my_group != group)(send)

        @pl.when(my_group == group)
        def _():
            slices[me] = sent[me]

    late_block(0, 0)
    late_block(1, 0)

    def early_at(step):
        return (ahead_of_last + (step + turn) % 4) % count

    @pl.when(early)
    def _():
        take_edges()
        block(early_at(2), 0)
        block(early_at(3), 0)

    @pl.when(part % 3 != 0)
    def _():
        take_edges()

    late_block(2, 0)
    late_block(3, 0)
    final_states(0)
    send_slices(0)
    project_quarters(opposite, (1, 2), (span, content + state_width), False)
    @pl.when(early)
    def _():
        for step in range(2, 4):
            block(early_at(step), 1)
            filter_outward(early_at(step))

    for step in range(4):
        late_block(step, 1)
    final_states(1)
    send_slices(1)

    def keep_entries(group):
        def onward(at, carried):
            return enter(at, 0, *carried)

        def back(at, carried):
            return enter(count - 1 - at, span, *carried)

        def enter(at, base, state, logs):
            added = block_states_ref[group, at, :, base : base + span]
            decay = block_logs_ref[group, at, :, base : base + span]
            block_states_ref[group, at, :, base : base + span] = state
            block_logs_ref[group, at, :, base : base + span] = logs
            return state * jnp.exp(decay) + added, logs + decay

        empty = jnp.zeros((STATE, span), f32)
        still = jnp.zeros((1, span), f32)
        for body in (onward, back):
            lax.fori_loop(0, count, body, (empty, still))

    lanes = lax.broadcasted_iota(jnp.int32, (BLOCK, LANES), 1)

    def diagonal(at, _):
        here = pl.ds(pl.multiple_of(at * BLOCK, BLOCK), BLOCK)
        within = within_ref[here, :]
        wide_gates[here, :] = silu(gates[here, :].astype(f32))
        for group in range(groups):
            intersect = lax.dot_general(
                outward_ref[here, group * STATE : (group + 1) * STATE],
                inward_ref[here, group * STATE : (group + 1) * STATE],
                (((1,), (1,)), ((), ())),
                preferred_element_type=f32,
            )
            products = []
            for head in range(group * ratio, (group + 1) * ratio):
                other = heads + head
                gap_ahead = within[:, head : head + 1] - rows_ref[head : head + 1, here]
                gap_behind = within[:, other : other + 1] - rows_ref[other : other + 1, here]
                step_ahead = rows_ref[2 * heads + head : 2 * heads + head + 1, here]
                step_behind = rows_ref[2 * heads + other : 2 * heads + other + 1, here]
                gap = jnp.where(row >= column, gap_ahead, gap_behind)
                step = jnp.where(
                    row > column,
                    step_ahead,
                    jnp.where(row < column, step_behind, step_ahead + step_behind),
                )
                mixing = (intersect * jnp.exp(gap) * step).astype(bf16)
                tile = head // 2 * 2 * HEAD_DIM
                products.append(
                    jnp.dot(
                        mixing,
                        signal_ref[here, tile : tile + LANES],
                        preferred_element_type=f32,
                    )
                )
            for two in range(ratio // 2):
                at_tile = (group * ratio + 2 * two) * HEAD_DIM
                total[here, at_tile : at_tile + LANES] = jnp.where(
                    lanes < HEAD_DIM, products[2 * two], products[2 * two + 1]
                )
        return 0


    def late_outward(step, _):
        filter_outward(late_at(step))
        return 0

    lax.fori_loop(0, 4, late_outward, 0)
    reverse = me // (stretches // 2)

    def scan_slices(group):
        arrived(all_logs.at[pl.ds(0, stretches - 1)], logs_receive.at[0])
        arrived(slices.at[pl.ds(0, stretches - 1)], scan_receive.at[0])

        def scan(step, state):
            for inner in range(4):
                at = 4 * step + inner
                source = at + reverse * (stretches - 1 - 2 * at)
                returned[source] = state.astype(bf16)
                logs = jnp.concatenate(
                    [all_logs[source, tile : tile + 1, :] for tile in range(span // LANES)],
                    axis=1,
                )
                state = state * jnp.exp(logs) + slices[source].astype(f32)
            return state

        lax.fori_loop(0, stretches // 4, scan, jnp.zeros((slice_rows, span), f32))
        for peer in peers:
            remote(
                returned.at[peer[0]],
                incoming.at[me],
                back_send.at[0],
                back_receive.at[group],
                peer,
            ).start()
        incoming[me] = returned[me]

    def take_incoming(group):
        scanners = 2 * handled

        @pl.when(my_group == group)
        def _():
            arrived(incoming.at[pl.ds(0, scanners - 1)], back_receive.at[group])

        @pl.when(my_group != group)
        def _():
            arrived(incoming.at[pl.ds(0, scanners)], back_receive.at[group])

    @pl.when(my_group == 0)
    def _():
        scan_slices(0)

    project_gate(opposite)
    for group in range(groups):
        keep_entries(group)
    lax.fori_loop(0, 3 * count // 4, diagonal, 0)

    @pl.when(my_group == 1)
    def _():
        scan_slices(1)

    lax.fori_loop(3 * count // 4, count, diagonal, 0)
    take_incoming(0)
    for _ in range(3):
        next(out_steps)
    def carried_in(way, group):
        first = (way * groups + group) * per_state
        return incoming[first : first + per_state].reshape(STATE, span).astype(f32)

    def finish(source, inner, group):
        at = source * (chunk // BLOCK) + inner
        here = pl.ds(pl.multiple_of(at * BLOCK, BLOCK), BLOCK)
        decays = jnp.exp(within_ref[here, :])
        wide = slice(group * span, (group + 1) * span)
        summed = total[here, wide]
        for way in range(2):
            base = way * span
            state = block_states_ref[group, at, :, base : base + span] + jnp.exp(
                block_logs_ref[group, at, :, base : base + span]
            ) * carried_in(way, group)
            carried = jnp.dot(
                outward_ref[here, group * STATE : (group + 1) * STATE],
                state.astype(bf16),
                preferred_element_type=f32,
            )
            summed += carried * spread(decays, way * heads + group * ratio, ratio)
        gated = summed * wide_gates[here, wide]
        scale = lax.rsqrt(jnp.mean(gated * gated, axis=-1, keepdims=True) + EPSILON)
        staged[group, source, pl.ds(inner * BLOCK, BLOCK), :] = (
            gated * scale * gain_ref[:, wide]
        ).astype(bf16)

    sides = (right, left)
    half_chunk = chunk // 2

    def half_of(at):
        return pl.ds(at * half_chunk, half_chunk)

    def send_mixed(group):
        for way in range(2):
            finish(opposite, way, group)
            remote(
                staged.at[group, opposite, half_of(way)],
                relay.at[group, way],
                mixed_send.at[0],
                relay_receive.at[2 * group + way],
                sides[way],
            ).start()
        for at in range(2):
            for way, target in enumerate((after, before)):
                finish(target, at, group)
                remote(
                    staged.at[group, target, half_of(at)],
                    mixed.at[group, part, half_of(at)],
                    mixed_send.at[0],
                    mixed_receive.at[2 * group + way],
                    sides[way],
                ).start()

    def pass_mixed(group):
        for way in range(2):
            arrived(relay.at[group, way], relay_receive.at[2 * group + way])
            remote(
                relay.at[group, way],
                mixed.at[group, (before, after)[way], half_of(way)],
                mixed_send.at[0],
                handed_receive.at[group],
                sides[way],
            ).start()

    send_mixed(0)
    take_incoming(1)
    send_mixed(1)
    pass_mixed(0)
    for group in range(groups):
        for at in range(2):
            finish(part, at, group)
    next(out_steps)
    pass_mixed(1)
    next(out_steps)

    def output(terms, first, last):
        broad = 8 * LANES

        def tile(at, _):
            columns = pl.ds(pl.multiple_of(at * broad, broad), broad)
            summed = 0.0 if first else summed_ref[:, columns]
            for block_of, group, source in terms:
                weight = jnp.concatenate(
                    [full_out[16 * at + 2 * place + group, source] for place in range(8)], axis=1
                )
                summed += jnp.dot(
                    block_of[group, source], weight, preferred_element_type=f32
                )
            if last:
                result_ref[:, columns] = summed.astype(bf16)
            else:
                summed_ref[:, columns] = summed
            return 0

        lax.fori_loop(0, features // broad, tile, 0)

    def take_sides(group):
        arrived(mixed.at[group, before], mixed_receive.at[2 * group])
        arrived(mixed.at[group, after], mixed_receive.at[2 * group + 1])

    take_sides(0)
    output(
        [(staged, 0, part), (staged, 1, part), (mixed, 0, before), (mixed, 0, after)],
        True,
        False,
    )
    take_sides(1)
    arrived(mixed.at[0, opposite], handed_receive.at[0])
    output([(mixed, 1, before), (mixed, 1, after), (mixed, 0, opposite)], False, False)
    arrived(mixed.at[1, opposite], handed_receive.at[1])
    output([(mixed, 1, opposite)], False, True)
    next(weights_steps)
    next(out_steps)
    pair.wait_send()
    left_here(full_out.at[0, pl.ds(0, 3)], cross_send.at[0])
    left_here(tokens.at[pl.ds(0, 3)], token_send.at[0])
    left_here(all_logs.at[pl.ds(0, stretches - 1)], logs_send.at[0])
    left_here(slices.at[pl.ds(0, stretches - 1)], scan_send.at[0])
    left_here(incoming.at[pl.ds(0, stretches - 1)], back_send.at[0])
    left_here(mixed, mixed_send.at[0])


def on_device(
    input_activations,
    norm_gain,
    w_gate,
    w_value,
    w_state_in,
    w_state_out,
    w_step_forward,
    w_step_backward,
    step_offset,
    fading_speed,
    conv_value,
    conv_state_in,
    conv_state_out,
    out_gain,
    w_out,
):
    stretches = lax.axis_size("sp")
    parts = lax.axis_size("tp")
    chunk, features = input_activations.shape
    extent = parts * chunk
    depth = w_gate.shape[0]
    content = w_value.shape[1]
    state_width = w_state_in.shape[1]
    heads = w_step_forward.shape[1]
    groups = state_width // STATE
    span = heads // groups * HEAD_DIM
    channels = content + 2 * state_width
    count = extent // BLOCK
    slice_rows = 2 * groups * STATE // stretches
    shift = math.log(extent * stretches)
    bf16, f32 = jnp.bfloat16, jnp.float32
    vmem, dma = pltpu.VMEM, pltpu.SemaphoreType.DMA
    space = pl.BlockSpec(memory_space=pltpu.VMEM)
    half_rows = w_out.shape[0] // 2
    inputs = (
        input_activations,
        norm_gain.reshape(1, features),
        w_gate,
        w_value,
        w_state_in,
        w_state_out,
        w_step_forward.T,
        w_step_backward.T,
        step_offset,
        fading_speed,
        conv_value,
        conv_state_in,
        conv_state_out,
        out_gain.reshape(1, content),
        w_out.T,
    )
    return pl.pallas_call(
        functools.partial(mixer_kernel, shift),
        out_shape=pltpu.VMEM((chunk, features), bf16),
        in_specs=[pl.BlockSpec(memory_space=pl.ANY)] * 15,
        out_specs=space,
        scratch_shapes=[
            vmem((parts, chunk, features), bf16),
            vmem((stretches * depth, channels + content + LANES), bf16),
            vmem((stretches, parts, half_rows, LANES), bf16),
            vmem((2, half_rows, LANES), bf16),
            vmem((half_rows, LANES), bf16),
            vmem((extent + 16, channels), f32),
            vmem((extent, content), bf16),
            vmem((extent, LANES), f32),
            vmem((chunk // 2, LANES), f32),
            vmem((2, 8, channels), f32),
            vmem((extent, content), bf16),
            vmem((extent, state_width), bf16),
            vmem((extent, state_width), bf16),
            vmem((extent, LANES), f32),
            vmem((4 * heads, extent), f32),
            vmem((groups, count, STATE, 2 * span), f32),
            vmem((groups, count, 1, 2 * span), f32),
            vmem((stretches, slice_rows, span), bf16),
            vmem((stretches, slice_rows, span), bf16),
            vmem((2 * groups, 8, LANES), f32),
            vmem((stretches, 8, LANES), f32),
            vmem((stretches, slice_rows, span), bf16),
            vmem((stretches, slice_rows, span), bf16),
            vmem((extent, content), f32),
            vmem((groups, parts, chunk, span), bf16),
            vmem((groups, parts, chunk, span), bf16),
            vmem((extent, content), f32),
            vmem((chunk, features), f32),
            vmem((groups, 2, chunk // 2, span), bf16),
            vmem((chunk, features), bf16),
            *[vmem(value.shape, value.dtype) for value in inputs[1:]],
            dma((1,)),
            dma((GATHER_WAITS,)),
            dma((1,)),
            dma((GATHER_WAITS,)),
            dma((1,)),
            dma((1,)),
            dma((1,)),
            dma((2,)),
            dma((1,)),
            dma((2, 3)),
            dma((2,)),
            dma((2,)),
            dma((2,)),
            dma((1,)),
            dma((1,)),
            dma((1,)),
            dma((1,)),
            dma((1,)),
            dma((2,)),
            dma((1,)),
            dma((4,)),
            dma((4,)),
            dma((2,)),
            dma((4,)),
            dma((14,)),
        ],
        cost_estimate=pl.CostEstimate(
            flops=int(3e10), bytes_accessed=1 << 20, transcendentals=0
        ),
        compiler_params=pltpu.CompilerParams(
            collective_id=1, has_side_effects=True, vmem_limit_bytes=VMEM_LIMIT
        ),
    )(*inputs)


def solution(mesh):
    return jax.shard_map(
        on_device,
        mesh=mesh,
        in_specs=(
            P(("sp", "tp"), None),
            P(),
            P("sp", "tp"),
            P("sp", "tp"),
            P("sp", "tp"),
            P("sp", "tp"),
            P("sp", "tp"),
            P("sp", "tp"),
            P(None, "tp"),
            P(None, "tp"),
            P(None, "tp"),
            P(None, "tp"),
            P(None, "tp"),
            P("tp"),
            P("tp", "sp"),
        ),
        out_specs=P(("sp", "tp"), None),
        check_vma=False,
    )
```
